256 devices in a mesh: grp: 2 (over z), sp: 16 (over y, core), tp: 8 (over x).
Axes of the slice: x: 8, y: 8, z: 2, core: 2. Of those that a mesh axis runs over, the one named last changes fastest.
The devices are a block of a 8x8x16 slice.
Arguments:
- residual: bfloat16 [32768, 2048], P(('grp', 'sp', 'tp')), parts along dimension 0, may hold values from -6 to 6
- grouped_value_heads: bfloat16 [32768, 2, 1024], P(('grp', 'sp'), None, 'tp'), parts along dimension 0, may hold values from -6 to 6
- output_gate_heads: bfloat16 [32768, 2, 1024], P(('grp', 'sp'), None, 'tp'), parts along dimension 0, may hold values from -6 to 6
- projected_key_query: bfloat16 [32768, 384], P(('grp', 'sp')), parts along dimension 0, may hold values from -6 to 6
- raw_step_size: bfloat16 [32768, 2, 16], P(('grp', 'sp'), None, 'tp'), parts along dimension 0, may hold values from -3 to 3
- step_size_bias: float32 [2, 16], P(None, 'tp'), may hold values from -1 to 0.5
- head_decay_logarithm: float32 [2, 16], P(None, 'tp'), may hold values from -16 to -2
- position_extra_decay: float32 [32768], P(('grp', 'sp')), parts along dimension 0, may hold values from -0.7 to 0
- head_skip_weight: float32 [2, 16], P(None, 'tp'), may hold values from 0.5 to 2
- value_kernel_taps: bfloat16 [4, 2, 1024], P(None, None, 'tp'), may hold values from -3 to 3
- key_query_kernel: bfloat16 [4, 384], replicated, may hold values from -3 to 3
- head_norm_gain: float32 [2, 1024], P(None, 'tp'), may hold values from 0.1 to 1.9
- output_matrix: bfloat16 [2, 1024, 2048], P(None, 'tp'), may hold values from -0.125 to 0.125
- expert_norm_gain: float32 [2048], replicated, may hold values from 0.1 to 1.9
- expert_gate_weight: bfloat16 [16, 2048, 4096], P('sp', None, 'tp'), may hold values from -0.125 to 0.125
- expert_up_weight: bfloat16 [16, 2048, 4096], P('sp', None, 'tp'), may hold values from -0.125 to 0.125
- expert_down_weight: bfloat16 [16, 4096, 2048], P('sp', 'tp'), may hold values from -0.09375 to 0.09375
- token_expert_choice: int32 [32768, 2], P(('grp', 'sp', 'tp')), parts along dimension 0, may hold values from 0 to 15, all different within a row; in each aligned block of 128 rows (0 to 127, 128 to 255, ...) at most 17 rows name the same one
- expert_output_weight: float32 [32768, 2], P(('grp', 'sp', 'tp')), parts along dimension 0, may hold values from 0.2 to 1
Outputs:
- layer_out: bfloat16 [32768, 2048], P(('grp', 'sp', 'tp')), parts along dimension 0
The draws below stay inside these ranges and needn't reach their ends.
There are 2 independent parts, one for each index of `grp`. The reference program is written for one: setup_inputs(seed, part) draws one part's arguments, and reference() takes and returns one part's arrays. A program takes and returns all parts, laid end to end along the dimension named above; an argument that names none is the same for every part. Nothing has to cross between parts.
Inputs may be any that keep to these rules, and one draw needn't show every extreme that they name: `token_expert_choice`: each row names two different experts. The token rows of one device name one expert at most 17 times.
All inputs are finite; a program needn't handle non-finite values.
Results may differ from the reference program's by a relative error of at most 0.015.
Values may be sent and summed in bfloat16 or wider, within the bound.
A program may use at most 128 MiB of HBM per device.

```python
import math
import jax
import jax.numpy as jnp
import numpy as np
from jax import lax

D = 2048
FF = 4096
GROUP_HEADS = 16
HEAD_DIM = 64
STATE_ONE = 64
STATE_TWO = 128
TAPS = 4
BLOCK = 128
ROWS_DEV = 128
SEQ_DEV = 1024
TOKENS = 16384
EXPERTS = 16
CAP = 17
N_TP = 8


def draw_raw_step_size(key, part):
    first, second, third = jax.random.split(jax.random.fold_in(key, 11), 3)
    segments = TOKENS // SEQ_DEV
    blocks = TOKENS // BLOCK
    segment_shift = jax.random.uniform(first, (segments, 1), jnp.float32, -1.0, 1.0)
    segment_shift = jnp.repeat(segment_shift, SEQ_DEV // BLOCK, axis=0)
    block_shift = jax.random.uniform(second, (blocks, 1), jnp.float32, -0.5, 0.5)
    grid_shape = (blocks, BLOCK * 2 * GROUP_HEADS)
    jitter = jnp.clip(0.6 * jax.random.normal(third, grid_shape, jnp.float32), -1.5, 1.5)
    return (segment_shift + block_shift + jitter).reshape(TOKENS, 2, GROUP_HEADS).astype(jnp.bfloat16)


def draw_head_decay_logarithm(key, part):
    first, second = jax.random.split(jax.random.fold_in(key, 23))
    slow_share = 0.5
    choose_slow = jax.random.uniform(first, (2, GROUP_HEADS), jnp.float32) < slow_share
    level = jax.random.uniform(second, (2, GROUP_HEADS), jnp.float32, 0.0, 1.0)
    slow_rate = jnp.log(0.3 / TOKENS) + level * jnp.log(5.0)
    fast_rate = jnp.log(0.03) + level * jnp.log(3.0)
    return jnp.where(choose_slow, slow_rate, fast_rate).astype(jnp.float32)


def draw_position_extra_decay(key, part):
    first, second = jax.random.split(jax.random.fold_in(key, 37))
    spots = jax.random.randint(first, (3,), 0, TOKENS)
    depth = jax.random.uniform(second, (3,), jnp.float32, jnp.log(0.5), jnp.log(0.8))
    places = jnp.arange(TOKENS)
    struck = places[:, None] == spots[None, :]
    return jnp.sum(jnp.where(struck, depth[None, :], 0.0), axis=1).astype(jnp.float32)


def block_levels(stream_key, extent, cuts, least, largest):
    def one(axis_at, blocks):
        steps = jax.random.uniform(jax.random.fold_in(jax.random.fold_in(stream_key, 6), axis_at), (blocks,), jnp.float32, least / len(cuts), largest / len(cuts))
        return jnp.repeat(jnp.exp(steps), extent[axis_at] // blocks).reshape((-1,) + (1,) * (len(extent) - axis_at - 1))

    loudness = one(*cuts[0])
    for cut in cuts[1:]:
        loudness = loudness * one(*cut)
    return loudness


def deal_out(own_key, own, number, rows, number_of, top, reach, lean):
    ranking = jax.random.permutation(own_key, number_of)
    heavy_load, ordinary = load_shares(number_of, rows * top, reach, lean, True), load_shares(number_of, rows * top, reach, lean, False)
    places = jnp.arange(number_of)

    def named(lengths, turn):
        used = int((lengths > 0).sum())
        fixed = max(1, used // 4)
        passed = fixed + (places - fixed + turn * (used - fixed)) % max(1, number_of - fixed)
        return jnp.zeros((number_of,), jnp.int32).at[ranking[jnp.where(places < fixed, places, passed)]].set(jnp.asarray(lengths, jnp.int32))

    lengths = jnp.where(number % 4 == 0, named(heavy_load, number // 4), named(ordinary, number - number // 4 - 1))
    mixed = jax.random.permutation(jax.random.fold_in(own, 3), number_of)
    donor, receiver = mixed[0:number_of // 2 * 2:2], mixed[1:number_of // 2 * 2:2]
    margin = jnp.minimum(lengths[donor] - 1, reach - lengths[receiver]) // 2
    margin = jnp.where((donor == ranking[0]) | (receiver == ranking[0]) | (lengths[receiver] == 0), 0, jnp.maximum(margin, 0))
    passed = jax.random.randint(jax.random.fold_in(own, 4), (number_of // 2,), 0, 1 << 20) % (margin + 1)
    lengths = lengths.at[donor].add(-passed).at[receiver].add(passed)
    items = jnp.searchsorted(jnp.cumsum(lengths), jnp.arange(rows * top), side="right").astype(jnp.int32)
    grid = items.reshape(top, rows).T
    grid = grid[jax.random.permutation(jax.random.fold_in(own, 1), rows)]
    turn = jax.random.randint(jax.random.fold_in(own, 2), (rows, 1), 0, top)
    return jnp.take_along_axis(grid, (jnp.arange(top)[None, :] + turn) % top, axis=1)


def load_shares(count, total, bound, lean, full):
    weights = [(1 << 20) // math.isqrt(standing ** lean) + 1 for standing in range(1, count + 1)]
    largest = bound if full else min(bound, max(-(-total // count), total * weights[0] // sum(weights)))
    least = 1 if total - largest >= count - 1 else 0
    holding, surplus = [largest] + [least] * (count - 1), total - largest - least * (count - 1)
    while surplus > 0:
        candidates = [i for i in range(1, count) if holding[i] < largest] or [i for i in range(1, count) if holding[i] < bound]
        whole, remaining = sum([weights[i] for i in candidates]), surplus
        for i in candidates:
            extra = min(bound - holding[i], max(1, remaining * weights[i] // whole), surplus)
            holding[i] = holding[i] + extra
            surplus = surplus - extra
    return np.array(holding)


def centred(own_key, shape, deviation, bound, shards=(), kind=jnp.bfloat16):
    entries = jax.random.normal(own_key, shape, jnp.float32) * deviation
    if len(shards) > 0:
        entries = block_levels(own_key, shape, shards, -0.22, 0.18) * entries
    return jnp.clip(entries, min=-bound, max=bound).astype(kind)


def setup_inputs(seed: int = 0, part: int = 0) -> dict:
    arg_keys = jax.random.split(jax.random.key(seed), 20)
    own_keys = jax.random.split(jax.random.fold_in(arg_keys[19], part), 20)
    residual = centred(own_keys[0], (TOKENS, D), 1.0, 6.0, ((0, 128),))
    grouped_value_heads = centred(own_keys[1], (TOKENS, 2, GROUP_HEADS * HEAD_DIM), 1.0, 6.0, ((0, 16), (2, 8)))
    output_gate_heads = centred(own_keys[2], (TOKENS, 2, GROUP_HEADS * HEAD_DIM), 1.0, 6.0, ((0, 16), (2, 8)))
    projected_key_query = centred(own_keys[3], (TOKENS, 2 * STATE_ONE + 2 * STATE_TWO), 1.0, 6.0, ((0, 16),))
    raw_step_size = draw_raw_step_size(jax.random.fold_in(jax.random.fold_in(arg_keys[19], part), 71), part)
    step_size_bias = jnp.clip(-1.0 + 1.5 * jax.random.uniform(arg_keys[5], (2, GROUP_HEADS), jnp.float32) ** block_levels(arg_keys[5], (2, GROUP_HEADS), ((1, 8),), -0.2, 0.2), -1.0, 0.5)
    head_decay_logarithm = draw_head_decay_logarithm(jax.random.fold_in(arg_keys[19], 71), part)
    position_extra_decay = draw_position_extra_decay(jax.random.fold_in(jax.random.fold_in(arg_keys[19], part), 71), part)
    head_skip_weight = jnp.clip(0.5 + 1.5 * jax.random.uniform(arg_keys[8], (2, GROUP_HEADS), jnp.float32) ** block_levels(arg_keys[8], (2, GROUP_HEADS), ((1, 8),), -0.2, 0.2), 0.5, 2.0)
    value_kernel_taps = centred(arg_keys[9], (TAPS, 2, GROUP_HEADS * HEAD_DIM), 0.5, 3.0, ((2, 8),))
    key_query_kernel = centred(arg_keys[10], (TAPS, 2 * STATE_ONE + 2 * STATE_TWO), 0.5, 3.0)
    head_norm_gain = jnp.clip(1.0 + 0.18 * jax.random.normal(arg_keys[11], (2, GROUP_HEADS * HEAD_DIM), jnp.float32), 0.1, 1.9)
    output_matrix = centred(arg_keys[12], (2, GROUP_HEADS * HEAD_DIM, D), (2 * GROUP_HEADS * HEAD_DIM) ** -0.5, 0.125, ((1, 8),))
    expert_norm_gain = jnp.clip(1.0 + 0.18 * jax.random.normal(arg_keys[13], (D,), jnp.float32), 0.1, 1.9)
    expert_gate_weight = centred(arg_keys[14], (EXPERTS, D, FF), D ** -0.5, 0.125, ((0, 16), (2, 8)))
    expert_up_weight = centred(arg_keys[15], (EXPERTS, D, FF), D ** -0.5, 0.125, ((0, 16), (2, 8)))
    expert_down_weight = centred(arg_keys[16], (EXPERTS, FF, D), FF ** -0.5, 0.09375, ((0, 16), (1, 8)))
    token_expert_choice_keys = jax.random.split(jax.random.fold_in(own_keys[17], 1), TOKENS // ROWS_DEV)
    token_expert_choice_turns = jax.random.permutation(jax.random.fold_in(own_keys[17], 3), TOKENS // ROWS_DEV)
    token_expert_choice = jax.vmap(lambda own, number: deal_out(jax.random.fold_in(own_keys[17], 2), own, number, ROWS_DEV, EXPERTS, 2, CAP, 1))(token_expert_choice_keys, token_expert_choice_turns).reshape((TOKENS, 2))
    expert_output_weight = jnp.clip(0.2 + 0.8 * jax.random.uniform(own_keys[18], (TOKENS, 2), jnp.float32) ** block_levels(own_keys[18], (TOKENS, 2), ((0, 128),), -0.2, 0.2), 0.2, 1.0)
    return dict(residual=residual, grouped_value_heads=grouped_value_heads, output_gate_heads=output_gate_heads, projected_key_query=projected_key_query, raw_step_size=raw_step_size, step_size_bias=step_size_bias, head_decay_logarithm=head_decay_logarithm, position_extra_decay=position_extra_decay, head_skip_weight=head_skip_weight, value_kernel_taps=value_kernel_taps, key_query_kernel=key_query_kernel, head_norm_gain=head_norm_gain, output_matrix=output_matrix, expert_norm_gain=expert_norm_gain, expert_gate_weight=expert_gate_weight, expert_up_weight=expert_up_weight, expert_down_weight=expert_down_weight, token_expert_choice=token_expert_choice, expert_output_weight=expert_output_weight)


EPSILON = 1e-06

def causal_conv(signal, tap_weights):
    tap_count = tap_weights.shape[0]
    length = signal.shape[0]
    padded = jnp.pad(signal, ((tap_count - 1, 0), (0, 0)))
    summed = jnp.zeros((length, signal.shape[1]), jnp.float32)
    for offset in range(tap_count):
        summed = summed + padded[offset:offset + length].astype(jnp.float32) * tap_weights[offset].astype(jnp.float32)
    return summed

def advance(carried, pair_item):
    block_state, fading_step = pair_item
    return (carried * fading_step[:, None, None] + block_state, carried)

def group_scan(value_rows, key_rows, query_rows, step_spacing, decay_logarithm, block_size):
    positions, head_count, head_width = value_rows.shape
    block_count = positions // block_size
    value_rows = value_rows.reshape(block_count, block_size, head_count, head_width).astype(jnp.float32)
    key_rows = key_rows.reshape(block_count, block_size, key_rows.shape[-1]).astype(jnp.float32)
    query_rows = query_rows.reshape(block_count, block_size, query_rows.shape[-1]).astype(jnp.float32)
    step_spacing = step_spacing.reshape(block_count, block_size, head_count)
    running = jnp.cumsum(decay_logarithm.reshape(block_count, block_size, head_count), axis=1)
    scores = jnp.einsum('kln,ksn->kls', query_rows, key_rows)
    causal = jnp.tril(jnp.ones((block_size, block_size), jnp.bool_))
    spread = running[:, :, None, :] - running[:, None, :, :]
    damping = jnp.exp(jnp.where(causal[None, :, :, None], spread, -jnp.inf))
    weights = (scores[:, :, :, None] * damping * step_spacing[:, None, :, :]).astype(jnp.bfloat16)
    near_part = jnp.einsum('klsh,kshp->klhp', weights.astype(jnp.float32), value_rows)
    fading = jnp.exp(running[:, -1:, :] - running) * step_spacing
    scaled_keys = (key_rows[:, :, None, :] * fading[:, :, :, None]).astype(jnp.bfloat16)
    states = jnp.einsum('kshn,kshp->khpn', scaled_keys.astype(jnp.float32), value_rows)
    anchor = jnp.zeros(states.shape[1:], jnp.float32)
    last_state, entering = lax.scan(advance, anchor, (states, jnp.exp(running[:, -1, :])))
    far_part = jnp.einsum('kln,khpn->klhp', query_rows, entering, precision=lax.Precision.HIGHEST)
    far_part = far_part * jnp.exp(running)[:, :, :, None]
    return (near_part + far_part).reshape(positions, head_count, head_width)

def reference(residual, grouped_value_heads, output_gate_heads, projected_key_query, raw_step_size, step_size_bias, head_decay_logarithm, position_extra_decay, head_skip_weight, value_kernel_taps, key_query_kernel, head_norm_gain, output_matrix, expert_norm_gain, expert_gate_weight, expert_up_weight, expert_down_weight, token_expert_choice, expert_output_weight):
    lane_count = 2 * GROUP_HEADS * HEAD_DIM
    flat_values = grouped_value_heads.reshape(TOKENS, lane_count)
    conv_heads = jax.nn.silu(causal_conv(flat_values, value_kernel_taps.reshape(TAPS, lane_count))).astype(jnp.bfloat16)
    conv_rows = jax.nn.silu(causal_conv(projected_key_query, key_query_kernel)).astype(jnp.bfloat16)
    step_spacing = jax.nn.softplus(raw_step_size.astype(jnp.float32) + step_size_bias[None])
    decay_logarithm = position_extra_decay[:, None, None] - jnp.exp(head_decay_logarithm)[None] * step_spacing
    value_heads = conv_heads.reshape(TOKENS, 2, GROUP_HEADS, HEAD_DIM)
    bounds = [0, STATE_ONE, 2 * STATE_ONE, 2 * STATE_ONE + STATE_TWO, 2 * STATE_ONE + 2 * STATE_TWO]
    group_parts = []
    for group_index in range(2):
        key_rows = conv_rows[:, bounds[2 * group_index]:bounds[2 * group_index + 1]]
        query_rows = conv_rows[:, bounds[2 * group_index + 1]:bounds[2 * group_index + 2]]
        group_parts.append(group_scan(value_heads[:, group_index], key_rows, query_rows, step_spacing[:, group_index], decay_logarithm[:, group_index], BLOCK))
    mixer_sum = jnp.stack(group_parts, axis=1) + head_skip_weight[None, :, :, None] * value_heads.astype(jnp.float32)
    gated_rows = mixer_sum * jax.nn.silu(output_gate_heads.astype(jnp.float32).reshape(TOKENS, 2, GROUP_HEADS, HEAD_DIM))
    scale_rows = lax.rsqrt(lax.optimization_barrier(jnp.mean(gated_rows * gated_rows, axis=3, keepdims=True)) + EPSILON)
    mixed_heads = (gated_rows * scale_rows * head_norm_gain.reshape(2, GROUP_HEADS, HEAD_DIM)).astype(jnp.bfloat16)
    mix_out = jnp.dot(mixed_heads.reshape(TOKENS, lane_count), output_matrix.reshape(lane_count, D), preferred_element_type=jnp.float32)
    stream = (residual.astype(jnp.float32) + mix_out).astype(jnp.bfloat16)
    wide_stream = stream.astype(jnp.float32)
    normed = (wide_stream * lax.rsqrt(lax.optimization_barrier(jnp.mean(wide_stream * wide_stream, axis=1, keepdims=True)) + EPSILON) * expert_norm_gain[None]).astype(jnp.bfloat16)
    sources = TOKENS // ROWS_DEV
    flat_ids = token_expert_choice.reshape(sources, 2 * ROWS_DEV)
    matches = (flat_ids[:, :, None] == jnp.arange(EXPERTS, dtype=jnp.int32)[None, None, :]).astype(jnp.int32)
    slot_rank = lax.optimization_barrier(jnp.sum((jnp.cumsum(matches, axis=1) - matches) * matches, axis=2))
    column = jnp.arange(sources, dtype=jnp.int32)[:, None] * CAP + slot_rank
    token_index = jnp.repeat(jnp.arange(TOKENS, dtype=jnp.int32).reshape(sources, ROWS_DEV), 2, axis=1)
    slot_table = jnp.zeros((EXPERTS, sources * CAP), jnp.int32).at[flat_ids.reshape(-1), column.reshape(-1)].set(token_index.reshape(-1))
    slice_width = FF // N_TP

    def one_expert(expert_index):
        gathered = jnp.take(normed, slot_table[expert_index], axis=0)
        gate_out = jnp.dot(gathered, expert_gate_weight[expert_index], preferred_element_type=jnp.float32)
        up_out = jnp.dot(gathered, expert_up_weight[expert_index], preferred_element_type=jnp.float32)
        hidden = (jax.nn.silu(gate_out) * up_out).astype(jnp.bfloat16)
        sliced = hidden.reshape(gathered.shape[0], N_TP, slice_width).astype(jnp.float32)
        down_slices = expert_down_weight[expert_index].reshape(N_TP, slice_width, D).astype(jnp.float32)
        pieces = jnp.einsum('rtf,tfd->rtd', sliced, down_slices).astype(jnp.bfloat16)
        pieces = lax.optimization_barrier(pieces).astype(jnp.float32)
        return lax.optimization_barrier(jnp.sum(pieces, axis=1)).astype(jnp.bfloat16)
    outputs = lax.map(one_expert, jnp.arange(EXPERTS, dtype=jnp.int32))
    picked = outputs[flat_ids.reshape(-1), column.reshape(-1)].reshape(TOKENS, 2, D).astype(jnp.float32)
    weighted = expert_output_weight[:, 0:1] * picked[:, 0] + expert_output_weight[:, 1:2] * picked[:, 1]
    return (wide_stream + weighted).astype(jnp.bfloat16)
```

```python
import functools

import jax
import jax.numpy as jnp
from jax import lax
from jax.experimental import pallas as pl
from jax.experimental.pallas import tpu as pltpu
from jax.sharding import PartitionSpec as P

HEAD_DIM = 64
STATE_ONE = 64
STATE_TWO = 128
BLOCK = 128


EPSILON = 1e-06


def passed_along(shard, axis, by):
    length = lax.axis_size(axis)
    pairs = [(i, i + by) for i in range(length) if 0 <= i + by < length]
    return lax.ppermute(shard, axis, pairs)


def sent_to_all(shard, axis):
    length = lax.axis_size(axis)
    return lax.all_to_all(
        jnp.broadcast_to(shard[None], (length, *shard.shape)), axis, 0, 0, tiled=True
    )


def all_in_one(shard, axis):
    leaves = jax.tree.leaves(shard)
    turns = sorted(range(len(leaves)), key=lambda k: -leaves[k].size)
    width = (1, *leaves[turns[0]].shape)[-1]
    lines = [
        jnp.pad(leaves[k].reshape(-1), (0, -leaves[k].size % width)).reshape(-1, width)
        for k in turns
    ]
    both, at, found = (sent_to_all(jnp.concatenate(lines), axis), 0, {})
    for k, line in zip(turns, lines):
        section = both[:, at : at + len(line)].reshape(len(both), -1)
        found[k] = section[:, : leaves[k].size].reshape(-1, *leaves[k].shape)
        at += len(line)
    numbers = iter(range(len(leaves)))
    return jax.tree.map(lambda _: found[next(numbers)], shard)


def joined_by_halves(pieces, combine):
    while len(jax.tree.leaves(pieces)[0]) > 1:
        pieces = jax.vmap(combine)(
            *(jax.tree.map(lambda part: part[side::2], pieces) for side in (0, 1))
        )
    return jax.tree.map(lambda part: part[0], pieces)


def entering_2(shard, axis, combine, identity):
    length, place = (lax.axis_size(axis), lax.axis_index(axis))
    passed = jnp.arange(length) < place

    def kept(part, zero, own):
        part = jnp.where(
            passed.reshape(-1, *(1 for _ in own.shape)),
            part.astype(own.dtype),
            jnp.asarray(zero, own.dtype),
        )
        return part

    pieces = all_in_one(
        jax.tree.map(
            lambda part, kind: part.astype(kind), shard, (jnp.bfloat16, jnp.bfloat16, jnp.bfloat16)
        ),
        axis,
    )
    return joined_by_halves(jax.tree.map(kept, pieces, identity, shard), combine)


def causal_taps(extended, tap_weights, length):
    summed = jnp.zeros((length, extended.shape[1]), jnp.float32)
    for offset in range(tap_weights.shape[0]):
        summed = summed + extended[offset : offset + length].astype(jnp.float32) * tap_weights[
            offset
        ].astype(jnp.float32)
    return summed


def advance(carried, pair_item):
    block_state, fading_step = pair_item
    return (carried * fading_step[:, None, None] + block_state, carried)


def local_blocks(value_rows, key_rows, query_rows, step_spacing, decay_logarithm):
    positions, head_count, head_width = value_rows.shape
    block_count = positions // BLOCK
    value_rows = value_rows.reshape(block_count, BLOCK, head_count, head_width)
    key_rows = key_rows.reshape(block_count, BLOCK, key_rows.shape[-1])
    query_rows = query_rows.reshape(block_count, BLOCK, query_rows.shape[-1])
    step_spacing = step_spacing.reshape(block_count, BLOCK, head_count)
    running = jnp.cumsum(decay_logarithm.reshape(block_count, BLOCK, head_count), axis=1)
    scores = jnp.einsum("kln,ksn->kls", query_rows, key_rows, preferred_element_type=jnp.float32)
    causal = jnp.tril(jnp.ones((BLOCK, BLOCK), jnp.bool_))
    spread = running[:, :, None, :] - running[:, None, :, :]
    damping = jnp.exp(jnp.where(causal[None, :, :, None], spread, -jnp.inf))
    weights = (scores[:, :, :, None] * damping * step_spacing[:, None, :, :]).astype(jnp.bfloat16)
    near_part = jnp.einsum(
        "klsh,kshp->klhp", weights, value_rows, preferred_element_type=jnp.float32
    )
    fading = jnp.exp(running[:, -1:, :] - running) * step_spacing
    scaled_keys = (key_rows.astype(jnp.float32)[:, :, None, :] * fading[:, :, :, None]).astype(
        jnp.bfloat16
    )
    states = jnp.einsum(
        "kshn,kshp->khpn", scaled_keys, value_rows, preferred_element_type=jnp.float32
    )
    block_ends = running[:, -1, :]
    anchor = jnp.zeros(states.shape[1:], jnp.float32)
    last_state, entering = lax.scan(advance, anchor, (states, jnp.exp(block_ends)))
    wide_queries = query_rows.astype(jnp.float32)
    far_part = jnp.einsum("kln,khpn->klhp", wide_queries, entering, precision=lax.Precision.HIGHEST)
    far_part = far_part * jnp.exp(running)[:, :, :, None]
    earlier_ends = jnp.cumsum(block_ends, axis=0) - block_ends
    carried_decay = jnp.exp(running + earlier_ends[:, None, :])
    return (
        near_part + far_part,
        last_state,
        jnp.sum(block_ends, axis=0),
        wide_queries,
        carried_decay,
    )


def join_states(earlier, later):
    early_decay, early_one, early_two = earlier
    late_decay, late_one, late_two = later
    return (
        early_decay + late_decay,
        early_one * jnp.exp(late_decay[0])[:, None, None] + late_one,
        early_two * jnp.exp(late_decay[1])[:, None, None] + late_two,
    )


MESH = pl.DeviceIdType.MESH
PIECE = 256
VMEM_LIMIT = 67043328


def expert_kernel(
    dims,
    stream_ref,
    gain_ref,
    choice_ref,
    share_ref,
    gate_hbm,
    up_hbm,
    down_hbm,
    out_ref,
    table,
    outbound,
    over_out,
    over_in,
    chunks,
    hidden,
    gate_up,
    down,
    sum_right,
    sum_left,
    totals,
    over_total,
    over_back,
    returned,
    over_ret,
    pick,
    load_sem,
    out_send,
    out_recv,
    over_send,
    over_recv,
    ring_send,
    ring_recv,
    sum_send,
    sum_recv,
    back_send,
    back_recv,
):
    f32, bf16 = jnp.float32, jnp.bfloat16
    places, columns, rows, main, over = dims["S"], dims["X"], dims["R"], dims["M"], dims["OV"]
    pieces, tiles, slots = dims["NP"], dims["NT"], dims["S"] * dims["M"]
    half = columns // 2
    me_x, me_s = lax.axis_index("tp"), lax.axis_index("sp")
    right = {"tp": lax.rem(me_x + 1, columns)}
    left = {"tp": lax.rem(me_x + columns - 1, columns)}

    def column(offset):
        return lax.rem(me_x + offset + columns, columns)

    def place(offset):
        return lax.rem(me_s + offset, places)

    def lines(index):
        return pl.ds(pl.multiple_of(index * main, main), main)

    def remote(src, dst, send, recv, device):
        return pltpu.make_async_remote_copy(
            src_ref=src, dst_ref=dst, send_sem=send, recv_sem=recv, device_id=device, device_id_type=MESH
        )

    loads = []
    for t in range(tiles):
        span = pl.ds(t * 128, 128)
        loads.append((gate_hbm.at[0, :, span], gate_up.at[t, :, pl.ds(0, 128)]))
        loads.append((up_hbm.at[0, :, span], gate_up.at[t, :, pl.ds(128, 128)]))
    for p in range(pieces):
        loads.append((down_hbm.at[0, :, pl.ds(p * PIECE, PIECE)], down.at[p]))
    loads = [pltpu.make_async_copy(a, b, load_sem.at[n]) for n, (a, b) in enumerate(loads)]
    for load in loads:
        load.start()

    barrier = pltpu.get_barrier_semaphore()
    for neighbour in (left, right):
        pl.semaphore_signal(barrier, inc=1, device_id=neighbour, device_id_type=MESH)
    for i in range(1, places):
        pl.semaphore_signal(barrier, inc=1, device_id={"sp": place(i)}, device_id_type=MESH)

    expert_at = lax.broadcasted_iota(jnp.int32, (over, rows), 0)
    token_a = lax.broadcasted_iota(jnp.int32, (rows, rows), 0)
    token_b = lax.broadcasted_iota(jnp.int32, (rows, rows), 1)
    choice = choice_ref[...]
    named = jnp.where((expert_at == choice[0:1]) | (expert_at == choice[1:2]), 1.0, 0.0)
    rank = jnp.dot(
        named.astype(bf16), jnp.where(token_a < token_b, 1.0, 0.0).astype(bf16), preferred_element_type=f32
    )
    slot_row = lax.broadcasted_iota(jnp.int32, (slots, over), 0)
    slot_expert = lax.broadcasted_iota(jnp.int32, (slots, over), 1) * main
    spread = jnp.where((slot_row >= slot_expert) & (slot_row < slot_expert + main), 1.0, 0.0).astype(bf16)
    named_x = jnp.dot(spread, named.astype(bf16), preferred_element_type=f32)
    rank_x = jnp.dot(spread, rank.astype(bf16), preferred_element_type=f32)
    turn = jnp.bitwise_and(lax.broadcasted_iota(jnp.int32, (slots, rows), 0), main - 1).astype(f32)
    put_main = jnp.where(rank_x == turn, named_x, 0.0).astype(bf16)
    put_over = jnp.where(rank == float(main), named, 0.0).astype(bf16)

    wide = stream_ref[...].astype(f32)
    scale = lax.rsqrt(jnp.mean(wide * wide, axis=1, keepdims=True) + EPSILON)
    normed = (wide * scale * gain_ref[...]).astype(bf16)
    for p in range(pieces):
        part = normed[:, p * PIECE : (p + 1) * PIECE]
        outbound[p] = jnp.dot(put_main, part, preferred_element_type=f32).astype(bf16)
        spill = jnp.dot(put_over, part, preferred_element_type=f32)
        for c in range(PIECE // 128):
            over_out[:, p * (PIECE // 128) + c, :] = spill[:, c * 128 : (c + 1) * 128]

    pl.semaphore_wait(barrier, 2 + places - 1)

    for i in range(1, places):
        remote(
            over_out.at[place(i)], over_in.at[me_s], over_send.at[0], over_recv.at[0], {"sp": place(i)}
        ).start()

    def send_out(p, carry):
        for i in range(1, places):
            remote(
                outbound.at[p, lines(place(i)), :],
                chunks.at[me_x, p, lines(me_s), :],
                out_send.at[p],
                out_recv.at[p],
                {"sp": place(i)},
            ).start()
        chunks[me_x, p, lines(me_s), :] = outbound[p, lines(me_s), :]
        return carry

    lax.fori_loop(0, pieces, send_out, 0)
    over_in[me_s] = over_out[me_s]
    if places < over:
        over_in[places:over] = jnp.zeros((over - places, *over_in.shape[1:]), f32)
        over_ret[places:over] = jnp.zeros((over - places, *over_ret.shape[1:]), f32)

    table[...] = jnp.zeros_like(table)
    table[0:2] = choice.astype(f32)
    table[2:4] = share_ref[...]
    turned = jnp.transpose(table[...])
    expert_to = lax.broadcasted_iota(jnp.int32, (rows, over), 1).astype(f32)
    named_k = [jnp.where(expert_to == turned[:, k : k + 1], 1.0, 0.0) for k in range(2)]
    rank_t = jnp.dot(
        jnp.where(token_b < token_a, 1.0, 0.0).astype(bf16),
        (named_k[0] + named_k[1]).astype(bf16),
        preferred_element_type=f32,
    )
    total_slots = slots + over
    slot_col = lax.broadcasted_iota(jnp.int32, (over, total_slots), 1)
    slot_exp = lax.broadcasted_iota(jnp.int32, (over, total_slots), 0)
    low = slot_exp * main
    spread_t = jnp.where(
        ((slot_col < slots) & (slot_col >= low) & (slot_col < low + main)) | (slot_col == slots + slot_exp), 1.0, 0.0
    ).astype(bf16)
    at = lax.broadcasted_iota(jnp.int32, (rows, total_slots), 1)
    turn_t = jnp.where(at < slots, jnp.bitwise_and(at, main - 1), main).astype(f32)
    rank_tx = jnp.dot(rank_t.astype(bf16), spread_t, preferred_element_type=f32)
    for k in range(2):
        named_tx = jnp.dot(named_k[k].astype(bf16), spread_t, preferred_element_type=f32)
        pick[k] = jnp.where(rank_tx == turn_t, named_tx, 0.0).astype(bf16)

    remote(
        over_out.at[0 : places - 1], over_in.at[0 : places - 1], over_send.at[0], over_recv.at[0], right
    ).wait_recv()
    for c in range(dims["NC"]):
        at_piece, at_lane = c // (PIECE // 128), (c % (PIECE // 128)) * 128
        chunks[me_x, at_piece, slots : slots + over, at_lane : at_lane + 128] = over_in[:, c, :].astype(bf16)

    def ring(way, step, p, col):
        return remote(
            chunks.at[col, p],
            chunks.at[col, p],
            ring_send.at[way, step, p],
            ring_recv.at[way, step, p],
            right if way == 0 else left,
        )

    def far(way, p):
        odd = lax.rem(p, 2)
        return half - odd if way == 0 else half - 1 + odd

    def unit(col, t):
        acc = jnp.dot(chunks[col, 0], gate_up[t, 0:PIECE, :], preferred_element_type=f32)
        for q in range(1, pieces):
            acc = acc + jnp.dot(
                chunks[col, q], gate_up[t, q * PIECE : (q + 1) * PIECE, :], preferred_element_type=f32
            )
        gate, up = acc[:, 0:128], acc[:, 128:256]
        value = gate * (1.0 / (1.0 + jnp.exp(-gate))) * up
        hidden[col, :, pl.ds(pl.multiple_of(t * 128, 128), 128)] = value.astype(bf16)

    def start_piece(p, carry):
        remote(
            outbound.at[p, 0 : (places - 1) * main, :],
            chunks.at[me_x, p, 0 : (places - 1) * main, :],
            out_send.at[p],
            out_recv.at[p],
            right,
        ).wait_recv()
        ring(0, 0, p, me_x).start()
        ring(1, 0, p, me_x).start()
        return carry

    lax.fori_loop(0, pieces, start_piece, 0)
    for load in loads:
        load.wait()

    for k in range(1, half + 1):

        def pass_on(p, carry, k=k):
            for way in range(2):
                col = column(-k if way == 0 else k)

                @pl.when(k <= far(way, p))
                def _():
                    ring(way, k - 1, p, col).wait_recv()

                if k < half:

                    @pl.when(k < far(way, p))
                    def _():
                        ring(way, k, p, col).start()

            if k == 1:

                @pl.when(lax.rem(p, 2) == 0)
                def _():
                    unit(me_x, lax.div(p, 2))

            else:
                side = lax.div(p, tiles)
                unit(column((2 * side - 1) * (k - 1)), lax.rem(p, tiles))
            return carry

        lax.fori_loop(0, pieces, pass_on, 0)

    def last_unit(t, carry):
        unit(column(half), t)
        return carry

    lax.fori_loop(0, tiles, last_unit, 0)

    def own(col, p):
        return jnp.dot(hidden[col], down[p], preferred_element_type=f32)

    def hop(way, j, p):
        buffer = sum_right if way == 0 else sum_left
        return remote(
            buffer.at[j, p],
            buffer.at[j - 1, p],
            sum_send.at[way, j - 1, p],
            sum_recv.at[way, j - 1, p],
            right if way == 0 else left,
        )

    def round_of(t, low_piece, high_piece):
        def body(p, carry):
            for way in range(2):
                buffer = sum_right if way == 0 else sum_left
                j = far(1 - way, p) - t

                def work(way=way, buffer=buffer, j=j):
                    value = own(column(j if way == 0 else -j), p)
                    if t > 0:
                        hop(way, j + 1, p).wait_recv()
                        value = value + buffer[j, p].astype(f32)
                    buffer[j, p] = value.astype(bf16)
                    hop(way, j, p).start()

                if t < half - 1:
                    work()
                else:
                    pl.when(j >= 1)(work)
            return carry

        lax.fori_loop(low_piece, high_piece, body, 0)

    def finish(low_piece, high_piece):
        def body(p, carry):
            value = own(me_x, p)
            hop(0, 1, p).wait_recv()
            hop(1, 1, p).wait_recv()
            value = value + sum_right[0, p].astype(f32) + sum_left[0, p].astype(f32)
            totals[p] = value[0:slots].astype(bf16)
            over_total[p] = value[slots : slots + over]
            returned[p, lines(me_s), :] = totals[p, lines(me_s), :]
            for i in range(1, places):
                remote(
                    totals.at[p, lines(place(i)), :],
                    returned.at[p, lines(me_s), :],
                    back_send.at[p],
                    back_recv.at[p],
                    {"sp": place(i)},
                ).start()
            return carry

        lax.fori_loop(low_piece, high_piece, body, 0)

    cut = pieces // 2
    for t in range(half - 1):
        round_of(t, 0, cut)
    round_of(0, cut, pieces)
    round_of(half - 1, 0, cut)
    for t in range(1, half):
        round_of(t, cut, pieces)
        if t == 1:
            finish(0, cut)
    if half == 1:
        finish(0, cut)
    finish(cut, pieces)

    for c in range(dims["NC"]):
        at_piece, at_lane = c // (PIECE // 128), (c % (PIECE // 128)) * 128
        over_back[:, c, :] = over_total[at_piece, :, at_lane : at_lane + 128]
    over_ret[me_s] = over_back[me_s]
    for i in range(1, places):
        remote(
            over_back.at[place(i)], over_ret.at[me_s], over_send.at[1], over_recv.at[1], {"sp": place(i)}
        ).start()

    first = turned[:, 2:3]
    second = turned[:, 3:4]
    remote(
        over_back.at[0 : places - 1], over_ret.at[0 : places - 1], over_send.at[1], over_recv.at[1], right
    ).wait_recv()
    for c in range(dims["NC"]):
        at_piece, at_lane = c // (PIECE // 128), (c % (PIECE // 128)) * 128
        returned[at_piece, slots : slots + over, at_lane : at_lane + 128] = over_ret[:, c, :].astype(bf16)

    def combine(p, carry):
        remote(
            totals.at[p, 0 : (places - 1) * main, :],
            returned.at[p, 0 : (places - 1) * main, :],
            back_send.at[p],
            back_recv.at[p],
            right,
        ).wait_recv()
        span = pl.ds(pl.multiple_of(p * PIECE, PIECE), PIECE)
        one = jnp.dot(pick[0], returned[p], preferred_element_type=f32)
        two = jnp.dot(pick[1], returned[p], preferred_element_type=f32)
        out_ref[:, span] = (stream_ref[:, span].astype(f32) + (first * one + second * two)).astype(bf16)
        return carry

    lax.fori_loop(0, pieces, combine, 0)

    for n, (a, b) in enumerate(((over_out, over_in), (over_back, over_ret))):
        remote(
            a.at[0 : places - 1], b.at[0 : places - 1], over_send.at[n], over_recv.at[n], right
        ).wait_send()

    def drain(p, carry):
        span = pl.ds(0, (places - 1) * main)
        remote(
            outbound.at[p, span, :], chunks.at[me_x, p, span, :], out_send.at[p], out_recv.at[p], right
        ).wait_send()
        remote(
            totals.at[p, span, :], returned.at[p, span, :], back_send.at[p], back_recv.at[p], right
        ).wait_send()
        for way in range(2):
            for k in range(half):
                pl.when(k < far(way, p))(lambda way=way, k=k: ring(way, k, p, me_x).wait_send())
                pl.when(k < far(1 - way, p))(lambda way=way, k=k: hop(way, k + 1, p).wait_send())
        return carry

    lax.fori_loop(0, pieces, drain, 0)


def expert_layer(stream, gain, choice, share, gate_weight, up_weight, down_weight, places, columns):
    rows, width = stream.shape
    units = gate_weight.shape[2]
    f32, bf16 = jnp.float32, jnp.bfloat16
    main = 2 * rows // places
    over = -(-places // 16) * 16
    pieces, tiles, lanes = width // PIECE, units // 128, width // 128
    half = columns // 2
    total = places * main + over
    dims = dict(S=places, X=columns, R=rows, M=main, OV=over, NP=pieces, NT=tiles, NC=lanes)
    dma = pltpu.SemaphoreType.DMA
    whole = pl.BlockSpec(memory_space=pltpu.VMEM)
    away = pl.BlockSpec(memory_space=pl.ANY)
    return pl.pallas_call(
        functools.partial(expert_kernel, dims),
        out_shape=jax.ShapeDtypeStruct((rows, width), bf16),
        in_specs=[whole, whole, whole, whole, away, away, away],
        out_specs=whole,
        scratch_shapes=[
            pltpu.VMEM((8, rows), f32),
            pltpu.VMEM((pieces, places * main, PIECE), bf16),
            pltpu.VMEM((over, lanes, 128), f32),
            pltpu.VMEM((over, lanes, 128), f32),
            pltpu.VMEM((columns, pieces, total, PIECE), bf16),
            pltpu.VMEM((columns, total, units), bf16),
            pltpu.VMEM((tiles, width, 256), bf16),
            pltpu.VMEM((pieces, units, PIECE), bf16),
            pltpu.VMEM((half + 1, pieces, total, PIECE), bf16),
            pltpu.VMEM((half + 1, pieces, total, PIECE), bf16),
            pltpu.VMEM((pieces, places * main, PIECE), bf16),
            pltpu.VMEM((pieces, over, PIECE), f32),
            pltpu.VMEM((over, lanes, 128), f32),
            pltpu.VMEM((pieces, total, PIECE), bf16),
            pltpu.VMEM((over, lanes, 128), f32),
            pltpu.VMEM((2, rows, total), bf16),
            dma((2 * tiles + pieces,)),
            dma((pieces,)),
            dma((pieces,)),
            dma((2,)),
            dma((2,)),
            dma((2, half, pieces)),
            dma((2, half, pieces)),
            dma((2, half + 1, pieces)),
            dma((2, half + 1, pieces)),
            dma((pieces,)),
            dma((pieces,)),
        ],
        compiler_params=pltpu.CompilerParams(
            collective_id=0, has_side_effects=True, vmem_limit_bytes=VMEM_LIMIT
        ),
        name="routed_experts",
    )(stream, gain, choice, share, gate_weight, up_weight, down_weight)


def local(
    residual,
    grouped_value_heads,
    output_gate_heads,
    projected_key_query,
    raw_step_size,
    step_size_bias,
    head_decay_logarithm,
    position_extra_decay,
    head_skip_weight,
    value_kernel_taps,
    key_query_kernel,
    head_norm_gain,
    output_matrix,
    expert_norm_gain,
    expert_gate_weight,
    expert_up_weight,
    expert_down_weight,
    token_expert_choice,
    expert_output_weight,
):
    positions = grouped_value_heads.shape[0]
    lane_width = grouped_value_heads.shape[2]
    local_heads = lane_width // HEAD_DIM
    both_lanes = 2 * lane_width
    rim_depth = key_query_kernel.shape[0] - 1
    flat_values = grouped_value_heads.reshape(positions, both_lanes)
    rim_rows = jnp.concatenate(
        [flat_values[positions - rim_depth :], projected_key_query[positions - rim_depth :]], axis=1
    )
    prior_rows = passed_along(rim_rows, "sp", 1)
    padded_values = jnp.concatenate([prior_rows[:, :both_lanes], flat_values], axis=0)
    padded_keys = jnp.concatenate([prior_rows[:, both_lanes:], projected_key_query], axis=0)
    conv_heads = jax.nn.silu(
        causal_taps(padded_values, value_kernel_taps.reshape(rim_depth + 1, both_lanes), positions)
    ).astype(jnp.bfloat16)
    conv_rows = jax.nn.silu(causal_taps(padded_keys, key_query_kernel, positions)).astype(
        jnp.bfloat16
    )
    step_spacing = jax.nn.softplus(raw_step_size.astype(jnp.float32) + step_size_bias[None])
    decay_logarithm = (
        position_extra_decay[:, None, None] - jnp.exp(head_decay_logarithm)[None] * step_spacing
    )
    value_heads = conv_heads.reshape(positions, 2, local_heads, HEAD_DIM)
    bounds = [0, STATE_ONE, 2 * STATE_ONE, 2 * STATE_ONE + STATE_TWO, 2 * STATE_ONE + 2 * STATE_TWO]
    local_parts = []
    end_states = []
    decay_totals = []
    query_list = []
    reach_list = []
    for group_index in range(2):
        key_rows = conv_rows[:, bounds[2 * group_index] : bounds[2 * group_index + 1]]
        query_rows = conv_rows[:, bounds[2 * group_index + 1] : bounds[2 * group_index + 2]]
        local_part, end_state, decay_total, wide_queries, carried_decay = local_blocks(
            value_heads[:, group_index],
            key_rows,
            query_rows,
            step_spacing[:, group_index],
            decay_logarithm[:, group_index],
        )
        local_parts.append(local_part)
        end_states.append(end_state)
        decay_totals.append(decay_total)
        query_list.append(wide_queries)
        reach_list.append(carried_decay)
    identity = (
        jnp.zeros((2, local_heads), jnp.float32),
        jnp.zeros_like(end_states[0]),
        jnp.zeros_like(end_states[1]),
    )
    prior_decay, enter_one, enter_two = entering_2(
        (jnp.stack(decay_totals), end_states[0], end_states[1]), "sp", join_states, identity
    )
    entered = [enter_one, enter_two]
    group_parts = []
    for group_index in range(2):
        carried_part = jnp.einsum(
            "kln,hpn->klhp",
            query_list[group_index],
            entered[group_index],
            precision=lax.Precision.HIGHEST,
        )
        carried_part = carried_part * reach_list[group_index][:, :, :, None]
        summed_part = local_parts[group_index] + carried_part
        group_parts.append(summed_part.reshape(positions, local_heads, HEAD_DIM))
    mixer_sum = jnp.stack(group_parts, axis=1) + head_skip_weight[
        None, :, :, None
    ] * value_heads.astype(jnp.float32)
    gated_rows = mixer_sum * jax.nn.silu(
        output_gate_heads.astype(jnp.float32).reshape(positions, 2, local_heads, HEAD_DIM)
    )
    scale_rows = lax.rsqrt(jnp.mean(gated_rows * gated_rows, axis=3, keepdims=True) + EPSILON)
    mixed_heads = (
        gated_rows * scale_rows * head_norm_gain.reshape(2, local_heads, HEAD_DIM)
    ).astype(jnp.bfloat16)
    mixed_heads = mixed_heads.reshape(positions, 2, lane_width)
    rows_here = residual.shape[0]
    model_width = output_matrix.shape[2]
    moved = lax.all_to_all(mixed_heads, "tp", split_axis=0, concat_axis=2, tiled=True)
    mix_out = jnp.einsum(
        "tgc,gcd->td",
        moved,
        lax.all_gather(output_matrix, "tp", axis=1, tiled=True),
        preferred_element_type=jnp.float32,
    )
    stream = (residual.astype(jnp.float32) + mix_out).astype(jnp.bfloat16)
    return expert_layer(
        stream,
        expert_norm_gain[None],
        token_expert_choice.T,
        expert_output_weight.T,
        expert_gate_weight,
        expert_up_weight,
        expert_down_weight,
        lax.axis_size("sp"),
        lax.axis_size("tp"),
    )


def solution(mesh):
    placed = (
        P(("grp", "sp", "tp"), None),
        P(("grp", "sp"), None, "tp"),
        P(("grp", "sp"), None, "tp"),
        P(("grp", "sp"), None),
        P(("grp", "sp"), None, "tp"),
        P(None, "tp"),
        P(None, "tp"),
        P(("grp", "sp")),
        P(None, "tp"),
        P(None, None, "tp"),
        P(),
        P(None, "tp"),
        P(None, "tp", None),
        P(),
        P("sp", None, "tp"),
        P("sp", None, "tp"),
        P("sp", "tp", None),
        P(("grp", "sp", "tp"), None),
        P(("grp", "sp", "tp"), None),
    )
    return jax.shard_map(
        local, mesh=mesh, in_specs=placed, out_specs=P(("grp", "sp", "tp"), None), check_vma=False
    )
```

```python
import functools

import jax
import jax.numpy as jnp
from jax import lax
from jax.experimental import pallas as pl
from jax.experimental.pallas import tpu as pltpu
from jax.sharding import PartitionSpec as P

HEAD_DIM = 64
STATE_ONE = 64
STATE_TWO = 128
BLOCK = 128
EPSILON = 1e-06
MESH = pl.DeviceIdType.MESH
PIECE = 256
VMEM_LIMIT = 67043328


def expert_kernel(
    dims,
    stream_ref,
    gain_ref,
    choice_ref,
    share_ref,
    gate_hbm,
    up_hbm,
    down_hbm,
    out_ref,
    table,
    outbound,
    over_out,
    over_in,
    chunks,
    hidden,
    gate_up,
    down,
    sum_right,
    sum_left,
    totals,
    over_total,
    over_back,
    returned,
    over_ret,
    pick,
    load_sem,
    out_send,
    out_recv,
    over_send,
    over_recv,
    ring_send,
    ring_recv,
    sum_send,
    sum_recv,
    back_send,
    back_recv,
):
    f32, bf16 = jnp.float32, jnp.bfloat16
    places, columns, rows, main, over = dims["S"], dims["X"], dims["R"], dims["M"], dims["OV"]
    pieces, tiles, slots = dims["NP"], dims["NT"], dims["S"] * dims["M"]
    half = columns // 2
    me_x, me_s = lax.axis_index("tp"), lax.axis_index("sp")
    right = {"tp": lax.rem(me_x + 1, columns)}
    left = {"tp": lax.rem(me_x + columns - 1, columns)}

    def column(offset):
        return lax.rem(me_x + offset + columns, columns)

    def place(offset):
        return lax.rem(me_s + offset, places)

    def lines(index):
        return pl.ds(pl.multiple_of(index * main, main), main)

    def remote(src, dst, send, recv, device):
        return pltpu.make_async_remote_copy(
            src_ref=src, dst_ref=dst, send_sem=send, recv_sem=recv, device_id=device, device_id_type=MESH
        )

    loads = []
    for t in range(tiles):
        span = pl.ds(t * 128, 128)
        loads.append((gate_hbm.at[0, :, span], gate_up.at[t, :, pl.ds(0, 128)]))
        loads.append((up_hbm.at[0, :, span], gate_up.at[t, :, pl.ds(128, 128)]))
    for p in range(pieces):
        loads.append((down_hbm.at[0, :, pl.ds(p * PIECE, PIECE)], down.at[p]))
    loads = [pltpu.make_async_copy(a, b, load_sem.at[n]) for n, (a, b) in enumerate(loads)]
    for load in loads:
        load.start()

    barrier = pltpu.get_barrier_semaphore()
    for neighbour in (left, right):
        pl.semaphore_signal(barrier, inc=1, device_id=neighbour, device_id_type=MESH)
    for i in range(1, places):
        pl.semaphore_signal(barrier, inc=1, device_id={"sp": place(i)}, device_id_type=MESH)

    expert_at = lax.broadcasted_iota(jnp.int32, (over, rows), 0)
    token_a = lax.broadcasted_iota(jnp.int32, (rows, rows), 0)
    token_b = lax.broadcasted_iota(jnp.int32, (rows, rows), 1)
    choice = choice_ref[...]
    named = jnp.where((expert_at == choice[0:1]) | (expert_at == choice[1:2]), 1.0, 0.0)
    rank = jnp.dot(
        named.astype(bf16), jnp.where(token_a < token_b, 1.0, 0.0).astype(bf16), preferred_element_type=f32
    )
    slot_row = lax.broadcasted_iota(jnp.int32, (slots, over), 0)
    slot_expert = lax.broadcasted_iota(jnp.int32, (slots, over), 1) * main
    spread = jnp.where((slot_row >= slot_expert) & (slot_row < slot_expert + main), 1.0, 0.0).astype(bf16)
    named_x = jnp.dot(spread, named.astype(bf16), preferred_element_type=f32)
    rank_x = jnp.dot(spread, rank.astype(bf16), preferred_element_type=f32)
    turn = jnp.bitwise_and(lax.broadcasted_iota(jnp.int32, (slots, rows), 0), main - 1).astype(f32)
    put_main = jnp.where(rank_x == turn, named_x, 0.0).astype(bf16)
    put_over = jnp.where(rank == float(main), named, 0.0).astype(bf16)

    wide = stream_ref[...].astype(f32)
    scale = lax.rsqrt(jnp.mean(wide * wide, axis=1, keepdims=True) + EPSILON)
    normed = (wide * scale * gain_ref[...]).astype(bf16)
    for p in range(pieces):
        part = normed[:, p * PIECE : (p + 1) * PIECE]
        outbound[p] = jnp.dot(put_main, part, preferred_element_type=f32).astype(bf16)
        spill = jnp.dot(put_over, part, preferred_element_type=f32)
        for c in range(PIECE // 128):
            over_out[:, p * (PIECE // 128) + c, :] = spill[:, c * 128 : (c + 1) * 128]

    pl.semaphore_wait(barrier, 2 + places - 1)

    for i in range(1, places):
        remote(
            over_out.at[place(i)], over_in.at[me_s], over_send.at[0], over_recv.at[0], {"sp": place(i)}
        ).start()

    def send_out(p, carry):
        for i in range(1, places):
            remote(
                outbound.at[p, lines(place(i)), :],
                chunks.at[me_x, p, lines(me_s), :],
                out_send.at[p],
                out_recv.at[p],
                {"sp": place(i)},
            ).start()
        chunks[me_x, p, lines(me_s), :] = outbound[p, lines(me_s), :]
        return carry

    lax.fori_loop(0, pieces, send_out, 0)
    over_in[me_s] = over_out[me_s]
    if places < over:
        over_in[places:over] = jnp.zeros((over - places, *over_in.shape[1:]), f32)
        over_ret[places:over] = jnp.zeros((over - places, *over_ret.shape[1:]), f32)

    table[...] = jnp.zeros_like(table)
    table[0:2] = choice.astype(f32)
    table[2:4] = share_ref[...]
    turned = jnp.transpose(table[...])
    expert_to = lax.broadcasted_iota(jnp.int32, (rows, over), 1).astype(f32)
    named_k = [jnp.where(expert_to == turned[:, k : k + 1], 1.0, 0.0) for k in range(2)]
    rank_t = jnp.dot(
        jnp.where(token_b < token_a, 1.0, 0.0).astype(bf16),
        (named_k[0] + named_k[1]).astype(bf16),
        preferred_element_type=f32,
    )
    total_slots = slots + over
    slot_col = lax.broadcasted_iota(jnp.int32, (over, total_slots), 1)
    slot_exp = lax.broadcasted_iota(jnp.int32, (over, total_slots), 0)
    low = slot_exp * main
    spread_t = jnp.where(
        ((slot_col < slots) & (slot_col >= low) & (slot_col < low + main)) | (slot_col == slots + slot_exp), 1.0, 0.0
    ).astype(bf16)
    at = lax.broadcasted_iota(jnp.int32, (rows, total_slots), 1)
    turn_t = jnp.where(at < slots, jnp.bitwise_and(at, main - 1), main).astype(f32)
    rank_tx = jnp.dot(rank_t.astype(bf16), spread_t, preferred_element_type=f32)
    for k in range(2):
        named_tx = jnp.dot(named_k[k].astype(bf16), spread_t, preferred_element_type=f32)
        pick[k] = jnp.where(rank_tx == turn_t, named_tx, 0.0).astype(bf16)

    remote(
        over_out.at[0 : places - 1], over_in.at[0 : places - 1], over_send.at[0], over_recv.at[0], right
    ).wait_recv()
    for c in range(dims["NC"]):
        at_piece, at_lane = c // (PIECE // 128), (c % (PIECE // 128)) * 128
        chunks[me_x, at_piece, slots : slots + over, at_lane : at_lane + 128] = over_in[:, c, :].astype(bf16)

    def ring(way, step, p, col):
        return remote(
            chunks.at[col, p],
            chunks.at[col, p],
            ring_send.at[way, step, p],
            ring_recv.at[way, step, p],
            right if way == 0 else left,
        )

    def far(way, p):
        odd = lax.rem(p, 2)
        return half - odd if way == 0 else half - 1 + odd

    def unit(col, t):
        acc = jnp.dot(chunks[col, 0], gate_up[t, 0:PIECE, :], preferred_element_type=f32)
        for q in range(1, pieces):
            acc = acc + jnp.dot(
                chunks[col, q], gate_up[t, q * PIECE : (q + 1) * PIECE, :], preferred_element_type=f32
            )
        gate, up = acc[:, 0:128], acc[:, 128:256]
        value = gate * (1.0 / (1.0 + jnp.exp(-gate))) * up
        hidden[col, :, pl.ds(pl.multiple_of(t * 128, 128), 128)] = value.astype(bf16)

    def start_piece(p, carry):
        remote(
            outbound.at[p, 0 : (places - 1) * main, :],
            chunks.at[me_x, p, 0 : (places - 1) * main, :],
            out_send.at[p],
            out_recv.at[p],
            right,
        ).wait_recv()
        ring(0, 0, p, me_x).start()
        ring(1, 0, p, me_x).start()
        return carry

    lax.fori_loop(0, pieces, start_piece, 0)
    for load in loads:
        load.wait()

    for k in range(1, half + 1):

        def pass_on(p, carry, k=k):
            for way in range(2):
                col = column(-k if way == 0 else k)

                @pl.when(k <= far(way, p))
                def _():
                    ring(way, k - 1, p, col).wait_recv()

                if k < half:

                    @pl.when(k < far(way, p))
                    def _():
                        ring(way, k, p, col).start()

            if k == 1:

                @pl.when(lax.rem(p, 2) == 0)
                def _():
                    unit(me_x, lax.div(p, 2))

            else:
                side = lax.div(p, tiles)
                unit(column((2 * side - 1) * (k - 1)), lax.rem(p, tiles))
            return carry

        lax.fori_loop(0, pieces, pass_on, 0)

    def last_unit(t, carry):
        unit(column(half), t)
        return carry

    lax.fori_loop(0, tiles, last_unit, 0)

    def own(col, p):
        return jnp.dot(hidden[col], down[p], preferred_element_type=f32)

    def hop(way, j, p):
        buffer = sum_right if way == 0 else sum_left
        return remote(
            buffer.at[j, p],
            buffer.at[j - 1, p],
            sum_send.at[way, j - 1, p],
            sum_recv.at[way, j - 1, p],
            right if way == 0 else left,
        )

    def round_of(t, low_piece, high_piece):
        def body(p, carry):
            for way in range(2):
                buffer = sum_right if way == 0 else sum_left
                j = far(1 - way, p) - t

                def work(way=way, buffer=buffer, j=j):
                    value = own(column(j if way == 0 else -j), p)
                    if t > 0:
                        hop(way, j + 1, p).wait_recv()
                        value = value + buffer[j, p].astype(f32)
                    buffer[j, p] = value.astype(bf16)
                    hop(way, j, p).start()

                if t < half - 1:
                    work()
                else:
                    pl.when(j >= 1)(work)
            return carry

        lax.fori_loop(low_piece, high_piece, body, 0)

    def finish(low_piece, high_piece):
        def body(p, carry):
            value = own(me_x, p)
            hop(0, 1, p).wait_recv()
            hop(1, 1, p).wait_recv()
            value = value + sum_right[0, p].astype(f32) + sum_left[0, p].astype(f32)
            totals[p] = value[0:slots].astype(bf16)
            over_total[p] = value[slots : slots + over]
            returned[p, lines(me_s), :] = totals[p, lines(me_s), :]
            for i in range(1, places):
                remote(
                    totals.at[p, lines(place(i)), :],
                    returned.at[p, lines(me_s), :],
                    back_send.at[p],
                    back_recv.at[p],
                    {"sp": place(i)},
                ).start()
            return carry

        lax.fori_loop(low_piece, high_piece, body, 0)

    cut = pieces // 2
    for t in range(half - 1):
        round_of(t, 0, cut)
    round_of(0, cut, pieces)
    round_of(half - 1, 0, cut)
    for t in range(1, half):
        round_of(t, cut, pieces)
        if t == 1:
            finish(0, cut)
    if half == 1:
        finish(0, cut)
    finish(cut, pieces)

    for c in range(dims["NC"]):
        at_piece, at_lane = c // (PIECE // 128), (c % (PIECE // 128)) * 128
        over_back[:, c, :] = over_total[at_piece, :, at_lane : at_lane + 128]
    over_ret[me_s] = over_back[me_s]
    for i in range(1, places):
        remote(
            over_back.at[place(i)], over_ret.at[me_s], over_send.at[1], over_recv.at[1], {"sp": place(i)}
        ).start()

    first = turned[:, 2:3]
    second = turned[:, 3:4]
    remote(
        over_back.at[0 : places - 1], over_ret.at[0 : places - 1], over_send.at[1], over_recv.at[1], right
    ).wait_recv()
    for c in range(dims["NC"]):
        at_piece, at_lane = c // (PIECE // 128), (c % (PIECE // 128)) * 128
        returned[at_piece, slots : slots + over, at_lane : at_lane + 128] = over_ret[:, c, :].astype(bf16)

    def combine(p, carry):
        remote(
            totals.at[p, 0 : (places - 1) * main, :],
            returned.at[p, 0 : (places - 1) * main, :],
            back_send.at[p],
            back_recv.at[p],
            right,
        ).wait_recv()
        span = pl.ds(pl.multiple_of(p * PIECE, PIECE), PIECE)
        one = jnp.dot(pick[0], returned[p], preferred_element_type=f32)
        two = jnp.dot(pick[1], returned[p], preferred_element_type=f32)
        out_ref[:, span] = (stream_ref[:, span].astype(f32) + (first * one + second * two)).astype(bf16)
        return carry

    lax.fori_loop(0, pieces, combine, 0)

    for n, (a, b) in enumerate(((over_out, over_in), (over_back, over_ret))):
        remote(
            a.at[0 : places - 1], b.at[0 : places - 1], over_send.at[n], over_recv.at[n], right
        ).wait_send()

    def drain(p, carry):
        span = pl.ds(0, (places - 1) * main)
        remote(
            outbound.at[p, span, :], chunks.at[me_x, p, span, :], out_send.at[p], out_recv.at[p], right
        ).wait_send()
        remote(
            totals.at[p, span, :], returned.at[p, span, :], back_send.at[p], back_recv.at[p], right
        ).wait_send()
        for way in range(2):
            for k in range(half):
                pl.when(k < far(way, p))(lambda way=way, k=k: ring(way, k, p, me_x).wait_send())
                pl.when(k < far(1 - way, p))(lambda way=way, k=k: hop(way, k + 1, p).wait_send())
        return carry

    lax.fori_loop(0, pieces, drain, 0)


def expert_layer(stream, gain, choice, share, gate_weight, up_weight, down_weight, places, columns):
    rows, width = stream.shape
    units = gate_weight.shape[2]
    f32, bf16 = jnp.float32, jnp.bfloat16
    main = 2 * rows // places
    over = -(-places // 16) * 16
    pieces, tiles, lanes = width // PIECE, units // 128, width // 128
    half = columns // 2
    total = places * main + over
    dims = dict(S=places, X=columns, R=rows, M=main, OV=over, NP=pieces, NT=tiles, NC=lanes)
    dma = pltpu.SemaphoreType.DMA
    whole = pl.BlockSpec(memory_space=pltpu.VMEM)
    away = pl.BlockSpec(memory_space=pl.ANY)
    return pl.pallas_call(
        functools.partial(expert_kernel, dims),
        out_shape=jax.ShapeDtypeStruct((rows, width), bf16),
        in_specs=[whole, whole, whole, whole, away, away, away],
        out_specs=whole,
        scratch_shapes=[
            pltpu.VMEM((8, rows), f32),
            pltpu.VMEM((pieces, places * main, PIECE), bf16),
            pltpu.VMEM((over, lanes, 128), f32),
            pltpu.VMEM((over, lanes, 128), f32),
            pltpu.VMEM((columns, pieces, total, PIECE), bf16),
            pltpu.VMEM((columns, total, units), bf16),
            pltpu.VMEM((tiles, width, 256), bf16),
            pltpu.VMEM((pieces, units, PIECE), bf16),
            pltpu.VMEM((half + 1, pieces, total, PIECE), bf16),
            pltpu.VMEM((half + 1, pieces, total, PIECE), bf16),
            pltpu.VMEM((pieces, places * main, PIECE), bf16),
            pltpu.VMEM((pieces, over, PIECE), f32),
            pltpu.VMEM((over, lanes, 128), f32),
            pltpu.VMEM((pieces, total, PIECE), bf16),
            pltpu.VMEM((over, lanes, 128), f32),
            pltpu.VMEM((2, rows, total), bf16),
            dma((2 * tiles + pieces,)),
            dma((pieces,)),
            dma((pieces,)),
            dma((2,)),
            dma((2,)),
            dma((2, half, pieces)),
            dma((2, half, pieces)),
            dma((2, half + 1, pieces)),
            dma((2, half + 1, pieces)),
            dma((pieces,)),
            dma((pieces,)),
        ],
        compiler_params=pltpu.CompilerParams(
            collective_id=0, has_side_effects=True, vmem_limit_bytes=VMEM_LIMIT
        ),
        name="routed_experts",
    )(stream, gain, choice, share, gate_weight, up_weight, down_weight)


def mixer_kernel(
    dims,
    residual_ref,
    value_hbm,
    gate_hbm,
    keys_hbm,
    raw_ref,
    bias_ref,
    log_ref,
    extra_ref,
    skip_ref,
    value_tap_ref,
    key_tap_ref,
    gain_ref,
    matrix_hbm,
    out_ref,
    value_in,
    gate_in,
    keys_in,
    value_rim,
    keys_rim,
    value_wide,
    keys_wide,
    gate_wide,
    conv_wide,
    x_s,
    kt_s,
    q_s,
    state_s,
    near_s,
    stride_s,
    run_s,
    fade_s,
    end_s,
    cols_s,
    own_pack,
    own_fade,
    mate_pack,
    mate_fade,
    chip_pack,
    chip_fade,
    all_pack,
    all_fade,
    enter_pack,
    carry_s,
    mixed_s,
    heads_in,
    matrix,
    acc_s,
    load_sem,
    rim_send,
    rim_recv,
    mate_send,
    mate_recv,
    chip_send,
    chip_recv,
    enter_send,
    enter_recv,
    head_send,
    head_recv,
    ring_send,
    ring_recv,
    pass_send,
    pass_recv,
):
    f32, bf16 = jnp.float32, jnp.bfloat16
    places, columns, width = dims["S"], dims["X"], dims["D"]
    blocks = columns
    rows = BLOCK
    half = columns // 2
    chips = places // 2
    me_x, me_s = lax.axis_index("tp"), lax.axis_index("sp")
    core = lax.rem(me_s, 2)
    me_y = lax.div(me_s, 2)
    right = {"tp": lax.rem(me_x + 1, columns)}
    left = {"tp": lax.rem(me_x + columns - 1, columns)}
    mate = {"sp": me_s + 1 - 2 * core}
    following = {"sp": lax.rem(me_s + 1, places)}
    previous = {"sp": lax.rem(me_s + places - 1, places)}

    def column(offset):
        return lax.rem(me_x + offset + columns, columns)

    def peer(offset):
        return {"sp": lax.rem(me_s + 2 * offset, places)}

    def remote(src, dst, send, recv, device):
        return pltpu.make_async_remote_copy(
            src_ref=src, dst_ref=dst, send_sem=send, recv_sem=recv, device_id=device, device_id_type=MESH
        )

    loads = [
        (matrix_hbm.at[0], matrix.at[me_x, pl.ds(0, rows), :]),
        (matrix_hbm.at[1], matrix.at[me_x, pl.ds(rows, rows), :]),
        (value_hbm, value_in),
        (keys_hbm, keys_in),
        (gate_hbm, gate_in),
    ]
    loads = [pltpu.make_async_copy(a, b, load_sem.at[n]) for n, (a, b) in enumerate(loads)]
    for load in loads:
        load.start()

    barrier = pltpu.get_barrier_semaphore()
    peers = [{"tp": column(i)} for i in range(1, columns)]
    peers += [peer(i) for i in range(1, chips)] + [following, previous]
    for device in peers:
        pl.semaphore_signal(barrier, inc=1, device_id=device, device_id_type=MESH)

    heads = 4
    for g in range(2):
        raw = raw_ref[g].astype(f32)
        for k in range(blocks):
            stride_s[heads * k + 2 * g : heads * k + 2 * g + 2, :] = raw[:, k * rows : (k + 1) * rows]
    for k in range(blocks):
        run_s[heads * k : heads * k + heads, :] = jnp.broadcast_to(extra_ref[k : k + 1, :], (heads, rows))
    head_of = jnp.bitwise_and(lax.broadcasted_iota(jnp.int32, (heads * blocks, rows), 0), heads - 1)

    def by_head(table):
        picked = jnp.full((heads * blocks, rows), table[1, 1], f32)
        for n in range(3):
            picked = jnp.where(head_of == n, table[n // 2, n % 2], picked)
        return picked

    shifted = stride_s[...] + by_head(bias_ref)
    stride = jnp.maximum(shifted, 0.0) + jnp.log1p(jnp.exp(-jnp.abs(shifted)))
    log_decay = run_s[...] - jnp.exp(by_head(log_ref)) * stride
    at_row = lax.broadcasted_iota(jnp.int32, (rows, rows), 0)
    at_lane = lax.broadcasted_iota(jnp.int32, (rows, rows), 1)
    running = jnp.dot(
        log_decay,
        jnp.where(at_row <= at_lane, 1.0, 0.0),
        preferred_element_type=f32,
        precision=lax.Precision.HIGHEST,
    )
    ends = jnp.broadcast_to(running[:, rows - 1 : rows], running.shape)
    stride_s[...] = stride
    run_s[...] = running
    fade_s[...] = jnp.exp(ends - running) * stride
    end_s[...] = jnp.exp(ends)
    turned = jnp.transpose(running)
    for k in range(blocks):
        cols_s[k, :, 0:heads] = turned[:, heads * k : heads * k + heads]

    first_head = lax.broadcasted_iota(jnp.int32, (rows, rows), 1) < HEAD_DIM

    def row_pair(table, k, g):
        low = table[pl.ds(heads * k + 2 * g, 1), :]
        high = table[pl.ds(heads * k + 2 * g + 1, 1), :]
        return jnp.where(first_head[0:1], low, high)

    pl.semaphore_wait(barrier, len(peers))
    for load in loads[:4]:
        load.wait()

    cut = width // 2
    mine = pl.ds(pl.multiple_of(core * rows, rows), rows)

    def ring(way, event, col):
        lanes = pl.ds(((event % 2) ^ way) * cut, cut)
        here = matrix.at[col, mine, lanes]
        return remote(
            here, here, ring_send.at[way, event], ring_recv.at[way, event], right if way == 0 else left
        )

    def passing(way, event, col):
        lanes = pl.ds(((event % 2) ^ way) * cut, cut)
        here = matrix.at[col, mine, lanes]
        return remote(here, here, pass_send.at[way, event], pass_recv.at[way, event], mate)

    for event in range(2):
        for way in range(2):
            if event < columns - 1:
                ring(way, event, me_x).start()

    def service(event):
        k = event // 2 + 1
        for way in range(2):
            col = column(-k if way == 0 else k)
            ring(way, event, col).wait_recv()
            if event + 2 < columns - 1:
                ring(way, event + 2, col).start()
            passing(way, event, col).start()

    rim_rows = 16
    positions = blocks * rows
    rims = [
        remote(
            value_in.at[pl.ds(2 * positions - rim_rows, rim_rows), :], value_rim, rim_send.at[0], rim_recv.at[0], following
        ),
        remote(keys_in.at[pl.ds(positions - rim_rows, rim_rows), :], keys_rim, rim_send.at[1], rim_recv.at[1], following),
    ]
    for rim in rims:
        rim.start()

    def silu(a):
        return a * (1.0 / (1.0 + jnp.exp(-a)))

    value_wide[rim_rows:, :] = value_in[...].astype(f32)
    keys_wide[rim_rows:, :] = keys_in[...].astype(f32)
    taps = value_tap_ref.shape[0] // 2
    value_tap = value_tap_ref[...].astype(f32)
    key_tap = key_tap_ref[...].astype(f32)
    even = jnp.bitwise_and(lax.broadcasted_iota(jnp.int32, (2 * rows, rows), 0), 1) == 0
    tap_rows = [jnp.where(even, value_tap[2 * j : 2 * j + 1], value_tap[2 * j + 1 : 2 * j + 2]) for j in range(taps)]

    def states_of(k):
        base = pl.multiple_of(k * 2 * rows, 2 * rows)
        window = value_wide[pl.ds(base, 2 * rows + rim_rows), :]
        total = jnp.zeros((2 * rows, rows), f32)
        for j in range(taps):
            start = rim_rows - 2 * (taps - 1 - j)
            total = total + window[start : start + 2 * rows] * tap_rows[j]
        conv_wide[...] = silu(total).astype(bf16).astype(f32)
        low = pl.multiple_of(k * rows, rows)
        window = keys_wide[pl.ds(low, rows + rim_rows), :]
        total = jnp.zeros((rows, keys_wide.shape[1]), f32)
        for j in range(taps):
            start = rim_rows - (taps - 1 - j)
            total = total + window[start : start + rows] * key_tap[j : j + 1]
        conv = silu(total).astype(bf16).astype(f32)
        both = conv[:, 0 : 2 * STATE_ONE]
        keys = [jnp.where(first_head, both, 0.0), conv[:, 2 * STATE_ONE : 2 * STATE_ONE + STATE_TWO]]
        asks = [pltpu.roll(both, STATE_ONE, 1), conv[:, 2 * STATE_ONE + STATE_TWO :]]
        for g in range(2):
            x = conv_wide[pl.ds(g, rows, stride=2), :].astype(bf16)
            key_t = jnp.transpose(keys[g])
            x_s[k, g] = x
            kt_s[k, g] = key_t.astype(bf16)
            q_s[k, g] = asks[g].astype(bf16)
            faded = jnp.concatenate(
                [key_t * fade_s[pl.ds(heads * k + 2 * g + h, 1), :] for h in range(2)], axis=0
            ).astype(bf16)
            state = jnp.dot(faded, x, preferred_element_type=f32)
            state_s[k, g] = jnp.where(first_head, state[:rows], state[rows:])

    def state_step(i, carry):
        states_of(i)
        return carry

    lax.fori_loop(1, blocks, state_step, 0)
    for rim in rims:
        rim.wait_recv()
    opening = me_s == 0
    value_wide[0:rim_rows, :] = jnp.where(opening, 0.0, value_rim[...].astype(f32))
    keys_wide[0:rim_rows, :] = jnp.where(opening, 0.0, keys_rim[...].astype(f32))
    states_of(0)

    packed = STATE_TWO + STATE_ONE
    piece = packed // 2

    def local_end(g):
        total = jnp.zeros((rows, rows), f32)
        faded = jnp.ones((1, rows), f32)
        for k in range(blocks):
            decay = row_pair(end_s, k, g)
            total = total * decay + state_s[k, g]
            faded = faded * decay
        return total, faded

    end_one, fade_one = local_end(0)
    end_two, fade_two = local_end(1)
    own = jnp.concatenate([end_two, end_one[:STATE_ONE]], axis=0)
    own_pack[...] = own.astype(bf16)
    own_fade[0:1, :] = fade_one
    own_fade[1:2, :] = fade_two
    own_fade[2:8, :] = jnp.zeros((6, rows), f32)
    mates = [
        remote(own_pack, mate_pack, mate_send.at[0], mate_recv.at[0], mate),
        remote(own_fade, mate_fade, mate_send.at[1], mate_recv.at[1], mate),
    ]
    for copy in mates:
        copy.start()
    service(0)
    for copy in mates:
        copy.wait_recv()
    is_low = core == 0
    low = jnp.where(is_low, own, mate_pack[...].astype(f32))
    high = jnp.where(is_low, mate_pack[...].astype(f32), own)
    mate_rows = mate_fade[...]
    own_rows = own_fade[...]
    high_rows = jnp.where(is_low, mate_rows, own_rows)
    in_two = lax.broadcasted_iota(jnp.int32, (packed, rows), 0) < STATE_TWO
    chip_pack[...] = (low * jnp.where(in_two, high_rows[1:2], high_rows[0:1]) + high).astype(bf16)
    chip_fade[...] = own_rows * mate_rows
    my_half = pl.ds(pl.multiple_of(core * piece, 16), piece)

    def to_chip(n, which):
        src = chip_pack.at[my_half, :] if which == 0 else chip_fade
        dst = all_pack.at[me_y] if which == 0 else all_fade.at[me_y]
        return remote(src, dst, chip_send.at[which, n], chip_recv.at[which, n], peer(n))

    for n in range(1, chips):
        for which in range(2):
            to_chip(n, which).start()

    below = at_row >= at_lane

    def near_step(k, carry):
        cols = cols_s[k]
        for g in range(2):
            scores = jnp.dot(q_s[k, g], kt_s[k, g], preferred_element_type=f32)
            parts = []
            for h in range(2):
                n = 2 * g + h
                gap = cols[:, n : n + 1] - run_s[pl.ds(heads * k + n, 1), :]
                damping = jnp.exp(jnp.where(below, gap, -1e30))
                parts.append((scores * damping * stride_s[pl.ds(heads * k + n, 1), :]).astype(bf16))
            near = jnp.dot(jnp.concatenate(parts, axis=0), x_s[k, g], preferred_element_type=f32)
            near_s[k, g] = jnp.where(first_head, near[:rows], near[rows:])
        return carry

    lax.fori_loop(0, blocks, near_step, 0)
    if columns > 2:
        service(1)
    loads[4].wait()

    for n in range(1, chips):
        for which in range(2):
            to_chip(n, which).wait_recv()
    row_at = lax.broadcasted_iota(jnp.int32, (piece, rows), 0) + core * piece
    half_two = row_at < STATE_TWO
    entering = jnp.zeros((piece, rows), f32)
    for y in range(chips):
        fades = all_fade[y]
        later = entering * jnp.where(half_two, fades[1:2], fades[0:1]) + all_pack[y].astype(f32)
        entering = jnp.where(y < me_y, later, entering)
    enter_pack[my_half, :] = entering.astype(bf16)
    here = enter_pack.at[my_half, :]
    enter_copy = remote(here, here, enter_send.at[0], enter_recv.at[0], mate)
    enter_copy.start()
    enter_copy.wait_recv()
    chip_state = enter_pack[...].astype(f32)
    after_low = chip_state * jnp.where(in_two, mate_rows[1:2], mate_rows[0:1]) + mate_pack[...].astype(f32)
    entered = jnp.where(is_low, chip_state, after_low)
    carry_s[1] = entered[:STATE_TWO]
    carry_s[0] = jnp.zeros((rows, rows), f32)
    carry_s[0, 0:STATE_ONE, :] = entered[STATE_TWO:]

    def head_copy(col):
        return remote(mixed_s.at[col], heads_in.at[me_x], head_send.at[col], head_recv.at[me_x], {"tp": col})

    def mix_step(k, carry):
        cols = jnp.exp(cols_s[k])
        gate_wide[...] = gate_in[pl.ds(pl.multiple_of(k * 2 * rows, 2 * rows), 2 * rows), :].astype(f32)
        for g in range(2):
            state = carry_s[g]
            coarse = state.astype(bf16)
            fine = (state - coarse.astype(f32)).astype(bf16)
            ask = q_s[k, g]
            far = jnp.dot(
                jnp.concatenate([ask, ask], axis=1),
                jnp.concatenate([coarse, fine], axis=0),
                preferred_element_type=f32,
            )
            reach = jnp.where(first_head, cols[:, 2 * g : 2 * g + 1], cols[:, 2 * g + 1 : 2 * g + 2])
            skip = jnp.where(first_head[0:1], skip_ref[g, 0], skip_ref[g, 1])
            mixed = near_s[k, g] + far * reach + skip * x_s[k, g].astype(f32)
            gate = gate_wide[pl.ds(g, rows, stride=2), :]
            gated = mixed * silu(gate)
            square = gated * gated
            one = jnp.sum(jnp.where(first_head, square, 0.0), axis=1, keepdims=True)
            two = jnp.sum(jnp.where(first_head, 0.0, square), axis=1, keepdims=True)
            scale = lax.rsqrt(jnp.where(first_head, one, two) * (1.0 / HEAD_DIM) + EPSILON)
            mixed_s[k, :, g * rows : (g + 1) * rows] = (gated * scale * gain_ref[g : g + 1, :]).astype(bf16)
            carry_s[g] = state * row_pair(end_s, k, g) + state_s[k, g]

        @pl.when(k != me_x)
        def _():
            head_copy(k).start()

        return carry

    lax.fori_loop(0, blocks, mix_step, 0)
    heads_in[me_x] = mixed_s[me_x]

    def arrived(col):
        return remote(mixed_s.at[col], heads_in.at[col], head_send.at[col], head_recv.at[col], {"tp": col})

    def product(col, first=False):
        for n in range(0, width, 512):
            part = jnp.dot(heads_in[col], matrix[col, :, n : n + 512], preferred_element_type=f32)
            acc_s[:, n : n + 512] = part if first else acc_s[:, n : n + 512] + part

    product(me_x, True)
    for event in range(2, columns - 1):
        service(event)
    for k in range(1, half + 1):
        for way in range(2):
            if way == 1 and k == half:
                continue
            for event in (2 * k - 2, 2 * k - 1):
                if event < columns - 1:
                    if k == half:
                        for side in range(2):
                            passing(side, event, column(k)).wait_recv()
                    else:
                        passing(way, event, column(k)).wait_recv()
            col = column(-k if way == 0 else k)
            arrived(col).wait_recv()
            product(col)
    out_ref[...] = (residual_ref[...].astype(f32) + acc_s[...]).astype(bf16)

    for copy in rims + mates + [enter_copy]:
        copy.wait_send()
    for n in range(1, chips):
        for which in range(2):
            to_chip(n, which).wait_send()
    for i in range(1, columns):
        head_copy(column(i)).wait_send()
    for event in range(columns - 1):
        for way in range(2):
            ring(way, event, me_x).wait_send()
            passing(way, event, me_x).wait_send()


def mixer_layer(
    residual, values, gates, keys, raw, bias, logarithm, extra, skip, value_taps, key_taps, gain, matrix, places, columns
):
    f32, bf16 = jnp.float32, jnp.bfloat16
    rows, width = residual.shape
    positions = values.shape[0]
    lanes = keys.shape[1]
    blocks = positions // BLOCK
    chips = places // 2
    packed = STATE_ONE + STATE_TWO
    dma = pltpu.SemaphoreType.DMA
    whole = pl.BlockSpec(memory_space=pltpu.VMEM)
    away = pl.BlockSpec(memory_space=pl.ANY)
    scalars = pl.BlockSpec(memory_space=pltpu.SMEM)
    square = (blocks, 2, BLOCK, BLOCK)
    return pl.pallas_call(
        functools.partial(mixer_kernel, dict(S=places, X=columns, D=width)),
        out_shape=jax.ShapeDtypeStruct((rows, width), bf16),
        in_specs=[
            whole, away, away, away, whole, scalars, scalars, whole, scalars, whole, whole, whole, away,
        ],
        out_specs=whole,
        scratch_shapes=[
            pltpu.VMEM((2 * positions, BLOCK), bf16),
            pltpu.VMEM((2 * positions, BLOCK), bf16),
            pltpu.VMEM((positions, lanes), bf16),
            pltpu.VMEM((16, BLOCK), bf16),
            pltpu.VMEM((16, lanes), bf16),
            pltpu.VMEM((2 * positions + 16, BLOCK), f32),
            pltpu.VMEM((positions + 16, lanes), f32),
            pltpu.VMEM((2 * BLOCK, BLOCK), f32),
            pltpu.VMEM((2 * BLOCK, BLOCK), f32),
            pltpu.VMEM(square, bf16),
            pltpu.VMEM(square, bf16),
            pltpu.VMEM(square, bf16),
            pltpu.VMEM(square, f32),
            pltpu.VMEM(square, f32),
            pltpu.VMEM((4 * blocks, BLOCK), f32),
            pltpu.VMEM((4 * blocks, BLOCK), f32),
            pltpu.VMEM((4 * blocks, BLOCK), f32),
            pltpu.VMEM((4 * blocks, BLOCK), f32),
            pltpu.VMEM((blocks, BLOCK, 4), f32),
            pltpu.VMEM((packed, BLOCK), bf16),
            pltpu.VMEM((8, BLOCK), f32),
            pltpu.VMEM((packed, BLOCK), bf16),
            pltpu.VMEM((8, BLOCK), f32),
            pltpu.VMEM((packed, BLOCK), bf16),
            pltpu.VMEM((8, BLOCK), f32),
            pltpu.VMEM((chips, packed // 2, BLOCK), bf16),
            pltpu.VMEM((chips, 8, BLOCK), f32),
            pltpu.VMEM((packed, BLOCK), bf16),
            pltpu.VMEM((2, BLOCK, BLOCK), f32),
            pltpu.VMEM((columns, BLOCK, 2 * BLOCK), bf16),
            pltpu.VMEM((columns, BLOCK, 2 * BLOCK), bf16),
            pltpu.VMEM((columns, 2 * BLOCK, width), bf16),
            pltpu.VMEM((rows, width), f32),
            dma((5,)),
            dma((2,)),
            dma((2,)),
            dma((2,)),
            dma((2,)),
            dma((2, chips)),
            dma((2, chips)),
            dma((1,)),
            dma((1,)),
            dma((columns,)),
            dma((columns,)),
            dma((2, columns - 1)),
            dma((2, columns - 1)),
            dma((2, columns - 1)),
            dma((2, columns - 1)),
        ],
        compiler_params=pltpu.CompilerParams(
            collective_id=1, has_side_effects=True, vmem_limit_bytes=VMEM_LIMIT
        ),
        name="mixer",
    )(
        residual,
        values.reshape(2 * positions, BLOCK),
        gates.reshape(2 * positions, BLOCK),
        keys,
        raw.transpose(1, 2, 0),
        bias,
        logarithm,
        extra.reshape(blocks, BLOCK),
        skip,
        value_taps.reshape(-1, BLOCK),
        key_taps,
        gain,
        matrix,
    )


def local(
    residual,
    grouped_value_heads,
    output_gate_heads,
    projected_key_query,
    raw_step_size,
    step_size_bias,
    head_decay_logarithm,
    position_extra_decay,
    head_skip_weight,
    value_kernel_taps,
    key_query_kernel,
    head_norm_gain,
    output_matrix,
    expert_norm_gain,
    expert_gate_weight,
    expert_up_weight,
    expert_down_weight,
    token_expert_choice,
    expert_output_weight,
):
    places, columns = lax.axis_size("sp"), lax.axis_size("tp")
    stream = mixer_layer(
        residual,
        grouped_value_heads,
        output_gate_heads,
        projected_key_query,
        raw_step_size,
        step_size_bias,
        head_decay_logarithm,
        position_extra_decay,
        head_skip_weight,
        value_kernel_taps,
        key_query_kernel,
        head_norm_gain,
        output_matrix,
        places,
        columns,
    )
    return expert_layer(
        stream,
        expert_norm_gain[None],
        token_expert_choice.T,
        expert_output_weight.T,
        expert_gate_weight,
        expert_up_weight,
        expert_down_weight,
        places,
        columns,
    )


def solution(mesh):
    placed = (
        P(("grp", "sp", "tp"), None),
        P(("grp", "sp"), None, "tp"),
        P(("grp", "sp"), None, "tp"),
        P(("grp", "sp"), None),
        P(("grp", "sp"), None, "tp"),
        P(None, "tp"),
        P(None, "tp"),
        P(("grp", "sp")),
        P(None, "tp"),
        P(None, None, "tp"),
        P(),
        P(None, "tp"),
        P(None, "tp", None),
        P(),
        P("sp", None, "tp"),
        P("sp", None, "tp"),
        P("sp", "tp", None),
        P(("grp", "sp", "tp"), None),
        P(("grp", "sp", "tp"), None),
    )
    return jax.shard_map(
        local, mesh=mesh, in_specs=placed, out_specs=P(("grp", "sp", "tp"), None), check_vma=False
    )
```

```python
import functools
import types

import jax
import jax.numpy as jnp
from jax import lax
from jax.experimental import pallas as pl
from jax.experimental.pallas import tpu as pltpu
from jax.sharding import PartitionSpec as P

HEAD_DIM = 64
STATE_ONE = 64
STATE_TWO = 128
BLOCK = 128
EPSILON = 1e-06

MESH = pl.DeviceIdType.MESH
PIECE = 256
HEADS = 4
VMEM_LIMIT = 67043328


def remote(src, dst, send, recv, device):
    return pltpu.make_async_remote_copy(
        src_ref=src, dst_ref=dst, send_sem=send, recv_sem=recv, device_id=device, device_id_type=MESH
    )


def silu(a):
    return a * (1.0 / (1.0 + jnp.exp(-a)))


def layer_kernel(dims, names, *refs):
    r = types.SimpleNamespace(**dict(zip(names, refs, strict=True)))
    f32, bf16 = jnp.float32, jnp.bfloat16
    places, columns, width, rows = dims.places, dims.columns, dims.width, BLOCK
    half, chips, blocks = columns // 2, places // 2, columns
    me_x, me_s = lax.axis_index("tp"), lax.axis_index("sp")
    core, me_y = lax.rem(me_s, 2), lax.div(me_s, 2)
    right = {"tp": lax.rem(me_x + 1, columns)}
    left = {"tp": lax.rem(me_x + columns - 1, columns)}
    mate = {"sp": me_s + 1 - 2 * core}
    following = {"sp": lax.rem(me_s + 1, places)}

    def column(offset):
        return lax.rem(me_x + offset + columns, columns)

    def place(offset):
        return lax.rem(me_s + offset, places)

    def peer(offset):
        return {"sp": lax.rem(me_s + 2 * offset, places)}

    def toward(way):
        return right if way == 0 else left

    loads = [
        (r.matrix_hbm.at[0], r.matrix.at[me_x, pl.ds(0, rows), :]),
        (r.matrix_hbm.at[1], r.matrix.at[me_x, pl.ds(rows, rows), :]),
        (r.value_hbm, r.value_in),
        (r.keys_hbm, r.keys_in),
        (r.gate_hbm, r.gate_in),
    ]
    early = len(loads)
    for t in range(dims.tiles):
        span = pl.ds(t * 128, 128)
        loads.append((r.expert_gate_hbm.at[0, :, span], r.gate_up.at[t, :, pl.ds(0, 128)]))
        loads.append((r.expert_up_hbm.at[0, :, span], r.gate_up.at[t, :, pl.ds(128, 128)]))
    for p in range(dims.pieces):
        loads.append((r.expert_down_hbm.at[0, :, pl.ds(p * PIECE, PIECE)], r.down.at[p]))
    loads = [pltpu.make_async_copy(a, b, r.load_sem.at[n]) for n, (a, b) in enumerate(loads)]
    for load in loads:
        load.start()

    barrier = pltpu.get_barrier_semaphore()
    peers = [{"tp": column(i)} for i in range(1, columns)] + [{"sp": place(i)} for i in range(1, places)]
    for device in peers:
        pl.semaphore_signal(barrier, inc=1, device_id=device, device_id_type=MESH)

    for g in range(2):
        raw = r.raw_ref[g].astype(f32)
        for k in range(blocks):
            r.stride_s[HEADS * k + 2 * g : HEADS * k + 2 * g + 2, :] = raw[:, k * rows : (k + 1) * rows]
    for k in range(blocks):
        r.run_s[HEADS * k : HEADS * k + HEADS, :] = jnp.broadcast_to(r.extra_ref[k : k + 1, :], (HEADS, rows))
    head_of = jnp.bitwise_and(lax.broadcasted_iota(jnp.int32, (HEADS * blocks, rows), 0), HEADS - 1)

    def by_head(table):
        picked = jnp.full((HEADS * blocks, rows), table[1, 1], f32)
        for n in range(3):
            picked = jnp.where(head_of == n, table[n // 2, n % 2], picked)
        return picked

    shifted = r.stride_s[...] + by_head(r.bias_ref)
    stride = jnp.maximum(shifted, 0.0) + jnp.log1p(jnp.exp(-jnp.abs(shifted)))
    log_decay = r.run_s[...] - jnp.exp(by_head(r.log_ref)) * stride
    at_row = lax.broadcasted_iota(jnp.int32, (rows, rows), 0)
    at_lane = lax.broadcasted_iota(jnp.int32, (rows, rows), 1)
    running = jnp.dot(
        log_decay,
        jnp.where(at_row <= at_lane, 1.0, 0.0),
        preferred_element_type=f32,
        precision=lax.Precision.HIGHEST,
    )
    ends = jnp.broadcast_to(running[:, rows - 1 : rows], running.shape)
    r.stride_s[...] = stride
    r.run_s[...] = running
    r.fade_s[...] = jnp.exp(ends - running) * stride
    r.end_s[...] = jnp.exp(ends)
    turned = jnp.transpose(running)
    for k in range(blocks):
        r.cols_s[k, :, 0:HEADS] = turned[:, HEADS * k : HEADS * k + HEADS]

    first_head = at_lane < HEAD_DIM

    def row_pair(table, k, g):
        low = table[pl.ds(HEADS * k + 2 * g, 1), :]
        high = table[pl.ds(HEADS * k + 2 * g + 1, 1), :]
        return jnp.where(first_head[0:1], low, high)

    r.tables[me_x] = jnp.zeros((8, rows), f32)
    r.tables[me_x, 0:2, :] = r.choice_ref[...].astype(f32)
    r.tables[me_x, 2:4, :] = r.share_ref[...]

    for load in loads[: early - 1]:
        load.wait()
    pl.semaphore_wait(barrier, len(peers))

    cut = width // 2
    mine = pl.ds(pl.multiple_of(core * rows, rows), rows)

    def matrix_ring(way, event, col):
        here = r.matrix.at[col, mine, pl.ds(((event % 2) ^ way) * cut, cut)]
        return remote(here, here, r.ring_send.at[way, event], r.ring_recv.at[way, event], toward(way))

    def matrix_pass(way, event, col):
        here = r.matrix.at[col, mine, pl.ds(((event % 2) ^ way) * cut, cut)]
        return remote(here, here, r.pass_send.at[way, event], r.pass_recv.at[way, event], mate)

    rim_rows = 16
    positions = blocks * rows
    rims = [
        remote(
            r.value_in.at[pl.ds(2 * positions - rim_rows, rim_rows), :],
            r.value_rim,
            r.rim_send.at[0],
            r.rim_recv.at[0],
            following,
        ),
        remote(
            r.keys_in.at[pl.ds(positions - rim_rows, rim_rows), :], r.keys_rim, r.rim_send.at[1], r.rim_recv.at[1], following
        ),
    ]
    for rim in rims:
        rim.start()

    def table_copy(offset):
        return remote(
            r.tables.at[me_x],
            r.tables.at[me_x],
            r.table_send.at[offset],
            r.table_recv.at[columns - offset],
            {"tp": column(offset)},
        )

    for i in range(1, columns):
        table_copy(i).start()
    for event in range(2):
        for way in range(2):
            if event < columns - 1:
                matrix_ring(way, event, me_x).start()

    def service(event):
        k = event // 2 + 1
        for way in range(2):
            col = column(-k if way == 0 else k)
            matrix_ring(way, event, col).wait_recv()
            if event + 2 < columns - 1:
                matrix_ring(way, event + 2, col).start()
            matrix_pass(way, event, col).start()

    r.value_wide[rim_rows:, :] = r.value_in[...].astype(f32)
    r.keys_wide[rim_rows:, :] = r.keys_in[...].astype(f32)
    taps = r.value_tap_ref.shape[0] // 2
    value_tap = r.value_tap_ref[...].astype(f32)
    key_tap = r.key_tap_ref[...].astype(f32)
    even = jnp.bitwise_and(lax.broadcasted_iota(jnp.int32, (2 * rows, rows), 0), 1) == 0
    tap_rows = [jnp.where(even, value_tap[2 * j : 2 * j + 1], value_tap[2 * j + 1 : 2 * j + 2]) for j in range(taps)]

    def states_of(k):
        window = r.value_wide[pl.ds(pl.multiple_of(k * 2 * rows, 2 * rows), 2 * rows + rim_rows), :]
        total = jnp.zeros((2 * rows, rows), f32)
        for j in range(taps):
            start = rim_rows - 2 * (taps - 1 - j)
            total = total + window[start : start + 2 * rows] * tap_rows[j]
        r.conv_wide[...] = silu(total).astype(bf16).astype(f32)
        window = r.keys_wide[pl.ds(pl.multiple_of(k * rows, rows), rows + rim_rows), :]
        total = jnp.zeros((rows, r.keys_wide.shape[1]), f32)
        for j in range(taps):
            start = rim_rows - (taps - 1 - j)
            total = total + window[start : start + rows] * key_tap[j : j + 1]
        conv = silu(total).astype(bf16).astype(f32)
        both = conv[:, 0 : 2 * STATE_ONE]
        keys = [jnp.where(first_head, both, 0.0), conv[:, 2 * STATE_ONE : 2 * STATE_ONE + STATE_TWO]]
        asks = [pltpu.roll(both, STATE_ONE, 1), conv[:, 2 * STATE_ONE + STATE_TWO :]]
        for g in range(2):
            x = r.conv_wide[pl.ds(g, rows, stride=2), :].astype(bf16)
            key_t = jnp.transpose(keys[g])
            r.x_s[k, g] = x
            r.kt_s[k, g] = key_t.astype(bf16)
            r.q_s[k, g] = asks[g].astype(bf16)
            faded = jnp.concatenate(
                [key_t * r.fade_s[pl.ds(HEADS * k + 2 * g + h, 1), :] for h in range(2)], axis=0
            ).astype(bf16)
            state = jnp.dot(faded, x, preferred_element_type=f32)
            r.state_s[k, g] = jnp.where(first_head, state[:rows], state[rows:])

    def state_step(i, carry):
        states_of(i)
        return carry

    lax.fori_loop(1, blocks, state_step, 0)
    for rim in rims:
        rim.wait_recv()
    opening = me_s == 0
    r.value_wide[0:rim_rows, :] = jnp.where(opening, 0.0, r.value_rim[...].astype(f32))
    r.keys_wide[0:rim_rows, :] = jnp.where(opening, 0.0, r.keys_rim[...].astype(f32))
    states_of(0)

    packed = STATE_TWO + STATE_ONE
    piece = packed // 2

    def local_end(g):
        total = jnp.zeros((rows, rows), f32)
        faded = jnp.ones((1, rows), f32)
        for k in range(blocks):
            decay = row_pair(r.end_s, k, g)
            total = total * decay + r.state_s[k, g]
            faded = faded * decay
        return total, faded

    end_one, fade_one = local_end(0)
    end_two, fade_two = local_end(1)
    own = jnp.concatenate([end_two, end_one[:STATE_ONE]], axis=0)
    r.own_pack[...] = own.astype(bf16)
    r.own_fade[0:1, :] = fade_one
    r.own_fade[1:2, :] = fade_two
    r.own_fade[2:8, :] = jnp.zeros((6, rows), f32)
    mates = [
        remote(r.own_pack, r.mate_pack, r.mate_send.at[0], r.mate_recv.at[0], mate),
        remote(r.own_fade, r.mate_fade, r.mate_send.at[1], r.mate_recv.at[1], mate),
    ]
    for copy in mates:
        copy.start()
    service(0)
    for copy in mates:
        copy.wait_recv()
    is_low = core == 0
    low = jnp.where(is_low, own, r.mate_pack[...].astype(f32))
    high = jnp.where(is_low, r.mate_pack[...].astype(f32), own)
    mate_rows = r.mate_fade[...]
    own_rows = r.own_fade[...]
    high_rows = jnp.where(is_low, mate_rows, own_rows)
    in_two = lax.broadcasted_iota(jnp.int32, (packed, rows), 0) < STATE_TWO
    r.chip_pack[...] = (low * jnp.where(in_two, high_rows[1:2], high_rows[0:1]) + high).astype(bf16)
    r.chip_fade[...] = own_rows * mate_rows
    my_half = pl.ds(pl.multiple_of(core * piece, 16), piece)

    def to_chip(n, which):
        src = r.chip_pack.at[my_half, :] if which == 0 else r.chip_fade
        dst = r.all_pack.at[me_y] if which == 0 else r.all_fade.at[me_y]
        return remote(src, dst, r.chip_send.at[which, n], r.chip_recv.at[which, n], peer(n))

    for n in range(1, chips):
        for which in range(2):
            to_chip(n, which).start()

    below = at_row >= at_lane

    def near_step(k, carry):
        cols = r.cols_s[k]
        for g in range(2):
            scores = jnp.dot(r.q_s[k, g], r.kt_s[k, g], preferred_element_type=f32)
            parts = []
            for h in range(2):
                n = 2 * g + h
                gap = cols[:, n : n + 1] - r.run_s[pl.ds(HEADS * k + n, 1), :]
                damping = jnp.exp(jnp.where(below, gap, -1e30))
                parts.append((scores * damping * r.stride_s[pl.ds(HEADS * k + n, 1), :]).astype(bf16))
            near = jnp.dot(jnp.concatenate(parts, axis=0), r.x_s[k, g], preferred_element_type=f32)
            r.near_s[k, g] = jnp.where(first_head, near[:rows], near[rows:])
        return carry

    lax.fori_loop(0, blocks, near_step, 0)
    if columns > 2:
        service(1)
    loads[early - 1].wait()

    for n in range(1, chips):
        for which in range(2):
            to_chip(n, which).wait_recv()
    row_at = lax.broadcasted_iota(jnp.int32, (piece, rows), 0) + core * piece
    half_two = row_at < STATE_TWO
    entering = jnp.zeros((piece, rows), f32)
    for y in range(chips):
        fades = r.all_fade[y]
        later = entering * jnp.where(half_two, fades[1:2], fades[0:1]) + r.all_pack[y].astype(f32)
        entering = jnp.where(y < me_y, later, entering)
    r.enter_pack[my_half, :] = entering.astype(bf16)
    here = r.enter_pack.at[my_half, :]
    enter_copy = remote(here, here, r.enter_send.at[0], r.enter_recv.at[0], mate)
    enter_copy.start()
    enter_copy.wait_recv()
    chip_state = r.enter_pack[...].astype(f32)
    after_low = chip_state * jnp.where(in_two, mate_rows[1:2], mate_rows[0:1]) + r.mate_pack[...].astype(f32)
    entered = jnp.where(is_low, chip_state, after_low)
    r.carry_s[1] = entered[:STATE_TWO]
    r.carry_s[0] = jnp.zeros((rows, rows), f32)
    r.carry_s[0, 0:STATE_ONE, :] = entered[STATE_TWO:]

    def head_copy(col):
        return remote(r.mixed_s.at[col], r.heads_in.at[me_x], r.head_send.at[col], r.head_recv.at[me_x], {"tp": col})

    def mix_step(k, carry):
        cols = jnp.exp(r.cols_s[k])
        r.gate_wide[...] = r.gate_in[pl.ds(pl.multiple_of(k * 2 * rows, 2 * rows), 2 * rows), :].astype(f32)
        for g in range(2):
            state = r.carry_s[g]
            coarse = state.astype(bf16)
            fine = (state - coarse.astype(f32)).astype(bf16)
            ask = r.q_s[k, g]
            far = jnp.dot(
                jnp.concatenate([ask, ask], axis=1),
                jnp.concatenate([coarse, fine], axis=0),
                preferred_element_type=f32,
            )
            reach = jnp.where(first_head, cols[:, 2 * g : 2 * g + 1], cols[:, 2 * g + 1 : 2 * g + 2])
            skip = jnp.where(first_head[0:1], r.skip_ref[g, 0], r.skip_ref[g, 1])
            mixed = r.near_s[k, g] + far * reach + skip * r.x_s[k, g].astype(f32)
            gated = mixed * silu(r.gate_wide[pl.ds(g, rows, stride=2), :])
            square = gated * gated
            one = jnp.sum(jnp.where(first_head, square, 0.0), axis=1, keepdims=True)
            two = jnp.sum(jnp.where(first_head, 0.0, square), axis=1, keepdims=True)
            scale = lax.rsqrt(jnp.where(first_head, one, two) * (1.0 / HEAD_DIM) + EPSILON)
            r.mixed_s[k, :, g * rows : (g + 1) * rows] = (gated * scale * r.head_gain_ref[g : g + 1, :]).astype(bf16)
            r.carry_s[g] = state * row_pair(r.end_s, k, g) + r.state_s[k, g]

        @pl.when(k != me_x)
        def _():
            head_copy(k).start()

        return carry

    lax.fori_loop(0, blocks, mix_step, 0)
    r.heads_in[me_x] = r.mixed_s[me_x]

    main, over, slots = dims.main, dims.over, places * dims.main
    total_slots = slots + over
    slot_row = lax.broadcasted_iota(jnp.int32, (total_slots, over), 0)
    slot_expert = lax.broadcasted_iota(jnp.int32, (total_slots, over), 1)
    spread = jnp.where(
        ((slot_row < slots) & (slot_row >= slot_expert * main) & (slot_row < slot_expert * main + main))
        | (slot_row == slots + slot_expert),
        1.0,
        0.0,
    ).astype(bf16)
    at = lax.broadcasted_iota(jnp.int32, (total_slots, rows), 0)
    turn = jnp.where(at < slots, jnp.bitwise_and(at, main - 1), main).astype(f32)
    expert_at = lax.broadcasted_iota(jnp.int32, (over, rows), 0).astype(f32)
    earlier = jnp.where(at_row < at_lane, 1.0, 0.0).astype(bf16)

    def make_put(col):
        table = r.tables[col]
        named = jnp.where((expert_at == table[0:1]) | (expert_at == table[1:2]), 1.0, 0.0)
        rank = jnp.dot(named.astype(bf16), earlier, preferred_element_type=f32)
        named_x = jnp.dot(spread, named.astype(bf16), preferred_element_type=f32)
        rank_x = jnp.dot(spread, rank.astype(bf16), preferred_element_type=f32)
        r.put[col] = jnp.where(rank_x == turn, named_x, 0.0).astype(bf16)

    for i in range(1, columns):
        table_copy(i).wait_recv()

    def put_step(col, carry):
        make_put(col)
        return carry

    lax.fori_loop(0, columns, put_step, 0)

    slot_col = lax.broadcasted_iota(jnp.int32, (over, total_slots), 1)
    slot_exp = lax.broadcasted_iota(jnp.int32, (over, total_slots), 0)
    spread_t = jnp.where(
        ((slot_col < slots) & (slot_col >= slot_exp * main) & (slot_col < slot_exp * main + main))
        | (slot_col == slots + slot_exp),
        1.0,
        0.0,
    ).astype(bf16)
    at_t = lax.broadcasted_iota(jnp.int32, (rows, total_slots), 1)
    turn_t = jnp.where(at_t < slots, jnp.bitwise_and(at_t, main - 1), main).astype(f32)
    expert_to = lax.broadcasted_iota(jnp.int32, (rows, over), 1).astype(f32)
    later_t = jnp.where(at_lane < at_row, 1.0, 0.0).astype(bf16)

    def make_pick(col):
        table = jnp.transpose(r.tables[col])
        named = [jnp.where(expert_to == table[:, k : k + 1], 1.0, 0.0) for k in range(2)]
        rank = jnp.dot(later_t, (named[0] + named[1]).astype(bf16), preferred_element_type=f32)
        rank_x = jnp.dot(rank.astype(bf16), spread_t, preferred_element_type=f32)
        for k in range(2):
            named_x = jnp.dot(named[k].astype(bf16), spread_t, preferred_element_type=f32)
            r.pick[col, k] = jnp.where(rank_x == turn_t, named_x, 0.0).astype(bf16)
            r.share_s[col, k] = jnp.broadcast_to(table[:, 2 + k : 3 + k], (rows, rows))

    def arrived(col):
        return remote(r.mixed_s.at[col], r.heads_in.at[col], r.head_send.at[col], r.head_recv.at[col], {"tp": col})

    def product(col, first=False):
        for n in range(0, width, 512):
            part = jnp.dot(r.heads_in[col], r.matrix[col, :, n : n + 512], preferred_element_type=f32)
            r.acc_s[:, n : n + 512] = part if first else r.acc_s[:, n : n + 512] + part

    product(me_x, True)
    for event in range(2, columns - 1):
        service(event)
    for k in range(1, half + 1):
        for way in range(2):
            if way == 1 and k == half:
                continue
            for event in (2 * k - 2, 2 * k - 1):
                if event < columns - 1:
                    for side in range(2) if k == half else (way,):
                        matrix_pass(side, event, column(k if side else -k)).wait_recv()
            col = column(-k if way == 0 else k)
            arrived(col).wait_recv()
            product(col)

    stream = (r.residual_ref[...].astype(f32) + r.acc_s[...]).astype(bf16)
    r.stream_s[...] = stream
    wide = stream.astype(f32)
    scale = lax.rsqrt(jnp.mean(wide * wide, axis=1, keepdims=True) + EPSILON)
    normed = (wide * scale * r.expert_gain_ref[...]).astype(bf16)

    direct, extra = dims.direct, dims.pieces - dims.direct
    pieces = dims.pieces
    lanes_of = PIECE // 128

    def lines(index):
        return pl.ds(pl.multiple_of(index * main, main), main)

    def far(way, p):
        odd = lax.rem(p, 2) if not isinstance(p, int) else p % 2
        return half - odd if way == 0 else half - 1 + odd

    for q in range(extra):
        r.tokens[me_x, q] = normed[:, (direct + q) * PIECE : (direct + q + 1) * PIECE]

    def token_ring(way, step, q, col):
        here = r.tokens.at[col, q]
        return remote(here, here, r.token_send.at[way, step, q], r.token_recv.at[way, step, q], toward(way))

    put_own = r.put[me_x]
    for p in range(direct):
        part = jnp.dot(put_own, normed[:, p * PIECE : (p + 1) * PIECE], preferred_element_type=f32)
        r.outbound[p] = part[:slots].astype(bf16)
        for c in range(lanes_of):
            r.over_out[:, p * lanes_of + c, :] = part[slots:, c * 128 : (c + 1) * 128]
    for q in range(extra):
        for way in range(2):
            token_ring(way, 0, q, me_x).start()

    for i in range(1, places):
        remote(
            r.over_out.at[place(i)], r.over_in.at[me_s], r.over_send.at[0], r.over_recv.at[0], {"sp": place(i)}
        ).start()

    def send_out(p, carry):
        for i in range(1, places):
            remote(
                r.outbound.at[p, lines(place(i)), :],
                r.chunks.at[me_x, p, lines(me_s), :],
                r.out_send.at[p],
                r.out_recv.at[p],
                {"sp": place(i)},
            ).start()
        r.chunks[me_x, p, lines(me_s), :] = r.outbound[p, lines(me_s), :]
        return carry

    lax.fori_loop(0, direct, send_out, 0)
    r.over_in[me_s] = r.over_out[me_s]
    if places < over:
        r.over_in[places:over] = jnp.zeros((over - places, *r.over_in.shape[1:]), f32)
        r.over_ret[places:over] = jnp.zeros((over - places, *r.over_ret.shape[1:]), f32)
        r.xover_in[:, places:over] = jnp.zeros((columns, over - places, *r.xover_in.shape[2:]), f32)
        r.xover_ret[:, places:over] = jnp.zeros((columns, over - places, *r.xover_ret.shape[2:]), f32)

    def route(offset):
        col = column(offset)
        for q in range(extra):
            part = jnp.dot(r.put[col], r.tokens[col, q], preferred_element_type=f32)
            r.xout[col, q] = part[:slots].astype(bf16)
            r.chunks[col, direct + q, lines(me_s), :] = r.xout[col, q, lines(me_s), :]
            for c in range(lanes_of):
                r.xover_out[offset, :, q * lanes_of + c, :] = part[slots:, c * 128 : (c + 1) * 128]
        r.xover_in[offset, me_s] = r.xover_out[offset, me_s]
        for i in range(1, places):
            remote(
                r.xout.at[col, :, lines(place(i)), :],
                r.chunks.at[col, pl.ds(direct, extra), lines(me_s), :],
                r.xout_send.at[offset],
                r.xout_recv.at[offset],
                {"sp": place(i)},
            ).start()
            remote(
                r.xover_out.at[offset, place(i)],
                r.xover_in.at[offset, me_s],
                r.xover_send.at[0, offset],
                r.xover_recv.at[0, offset],
                {"sp": place(i)},
            ).start()

    def routed(offset):
        col = column(offset)
        most = pl.ds(0, (places - 1) * main)
        return (
            remote(
                r.xout.at[col, :, most, :],
                r.chunks.at[col, pl.ds(direct, extra), most, :],
                r.xout_send.at[offset],
                r.xout_recv.at[offset],
                right,
            ),
            remote(
                r.xover_out.at[offset, 0 : places - 1],
                r.xover_in.at[offset, 0 : places - 1],
                r.xover_send.at[0, offset],
                r.xover_recv.at[0, offset],
                right,
            ),
        )

    def take_routed(offset):
        col = column(offset)
        for copy in routed(offset):
            copy.wait_recv()
        for q in range(extra):
            for c in range(lanes_of):
                r.chunks[col, direct + q, slots:, c * 128 : (c + 1) * 128] = r.xover_in[
                    offset, :, q * lanes_of + c, :
                ].astype(bf16)

    route(0)

    def token_event(k):
        for q in range(extra):
            for way in range(2):
                if k <= far(way, q):
                    col = column(-k if way == 0 else k)
                    token_ring(way, k - 1, q, col).wait_recv()
                    if k < far(way, q):
                        token_ring(way, k, q, col).start()
        if k < half:
            route(columns - k)
        route(k)

    def chunk_ring(way, step, p, col):
        here = r.chunks.at[col, p]
        return remote(here, here, r.chunk_send.at[way, step, p], r.chunk_recv.at[way, step, p], toward(way))

    def out_arrived(p):
        most = pl.ds(0, (places - 1) * main)
        return remote(
            r.outbound.at[p, most, :], r.chunks.at[me_x, p, most, :], r.out_send.at[p], r.out_recv.at[p], right
        )

    def start_piece(p):
        out_arrived(p).wait_recv()
        chunk_ring(0, 0, p, me_x).start()
        chunk_ring(1, 0, p, me_x).start()

    remote(
        r.over_out.at[0 : places - 1], r.over_in.at[0 : places - 1], r.over_send.at[0], r.over_recv.at[0], right
    ).wait_recv()
    for c in range(direct * lanes_of):
        at_lanes = (c % lanes_of) * 128
        r.chunks[me_x, c // lanes_of, slots:, at_lanes : at_lanes + 128] = r.over_in[:, c, :].astype(bf16)
    for n in range(max(direct, half)):
        if n < direct:
            start_piece(n)
        if n < half:
            token_event(n + 1)

    def offset_of(n):
        k = lax.div(n + 1, 2)
        return jnp.where(lax.rem(n, 2) == 1, lax.rem(columns - k, columns), k)

    def unit(n, t):
        offset = offset_of(n)
        col = column(offset)
        pl.when(t == 0)(lambda: take_routed(offset))
        acc = jnp.dot(r.chunks[col, 0], r.gate_up[t, 0:PIECE, :], preferred_element_type=f32)
        for q in range(1, pieces):
            acc = acc + jnp.dot(
                r.chunks[col, q], r.gate_up[t, q * PIECE : (q + 1) * PIECE, :], preferred_element_type=f32
            )
        value = silu(acc[:, 0:128]) * acc[:, 128:256]
        r.hidden[col, :, pl.ds(pl.multiple_of(t * 128, 128), 128)] = value.astype(bf16)
        pl.when(t == dims.tiles - 1)(lambda: give_back(offset))

    def own(col, p):
        return jnp.dot(r.hidden[col], r.down[p], preferred_element_type=f32)

    def give_back(offset):
        col = column(offset)
        for q in range(extra):
            part = own(col, direct + q)
            r.xback[col, q] = part[:slots].astype(bf16)
            r.xret[col, q, lines(me_s), :] = r.xback[col, q, lines(me_s), :]
            for c in range(lanes_of):
                r.xover_back[offset, :, q * lanes_of + c, :] = part[slots:, c * 128 : (c + 1) * 128]
        r.xover_ret[offset, me_s] = r.xover_back[offset, me_s]
        for i in range(1, places):
            remote(
                r.xback.at[col, :, lines(place(i)), :],
                r.xret.at[col, :, lines(me_s), :],
                r.xback_send.at[offset],
                r.xback_recv.at[offset],
                {"sp": place(i)},
            ).start()
            remote(
                r.xover_back.at[offset, place(i)],
                r.xover_ret.at[offset, me_s],
                r.xover_send.at[1, offset],
                r.xover_recv.at[1, offset],
                {"sp": place(i)},
            ).start()

    def given_back(offset):
        col = column(offset)
        most = pl.ds(0, (places - 1) * main)
        return (
            remote(
                r.xback.at[col, :, most, :],
                r.xret.at[col, :, most, :],
                r.xback_send.at[offset],
                r.xback_recv.at[offset],
                right,
            ),
            remote(
                r.xover_back.at[offset, 0 : places - 1],
                r.xover_ret.at[offset, 0 : places - 1],
                r.xover_send.at[1, offset],
                r.xover_recv.at[1, offset],
                right,
            ),
        )

    for load in loads[early:]:
        load.wait()

    def units(low, high):
        def body(v, carry):
            unit(lax.div(v, dims.tiles), lax.rem(v, dims.tiles))
            return carry

        lax.fori_loop(low, high, body, 0)

    share_of = dims.schedule
    for k in range(1, half + 1):
        first, last = share_of[k - 1] * dims.tiles, share_of[k] * dims.tiles

        def pass_on(p, carry, k=k, first=first, last=last):
            for way in range(2):
                col = column(-k if way == 0 else k)

                @pl.when(k <= far(way, p))
                def _():
                    chunk_ring(way, k - 1, p, col).wait_recv()

                if k < half:

                    @pl.when(k < far(way, p))
                    def _():
                        chunk_ring(way, k, p, col).start()

            if last > first:
                units(
                    first + lax.div(p * (last - first), direct), first + lax.div((p + 1) * (last - first), direct)
                )
            return carry

        lax.fori_loop(0, direct, pass_on, 0)
        if k == 1:
            lax.fori_loop(0, columns, lambda col, carry: (make_pick(col), carry)[1], 0)
    units(share_of[half] * dims.tiles, columns * dims.tiles)

    def hop(way, j, p):
        buffer = r.sum_right if way == 0 else r.sum_left
        return remote(
            buffer.at[j, p],
            buffer.at[j - 1, p],
            r.sum_send.at[way, j - 1, p],
            r.sum_recv.at[way, j - 1, p],
            toward(way),
        )

    def round_of(t, low_piece, high_piece):
        def body(p, carry):
            for way in range(2):
                buffer = r.sum_right if way == 0 else r.sum_left
                j = far(1 - way, p) - t

                def work(way=way, buffer=buffer, j=j):
                    value = own(column(j if way == 0 else -j), p)
                    if t > 0:
                        hop(way, j + 1, p).wait_recv()
                        value = value + buffer[j, p].astype(f32)
                    buffer[j, p] = value.astype(bf16)
                    hop(way, j, p).start()

                if t < half - 1:
                    work()
                else:
                    pl.when(j >= 1)(work)
            return carry

        lax.fori_loop(low_piece, high_piece, body, 0)

    def finish(p, carry):
        value = own(me_x, p)
        hop(0, 1, p).wait_recv()
        hop(1, 1, p).wait_recv()
        value = value + r.sum_right[0, p].astype(f32) + r.sum_left[0, p].astype(f32)
        r.totals[p] = value[0:slots].astype(bf16)
        r.over_total[p] = value[slots:]
        r.returned[p, lines(me_s), :] = r.totals[p, lines(me_s), :]
        for i in range(1, places):
            remote(
                r.totals.at[p, lines(place(i)), :],
                r.returned.at[p, lines(me_s), :],
                r.back_send.at[p],
                r.back_recv.at[p],
                {"sp": place(i)},
            ).start()
        return carry

    def weighted(col, table, q):
        one = jnp.dot(r.pick[col, 0], table[q], preferred_element_type=f32)
        two = jnp.dot(r.pick[col, 1], table[q], preferred_element_type=f32)
        first, second = r.share_s[col, 0], r.share_s[col, 1]
        return jnp.concatenate([first] * lanes_of, axis=1) * one + jnp.concatenate([second] * lanes_of, axis=1) * two

    def take_back(offset):
        col = column(offset)
        for copy in given_back(offset):
            copy.wait_recv()
        for q in range(extra):
            for c in range(lanes_of):
                r.xret[col, q, slots:, c * 128 : (c + 1) * 128] = r.xover_ret[
                    offset, :, q * lanes_of + c, :
                ].astype(bf16)

    def token_hop(way, j, q):
        buffer = r.xsum_right if way == 0 else r.xsum_left
        return remote(
            buffer.at[j, q],
            buffer.at[j - 1, q],
            r.xsum_send.at[way, j - 1, q],
            r.xsum_recv.at[way, j - 1, q],
            toward(way),
        )

    taken = set()

    def token_round(t):
        for q in range(extra):
            for way in range(2):
                buffer = r.xsum_right if way == 0 else r.xsum_left
                j = far(1 - way, q) - t
                if j < 1:
                    continue
                offset = j if way == 0 else columns - j
                if offset not in taken:
                    taken.add(offset)
                    take_back(offset)
                col = column(offset)
                value = weighted(col, r.xret.at[col], q)
                if t > 0:
                    token_hop(way, j + 1, q).wait_recv()
                    value = value + buffer[j, q].astype(f32)
                buffer[j, q] = value.astype(bf16)
                token_hop(way, j, q).start()

    for t in range(half - 1):
        round_of(t, 0, direct)
    token_round(0)
    round_of(half - 1, 0, direct)
    if half > 1:
        token_round(1)
    lax.fori_loop(0, direct, finish, 0)
    for c in range(direct * lanes_of):
        at_lanes = (c % lanes_of) * 128
        r.over_back[:, c, :] = r.over_total[c // lanes_of, :, at_lanes : at_lanes + 128]
    r.over_ret[me_s] = r.over_back[me_s]
    for i in range(1, places):
        remote(
            r.over_back.at[place(i)], r.over_ret.at[me_s], r.over_send.at[1], r.over_recv.at[1], {"sp": place(i)}
        ).start()
    for t in range(2, half):
        token_round(t)
    take_back(0)
    for q in range(extra):
        value = weighted(me_x, r.xret.at[me_x], q)
        for way in range(2):
            token_hop(way, 1, q).wait_recv()
        value = value + r.xsum_right[0, q].astype(f32) + r.xsum_left[0, q].astype(f32)
        span = slice((direct + q) * PIECE, (direct + q + 1) * PIECE)
        r.out_ref[:, span] = (r.stream_s[:, span].astype(f32) + value).astype(bf16)

    remote(
        r.over_back.at[0 : places - 1], r.over_ret.at[0 : places - 1], r.over_send.at[1], r.over_recv.at[1], right
    ).wait_recv()
    for c in range(direct * lanes_of):
        at_lanes = (c % lanes_of) * 128
        r.returned[c // lanes_of, slots:, at_lanes : at_lanes + 128] = r.over_ret[:, c, :].astype(bf16)

    def back_arrived(p):
        most = pl.ds(0, (places - 1) * main)
        return remote(
            r.totals.at[p, most, :], r.returned.at[p, most, :], r.back_send.at[p], r.back_recv.at[p], right
        )

    def combine(p, carry):
        back_arrived(p).wait_recv()
        span = pl.ds(pl.multiple_of(p * PIECE, PIECE), PIECE)
        value = weighted(me_x, r.returned, p)
        r.out_ref[:, span] = (r.stream_s[:, span].astype(f32) + value).astype(bf16)
        return carry

    lax.fori_loop(0, direct, combine, 0)

    for copy in rims + mates + [enter_copy]:
        copy.wait_send()
    for n in range(1, chips):
        for which in range(2):
            to_chip(n, which).wait_send()
    for i in range(1, columns):
        head_copy(column(i)).wait_send()
        table_copy(i).wait_send()
    for event in range(columns - 1):
        for way in range(2):
            matrix_ring(way, event, me_x).wait_send()
            matrix_pass(way, event, me_x).wait_send()
    for n, (a, b) in enumerate(((r.over_out, r.over_in), (r.over_back, r.over_ret))):
        remote(a.at[0 : places - 1], b.at[0 : places - 1], r.over_send.at[n], r.over_recv.at[n], right).wait_send()
    for q in range(extra):
        for way in range(2):
            for k in range(far(way, q)):
                token_ring(way, k, q, me_x).wait_send()
            for k in range(far(1 - way, q)):
                token_hop(way, k + 1, q).wait_send()

    def drain_columns(offset, carry):
        for copy in routed(offset) + given_back(offset):
            copy.wait_send()
        return carry

    lax.fori_loop(0, columns, drain_columns, 0)

    def drain(p, carry):
        out_arrived(p).wait_send()
        back_arrived(p).wait_send()
        for way in range(2):
            for k in range(half):
                pl.when(k < far(way, p))(lambda way=way, k=k: chunk_ring(way, k, p, me_x).wait_send())
                pl.when(k < far(1 - way, p))(lambda way=way, k=k: hop(way, k + 1, p).wait_send())
        return carry

    lax.fori_loop(0, direct, drain, 0)


def layer(places, columns, **given):
    f32, bf16 = jnp.float32, jnp.bfloat16
    rows, width = given["residual_ref"].shape
    units = given["expert_gate_hbm"].shape[2]
    lanes = given["keys_hbm"].shape[1]
    positions = columns * BLOCK
    half, chips, blocks = columns // 2, places // 2, columns
    main = 2 * rows // places
    over = -(-places // 16) * 16
    pieces = width // PIECE
    extra = max(1, pieces // 4)
    direct = pieces - extra
    tiles, total = units // 128, places * main + over
    schedule = (0, 0, 1, 5, 7) if half == 4 else (0,) + (0,) * (half - 1) + (1,)
    dims = types.SimpleNamespace(
        places=places, columns=columns, width=width, main=main, over=over, pieces=pieces, direct=direct, tiles=tiles,
        schedule=schedule,
    )
    packed = STATE_ONE + STATE_TWO
    square = (blocks, 2, BLOCK, BLOCK)
    ring = columns - 1
    vmem = lambda *shape, dtype=bf16: pltpu.VMEM(shape, dtype)
    dma = lambda *shape: pltpu.SemaphoreType.DMA(shape)
    spaces = {"ref": pltpu.VMEM, "hbm": pl.ANY}
    in_specs = [
        pl.BlockSpec(memory_space=pltpu.SMEM if a.shape == (2, 2) else spaces[name[-3:]]) for name, a in given.items()
    ]
    lane_rows = PIECE // 128
    scratch = dict(
        value_in=vmem(2 * positions, BLOCK),
        gate_in=vmem(2 * positions, BLOCK),
        keys_in=vmem(positions, lanes),
        value_rim=vmem(16, BLOCK),
        keys_rim=vmem(16, lanes),
        value_wide=vmem(2 * positions + 16, BLOCK, dtype=f32),
        keys_wide=vmem(positions + 16, lanes, dtype=f32),
        gate_wide=vmem(2 * BLOCK, BLOCK, dtype=f32),
        conv_wide=vmem(2 * BLOCK, BLOCK, dtype=f32),
        x_s=vmem(*square),
        kt_s=vmem(*square),
        q_s=vmem(*square),
        state_s=vmem(*square, dtype=f32),
        near_s=vmem(*square, dtype=f32),
        stride_s=vmem(HEADS * blocks, BLOCK, dtype=f32),
        run_s=vmem(HEADS * blocks, BLOCK, dtype=f32),
        fade_s=vmem(HEADS * blocks, BLOCK, dtype=f32),
        end_s=vmem(HEADS * blocks, BLOCK, dtype=f32),
        cols_s=vmem(blocks, BLOCK, HEADS, dtype=f32),
        own_pack=vmem(packed, BLOCK),
        own_fade=vmem(8, BLOCK, dtype=f32),
        mate_pack=vmem(packed, BLOCK),
        mate_fade=vmem(8, BLOCK, dtype=f32),
        chip_pack=vmem(packed, BLOCK),
        chip_fade=vmem(8, BLOCK, dtype=f32),
        all_pack=vmem(chips, packed // 2, BLOCK),
        all_fade=vmem(chips, 8, BLOCK, dtype=f32),
        enter_pack=vmem(packed, BLOCK),
        carry_s=vmem(2, BLOCK, BLOCK, dtype=f32),
        mixed_s=vmem(columns, BLOCK, 2 * BLOCK),
        heads_in=vmem(columns, BLOCK, 2 * BLOCK),
        matrix=vmem(columns, 2 * BLOCK, width),
        acc_s=vmem(rows, width, dtype=f32),
        stream_s=vmem(rows, width),
        tables=vmem(columns, 8, rows, dtype=f32),
        put=vmem(columns, total, rows),
        pick=vmem(columns, 2, rows, total),
        share_s=vmem(columns, 2, rows, 128, dtype=f32),
        tokens=vmem(columns, extra, rows, PIECE),
        outbound=vmem(direct, places * main, PIECE),
        over_out=vmem(over, direct * lane_rows, 128, dtype=f32),
        over_in=vmem(over, direct * lane_rows, 128, dtype=f32),
        over_back=vmem(over, direct * lane_rows, 128, dtype=f32),
        over_ret=vmem(over, direct * lane_rows, 128, dtype=f32),
        over_total=vmem(direct, over, PIECE, dtype=f32),
        xout=vmem(columns, extra, places * main, PIECE),
        xback=vmem(columns, extra, places * main, PIECE),
        xret=vmem(columns, extra, total, PIECE),
        xover_out=vmem(columns, over, extra * lane_rows, 128, dtype=f32),
        xover_in=vmem(columns, over, extra * lane_rows, 128, dtype=f32),
        xover_back=vmem(columns, over, extra * lane_rows, 128, dtype=f32),
        xover_ret=vmem(columns, over, extra * lane_rows, 128, dtype=f32),
        chunks=vmem(columns, pieces, total, PIECE),
        hidden=vmem(columns, total, units),
        gate_up=vmem(tiles, width, 256),
        down=vmem(pieces, units, PIECE),
        sum_right=vmem(half + 1, direct, total, PIECE),
        sum_left=vmem(half + 1, direct, total, PIECE),
        xsum_right=vmem(half + 1, extra, rows, PIECE),
        xsum_left=vmem(half + 1, extra, rows, PIECE),
        totals=vmem(direct, places * main, PIECE),
        returned=vmem(direct, total, PIECE),
        load_sem=dma(5 + 2 * tiles + pieces),
    )
    for name, shape in dict(
        rim=(2,), mate=(2,), chip=(2, chips), enter=(1,), head=(columns,), table=(columns,), ring=(2, ring),
        over=(2,), token=(2, half, extra), out=(direct,), xout=(columns,), xover=(2, columns), chunk=(2, half, direct),
        xback=(columns,), sum=(2, half + 1, direct), xsum=(2, half + 1, extra), back=(direct,),
    ).items():
        scratch[name + "_send"], scratch[name + "_recv"] = dma(*shape), dma(*shape)
    scratch["pass_send"], scratch["pass_recv"] = dma(2, ring), dma(2, ring)
    names = [*given, "out_ref", *scratch]
    return pl.pallas_call(
        functools.partial(layer_kernel, dims, names),
        out_shape=jax.ShapeDtypeStruct((rows, width), bf16),
        in_specs=in_specs,
        out_specs=pl.BlockSpec(memory_space=pltpu.VMEM),
        scratch_shapes=list(scratch.values()),
        compiler_params=pltpu.CompilerParams(
            collective_id=0, has_side_effects=True, vmem_limit_bytes=VMEM_LIMIT
        ),
        name="layer",
    )(*given.values())


def local(
    residual,
    grouped_value_heads,
    output_gate_heads,
    projected_key_query,
    raw_step_size,
    step_size_bias,
    head_decay_logarithm,
    position_extra_decay,
    head_skip_weight,
    value_kernel_taps,
    key_query_kernel,
    head_norm_gain,
    output_matrix,
    expert_norm_gain,
    expert_gate_weight,
    expert_up_weight,
    expert_down_weight,
    token_expert_choice,
    expert_output_weight,
):
    return layer(
        lax.axis_size("sp"),
        lax.axis_size("tp"),
        residual_ref=residual,
        value_hbm=grouped_value_heads.reshape(-1, BLOCK),
        gate_hbm=output_gate_heads.reshape(-1, BLOCK),
        keys_hbm=projected_key_query,
        raw_ref=raw_step_size.transpose(1, 2, 0),
        bias_ref=step_size_bias,
        log_ref=head_decay_logarithm,
        extra_ref=position_extra_decay.reshape(-1, BLOCK),
        skip_ref=head_skip_weight,
        value_tap_ref=value_kernel_taps.reshape(-1, BLOCK),
        key_tap_ref=key_query_kernel,
        head_gain_ref=head_norm_gain,
        matrix_hbm=output_matrix,
        expert_gain_ref=expert_norm_gain[None],
        choice_ref=token_expert_choice.T,
        share_ref=expert_output_weight.T,
        expert_gate_hbm=expert_gate_weight,
        expert_up_hbm=expert_up_weight,
        expert_down_hbm=expert_down_weight,
    )


def solution(mesh):
    placed = (
        P(("grp", "sp", "tp"), None),
        P(("grp", "sp"), None, "tp"),
        P(("grp", "sp"), None, "tp"),
        P(("grp", "sp"), None),
        P(("grp", "sp"), None, "tp"),
        P(None, "tp"),
        P(None, "tp"),
        P(("grp", "sp")),
        P(None, "tp"),
        P(None, None, "tp"),
        P(),
        P(None, "tp"),
        P(None, "tp", None),
        P(),
        P("sp", None, "tp"),
        P("sp", None, "tp"),
        P("sp", "tp", None),
        P(("grp", "sp", "tp"), None),
        P(("grp", "sp", "tp"), None),
    )
    return jax.shard_map(
        local, mesh=mesh, in_specs=placed, out_specs=P(("grp", "sp", "tp"), None), check_vma=False
    )
```

```python
import functools
import types

import jax
import jax.numpy as jnp
from jax import lax
from jax.experimental import pallas as pl
from jax.experimental.pallas import tpu as pltpu
from jax.sharding import PartitionSpec as P

HEAD_DIM = 64
STATE_ONE = 64
STATE_TWO = 128
BLOCK = 128
EPSILON = 1e-06

MESH = pl.DeviceIdType.MESH
PIECE = 256
HEADS = 4
VMEM_LIMIT = 67043328


def remote(src, dst, send, recv, device):
    return pltpu.make_async_remote_copy(
        src_ref=src, dst_ref=dst, send_sem=send, recv_sem=recv, device_id=device, device_id_type=MESH
    )


def silu(a):
    return a * (1.0 / (1.0 + jnp.exp(-a)))


def layer_kernel(dims, names, *refs):
    r = types.SimpleNamespace(**dict(zip(names, refs, strict=True)))
    f32, bf16 = jnp.float32, jnp.bfloat16
    places, columns, width, rows = dims.places, dims.columns, dims.width, BLOCK
    half, chips, blocks = columns // 2, places // 2, columns
    me_x, me_s = lax.axis_index("tp"), lax.axis_index("sp")
    core, me_y = lax.rem(me_s, 2), lax.div(me_s, 2)
    right = {"tp": lax.rem(me_x + 1, columns)}
    left = {"tp": lax.rem(me_x + columns - 1, columns)}
    mate = {"sp": me_s + 1 - 2 * core}
    following = {"sp": lax.rem(me_s + 1, places)}

    def column(offset):
        return lax.rem(me_x + offset + columns, columns)

    def place(offset):
        return lax.rem(me_s + offset, places)

    def peer(offset):
        return {"sp": lax.rem(me_s + 2 * offset, places)}

    def toward(way):
        return right if way == 0 else left

    loads = [
        (r.matrix_hbm.at[0], r.matrix.at[me_x, pl.ds(0, rows), :]),
        (r.matrix_hbm.at[1], r.matrix.at[me_x, pl.ds(rows, rows), :]),
        (r.value_hbm, r.value_in),
        (r.keys_hbm, r.keys_in),
        (r.gate_hbm, r.gate_in),
    ]
    early = len(loads)
    for t in range(dims.tiles):
        span = pl.ds(t * 128, 128)
        loads.append((r.expert_gate_hbm.at[0, :, span], r.gate_up.at[t, :, pl.ds(0, 128)]))
        loads.append((r.expert_up_hbm.at[0, :, span], r.gate_up.at[t, :, pl.ds(128, 128)]))
    for p in range(dims.pieces):
        loads.append((r.expert_down_hbm.at[0, :, pl.ds(p * PIECE, PIECE)], r.down.at[p]))
    loads = [pltpu.make_async_copy(a, b, r.load_sem.at[n]) for n, (a, b) in enumerate(loads)]
    for load in loads:
        load.start()

    barrier = pltpu.get_barrier_semaphore()
    peers = [{"tp": column(i)} for i in range(1, columns)] + [{"sp": place(i)} for i in range(1, places)]
    for device in peers:
        pl.semaphore_signal(barrier, inc=1, device_id=device, device_id_type=MESH)

    for g in range(2):
        raw = r.raw_ref[g].astype(f32)
        for k in range(blocks):
            r.stride_s[HEADS * k + 2 * g : HEADS * k + 2 * g + 2, :] = raw[:, k * rows : (k + 1) * rows]
    for k in range(blocks):
        r.run_s[HEADS * k : HEADS * k + HEADS, :] = jnp.broadcast_to(r.extra_ref[k : k + 1, :], (HEADS, rows))
    head_of = jnp.bitwise_and(lax.broadcasted_iota(jnp.int32, (HEADS * blocks, rows), 0), HEADS - 1)

    def by_head(table):
        picked = jnp.full((HEADS * blocks, rows), table[1, 1], f32)
        for n in range(3):
            picked = jnp.where(head_of == n, table[n // 2, n % 2], picked)
        return picked

    shifted = r.stride_s[...] + by_head(r.bias_ref)
    stride = jnp.maximum(shifted, 0.0) + jnp.log1p(jnp.exp(-jnp.abs(shifted)))
    log_decay = r.run_s[...] - jnp.exp(by_head(r.log_ref)) * stride
    at_row = lax.broadcasted_iota(jnp.int32, (rows, rows), 0)
    at_lane = lax.broadcasted_iota(jnp.int32, (rows, rows), 1)
    running = jnp.dot(
        log_decay,
        jnp.where(at_row <= at_lane, 1.0, 0.0),
        preferred_element_type=f32,
        precision=lax.Precision.HIGHEST,
    )
    ends = jnp.broadcast_to(running[:, rows - 1 : rows], running.shape)
    r.stride_s[...] = stride
    r.run_s[...] = running
    r.fade_s[...] = jnp.exp(ends - running) * stride
    r.end_s[...] = jnp.exp(ends)
    turned = jnp.transpose(running)
    for k in range(blocks):
        r.cols_s[k, :, 0:HEADS] = turned[:, HEADS * k : HEADS * k + HEADS]

    first_head = at_lane < HEAD_DIM

    def row_pair(table, k, g):
        low = table[pl.ds(HEADS * k + 2 * g, 1), :]
        high = table[pl.ds(HEADS * k + 2 * g + 1, 1), :]
        return jnp.where(first_head[0:1], low, high)

    r.tables[me_x] = jnp.zeros((8, rows), f32)
    r.tables[me_x, 0:2, :] = r.choice_ref[...].astype(f32)
    r.tables[me_x, 2:4, :] = r.share_ref[...]

    for load in loads[: early - 1]:
        load.wait()
    pl.semaphore_wait(barrier, len(peers))

    cut = width // 2
    mine = pl.ds(pl.multiple_of(core * rows, rows), rows)

    def matrix_ring(way, event, col):
        here = r.matrix.at[col, mine, pl.ds(((event % 2) ^ way) * cut, cut)]
        return remote(here, here, r.ring_send.at[way, event], r.ring_recv.at[way, event], toward(way))

    def matrix_pass(way, event, col):
        here = r.matrix.at[col, mine, pl.ds(((event % 2) ^ way) * cut, cut)]
        return remote(here, here, r.pass_send.at[way, event], r.pass_recv.at[way, event], mate)

    rim_rows = 16
    positions = blocks * rows
    rims = [
        remote(
            r.value_in.at[pl.ds(2 * positions - rim_rows, rim_rows), :],
            r.value_rim,
            r.rim_send.at[0],
            r.rim_recv.at[0],
            following,
        ),
        remote(
            r.keys_in.at[pl.ds(positions - rim_rows, rim_rows), :], r.keys_rim, r.rim_send.at[1], r.rim_recv.at[1], following
        ),
    ]
    for rim in rims:
        rim.start()

    def table_copy(offset):
        return remote(
            r.tables.at[me_x],
            r.tables.at[me_x],
            r.table_send.at[offset],
            r.table_recv.at[columns - offset],
            {"tp": column(offset)},
        )

    for i in range(1, columns):
        table_copy(i).start()
    for event in range(2):
        for way in range(2):
            if event < columns - 1:
                matrix_ring(way, event, me_x).start()

    def service(event):
        k = event // 2 + 1
        for way in range(2):
            col = column(-k if way == 0 else k)
            matrix_ring(way, event, col).wait_recv()
            if event + 2 < columns - 1:
                matrix_ring(way, event + 2, col).start()
            matrix_pass(way, event, col).start()

    r.value_wide[rim_rows:, :] = r.value_in[...].astype(f32)
    r.keys_wide[rim_rows:, :] = r.keys_in[...].astype(f32)
    taps = r.value_tap_ref.shape[0] // 2
    value_tap = r.value_tap_ref[...].astype(f32)
    key_tap = r.key_tap_ref[...].astype(f32)
    even = jnp.bitwise_and(lax.broadcasted_iota(jnp.int32, (2 * rows, rows), 0), 1) == 0
    tap_rows = [jnp.where(even, value_tap[2 * j : 2 * j + 1], value_tap[2 * j + 1 : 2 * j + 2]) for j in range(taps)]

    def states_of(k):
        window = r.value_wide[pl.ds(pl.multiple_of(k * 2 * rows, 2 * rows), 2 * rows + rim_rows), :]
        total = jnp.zeros((2 * rows, rows), f32)
        for j in range(taps):
            start = rim_rows - 2 * (taps - 1 - j)
            total = total + window[start : start + 2 * rows] * tap_rows[j]
        r.conv_wide[...] = silu(total).astype(bf16).astype(f32)
        window = r.keys_wide[pl.ds(pl.multiple_of(k * rows, rows), rows + rim_rows), :]
        total = jnp.zeros((rows, r.keys_wide.shape[1]), f32)
        for j in range(taps):
            start = rim_rows - (taps - 1 - j)
            total = total + window[start : start + rows] * key_tap[j : j + 1]
        conv = silu(total).astype(bf16).astype(f32)
        both = conv[:, 0 : 2 * STATE_ONE]
        keys = [jnp.where(first_head, both, 0.0), conv[:, 2 * STATE_ONE : 2 * STATE_ONE + STATE_TWO]]
        asks = [pltpu.roll(both, STATE_ONE, 1), conv[:, 2 * STATE_ONE + STATE_TWO :]]
        for g in range(2):
            x = r.conv_wide[pl.ds(g, rows, stride=2), :].astype(bf16)
            key_t = jnp.transpose(keys[g])
            r.x_s[k, g] = x
            r.kt_s[k, g] = key_t.astype(bf16)
            r.q_s[k, g] = asks[g].astype(bf16)
            faded = jnp.concatenate(
                [key_t * r.fade_s[pl.ds(HEADS * k + 2 * g + h, 1), :] for h in range(2)], axis=0
            ).astype(bf16)
            state = jnp.dot(faded, x, preferred_element_type=f32)
            r.state_s[k, g] = jnp.where(first_head, state[:rows], state[rows:])

    def state_step(i, carry):
        states_of(i)
        return carry

    lax.fori_loop(1, blocks, state_step, 0)
    for rim in rims:
        rim.wait_recv()
    opening = me_s == 0
    r.value_wide[0:rim_rows, :] = jnp.where(opening, 0.0, r.value_rim[...].astype(f32))
    r.keys_wide[0:rim_rows, :] = jnp.where(opening, 0.0, r.keys_rim[...].astype(f32))
    states_of(0)

    packed = STATE_TWO + STATE_ONE
    piece = packed // 2

    def local_end(g):
        total = jnp.zeros((rows, rows), f32)
        faded = jnp.ones((1, rows), f32)
        for k in range(blocks):
            decay = row_pair(r.end_s, k, g)
            total = total * decay + r.state_s[k, g]
            faded = faded * decay
        return total, faded

    end_one, fade_one = local_end(0)
    end_two, fade_two = local_end(1)
    own = jnp.concatenate([end_two, end_one[:STATE_ONE]], axis=0)
    r.own_pack[...] = own.astype(bf16)
    r.own_fade[0:1, :] = fade_one
    r.own_fade[1:2, :] = fade_two
    r.own_fade[2:8, :] = jnp.zeros((6, rows), f32)
    mates = [
        remote(r.own_pack, r.mate_pack, r.mate_send.at[0], r.mate_recv.at[0], mate),
        remote(r.own_fade, r.mate_fade, r.mate_send.at[1], r.mate_recv.at[1], mate),
    ]
    for copy in mates:
        copy.start()
    service(0)
    for copy in mates:
        copy.wait_recv()
    is_low = core == 0
    low = jnp.where(is_low, own, r.mate_pack[...].astype(f32))
    high = jnp.where(is_low, r.mate_pack[...].astype(f32), own)
    mate_rows = r.mate_fade[...]
    own_rows = r.own_fade[...]
    high_rows = jnp.where(is_low, mate_rows, own_rows)
    in_two = lax.broadcasted_iota(jnp.int32, (packed, rows), 0) < STATE_TWO
    r.chip_pack[...] = (low * jnp.where(in_two, high_rows[1:2], high_rows[0:1]) + high).astype(bf16)
    r.chip_fade[...] = own_rows * mate_rows
    my_half = pl.ds(pl.multiple_of(core * piece, 16), piece)

    def to_chip(n, which):
        src = r.chip_pack.at[my_half, :] if which == 0 else r.chip_fade
        dst = r.all_pack.at[me_y] if which == 0 else r.all_fade.at[me_y]
        return remote(src, dst, r.chip_send.at[which, n], r.chip_recv.at[which, n], peer(n))

    for n in range(1, chips):
        for which in range(2):
            to_chip(n, which).start()

    below = at_row >= at_lane

    def near_step(k, carry):
        cols = r.cols_s[k]
        for g in range(2):
            scores = jnp.dot(r.q_s[k, g], r.kt_s[k, g], preferred_element_type=f32)
            parts = []
            for h in range(2):
                n = 2 * g + h
                gap = cols[:, n : n + 1] - r.run_s[pl.ds(HEADS * k + n, 1), :]
                damping = jnp.exp(jnp.where(below, gap, -1e30))
                parts.append((scores * damping * r.stride_s[pl.ds(HEADS * k + n, 1), :]).astype(bf16))
            near = jnp.dot(jnp.concatenate(parts, axis=0), r.x_s[k, g], preferred_element_type=f32)
            r.near_s[k, g] = jnp.where(first_head, near[:rows], near[rows:])
        return carry

    lax.fori_loop(0, blocks, near_step, 0)
    if columns > 2:
        service(1)
    loads[early - 1].wait()

    for n in range(1, chips):
        for which in range(2):
            to_chip(n, which).wait_recv()
    row_at = lax.broadcasted_iota(jnp.int32, (piece, rows), 0) + core * piece
    half_two = row_at < STATE_TWO
    entering = jnp.zeros((piece, rows), f32)
    for y in range(chips):
        fades = r.all_fade[y]
        later = entering * jnp.where(half_two, fades[1:2], fades[0:1]) + r.all_pack[y].astype(f32)
        entering = jnp.where(y < me_y, later, entering)
    r.enter_pack[my_half, :] = entering.astype(bf16)
    here = r.enter_pack.at[my_half, :]
    enter_copy = remote(here, here, r.enter_send.at[0], r.enter_recv.at[0], mate)
    enter_copy.start()
    enter_copy.wait_recv()
    chip_state = r.enter_pack[...].astype(f32)
    after_low = chip_state * jnp.where(in_two, mate_rows[1:2], mate_rows[0:1]) + r.mate_pack[...].astype(f32)
    entered = jnp.where(is_low, chip_state, after_low)
    r.carry_s[1] = entered[:STATE_TWO]
    r.carry_s[0] = jnp.zeros((rows, rows), f32)
    r.carry_s[0, 0:STATE_ONE, :] = entered[STATE_TWO:]

    def head_copy(col):
        return remote(r.mixed_s.at[col], r.heads_in.at[me_x], r.head_send.at[col], r.head_recv.at[me_x], {"tp": col})

    def mix_step(k, carry):
        cols = jnp.exp(r.cols_s[k])
        r.gate_wide[...] = r.gate_in[pl.ds(pl.multiple_of(k * 2 * rows, 2 * rows), 2 * rows), :].astype(f32)
        for g in range(2):
            state = r.carry_s[g]
            coarse = state.astype(bf16)
            fine = (state - coarse.astype(f32)).astype(bf16)
            ask = r.q_s[k, g]
            far = jnp.dot(
                jnp.concatenate([ask, ask], axis=1),
                jnp.concatenate([coarse, fine], axis=0),
                preferred_element_type=f32,
            )
            reach = jnp.where(first_head, cols[:, 2 * g : 2 * g + 1], cols[:, 2 * g + 1 : 2 * g + 2])
            skip = jnp.where(first_head[0:1], r.skip_ref[g, 0], r.skip_ref[g, 1])
            mixed = r.near_s[k, g] + far * reach + skip * r.x_s[k, g].astype(f32)
            gated = mixed * silu(r.gate_wide[pl.ds(g, rows, stride=2), :])
            square = gated * gated
            one = jnp.sum(jnp.where(first_head, square, 0.0), axis=1, keepdims=True)
            two = jnp.sum(jnp.where(first_head, 0.0, square), axis=1, keepdims=True)
            scale = lax.rsqrt(jnp.where(first_head, one, two) * (1.0 / HEAD_DIM) + EPSILON)
            r.mixed_s[k, :, g * rows : (g + 1) * rows] = (gated * scale * r.head_gain_ref[g : g + 1, :]).astype(bf16)
            r.carry_s[g] = state * row_pair(r.end_s, k, g) + r.state_s[k, g]

        @pl.when(k != me_x)
        def _():
            head_copy(k).start()

        return carry

    lax.fori_loop(0, blocks, mix_step, 0)
    r.heads_in[me_x] = r.mixed_s[me_x]

    main, over, slots = dims.main, dims.over, places * dims.main
    total_slots = slots + over
    slot_row = lax.broadcasted_iota(jnp.int32, (total_slots, over), 0)
    slot_expert = lax.broadcasted_iota(jnp.int32, (total_slots, over), 1)
    spread = jnp.where(
        ((slot_row < slots) & (slot_row >= slot_expert * main) & (slot_row < slot_expert * main + main))
        | (slot_row == slots + slot_expert),
        1.0,
        0.0,
    ).astype(bf16)
    at = lax.broadcasted_iota(jnp.int32, (total_slots, rows), 0)
    turn = jnp.where(at < slots, jnp.bitwise_and(at, main - 1), main).astype(f32)
    expert_at = lax.broadcasted_iota(jnp.int32, (over, rows), 0).astype(f32)
    earlier = jnp.where(at_row < at_lane, 1.0, 0.0).astype(bf16)

    def make_put(col):
        table = r.tables[col]
        named = jnp.where((expert_at == table[0:1]) | (expert_at == table[1:2]), 1.0, 0.0)
        rank = jnp.dot(named.astype(bf16), earlier, preferred_element_type=f32)
        named_x = jnp.dot(spread, named.astype(bf16), preferred_element_type=f32)
        rank_x = jnp.dot(spread, rank.astype(bf16), preferred_element_type=f32)
        r.put[col] = jnp.where(rank_x == turn, named_x, 0.0).astype(bf16)

    for i in range(1, columns):
        table_copy(i).wait_recv()

    def put_step(col, carry):
        make_put(col)
        return carry

    lax.fori_loop(0, columns, put_step, 0)

    slot_col = lax.broadcasted_iota(jnp.int32, (over, total_slots), 1)
    slot_exp = lax.broadcasted_iota(jnp.int32, (over, total_slots), 0)
    spread_t = jnp.where(
        ((slot_col < slots) & (slot_col >= slot_exp * main) & (slot_col < slot_exp * main + main))
        | (slot_col == slots + slot_exp),
        1.0,
        0.0,
    ).astype(bf16)
    at_t = lax.broadcasted_iota(jnp.int32, (rows, total_slots), 1)
    turn_t = jnp.where(at_t < slots, jnp.bitwise_and(at_t, main - 1), main).astype(f32)
    expert_to = lax.broadcasted_iota(jnp.int32, (rows, over), 1).astype(f32)
    later_t = jnp.where(at_lane < at_row, 1.0, 0.0).astype(bf16)

    def make_pick(col):
        table = jnp.transpose(r.tables[col])
        named = [jnp.where(expert_to == table[:, k : k + 1], 1.0, 0.0) for k in range(2)]
        rank = jnp.dot(later_t, (named[0] + named[1]).astype(bf16), preferred_element_type=f32)
        rank_x = jnp.dot(rank.astype(bf16), spread_t, preferred_element_type=f32)
        for k in range(2):
            named_x = jnp.dot(named[k].astype(bf16), spread_t, preferred_element_type=f32)
            r.pick[col, k] = jnp.where(rank_x == turn_t, named_x, 0.0).astype(bf16)
            r.share_s[col, k] = jnp.broadcast_to(table[:, 2 + k : 3 + k], (rows, rows))

    def arrived(col):
        return remote(r.mixed_s.at[col], r.heads_in.at[col], r.head_send.at[col], r.head_recv.at[col], {"tp": col})

    def product(col, first=False):
        for n in range(0, width, 512):
            part = jnp.dot(r.heads_in[col], r.matrix[col, :, n : n + 512], preferred_element_type=f32)
            r.acc_s[:, n : n + 512] = part if first else r.acc_s[:, n : n + 512] + part

    product(me_x, True)
    for event in range(2, columns - 1):
        service(event)
    for k in range(1, half + 1):
        for way in range(2):
            if way == 1 and k == half:
                continue
            for event in (2 * k - 2, 2 * k - 1):
                if event < columns - 1:
                    for side in range(2) if k == half else (way,):
                        matrix_pass(side, event, column(k if side else -k)).wait_recv()
            col = column(-k if way == 0 else k)
            arrived(col).wait_recv()
            product(col)

    stream = (r.residual_ref[...].astype(f32) + r.acc_s[...]).astype(bf16)
    r.stream_s[...] = stream
    wide = stream.astype(f32)
    scale = lax.rsqrt(jnp.mean(wide * wide, axis=1, keepdims=True) + EPSILON)
    normed = (wide * scale * r.expert_gain_ref[...]).astype(bf16)

    direct, extra = dims.direct, dims.pieces - dims.direct
    pieces = dims.pieces
    lanes_of = PIECE // 128

    def lines(index):
        return pl.ds(pl.multiple_of(index * main, main), main)

    def far(way, p):
        odd = lax.rem(p, 2) if not isinstance(p, int) else p % 2
        return half - odd if way == 0 else half - 1 + odd

    for q in range(extra):
        r.tokens[me_x, q] = normed[:, (direct + q) * PIECE : (direct + q + 1) * PIECE]

    def token_ring(way, step, q, col):
        here = r.tokens.at[col, q]
        return remote(here, here, r.token_send.at[way, step, q], r.token_recv.at[way, step, q], toward(way))

    put_own = r.put[me_x]
    for p in range(direct):
        part = jnp.dot(put_own, normed[:, p * PIECE : (p + 1) * PIECE], preferred_element_type=f32)
        r.outbound[p] = part[:slots].astype(bf16)
        for c in range(lanes_of):
            r.over_out[:, p * lanes_of + c, :] = part[slots:, c * 128 : (c + 1) * 128]
    for q in range(extra):
        for way in range(2):
            token_ring(way, 0, q, me_x).start()

    def send_out(p, carry):
        for i in range(1, places):
            remote(
                r.outbound.at[p, lines(place(i)), :],
                r.chunks.at[me_x, p, lines(me_s), :],
                r.out_send.at[p],
                r.out_recv.at[p],
                {"sp": place(i)},
            ).start()
        r.chunks[me_x, p, lines(me_s), :] = r.outbound[p, lines(me_s), :]
        return carry

    lax.fori_loop(0, direct, send_out, 0)
    for i in range(1, places):
        remote(
            r.over_out.at[place(i)], r.over_in.at[me_s], r.over_send.at[0], r.over_recv.at[0], {"sp": place(i)}
        ).start()
    r.over_in[me_s] = r.over_out[me_s]
    if places < over:
        r.over_in[places:over] = jnp.zeros((over - places, *r.over_in.shape[1:]), f32)
        r.over_ret[places:over] = jnp.zeros((over - places, *r.over_ret.shape[1:]), f32)
        r.xover_in[:, places:over] = jnp.zeros((columns, over - places, *r.xover_in.shape[2:]), f32)
        r.xover_ret[:, places:over] = jnp.zeros((columns, over - places, *r.xover_ret.shape[2:]), f32)

    def route(offset):
        col = column(offset)
        for q in range(extra):
            part = jnp.dot(r.put[col], r.tokens[col, q], preferred_element_type=f32)
            r.xout[col, q] = part[:slots].astype(bf16)
            r.chunks[col, direct + q, lines(me_s), :] = r.xout[col, q, lines(me_s), :]
            for c in range(lanes_of):
                r.xover_out[offset, :, q * lanes_of + c, :] = part[slots:, c * 128 : (c + 1) * 128]
        r.xover_in[offset, me_s] = r.xover_out[offset, me_s]
        for i in range(1, places):
            remote(
                r.xout.at[col, :, lines(place(i)), :],
                r.chunks.at[col, pl.ds(direct, extra), lines(me_s), :],
                r.xout_send.at[offset],
                r.xout_recv.at[offset],
                {"sp": place(i)},
            ).start()
            remote(
                r.xover_out.at[offset, place(i)],
                r.xover_in.at[offset, me_s],
                r.xover_send.at[0, offset],
                r.xover_recv.at[0, offset],
                {"sp": place(i)},
            ).start()

    def routed(offset):
        col = column(offset)
        most = pl.ds(0, (places - 1) * main)
        return (
            remote(
                r.xout.at[col, :, most, :],
                r.chunks.at[col, pl.ds(direct, extra), most, :],
                r.xout_send.at[offset],
                r.xout_recv.at[offset],
                right,
            ),
            remote(
                r.xover_out.at[offset, 0 : places - 1],
                r.xover_in.at[offset, 0 : places - 1],
                r.xover_send.at[0, offset],
                r.xover_recv.at[0, offset],
                right,
            ),
        )

    def take_routed(offset):
        col = column(offset)
        for copy in routed(offset):
            copy.wait_recv()
        for q in range(extra):
            for c in range(lanes_of):
                r.chunks[col, direct + q, slots:, c * 128 : (c + 1) * 128] = r.xover_in[
                    offset, :, q * lanes_of + c, :
                ].astype(bf16)

    route(0)

    def token_event(k):
        for q in range(extra):
            for way in range(2):
                if k <= far(way, q):
                    col = column(-k if way == 0 else k)
                    token_ring(way, k - 1, q, col).wait_recv()
                    if k < far(way, q):
                        token_ring(way, k, q, col).start()
        if k < half:
            route(columns - k)
        route(k)

    def chunk_ring(way, step, p, col):
        here = r.chunks.at[col, p, pl.ds(0, slots), :]
        return remote(here, here, r.chunk_send.at[way, step, p], r.chunk_recv.at[way, step, p], toward(way))

    def over_ring(way, step, col):
        here = r.chunks.at[col, pl.ds(0, direct), pl.ds(slots, over), :]
        return remote(here, here, r.tail_send.at[way, step], r.tail_recv.at[way, step], toward(way))

    def out_arrived(p):
        most = pl.ds(0, (places - 1) * main)
        return remote(
            r.outbound.at[p, most, :], r.chunks.at[me_x, p, most, :], r.out_send.at[p], r.out_recv.at[p], right
        )

    def start_piece(p):
        out_arrived(p).wait_recv()
        chunk_ring(0, 0, p, me_x).start()
        chunk_ring(1, 0, p, me_x).start()

    def start_over():
        remote(
            r.over_out.at[0 : places - 1], r.over_in.at[0 : places - 1], r.over_send.at[0], r.over_recv.at[0], right
        ).wait_recv()
        for c in range(direct * lanes_of):
            at_lanes = (c % lanes_of) * 128
            r.chunks[me_x, c // lanes_of, slots:, at_lanes : at_lanes + 128] = r.over_in[:, c, :].astype(bf16)
        for way in range(2):
            over_ring(way, 0, me_x).start()

    for copy in rims + mates + [enter_copy]:
        copy.wait_send()
    for n in range(1, chips):
        for which in range(2):
            to_chip(n, which).wait_send()
    for i in range(1, columns):
        head_copy(column(i)).wait_send()
        table_copy(i).wait_send()
    for event in range(columns - 1):
        for way in range(2):
            matrix_ring(way, event, me_x).wait_send()
            matrix_pass(way, event, me_x).wait_send()

    for step in dims.opening:
        if step > 0:
            token_event(step)
        elif -step < direct:
            start_piece(-step)
    start_over()

    def offset_of(n):
        k = lax.div(n + 1, 2)
        return jnp.where(lax.rem(n, 2) == 1, lax.rem(columns - k, columns), k)

    def unit(n, t):
        offset = offset_of(n)
        col = column(offset)
        pl.when(t == 0)(lambda: take_routed(offset))
        acc = jnp.dot(r.chunks[col, 0], r.gate_up[t, 0:PIECE, :], preferred_element_type=f32)
        for q in range(1, pieces):
            acc = acc + jnp.dot(
                r.chunks[col, q], r.gate_up[t, q * PIECE : (q + 1) * PIECE, :], preferred_element_type=f32
            )
        value = silu(acc[:, 0:128]) * acc[:, 128:256]
        r.hidden[col, :, pl.ds(pl.multiple_of(t * 128, 128), 128)] = value.astype(bf16)
        pl.when(t == dims.tiles - 1)(lambda: give_back(offset))

    def own(col, p):
        return jnp.dot(r.hidden[col], r.down[p], preferred_element_type=f32)

    def give_back(offset):
        col = column(offset)
        for q in range(extra):
            part = own(col, direct + q)
            r.xback[col, q] = part[:slots].astype(bf16)
            r.xret[col, q, lines(me_s), :] = r.xback[col, q, lines(me_s), :]
            for c in range(lanes_of):
                r.xover_back[offset, :, q * lanes_of + c, :] = part[slots:, c * 128 : (c + 1) * 128]
        r.xover_ret[offset, me_s] = r.xover_back[offset, me_s]
        for i in range(1, places):
            remote(
                r.xback.at[col, :, lines(place(i)), :],
                r.xret.at[col, :, lines(me_s), :],
                r.xback_send.at[offset],
                r.xback_recv.at[offset],
                {"sp": place(i)},
            ).start()
            remote(
                r.xover_back.at[offset, place(i)],
                r.xover_ret.at[offset, me_s],
                r.xover_send.at[1, offset],
                r.xover_recv.at[1, offset],
                {"sp": place(i)},
            ).start()

    def given_back(offset):
        col = column(offset)
        most = pl.ds(0, (places - 1) * main)
        return (
            remote(
                r.xback.at[col, :, most, :],
                r.xret.at[col, :, most, :],
                r.xback_send.at[offset],
                r.xback_recv.at[offset],
                right,
            ),
            remote(
                r.xover_back.at[offset, 0 : places - 1],
                r.xover_ret.at[offset, 0 : places - 1],
                r.xover_send.at[1, offset],
                r.xover_recv.at[1, offset],
                right,
            ),
        )

    for load in loads[early:]:
        load.wait()

    def units(low, high):
        def body(v, carry):
            unit(lax.div(v, dims.tiles), lax.rem(v, dims.tiles))
            return carry

        lax.fori_loop(low, high, body, 0)

    def hop(way, j, p):
        return remote(
            r.sums.at[way, j, p],
            r.sums.at[way, j - 1, p],
            r.sum_send.at[way, j - 1, p],
            r.sum_recv.at[way, j - 1, p],
            {"tp": column(1 - 2 * way)},
        )

    def chains(long, step, group):
        j = half - step if long else half - 1 - step

        def body(p, carry):
            odd = lax.rem(p, 2)
            way = 1 - odd if long else odd
            value = own(column(j * (1 - 2 * way)), p)
            if step > 0:
                hop(way, j + 1, p).wait_recv()
                value = value + r.sums[way, j, p].astype(f32)
            r.sums[way, j, p] = value.astype(bf16)
            hop(way, j, p).start()
            return carry

        lax.fori_loop(*group, body, 0)

    share_of = dims.schedule
    for k in range(1, half + 1):
        first, last = share_of[k - 1] * dims.tiles, share_of[k] * dims.tiles

        if k == half and half > 1:
            units(first, last)
            first = last
            for group in dims.groups:
                chains(False, 0, group)

        def pass_on(p, carry, k=k, first=first, last=last):
            for way in range(2):
                col = column(-k if way == 0 else k)

                @pl.when(k <= far(way, p))
                def _():
                    chunk_ring(way, k - 1, p, col).wait_recv()

                if k < half:

                    @pl.when(k < far(way, p))
                    def _():
                        chunk_ring(way, k, p, col).start()

            if last > first:
                units(
                    first + lax.div(p * (last - first), direct), first + lax.div((p + 1) * (last - first), direct)
                )
            return carry

        lax.fori_loop(0, direct, pass_on, 0)
        for way in range(2):
            if k <= far(way, 0):
                col = column(-k if way == 0 else k)
                over_ring(way, k - 1, col).wait_recv()
                if k < far(way, 0):
                    over_ring(way, k, col).start()
        if k == 1:
            lax.fori_loop(0, columns, lambda col, carry: (make_pick(col), carry)[1], 0)
    units(share_of[half] * dims.tiles, columns * dims.tiles)

    def finish(p, carry):
        value = own(me_x, p)
        hop(0, 1, p).wait_recv()
        hop(1, 1, p).wait_recv()
        value = value + r.sums[0, 0, p].astype(f32) + r.sums[1, 0, p].astype(f32)
        r.totals[p] = value[0:slots].astype(bf16)
        r.over_total[p] = value[slots:]
        r.returned[p, lines(me_s), :] = r.totals[p, lines(me_s), :]
        for i in range(1, places):
            remote(
                r.totals.at[p, lines(place(i)), :],
                r.returned.at[p, lines(me_s), :],
                r.back_send.at[p],
                r.back_recv.at[p],
                {"sp": place(i)},
            ).start()
        return carry

    def weighted(col, table, q):
        one = jnp.dot(r.pick[col, 0], table[q], preferred_element_type=f32)
        two = jnp.dot(r.pick[col, 1], table[q], preferred_element_type=f32)
        first, second = r.share_s[col, 0], r.share_s[col, 1]
        return jnp.concatenate([first] * lanes_of, axis=1) * one + jnp.concatenate([second] * lanes_of, axis=1) * two

    def take_back(offset):
        col = column(offset)
        for copy in given_back(offset):
            copy.wait_recv()
        for q in range(extra):
            for c in range(lanes_of):
                r.xret[col, q, slots:, c * 128 : (c + 1) * 128] = r.xover_ret[
                    offset, :, q * lanes_of + c, :
                ].astype(bf16)

    def token_hop(way, j, q):
        buffer = r.xsum_right if way == 0 else r.xsum_left
        return remote(
            buffer.at[j, q],
            buffer.at[j - 1, q],
            r.xsum_send.at[way, j - 1, q],
            r.xsum_recv.at[way, j - 1, q],
            toward(way),
        )

    taken = set()

    def token_round(t):
        for q in range(extra):
            for way in range(2):
                buffer = r.xsum_right if way == 0 else r.xsum_left
                j = far(1 - way, q) - t
                if j < 1:
                    continue
                offset = j if way == 0 else columns - j
                if offset not in taken:
                    taken.add(offset)
                    take_back(offset)
                col = column(offset)
                value = weighted(col, r.xret.at[col], q)
                if t > 0:
                    token_hop(way, j + 1, q).wait_recv()
                    value = value + buffer[j, q].astype(f32)
                buffer[j, q] = value.astype(bf16)
                token_hop(way, j, q).start()

    for group in dims.groups:
        chains(True, 0, group)
    remote(
        r.over_out.at[0 : places - 1], r.over_in.at[0 : places - 1], r.over_send.at[0], r.over_recv.at[0], right
    ).wait_send()
    for way in range(2):
        for q in range(extra):
            for k in range(far(way, q)):
                token_ring(way, k, q, me_x).wait_send()
        for k in range(far(way, 0)):
            over_ring(way, k, me_x).wait_send()

    def drain_gather(p, carry):
        out_arrived(p).wait_send()
        for way in range(2):
            for k in range(half):
                pl.when(k < far(way, p))(lambda way=way, k=k: chunk_ring(way, k, p, me_x).wait_send())
        return carry

    lax.fori_loop(0, direct, drain_gather, 0)

    def drain_routed(offset, carry):
        for copy in routed(offset):
            copy.wait_send()
        return carry

    lax.fori_loop(0, columns, drain_routed, 0)
    for kind, step, group in dims.closing:
        if kind == "short":
            chains(False, step, group)
        elif kind == "long":
            chains(True, step, group)
        elif kind == "token":
            token_round(step)
        else:
            lax.fori_loop(*group, finish, 0)
    for c in range(direct * lanes_of):
        at_lanes = (c % lanes_of) * 128
        r.over_back[:, c, :] = r.over_total[c // lanes_of, :, at_lanes : at_lanes + 128]
    r.over_ret[me_s] = r.over_back[me_s]
    for i in range(1, places):
        remote(
            r.over_back.at[place(i)], r.over_ret.at[me_s], r.over_send.at[1], r.over_recv.at[1], {"sp": place(i)}
        ).start()

    def drain_back(offset, carry):
        for copy in given_back(offset):
            copy.wait_send()
        return carry

    lax.fori_loop(0, columns, drain_back, 0)

    def drain_sums(p, carry):
        for way in range(2):
            for k in range(half):
                pl.when(k < far(1 - way, p))(lambda way=way, k=k: hop(way, k + 1, p).wait_send())
        return carry

    lax.fori_loop(0, direct, drain_sums, 0)
    token_round(half - 1)
    take_back(0)
    for q in range(extra):
        value = weighted(me_x, r.xret.at[me_x], q)
        for way in range(2):
            token_hop(way, 1, q).wait_recv()
        value = value + r.xsum_right[0, q].astype(f32) + r.xsum_left[0, q].astype(f32)
        span = slice((direct + q) * PIECE, (direct + q + 1) * PIECE)
        r.out_ref[:, span] = (r.stream_s[:, span].astype(f32) + value).astype(bf16)

    remote(
        r.over_back.at[0 : places - 1], r.over_ret.at[0 : places - 1], r.over_send.at[1], r.over_recv.at[1], right
    ).wait_recv()
    for c in range(direct * lanes_of):
        at_lanes = (c % lanes_of) * 128
        r.returned[c // lanes_of, slots:, at_lanes : at_lanes + 128] = r.over_ret[:, c, :].astype(bf16)

    def back_arrived(p):
        most = pl.ds(0, (places - 1) * main)
        return remote(
            r.totals.at[p, most, :], r.returned.at[p, most, :], r.back_send.at[p], r.back_recv.at[p], right
        )

    def combine(p, carry):
        back_arrived(p).wait_recv()
        span = pl.ds(pl.multiple_of(p * PIECE, PIECE), PIECE)
        value = weighted(me_x, r.returned, p)
        r.out_ref[:, span] = (r.stream_s[:, span].astype(f32) + value).astype(bf16)
        return carry

    lax.fori_loop(0, direct, combine, 0)

    remote(
        r.over_back.at[0 : places - 1], r.over_ret.at[0 : places - 1], r.over_send.at[1], r.over_recv.at[1], right
    ).wait_send()
    for q in range(extra):
        for way in range(2):
            for k in range(far(1 - way, q)):
                token_hop(way, k + 1, q).wait_send()
    for p in range(direct):
        back_arrived(p).wait_send()

def layer(places, columns, **given):
    f32, bf16 = jnp.float32, jnp.bfloat16
    rows, width = given["residual_ref"].shape
    units = given["expert_gate_hbm"].shape[2]
    lanes = given["keys_hbm"].shape[1]
    positions = columns * BLOCK
    half, chips, blocks = columns // 2, places // 2, columns
    main = 2 * rows // places
    over = -(-places // 16) * 16
    pieces = width // PIECE
    extra = max(1, pieces // 4)
    direct = pieces - extra
    tiles, total = units // 128, places * main + over
    schedule = (0, 0, 1, 5, 7) if half == 4 else (0,) * half + (columns - 1,)
    opening = (1, 0, 2, -1, -2, 3, -3, -4, 4, -5) if half == 4 else (*range(1, half + 1), *range(0, -direct, -1))
    groups = [(low, min(low + 2, direct)) for low in range(0, direct, 2)]
    closing = []
    for n, group in enumerate(groups):
        last = n == len(groups) - 1
        for step in range(1, half):
            if step < half - 1:
                closing.append(("short", step, group))
            closing.append(("long", step, group))
            if last and step < half:
                closing.append(("token", step - 1, None))
        if n > 0:
            closing.insert(len(closing) - half, ("finish", None, groups[n - 1]))
    closing.append(("finish", None, groups[-1]))
    dims = types.SimpleNamespace(
        places=places, columns=columns, width=width, main=main, over=over, pieces=pieces, direct=direct, tiles=tiles,
        schedule=schedule, opening=opening, groups=groups, closing=closing,
    )
    packed = STATE_ONE + STATE_TWO
    square = (blocks, 2, BLOCK, BLOCK)
    ring = columns - 1
    vmem = lambda *shape, dtype=bf16: pltpu.VMEM(shape, dtype)
    dma = lambda *shape: pltpu.SemaphoreType.DMA(shape)
    spaces = {"ref": pltpu.VMEM, "hbm": pl.ANY}
    in_specs = [
        pl.BlockSpec(memory_space=pltpu.SMEM if a.shape == (2, 2) else spaces[name[-3:]]) for name, a in given.items()
    ]
    lane_rows = PIECE // 128
    scratch = dict(
        value_in=vmem(2 * positions, BLOCK),
        gate_in=vmem(2 * positions, BLOCK),
        keys_in=vmem(positions, lanes),
        value_rim=vmem(16, BLOCK),
        keys_rim=vmem(16, lanes),
        value_wide=vmem(2 * positions + 16, BLOCK, dtype=f32),
        keys_wide=vmem(positions + 16, lanes, dtype=f32),
        gate_wide=vmem(2 * BLOCK, BLOCK, dtype=f32),
        conv_wide=vmem(2 * BLOCK, BLOCK, dtype=f32),
        x_s=vmem(*square),
        kt_s=vmem(*square),
        q_s=vmem(*square),
        state_s=vmem(*square, dtype=f32),
        near_s=vmem(*square, dtype=f32),
        stride_s=vmem(HEADS * blocks, BLOCK, dtype=f32),
        run_s=vmem(HEADS * blocks, BLOCK, dtype=f32),
        fade_s=vmem(HEADS * blocks, BLOCK, dtype=f32),
        end_s=vmem(HEADS * blocks, BLOCK, dtype=f32),
        cols_s=vmem(blocks, BLOCK, HEADS, dtype=f32),
        own_pack=vmem(packed, BLOCK),
        own_fade=vmem(8, BLOCK, dtype=f32),
        mate_pack=vmem(packed, BLOCK),
        mate_fade=vmem(8, BLOCK, dtype=f32),
        chip_pack=vmem(packed, BLOCK),
        chip_fade=vmem(8, BLOCK, dtype=f32),
        all_pack=vmem(chips, packed // 2, BLOCK),
        all_fade=vmem(chips, 8, BLOCK, dtype=f32),
        enter_pack=vmem(packed, BLOCK),
        carry_s=vmem(2, BLOCK, BLOCK, dtype=f32),
        mixed_s=vmem(columns, BLOCK, 2 * BLOCK),
        heads_in=vmem(columns, BLOCK, 2 * BLOCK),
        matrix=vmem(columns, 2 * BLOCK, width),
        acc_s=vmem(rows, width, dtype=f32),
        stream_s=vmem(rows, width),
        tables=vmem(columns, 8, rows, dtype=f32),
        put=vmem(columns, total, rows),
        pick=vmem(columns, 2, rows, total),
        share_s=vmem(columns, 2, rows, 128, dtype=f32),
        tokens=vmem(columns, extra, rows, PIECE),
        outbound=vmem(direct, places * main, PIECE),
        over_out=vmem(over, direct * lane_rows, 128, dtype=f32),
        over_in=vmem(over, direct * lane_rows, 128, dtype=f32),
        over_back=vmem(over, direct * lane_rows, 128, dtype=f32),
        over_ret=vmem(over, direct * lane_rows, 128, dtype=f32),
        over_total=vmem(direct, over, PIECE, dtype=f32),
        xout=vmem(columns, extra, places * main, PIECE),
        xback=vmem(columns, extra, places * main, PIECE),
        xret=vmem(columns, extra, total, PIECE),
        xover_out=vmem(columns, over, extra * lane_rows, 128, dtype=f32),
        xover_in=vmem(columns, over, extra * lane_rows, 128, dtype=f32),
        xover_back=vmem(columns, over, extra * lane_rows, 128, dtype=f32),
        xover_ret=vmem(columns, over, extra * lane_rows, 128, dtype=f32),
        chunks=vmem(columns, pieces, total, PIECE),
        hidden=vmem(columns, total, units),
        gate_up=vmem(tiles, width, 256),
        down=vmem(pieces, units, PIECE),
        sums=vmem(2, half + 1, direct, total, PIECE),
        xsum_right=vmem(half + 1, extra, rows, PIECE),
        xsum_left=vmem(half + 1, extra, rows, PIECE),
        totals=vmem(direct, places * main, PIECE),
        returned=vmem(direct, total, PIECE),
        load_sem=dma(5 + 2 * tiles + pieces),
    )
    for name, shape in dict(
        rim=(2,), mate=(2,), chip=(2, chips), enter=(1,), head=(columns,), table=(columns,), ring=(2, ring),
        over=(2,), token=(2, half, extra), out=(direct,), xout=(columns,), xover=(2, columns), chunk=(2, half, direct),
        xback=(columns,), sum=(2, half + 1, direct), xsum=(2, half + 1, extra), back=(direct,), tail=(2, half),
    ).items():
        scratch[name + "_send"], scratch[name + "_recv"] = dma(*shape), dma(*shape)
    scratch["pass_send"], scratch["pass_recv"] = dma(2, ring), dma(2, ring)
    names = [*given, "out_ref", *scratch]
    return pl.pallas_call(
        functools.partial(layer_kernel, dims, names),
        out_shape=jax.ShapeDtypeStruct((rows, width), bf16),
        in_specs=in_specs,
        out_specs=pl.BlockSpec(memory_space=pltpu.VMEM),
        scratch_shapes=list(scratch.values()),
        compiler_params=pltpu.CompilerParams(
            collective_id=0, has_side_effects=True, vmem_limit_bytes=VMEM_LIMIT
        ),
        name="layer",
    )(*given.values())


def local(
    residual,
    grouped_value_heads,
    output_gate_heads,
    projected_key_query,
    raw_step_size,
    step_size_bias,
    head_decay_logarithm,
    position_extra_decay,
    head_skip_weight,
    value_kernel_taps,
    key_query_kernel,
    head_norm_gain,
    output_matrix,
    expert_norm_gain,
    expert_gate_weight,
    expert_up_weight,
    expert_down_weight,
    token_expert_choice,
    expert_output_weight,
):
    return layer(
        lax.axis_size("sp"),
        lax.axis_size("tp"),
        residual_ref=residual,
        value_hbm=grouped_value_heads.reshape(-1, BLOCK),
        gate_hbm=output_gate_heads.reshape(-1, BLOCK),
        keys_hbm=projected_key_query,
        raw_ref=raw_step_size.transpose(1, 2, 0),
        bias_ref=step_size_bias,
        log_ref=head_decay_logarithm,
        extra_ref=position_extra_decay.reshape(-1, BLOCK),
        skip_ref=head_skip_weight,
        value_tap_ref=value_kernel_taps.reshape(-1, BLOCK),
        key_tap_ref=key_query_kernel,
        head_gain_ref=head_norm_gain,
        matrix_hbm=output_matrix,
        expert_gain_ref=expert_norm_gain[None],
        choice_ref=token_expert_choice.T,
        share_ref=expert_output_weight.T,
        expert_gate_hbm=expert_gate_weight,
        expert_up_hbm=expert_up_weight,
        expert_down_hbm=expert_down_weight,
    )


def solution(mesh):
    placed = (
        P(("grp", "sp", "tp"), None),
        P(("grp", "sp"), None, "tp"),
        P(("grp", "sp"), None, "tp"),
        P(("grp", "sp"), None),
        P(("grp", "sp"), None, "tp"),
        P(None, "tp"),
        P(None, "tp"),
        P(("grp", "sp")),
        P(None, "tp"),
        P(None, None, "tp"),
        P(),
        P(None, "tp"),
        P(None, "tp", None),
        P(),
        P("sp", None, "tp"),
        P("sp", None, "tp"),
        P("sp", "tp", None),
        P(("grp", "sp", "tp"), None),
        P(("grp", "sp", "tp"), None),
    )
    return jax.shard_map(
        local, mesh=mesh, in_specs=placed, out_specs=P(("grp", "sp", "tp"), None), check_vma=False
    )
```

```python
import functools
import types

import jax
import jax.numpy as jnp
from jax import lax
from jax.experimental import pallas as pl
from jax.experimental.pallas import tpu as pltpu
from jax.sharding import PartitionSpec as P

HEAD_DIM = 64
STATE_ONE = 64
STATE_TWO = 128
BLOCK = 128
EPSILON = 1e-06

MESH = pl.DeviceIdType.MESH
PIECE = 256
HEADS = 4
RING_SHARE = 6
VMEM_LIMIT = 67043328


def remote(src, dst, send, recv, device):
    return pltpu.make_async_remote_copy(
        src_ref=src, dst_ref=dst, send_sem=send, recv_sem=recv, device_id=device, device_id_type=MESH
    )


def silu(a):
    return a * (1.0 / (1.0 + jnp.exp(-a)))


def layer_kernel(dims, names, *refs):
    r = types.SimpleNamespace(**dict(zip(names, refs, strict=True)))
    f32, bf16 = jnp.float32, jnp.bfloat16
    places, columns, width, rows = dims.places, dims.columns, dims.width, BLOCK
    half, chips, blocks = columns // 2, places // 2, columns
    me_x, me_s = lax.axis_index("tp"), lax.axis_index("sp")
    core, me_y = lax.rem(me_s, 2), lax.div(me_s, 2)
    right = {"tp": lax.rem(me_x + 1, columns)}
    left = {"tp": lax.rem(me_x + columns - 1, columns)}
    mate = {"sp": me_s + 1 - 2 * core}
    following = {"sp": lax.rem(me_s + 1, places)}

    def column(offset):
        return lax.rem(me_x + offset + columns, columns)

    def place(offset):
        return lax.rem(me_s + offset, places)

    def peer(offset):
        return {"sp": lax.rem(me_s + 2 * offset, places)}

    def toward(way):
        return right if way == 0 else left

    ring_part, slab = dims.ring_part, rows // chips
    mine = pl.multiple_of(core * rows, rows)

    def slab_rows(y):
        return pl.ds(pl.multiple_of(mine + y * slab, 16), slab)

    on_ring, on_grid = pl.ds(0, ring_part), pl.ds(ring_part, width - ring_part)
    loads = [
        (r.matrix_hbm.at[0], r.matrix.at[0, pl.ds(0, rows), :]),
        (r.matrix_hbm.at[1], r.matrix.at[0, pl.ds(rows, rows), :]),
        (r.value_hbm, r.value_in),
        (r.keys_hbm, r.keys_in),
        (r.gate_hbm, r.gate_in),
    ]
    loads = [pltpu.make_async_copy(a, b, r.load_sem.at[n]) for n, (a, b) in enumerate(loads)]
    for load in loads:
        load.start()
    for t in range(dims.tiles):
        span = pl.ds(t * 128, 128)
        for n, weight in enumerate((r.expert_gate_hbm, r.expert_up_hbm)):
            pltpu.make_async_copy(
                weight.at[0, :, span], r.gate_up.at[t, :, pl.ds(n * 128, 128)], r.weight_sem.at[0]
            ).start()
    for p in range(dims.pieces):
        pltpu.make_async_copy(
            r.expert_down_hbm.at[0, :, pl.ds(p * PIECE, PIECE)], r.down.at[p], r.weight_sem.at[1]
        ).start()

    barrier = pltpu.get_barrier_semaphore()
    peers = [{"tp": column(i)} for i in range(1, columns)] + [{"sp": place(i)} for i in range(1, places)]
    for device in peers:
        pl.semaphore_signal(barrier, inc=1, device_id=device, device_id_type=MESH)

    for g in range(2):
        raw = r.raw_ref[g].astype(f32)
        for k in range(blocks):
            r.stride_s[HEADS * k + 2 * g : HEADS * k + 2 * g + 2, :] = raw[:, k * rows : (k + 1) * rows]
    for k in range(blocks):
        r.run_s[HEADS * k : HEADS * k + HEADS, :] = jnp.broadcast_to(r.extra_ref[k : k + 1, :], (HEADS, rows))
    head_of = jnp.bitwise_and(lax.broadcasted_iota(jnp.int32, (HEADS * blocks, rows), 0), HEADS - 1)

    def by_head(table):
        picked = jnp.full((HEADS * blocks, rows), table[1, 1], f32)
        for n in range(3):
            picked = jnp.where(head_of == n, table[n // 2, n % 2], picked)
        return picked

    shifted = r.stride_s[...] + by_head(r.bias_ref)
    stride = jnp.maximum(shifted, 0.0) + jnp.log1p(jnp.exp(-jnp.abs(shifted)))
    log_decay = r.run_s[...] - jnp.exp(by_head(r.log_ref)) * stride
    at_row = lax.broadcasted_iota(jnp.int32, (rows, rows), 0)
    at_lane = lax.broadcasted_iota(jnp.int32, (rows, rows), 1)
    running = jnp.dot(
        log_decay,
        jnp.where(at_row <= at_lane, 1.0, 0.0),
        preferred_element_type=f32,
        precision=lax.Precision.HIGHEST,
    )
    ends = jnp.broadcast_to(running[:, rows - 1 : rows], running.shape)
    r.stride_s[...] = stride
    r.run_s[...] = running
    r.fade_s[...] = jnp.exp(ends - running) * stride
    r.end_s[...] = jnp.exp(ends)
    turned = jnp.transpose(running)
    for k in range(blocks):
        r.cols_s[k, :, 0:HEADS] = turned[:, HEADS * k : HEADS * k + HEADS]

    first_head = at_lane < HEAD_DIM

    def row_pair(table, k, g):
        low = table[pl.ds(HEADS * k + 2 * g, 1), :]
        high = table[pl.ds(HEADS * k + 2 * g + 1, 1), :]
        return jnp.where(first_head[0:1], low, high)

    r.tables[me_x] = jnp.zeros((8, rows), f32)
    r.tables[me_x, 0:2, :] = r.choice_ref[...].astype(f32)
    r.tables[me_x, 2:4, :] = r.share_ref[...]

    for load in loads[:-1]:
        load.wait()
    pl.semaphore_wait(barrier, len(peers))

    def matrix_block(way, event, k):
        piece = (event % 2) ^ way
        block = (columns - k if way == 0 else k) % columns
        return r.matrix.at[block, pl.ds(pl.multiple_of(mine + piece * (rows // 2), 16), rows // 2), on_ring]

    def matrix_ring(way, event):
        k = event // 2
        return remote(
            matrix_block(way, event, k),
            matrix_block(way, event, k + 1),
            r.ring_send.at[0],
            r.ring_recv.at[way, event],
            toward(way),
        )

    def slab_copy(offset):
        return remote(
            r.matrix.at[0, slab_rows(me_y), on_grid],
            r.matrix.at[columns - offset, slab_rows(me_y), on_grid],
            r.slab_send.at[0],
            r.slab_recv.at[0],
            {"tp": column(offset)},
        )

    def grid_view(way, event, y):
        blocks_of = pl.ds(1, half) if (event % 2) ^ way == 0 else pl.ds(1 + half, half - 1)
        return r.matrix.at[blocks_of, slab_rows(y), on_grid]

    def grid_ring(way, event, y):
        here = grid_view(way, event, y)
        return remote(
            here, here, r.grid_send.at[0], r.grid_recv.at[way, event], peer(1) if way == 0 else peer(chips - 1)
        )

    def to_mate(here, which):
        return remote(here, here, r.pass_send.at[which], r.pass_recv.at[which], mate)

    most_columns, other_blocks = pl.ds(0, columns - 1), pl.ds(1, columns - 1)
    ring_total = r.matrix.at[other_blocks, pl.ds(0, rows), on_ring]
    grid_total = r.matrix.at[other_blocks, pl.ds(0, (chips - 1) * slab), on_grid]
    slab_total = r.matrix.at[other_blocks, pl.ds(0, slab), on_grid]
    pass_totals = (ring_total, r.matrix.at[other_blocks, pl.ds(0, rows), on_grid])

    rim_rows = 16
    positions = blocks * rows
    rims = [
        remote(
            r.value_in.at[pl.ds(2 * positions - rim_rows, rim_rows), :],
            r.value_rim,
            r.rim_send.at[0],
            r.rim_recv.at[0],
            following,
        ),
        remote(
            r.keys_in.at[pl.ds(positions - rim_rows, rim_rows), :], r.keys_rim, r.rim_send.at[1], r.rim_recv.at[1], following
        ),
    ]
    for rim in rims:
        rim.start()

    def table_copy(offset):
        here = r.tables.at[me_x]
        return remote(here, here, r.table_send.at[0], r.table_recv.at[0], {"tp": column(offset)})

    for i in range(1, columns):
        table_copy(i).start()
    for i in range(1, columns):
        slab_copy(i).start()
    for event in range(2):
        for way in range(2):
            if event < columns - 1:
                matrix_ring(way, event).start()
    tables_total = remote(
        r.tables.at[most_columns], r.tables.at[most_columns], r.table_send.at[0], r.table_recv.at[0], right
    )

    def serve_ring(event):
        for way in range(2):
            matrix_ring(way, event).wait_recv()
            if event + 2 < columns - 1:
                matrix_ring(way, event + 2).start()
            to_mate(matrix_block(way, event, event // 2 + 1), 0).start()

    def serve_slab():
        remote(slab_total, slab_total, r.slab_send.at[0], r.slab_recv.at[0], right).wait_recv()
        for event in range(2):
            for way in range(2):
                if event < chips - 1:
                    grid_ring(way, event, me_y).start()
        to_mate(r.matrix.at[other_blocks, slab_rows(me_y), on_grid], 1).start()

    def serve_grid(event):
        k = event // 2 + 1
        for way in range(2):
            y = lax.rem(me_y + (chips - k if way == 0 else k), chips)
            grid_ring(way, event, y).wait_recv()
            if event + 2 < chips - 1:
                grid_ring(way, event + 2, y).start()
            to_mate(grid_view(way, event, y), 1).start()

    waiting = [("x", e) for e in range(columns - 1)] + [("y", e) for e in range(chips - 1)]

    def serve(*steps):
        for step in steps:
            if step in waiting:
                waiting.remove(step)
                (serve_ring if step[0] == "x" else serve_grid)(step[1])

    r.value_wide[rim_rows:, :] = r.value_in[...].astype(f32)
    r.keys_wide[rim_rows:, :] = r.keys_in[...].astype(f32)
    taps = r.value_tap_ref.shape[0] // 2
    value_tap = r.value_tap_ref[...].astype(f32)
    key_tap = r.key_tap_ref[...].astype(f32)
    even = jnp.bitwise_and(lax.broadcasted_iota(jnp.int32, (2 * rows, rows), 0), 1) == 0
    tap_rows = [jnp.where(even, value_tap[2 * j : 2 * j + 1], value_tap[2 * j + 1 : 2 * j + 2]) for j in range(taps)]

    def states_of(k):
        window = r.value_wide[pl.ds(pl.multiple_of(k * 2 * rows, 2 * rows), 2 * rows + rim_rows), :]
        total = jnp.zeros((2 * rows, rows), f32)
        for j in range(taps):
            start = rim_rows - 2 * (taps - 1 - j)
            total = total + window[start : start + 2 * rows] * tap_rows[j]
        r.conv_wide[...] = silu(total).astype(bf16).astype(f32)
        window = r.keys_wide[pl.ds(pl.multiple_of(k * rows, rows), rows + rim_rows), :]
        total = jnp.zeros((rows, r.keys_wide.shape[1]), f32)
        for j in range(taps):
            start = rim_rows - (taps - 1 - j)
            total = total + window[start : start + rows] * key_tap[j : j + 1]
        conv = silu(total).astype(bf16).astype(f32)
        both = conv[:, 0 : 2 * STATE_ONE]
        keys = [jnp.where(first_head, both, 0.0), conv[:, 2 * STATE_ONE : 2 * STATE_ONE + STATE_TWO]]
        asks = [pltpu.roll(both, STATE_ONE, 1), conv[:, 2 * STATE_ONE + STATE_TWO :]]
        for g in range(2):
            x = r.conv_wide[pl.ds(g, rows, stride=2), :].astype(bf16)
            key_t = jnp.transpose(keys[g])
            r.x_s[k, g] = x
            r.kt_s[k, g] = key_t.astype(bf16)
            r.q_s[k, g] = asks[g].astype(bf16)
            faded = jnp.concatenate(
                [key_t * r.fade_s[pl.ds(HEADS * k + 2 * g + h, 1), :] for h in range(2)], axis=0
            ).astype(bf16)
            state = jnp.dot(faded, x, preferred_element_type=f32)
            r.state_s[k, g] = jnp.where(first_head, state[:rows], state[rows:])

    def state_step(i, carry):
        states_of(i)
        return carry

    lax.fori_loop(1, blocks, state_step, 0)
    for rim in rims:
        rim.wait_recv()
    opening = me_s == 0
    r.value_wide[0:rim_rows, :] = jnp.where(opening, 0.0, r.value_rim[...].astype(f32))
    r.keys_wide[0:rim_rows, :] = jnp.where(opening, 0.0, r.keys_rim[...].astype(f32))
    states_of(0)

    packed = STATE_TWO + STATE_ONE
    piece = packed // 2

    def local_end(g):
        total = jnp.zeros((rows, rows), f32)
        faded = jnp.ones((1, rows), f32)
        for k in range(blocks):
            decay = row_pair(r.end_s, k, g)
            total = total * decay + r.state_s[k, g]
            faded = faded * decay
        return total, faded

    end_one, fade_one = local_end(0)
    end_two, fade_two = local_end(1)
    own = jnp.concatenate([end_two, end_one[:STATE_ONE]], axis=0)
    r.own_pack[...] = own.astype(bf16)
    r.own_fade[0:1, :] = fade_one
    r.own_fade[1:2, :] = fade_two
    r.own_fade[2:8, :] = jnp.zeros((6, rows), f32)
    mates = [
        remote(r.own_pack, r.mate_pack, r.mate_send.at[0], r.mate_recv.at[0], mate),
        remote(r.own_fade, r.mate_fade, r.mate_send.at[1], r.mate_recv.at[1], mate),
    ]
    for copy in mates:
        copy.start()
    for copy in mates:
        copy.wait_recv()
    is_low = core == 0
    low = jnp.where(is_low, own, r.mate_pack[...].astype(f32))
    high = jnp.where(is_low, r.mate_pack[...].astype(f32), own)
    mate_rows = r.mate_fade[...]
    own_rows = r.own_fade[...]
    high_rows = jnp.where(is_low, mate_rows, own_rows)
    in_two = lax.broadcasted_iota(jnp.int32, (packed, rows), 0) < STATE_TWO
    r.chip_pack[...] = (low * jnp.where(in_two, high_rows[1:2], high_rows[0:1]) + high).astype(bf16)
    r.chip_fade[...] = own_rows * mate_rows
    my_half = pl.ds(pl.multiple_of(core * piece, 16), piece)

    def to_chip(n, which):
        src = r.chip_pack.at[my_half, :] if which == 0 else r.chip_fade
        dst = r.all_pack.at[me_y] if which == 0 else r.all_fade.at[me_y]
        return remote(src, dst, r.chip_send.at[which, n], r.chip_recv.at[which, n], peer(n))

    for n in range(1, chips):

        @pl.when(me_y + n < chips)
        def _():
            for which in range(2):
                to_chip(n, which).start()


    below = at_row >= at_lane

    def near_step(k, carry):
        cols = r.cols_s[k]
        for g in range(2):
            scores = jnp.dot(r.q_s[k, g], r.kt_s[k, g], preferred_element_type=f32)
            parts = []
            for h in range(2):
                n = 2 * g + h
                gap = cols[:, n : n + 1] - r.run_s[pl.ds(HEADS * k + n, 1), :]
                damping = jnp.exp(jnp.where(below, gap, -1e30))
                parts.append((scores * damping * r.stride_s[pl.ds(HEADS * k + n, 1), :]).astype(bf16))
            near = jnp.dot(jnp.concatenate(parts, axis=0), r.x_s[k, g], preferred_element_type=f32)
            r.near_s[k, g] = jnp.where(first_head, near[:rows], near[rows:])
        return carry

    lax.fori_loop(0, blocks, near_step, 0)
    serve_slab()
    serve(*dims.serving[0])
    main, over, slots = dims.main, dims.over, places * dims.main
    total_slots = slots + over
    slot_row = lax.broadcasted_iota(jnp.int32, (total_slots, over), 0)
    slot_expert = lax.broadcasted_iota(jnp.int32, (total_slots, over), 1)
    spread = jnp.where(
        ((slot_row < slots) & (slot_row >= slot_expert * main) & (slot_row < slot_expert * main + main))
        | (slot_row == slots + slot_expert),
        1.0,
        0.0,
    ).astype(bf16)
    at = lax.broadcasted_iota(jnp.int32, (total_slots, rows), 0)
    turn = jnp.where(at < slots, jnp.bitwise_and(at, main - 1), main).astype(f32)
    expert_at = lax.broadcasted_iota(jnp.int32, (over, rows), 0).astype(f32)
    earlier = jnp.where(at_row < at_lane, 1.0, 0.0).astype(bf16)

    def make_put(col):
        table = r.tables[col]
        named = jnp.where((expert_at == table[0:1]) | (expert_at == table[1:2]), 1.0, 0.0)
        rank = jnp.dot(named.astype(bf16), earlier, preferred_element_type=f32)
        named_x = jnp.dot(spread, named.astype(bf16), preferred_element_type=f32)
        rank_x = jnp.dot(spread, rank.astype(bf16), preferred_element_type=f32)
        r.put[col] = jnp.where(rank_x == turn, named_x, 0.0).astype(bf16)

    tables_total.wait_recv()

    def put_step(col, carry):
        make_put(col)
        return carry

    lax.fori_loop(0, columns, put_step, 0)

    loads[-1].wait()
    serve(*dims.serving[1])
    for n in range(1, chips):

        @pl.when(me_y >= n)
        def _():
            for which in range(2):
                to_chip(n, which).wait_recv()

    row_at = lax.broadcasted_iota(jnp.int32, (piece, rows), 0) + core * piece
    half_two = row_at < STATE_TWO
    entering = jnp.zeros((piece, rows), f32)
    for y in range(chips):
        fades = r.all_fade[y]
        later = entering * jnp.where(half_two, fades[1:2], fades[0:1]) + r.all_pack[y].astype(f32)
        entering = jnp.where(y < me_y, later, entering)
    r.enter_pack[my_half, :] = entering.astype(bf16)
    here = r.enter_pack.at[my_half, :]
    enter_copy = remote(here, here, r.enter_send.at[0], r.enter_recv.at[0], mate)
    enter_copy.start()
    enter_copy.wait_recv()
    chip_state = r.enter_pack[...].astype(f32)
    after_low = chip_state * jnp.where(in_two, mate_rows[1:2], mate_rows[0:1]) + r.mate_pack[...].astype(f32)
    entered = jnp.where(is_low, chip_state, after_low)
    r.carry_s[1] = entered[:STATE_TWO]
    r.carry_s[0] = jnp.zeros((rows, rows), f32)
    r.carry_s[0, 0:STATE_ONE, :] = entered[STATE_TWO:]

    serve(*dims.serving[2])
    def head_copy(col):
        return remote(r.mixed_s.at[col], r.heads_in.at[me_x], r.head_send.at[0], r.head_recv.at[0], {"tp": col})

    def mix_step(k, carry):
        cols = jnp.exp(r.cols_s[k])
        r.gate_wide[...] = r.gate_in[pl.ds(pl.multiple_of(k * 2 * rows, 2 * rows), 2 * rows), :].astype(f32)
        for g in range(2):
            state = r.carry_s[g]
            coarse = state.astype(bf16)
            fine = (state - coarse.astype(f32)).astype(bf16)
            ask = r.q_s[k, g]
            far = jnp.dot(
                jnp.concatenate([ask, ask], axis=1),
                jnp.concatenate([coarse, fine], axis=0),
                preferred_element_type=f32,
            )
            reach = jnp.where(first_head, cols[:, 2 * g : 2 * g + 1], cols[:, 2 * g + 1 : 2 * g + 2])
            skip = jnp.where(first_head[0:1], r.skip_ref[g, 0], r.skip_ref[g, 1])
            mixed = r.near_s[k, g] + far * reach + skip * r.x_s[k, g].astype(f32)
            gated = mixed * silu(r.gate_wide[pl.ds(g, rows, stride=2), :])
            square = gated * gated
            one = jnp.sum(jnp.where(first_head, square, 0.0), axis=1, keepdims=True)
            two = jnp.sum(jnp.where(first_head, 0.0, square), axis=1, keepdims=True)
            scale = lax.rsqrt(jnp.where(first_head, one, two) * (1.0 / HEAD_DIM) + EPSILON)
            r.mixed_s[k, :, g * rows : (g + 1) * rows] = (gated * scale * r.head_gain_ref[g : g + 1, :]).astype(bf16)
            r.carry_s[g] = state * row_pair(r.end_s, k, g) + r.state_s[k, g]

        @pl.when(k != me_x)
        def _():
            head_copy(k).start()

        return carry

    lax.fori_loop(0, blocks, mix_step, 0)
    r.heads_in[me_x] = r.mixed_s[me_x]

    slot_col = lax.broadcasted_iota(jnp.int32, (over, total_slots), 1)
    slot_exp = lax.broadcasted_iota(jnp.int32, (over, total_slots), 0)
    spread_t = jnp.where(
        ((slot_col < slots) & (slot_col >= slot_exp * main) & (slot_col < slot_exp * main + main))
        | (slot_col == slots + slot_exp),
        1.0,
        0.0,
    ).astype(bf16)
    at_t = lax.broadcasted_iota(jnp.int32, (rows, total_slots), 1)
    turn_t = jnp.where(at_t < slots, jnp.bitwise_and(at_t, main - 1), main).astype(f32)
    expert_to = lax.broadcasted_iota(jnp.int32, (rows, over), 1).astype(f32)
    later_t = jnp.where(at_lane < at_row, 1.0, 0.0).astype(bf16)

    def make_pick(col):
        table = jnp.transpose(r.tables[col])
        named = [jnp.where(expert_to == table[:, k : k + 1], 1.0, 0.0) for k in range(2)]
        rank = jnp.dot(later_t, (named[0] + named[1]).astype(bf16), preferred_element_type=f32)
        rank_x = jnp.dot(rank.astype(bf16), spread_t, preferred_element_type=f32)
        for k in range(2):
            named_x = jnp.dot(named[k].astype(bf16), spread_t, preferred_element_type=f32)
            r.pick[col, k] = jnp.where(rank_x == turn_t, named_x, 0.0).astype(bf16)
            r.share_s[col, k] = jnp.broadcast_to(table[:, 2 + k : 3 + k], (rows, rows))

    def product(block, first):
        for n in range(0, width, 512):
            span = slice(n, n + 512)
            part = jnp.dot(r.heads_in[column(block)], r.matrix[block, :, span], preferred_element_type=f32)
            r.acc_s[:, span] = part if first else r.acc_s[:, span] + part

    serve(*dims.serving[3])
    serve(*list(waiting))
    heads_total = remote(
        r.mixed_s.at[most_columns], r.heads_in.at[most_columns], r.head_send.at[0], r.head_recv.at[0], right
    )
    heads_total.wait_recv()
    remote(pass_totals[0], pass_totals[0], r.pass_send.at[0], r.pass_recv.at[0], mate).wait_recv()
    remote(pass_totals[1], pass_totals[1], r.pass_send.at[1], r.pass_recv.at[1], mate).wait_recv()
    for block in range(columns):
        product(block, block == 0)

    stream = (r.residual_ref[...].astype(f32) + r.acc_s[...]).astype(bf16)
    r.stream_s[...] = stream
    wide = stream.astype(f32)
    scale = lax.rsqrt(jnp.mean(wide * wide, axis=1, keepdims=True) + EPSILON)
    normed = (wide * scale * r.expert_gain_ref[...]).astype(bf16)

    direct, extra = dims.direct, dims.pieces - dims.direct
    pieces = dims.pieces
    lanes_of = PIECE // 128

    def lines(index):
        return pl.ds(pl.multiple_of(index * main, main), main)

    def far(way, p):
        odd = lax.rem(p, 2) if not isinstance(p, int) else p % 2
        return half - odd if way == 0 else half - 1 + odd

    for q in range(extra):
        r.tokens[me_x, q] = normed[:, (direct + q) * PIECE : (direct + q + 1) * PIECE]

    def token_ring(way, step, q, col):
        here = r.tokens.at[col, q]
        return remote(here, here, r.token_send.at[0], r.token_recv.at[way, step, q], toward(way))

    put_own = r.put[me_x]
    for p in range(direct):
        part = jnp.dot(put_own, normed[:, p * PIECE : (p + 1) * PIECE], preferred_element_type=f32)
        r.outbound[p] = part[:slots].astype(bf16)
        for c in range(lanes_of):
            r.over_out[:, p * lanes_of + c, :] = part[slots:, c * 128 : (c + 1) * 128]
    for q in range(extra):
        for way in range(2):
            token_ring(way, 0, q, me_x).start()

    def send_out(p, carry):
        for i in range(1, places):
            remote(
                r.outbound.at[p, lines(place(i)), :],
                r.chunks.at[me_x, p, lines(me_s), :],
                r.out_send.at[0],
                r.out_recv.at[p],
                {"sp": place(i)},
            ).start()
        r.chunks[me_x, p, lines(me_s), :] = r.outbound[p, lines(me_s), :]
        return carry

    lax.fori_loop(0, direct, send_out, 0)
    for i in range(1, places):
        remote(
            r.over_out.at[place(i)], r.over_in.at[me_s], r.over_send.at[0], r.over_recv.at[0], {"sp": place(i)}
        ).start()
    r.over_in[me_s] = r.over_out[me_s]
    if places < over:
        r.over_in[places:over] = jnp.zeros((over - places, *r.over_in.shape[1:]), f32)
        r.over_ret[places:over] = jnp.zeros((over - places, *r.over_ret.shape[1:]), f32)
        r.xover_in[:, places:over] = jnp.zeros((columns, over - places, *r.xover_in.shape[2:]), f32)
        r.xover_ret[:, places:over] = jnp.zeros((columns, over - places, *r.xover_ret.shape[2:]), f32)

    def route(offset):
        col = column(offset)
        for q in range(extra):
            part = jnp.dot(r.put[col], r.tokens[col, q], preferred_element_type=f32)
            r.xout[col, q] = part[:slots].astype(bf16)
            r.chunks[col, direct + q, lines(me_s), :] = r.xout[col, q, lines(me_s), :]
            for c in range(lanes_of):
                r.xover_out[offset, :, q * lanes_of + c, :] = part[slots:, c * 128 : (c + 1) * 128]
        r.xover_in[offset, me_s] = r.xover_out[offset, me_s]
        for i in range(1, places):
            remote(
                r.xout.at[col, :, lines(place(i)), :],
                r.chunks.at[col, pl.ds(direct, extra), lines(me_s), :],
                r.xout_send.at[0],
                r.xout_recv.at[offset],
                {"sp": place(i)},
            ).start()
            remote(
                r.xover_out.at[offset, place(i)],
                r.xover_in.at[offset, me_s],
                r.xover_send.at[0],
                r.xover_recv.at[0, offset],
                {"sp": place(i)},
            ).start()

    def routed(offset):
        col = column(offset)
        most = pl.ds(0, (places - 1) * main)
        return (
            remote(
                r.xout.at[col, :, most, :],
                r.chunks.at[col, pl.ds(direct, extra), most, :],
                r.xout_send.at[0],
                r.xout_recv.at[offset],
                right,
            ),
            remote(
                r.xover_out.at[offset, 0 : places - 1],
                r.xover_in.at[offset, 0 : places - 1],
                r.xover_send.at[0],
                r.xover_recv.at[0, offset],
                right,
            ),
        )

    def take_routed(offset):
        col = column(offset)
        for copy in routed(offset):
            copy.wait_recv()
        for q in range(extra):
            for c in range(lanes_of):
                r.chunks[col, direct + q, slots:, c * 128 : (c + 1) * 128] = r.xover_in[
                    offset, :, q * lanes_of + c, :
                ].astype(bf16)

    route(0)

    def token_event(k):
        for q in range(extra):
            for way in range(2):
                if k <= far(way, q):
                    col = column(-k if way == 0 else k)
                    token_ring(way, k - 1, q, col).wait_recv()
                    if k < far(way, q):
                        token_ring(way, k, q, col).start()
        if k < half:
            route(columns - k)
        route(k)

    def chunk_ring(way, step, p, col):
        here = r.chunks.at[col, p, pl.ds(0, slots), :]
        return remote(here, here, r.chunk_send.at[0], r.chunk_recv.at[way, step, p], toward(way))

    def over_ring(way, step, col):
        here = r.chunks.at[col, pl.ds(0, direct), pl.ds(slots, over), :]
        return remote(here, here, r.tail_send.at[0], r.tail_recv.at[way, step], toward(way))

    def out_arrived(p):
        most = pl.ds(0, (places - 1) * main)
        return remote(
            r.outbound.at[p, most, :], r.chunks.at[me_x, p, most, :], r.out_send.at[0], r.out_recv.at[p], right
        )

    def start_piece(p):
        out_arrived(p).wait_recv()
        chunk_ring(0, 0, p, me_x).start()
        chunk_ring(1, 0, p, me_x).start()

    def start_over():
        remote(
            r.over_out.at[0 : places - 1], r.over_in.at[0 : places - 1], r.over_send.at[0], r.over_recv.at[0], right
        ).wait_recv()
        for c in range(direct * lanes_of):
            at_lanes = (c % lanes_of) * 128
            r.chunks[me_x, c // lanes_of, slots:, at_lanes : at_lanes + 128] = r.over_in[:, c, :].astype(bf16)
        for way in range(2):
            over_ring(way, 0, me_x).start()

    for copy in rims + mates + [enter_copy]:
        copy.wait_send()
    for n in range(1, chips):

        @pl.when(me_y + n < chips)
        def _():
            for which in range(2):
                to_chip(n, which).wait_send()

    heads_total.wait_send()
    tables_total.wait_send()
    remote(ring_total, ring_total, r.ring_send.at[0], r.ring_recv.at[0, 0], right).wait_send()
    remote(slab_total, slab_total, r.slab_send.at[0], r.slab_recv.at[0], right).wait_send()
    remote(grid_total, grid_total, r.grid_send.at[0], r.grid_recv.at[0, 0], right).wait_send()
    for which in range(2):
        view = pass_totals[which]
        remote(view, view, r.pass_send.at[which], r.pass_recv.at[which], mate).wait_send()

    for step in dims.opening:
        if step > 0:
            token_event(step)
        elif -step < direct:
            start_piece(-step)
    start_over()

    def offset_of(n):
        k = lax.div(n + 1, 2)
        return jnp.where(lax.rem(n, 2) == 1, lax.rem(columns - k, columns), k)

    def unit(n, t):
        offset = offset_of(n)
        col = column(offset)
        pl.when(t == 0)(lambda: take_routed(offset))
        acc = jnp.dot(r.chunks[col, 0], r.gate_up[t, 0:PIECE, :], preferred_element_type=f32)
        for q in range(1, pieces):
            acc = acc + jnp.dot(
                r.chunks[col, q], r.gate_up[t, q * PIECE : (q + 1) * PIECE, :], preferred_element_type=f32
            )
        value = silu(acc[:, 0:128]) * acc[:, 128:256]
        r.hidden[col, :, pl.ds(pl.multiple_of(t * 128, 128), 128)] = value.astype(bf16)
        pl.when(t == dims.tiles - 1)(lambda: give_back(offset))

    def own(col, p):
        return jnp.dot(r.hidden[col], r.down[p], preferred_element_type=f32)

    def give_back(offset):
        col = column(offset)
        for q in range(extra):
            part = own(col, direct + q)
            r.xback[col, q] = part[:slots].astype(bf16)
            r.xret[col, q, lines(me_s), :] = r.xback[col, q, lines(me_s), :]
            for c in range(lanes_of):
                r.xover_back[offset, :, q * lanes_of + c, :] = part[slots:, c * 128 : (c + 1) * 128]
        r.xover_ret[offset, me_s] = r.xover_back[offset, me_s]
        for i in range(1, places):
            remote(
                r.xback.at[col, :, lines(place(i)), :],
                r.xret.at[col, :, lines(me_s), :],
                r.xback_send.at[0],
                r.xback_recv.at[offset],
                {"sp": place(i)},
            ).start()
            remote(
                r.xover_back.at[offset, place(i)],
                r.xover_ret.at[offset, me_s],
                r.xover_send.at[1],
                r.xover_recv.at[1, offset],
                {"sp": place(i)},
            ).start()

    def given_back(offset):
        col = column(offset)
        most = pl.ds(0, (places - 1) * main)
        return (
            remote(
                r.xback.at[col, :, most, :],
                r.xret.at[col, :, most, :],
                r.xback_send.at[0],
                r.xback_recv.at[offset],
                right,
            ),
            remote(
                r.xover_back.at[offset, 0 : places - 1],
                r.xover_ret.at[offset, 0 : places - 1],
                r.xover_send.at[1],
                r.xover_recv.at[1, offset],
                right,
            ),
        )

    for n, weights in enumerate((r.gate_up, r.down)):
        pltpu.make_async_copy(weights, weights, r.weight_sem.at[n]).wait()

    def units(low, high):
        def body(v, carry):
            unit(lax.div(v, dims.tiles), lax.rem(v, dims.tiles))
            return carry

        lax.fori_loop(low, high, body, 0)

    def hop(way, j, p):
        return remote(
            r.sums.at[way, j, p],
            r.sums.at[way, j - 1, p],
            r.sum_send.at[0],
            r.sum_recv.at[way, j - 1, p],
            {"tp": column(1 - 2 * way)},
        )

    def chains(long, step, group):
        j = half - step if long else half - 1 - step

        def body(p, carry):
            odd = lax.rem(p, 2)
            way = 1 - odd if long else odd
            value = own(column(j * (1 - 2 * way)), p)
            if step > 0:
                hop(way, j + 1, p).wait_recv()
                value = value + r.sums[way, j, p].astype(f32)
            r.sums[way, j, p] = value.astype(bf16)
            hop(way, j, p).start()
            return carry

        lax.fori_loop(*group, body, 0)

    share_of = dims.schedule
    for k in range(1, half + 1):
        first, last = share_of[k - 1] * dims.tiles, share_of[k] * dims.tiles

        if k == half and half > 1:
            units(first, last)
            first = last
            for group in dims.groups:
                chains(False, 0, group)

        def pass_on(p, carry, k=k, first=first, last=last):
            for way in range(2):
                col = column(-k if way == 0 else k)

                @pl.when(k <= far(way, p))
                def _():
                    chunk_ring(way, k - 1, p, col).wait_recv()

                if k < half:

                    @pl.when(k < far(way, p))
                    def _():
                        chunk_ring(way, k, p, col).start()

            if last > first:
                units(
                    first + lax.div(p * (last - first), direct), first + lax.div((p + 1) * (last - first), direct)
                )
            return carry

        lax.fori_loop(0, direct, pass_on, 0)
        for way in range(2):
            if k <= far(way, 0):
                col = column(-k if way == 0 else k)
                over_ring(way, k - 1, col).wait_recv()
                if k < far(way, 0):
                    over_ring(way, k, col).start()
        if k == 1:
            lax.fori_loop(0, columns, lambda col, carry: (make_pick(col), carry)[1], 0)
    units(share_of[half] * dims.tiles, columns * dims.tiles)

    def finish(p, carry):
        value = own(me_x, p)
        hop(0, 1, p).wait_recv()
        hop(1, 1, p).wait_recv()
        value = value + r.sums[0, 0, p].astype(f32) + r.sums[1, 0, p].astype(f32)
        r.totals[p] = value[0:slots].astype(bf16)
        r.over_total[p] = value[slots:]
        r.returned[p, lines(me_s), :] = r.totals[p, lines(me_s), :]
        for i in range(1, places):
            remote(
                r.totals.at[p, lines(place(i)), :],
                r.returned.at[p, lines(me_s), :],
                r.back_send.at[0],
                r.back_recv.at[p],
                {"sp": place(i)},
            ).start()
        return carry

    def weighted(col, table, q):
        one = jnp.dot(r.pick[col, 0], table[q], preferred_element_type=f32)
        two = jnp.dot(r.pick[col, 1], table[q], preferred_element_type=f32)
        first, second = r.share_s[col, 0], r.share_s[col, 1]
        return jnp.concatenate([first] * lanes_of, axis=1) * one + jnp.concatenate([second] * lanes_of, axis=1) * two

    def take_back(offset):
        col = column(offset)
        for copy in given_back(offset):
            copy.wait_recv()
        for q in range(extra):
            for c in range(lanes_of):
                r.xret[col, q, slots:, c * 128 : (c + 1) * 128] = r.xover_ret[
                    offset, :, q * lanes_of + c, :
                ].astype(bf16)

    def token_hop(way, j, q):
        buffer = r.xsum_right if way == 0 else r.xsum_left
        return remote(
            buffer.at[j, q],
            buffer.at[j - 1, q],
            r.xsum_send.at[0],
            r.xsum_recv.at[way, j - 1, q],
            toward(way),
        )

    taken = set()

    def token_round(t):
        for q in range(extra):
            for way in range(2):
                buffer = r.xsum_right if way == 0 else r.xsum_left
                j = far(1 - way, q) - t
                if j < 1:
                    continue
                offset = j if way == 0 else columns - j
                if offset not in taken:
                    taken.add(offset)
                    take_back(offset)
                col = column(offset)
                value = weighted(col, r.xret.at[col], q)
                if t > 0:
                    token_hop(way, j + 1, q).wait_recv()
                    value = value + buffer[j, q].astype(f32)
                buffer[j, q] = value.astype(bf16)
                token_hop(way, j, q).start()

    for group in dims.groups:
        chains(True, 0, group)
    def left_by_now(view, send, recv):
        remote(view, view, send, recv, right).wait_send()

    most_places, most_lines = pl.ds(0, places - 1), pl.ds(0, (places - 1) * main)
    chunks_total = r.chunks.at[most_columns, pl.ds(0, direct), pl.ds(0, slots), :]
    left_by_now(r.over_out.at[most_places], r.over_send.at[0], r.over_recv.at[0])
    left_by_now(r.tokens.at[most_columns], r.token_send.at[0], r.token_recv.at[0, 0, 0])
    left_by_now(r.chunks.at[most_columns, pl.ds(0, direct), pl.ds(slots, over), :], r.tail_send.at[0], r.tail_recv.at[0, 0])
    left_by_now(chunks_total, r.chunk_send.at[0], r.chunk_recv.at[0, 0, 0])
    left_by_now(r.outbound.at[:, most_lines, :], r.out_send.at[0], r.out_recv.at[0])
    left_by_now(r.xout.at[:, :, most_lines, :], r.xout_send.at[0], r.xout_recv.at[0])
    left_by_now(r.xover_out.at[:, most_places], r.xover_send.at[0], r.xover_recv.at[0, 0])
    for kind, step, group in dims.closing:
        if kind == "short":
            chains(False, step, group)
        elif kind == "long":
            chains(True, step, group)
        elif kind == "token":
            token_round(step)
        else:
            lax.fori_loop(*group, finish, 0)
    for c in range(direct * lanes_of):
        at_lanes = (c % lanes_of) * 128
        r.over_back[:, c, :] = r.over_total[c // lanes_of, :, at_lanes : at_lanes + 128]
    r.over_ret[me_s] = r.over_back[me_s]
    for i in range(1, places):
        remote(
            r.over_back.at[place(i)], r.over_ret.at[me_s], r.over_send.at[1], r.over_recv.at[1], {"sp": place(i)}
        ).start()

    left_by_now(r.xback.at[:, :, most_lines, :], r.xback_send.at[0], r.xback_recv.at[0])
    left_by_now(r.xover_back.at[:, most_places], r.xover_send.at[1], r.xover_recv.at[1, 0])
    left_by_now(r.chunks.at[most_columns, pl.ds(0, direct)], r.sum_send.at[0], r.sum_recv.at[0, 0, 0])
    token_round(half - 1)
    take_back(0)
    for q in range(extra):
        value = weighted(me_x, r.xret.at[me_x], q)
        for way in range(2):
            token_hop(way, 1, q).wait_recv()
        value = value + r.xsum_right[0, q].astype(f32) + r.xsum_left[0, q].astype(f32)
        span = slice((direct + q) * PIECE, (direct + q + 1) * PIECE)
        r.out_ref[:, span] = (r.stream_s[:, span].astype(f32) + value).astype(bf16)

    remote(
        r.over_back.at[0 : places - 1], r.over_ret.at[0 : places - 1], r.over_send.at[1], r.over_recv.at[1], right
    ).wait_recv()
    for c in range(direct * lanes_of):
        at_lanes = (c % lanes_of) * 128
        r.returned[c // lanes_of, slots:, at_lanes : at_lanes + 128] = r.over_ret[:, c, :].astype(bf16)

    def back_arrived(p):
        most = pl.ds(0, (places - 1) * main)
        return remote(
            r.totals.at[p, most, :], r.returned.at[p, most, :], r.back_send.at[0], r.back_recv.at[p], right
        )

    def combine(p, carry):
        back_arrived(p).wait_recv()
        span = pl.ds(pl.multiple_of(p * PIECE, PIECE), PIECE)
        value = weighted(me_x, r.returned, p)
        r.out_ref[:, span] = (r.stream_s[:, span].astype(f32) + value).astype(bf16)
        return carry

    lax.fori_loop(0, direct, combine, 0)

    left_by_now(r.over_back.at[most_places], r.over_send.at[1], r.over_recv.at[1])
    left_by_now(r.tokens.at[most_columns], r.xsum_send.at[0], r.xsum_recv.at[0, 0, 0])
    left_by_now(r.totals.at[:, most_lines, :], r.back_send.at[0], r.back_recv.at[0])


def layer(places, columns, **given):
    f32, bf16 = jnp.float32, jnp.bfloat16
    rows, width = given["residual_ref"].shape
    units = given["expert_gate_hbm"].shape[2]
    lanes = given["keys_hbm"].shape[1]
    positions = columns * BLOCK
    half, chips, blocks = columns // 2, places // 2, columns
    main = 2 * rows // places
    over = -(-places // 16) * 16
    pieces = width // PIECE
    extra = max(1, pieces // 4)
    direct = pieces - extra
    tiles, total = units // 128, places * main + over
    ring_part = width * RING_SHARE // 16 // 128 * 128
    schedule = (0, 0, 1, 5, 7) if half == 4 else (0,) * half + (columns - 1,)
    opening = (1, 0, 2, -1, -2, 3, -3, -4, 4, -5) if half == 4 else (*range(1, half + 1), *range(0, -direct, -1))
    serving = [
        [("x", 0)],
        [("x", 1), ("y", 0)],
        [("x", 2), ("y", 1)],
        [("x", 3), ("y", 2), ("x", 4), ("y", 3), ("y", 4), ("y", 5), ("x", 5), ("x", 6), ("y", 6)],
    ]
    groups = [(low, min(low + 2, direct)) for low in range(0, direct, 2)]
    closing = []
    for n, group in enumerate(groups):
        last = n == len(groups) - 1
        for step in range(1, half):
            if step < half - 1:
                closing.append(("short", step, group))
            closing.append(("long", step, group))
            if last and step < half:
                closing.append(("token", step - 1, None))
        if n > 0:
            closing.insert(len(closing) - half, ("finish", None, groups[n - 1]))
    closing.append(("finish", None, groups[-1]))
    dims = types.SimpleNamespace(
        places=places, columns=columns, width=width, main=main, over=over, pieces=pieces, direct=direct, tiles=tiles,
        schedule=schedule, opening=opening, groups=groups, closing=closing, ring_part=ring_part, serving=serving,
    )
    packed = STATE_ONE + STATE_TWO
    square = (blocks, 2, BLOCK, BLOCK)
    vmem = lambda *shape, dtype=bf16: pltpu.VMEM(shape, dtype)
    dma = lambda *shape: pltpu.SemaphoreType.DMA(shape)
    spaces = {"ref": pltpu.VMEM, "hbm": pl.ANY}
    in_specs = [
        pl.BlockSpec(memory_space=pltpu.SMEM if a.shape == (2, 2) else spaces[name[-3:]]) for name, a in given.items()
    ]
    lane_rows = PIECE // 128
    scratch = dict(
        value_in=vmem(2 * positions, BLOCK),
        gate_in=vmem(2 * positions, BLOCK),
        keys_in=vmem(positions, lanes),
        value_rim=vmem(16, BLOCK),
        keys_rim=vmem(16, lanes),
        value_wide=vmem(2 * positions + 16, BLOCK, dtype=f32),
        keys_wide=vmem(positions + 16, lanes, dtype=f32),
        gate_wide=vmem(2 * BLOCK, BLOCK, dtype=f32),
        conv_wide=vmem(2 * BLOCK, BLOCK, dtype=f32),
        x_s=vmem(*square),
        kt_s=vmem(*square),
        q_s=vmem(*square),
        state_s=vmem(*square, dtype=f32),
        near_s=vmem(*square, dtype=f32),
        stride_s=vmem(HEADS * blocks, BLOCK, dtype=f32),
        run_s=vmem(HEADS * blocks, BLOCK, dtype=f32),
        fade_s=vmem(HEADS * blocks, BLOCK, dtype=f32),
        end_s=vmem(HEADS * blocks, BLOCK, dtype=f32),
        cols_s=vmem(blocks, BLOCK, HEADS, dtype=f32),
        own_pack=vmem(packed, BLOCK),
        own_fade=vmem(8, BLOCK, dtype=f32),
        mate_pack=vmem(packed, BLOCK),
        mate_fade=vmem(8, BLOCK, dtype=f32),
        chip_pack=vmem(packed, BLOCK),
        chip_fade=vmem(8, BLOCK, dtype=f32),
        all_pack=vmem(chips, packed // 2, BLOCK),
        all_fade=vmem(chips, 8, BLOCK, dtype=f32),
        enter_pack=vmem(packed, BLOCK),
        carry_s=vmem(2, BLOCK, BLOCK, dtype=f32),
        mixed_s=vmem(columns, BLOCK, 2 * BLOCK),
        heads_in=vmem(columns, BLOCK, 2 * BLOCK),
        matrix=vmem(columns, 2 * BLOCK, width),
        acc_s=vmem(rows, width, dtype=f32),
        stream_s=vmem(rows, width),
        tables=vmem(columns, 8, rows, dtype=f32),
        put=vmem(columns, total, rows),
        pick=vmem(columns, 2, rows, total),
        share_s=vmem(columns, 2, rows, 128, dtype=f32),
        tokens=vmem(columns, extra, rows, PIECE),
        outbound=vmem(direct, places * main, PIECE),
        over_out=vmem(over, direct * lane_rows, 128, dtype=f32),
        over_in=vmem(over, direct * lane_rows, 128, dtype=f32),
        over_back=vmem(over, direct * lane_rows, 128, dtype=f32),
        over_ret=vmem(over, direct * lane_rows, 128, dtype=f32),
        over_total=vmem(direct, over, PIECE, dtype=f32),
        xout=vmem(columns, extra, places * main, PIECE),
        xback=vmem(columns, extra, places * main, PIECE),
        xret=vmem(columns, extra, total, PIECE),
        xover_out=vmem(columns, over, extra * lane_rows, 128, dtype=f32),
        xover_in=vmem(columns, over, extra * lane_rows, 128, dtype=f32),
        xover_back=vmem(columns, over, extra * lane_rows, 128, dtype=f32),
        xover_ret=vmem(columns, over, extra * lane_rows, 128, dtype=f32),
        chunks=vmem(columns, pieces, total, PIECE),
        hidden=vmem(columns, total, units),
        gate_up=vmem(tiles, width, 256),
        down=vmem(pieces, units, PIECE),
        sums=vmem(2, half + 1, direct, total, PIECE),
        xsum_right=vmem(half + 1, extra, rows, PIECE),
        xsum_left=vmem(half + 1, extra, rows, PIECE),
        totals=vmem(direct, places * main, PIECE),
        returned=vmem(direct, total, PIECE),
        load_sem=dma(5),
        weight_sem=dma(2),
    )
    steps = (2, half)
    for name, send, recv in (
        ("rim", (2,), (2,)),
        ("mate", (2,), (2,)),
        ("chip", (2, chips), (2, chips)),
        ("enter", (1,), (1,)),
        ("head", (1,), (1,)),
        ("table", (1,), (1,)),
        ("ring", (1,), (2, columns - 1)),
        ("slab", (1,), (1,)),
        ("grid", (1,), (2, chips - 1)),
        ("pass", (2,), (2,)),
        ("over", (2,), (2,)),
        ("token", (1,), (*steps, extra)),
        ("out", (1,), (direct,)),
        ("xout", (1,), (columns,)),
        ("xover", (2,), (2, columns)),
        ("chunk", (1,), (*steps, direct)),
        ("tail", (1,), steps),
        ("xback", (1,), (columns,)),
        ("sum", (1,), (*steps, direct)),
        ("xsum", (1,), (*steps, extra)),
        ("back", (1,), (direct,)),
    ):
        scratch[name + "_send"], scratch[name + "_recv"] = dma(*send), dma(*recv)
    names = [*given, "out_ref", *scratch]
    return pl.pallas_call(
        functools.partial(layer_kernel, dims, names),
        out_shape=jax.ShapeDtypeStruct((rows, width), bf16),
        in_specs=in_specs,
        out_specs=pl.BlockSpec(memory_space=pltpu.VMEM),
        scratch_shapes=list(scratch.values()),
        compiler_params=pltpu.CompilerParams(
            collective_id=0, has_side_effects=True, vmem_limit_bytes=VMEM_LIMIT
        ),
        name="layer",
    )(*given.values())


def local(
    residual,
    grouped_value_heads,
    output_gate_heads,
    projected_key_query,
    raw_step_size,
    step_size_bias,
    head_decay_logarithm,
    position_extra_decay,
    head_skip_weight,
    value_kernel_taps,
    key_query_kernel,
    head_norm_gain,
    output_matrix,
    expert_norm_gain,
    expert_gate_weight,
    expert_up_weight,
    expert_down_weight,
    token_expert_choice,
    expert_output_weight,
):
    return layer(
        lax.axis_size("sp"),
        lax.axis_size("tp"),
        residual_ref=residual,
        value_hbm=grouped_value_heads.reshape(-1, BLOCK),
        gate_hbm=output_gate_heads.reshape(-1, BLOCK),
        keys_hbm=projected_key_query,
        raw_ref=raw_step_size.transpose(1, 2, 0),
        bias_ref=step_size_bias,
        log_ref=head_decay_logarithm,
        extra_ref=position_extra_decay.reshape(-1, BLOCK),
        skip_ref=head_skip_weight,
        value_tap_ref=value_kernel_taps.reshape(-1, BLOCK),
        key_tap_ref=key_query_kernel,
        head_gain_ref=head_norm_gain,
        matrix_hbm=output_matrix,
        expert_gain_ref=expert_norm_gain[None],
        choice_ref=token_expert_choice.T,
        share_ref=expert_output_weight.T,
        expert_gate_hbm=expert_gate_weight,
        expert_up_hbm=expert_up_weight,
        expert_down_hbm=expert_down_weight,
    )


def solution(mesh):
    placed = (
        P(("grp", "sp", "tp"), None),
        P(("grp", "sp"), None, "tp"),
        P(("grp", "sp"), None, "tp"),
        P(("grp", "sp"), None),
        P(("grp", "sp"), None, "tp"),
        P(None, "tp"),
        P(None, "tp"),
        P(("grp", "sp")),
        P(None, "tp"),
        P(None, None, "tp"),
        P(),
        P(None, "tp"),
        P(None, "tp", None),
        P(),
        P("sp", None, "tp"),
        P("sp", None, "tp"),
        P("sp", "tp", None),
        P(("grp", "sp", "tp"), None),
        P(("grp", "sp", "tp"), None),
    )
    return jax.shard_map(
        local, mesh=mesh, in_specs=placed, out_specs=P(("grp", "sp", "tp"), None), check_vma=False
    )
```

```python
import functools
import types

import jax
import jax.numpy as jnp
from jax import lax
from jax.experimental import pallas as pl
from jax.experimental.pallas import tpu as pltpu
from jax.sharding import PartitionSpec as P

HEAD_DIM = 64
STATE_ONE = 64
STATE_TWO = 128
BLOCK = 128
EPSILON = 1e-06

MESH = pl.DeviceIdType.MESH
PIECE = 256
HEADS = 4
RING_SHARE = 7
VMEM_LIMIT = 67043328


def remote(src, dst, send, recv, device):
    return pltpu.make_async_remote_copy(
        src_ref=src, dst_ref=dst, send_sem=send, recv_sem=recv, device_id=device, device_id_type=MESH
    )


def silu(a):
    return a * (1.0 / (1.0 + jnp.exp(-a)))


def layer_kernel(dims, names, *refs):
    r = types.SimpleNamespace(**dict(zip(names, refs, strict=True)))
    f32, bf16 = jnp.float32, jnp.bfloat16
    places, columns, width, rows = dims.places, dims.columns, dims.width, BLOCK
    half, chips, blocks = columns // 2, places // 2, columns
    me_x, me_s = lax.axis_index("tp"), lax.axis_index("sp")
    core, me_y = lax.rem(me_s, 2), lax.div(me_s, 2)
    right = {"tp": lax.rem(me_x + 1, columns)}
    left = {"tp": lax.rem(me_x + columns - 1, columns)}
    mate = {"sp": me_s + 1 - 2 * core}
    following = {"sp": lax.rem(me_s + 1, places)}

    def column(offset):
        return lax.rem(me_x + offset + columns, columns)

    def place(offset):
        return lax.rem(me_s + offset, places)

    def peer(offset):
        return {"sp": lax.rem(me_s + 2 * offset, places)}

    def toward(way):
        return right if way == 0 else left

    barrier = pltpu.get_barrier_semaphore()
    peers = [{"tp": column(i)} for i in range(1, columns)] + [{"sp": place(i)} for i in range(1, places)]
    for device in peers:
        pl.semaphore_signal(barrier, inc=1, device_id=device, device_id_type=MESH)

    ring_part, slab = dims.ring_part, rows // chips
    mine = pl.multiple_of(core * rows, rows)

    def slab_rows(y):
        return pl.ds(pl.multiple_of(mine + y * slab, 16), slab)

    on_ring, on_grid = pl.ds(0, ring_part), pl.ds(ring_part, width - ring_part)
    loads = [
        (r.matrix_hbm.at[0], r.matrix.at[0, pl.ds(0, rows), :]),
        (r.matrix_hbm.at[1], r.matrix.at[0, pl.ds(rows, rows), :]),
        (r.value_hbm, r.value_in),
        (r.keys_hbm, r.keys_in),
        (r.gate_hbm, r.gate_in),
        (r.residual_hbm, r.residual_in),
    ]
    loads = [pltpu.make_async_copy(a, b, r.load_sem.at[n]) for n, (a, b) in enumerate(loads)]
    for load in loads:
        load.start()
    r.tables[me_x] = jnp.zeros((8, rows), f32)
    r.tables[me_x, 0:2, :] = r.choice_ref[...].astype(f32)
    r.tables[me_x, 2:4, :] = r.share_ref[...]

    for load in loads[:-2]:
        load.wait()
    pl.semaphore_wait(barrier, len(peers))

    def matrix_block(way, event, k, sub):
        piece = ((event % 2) ^ way) * 2 + sub
        block = (columns - k if way == 0 else k) % columns
        return r.matrix.at[block, pl.ds(pl.multiple_of(mine + piece * (rows // 4), 16), rows // 4), on_ring]

    def matrix_ring(way, event, sub):
        k = event // 2
        return remote(
            matrix_block(way, event, k, sub),
            matrix_block(way, event, k + 1, sub),
            r.ring_send.at[0],
            r.ring_recv.at[way, event, sub],
            toward(way),
        )

    def slab_copy(offset):
        return remote(
            r.matrix.at[0, slab_rows(me_y), on_grid],
            r.matrix.at[columns - offset, slab_rows(me_y), on_grid],
            r.slab_send.at[0],
            r.slab_recv.at[0],
            {"tp": column(offset)},
        )

    def grid_view(way, event, y):
        blocks_of = pl.ds(1, half) if (event % 2) ^ way == 0 else pl.ds(1 + half, half - 1)
        return r.matrix.at[blocks_of, slab_rows(y), on_grid]

    def grid_ring(way, event, y):
        here = grid_view(way, event, y)
        return remote(
            here, here, r.grid_send.at[0], r.grid_recv.at[way, event], peer(1) if way == 0 else peer(chips - 1)
        )

    def to_mate(here, which):
        return remote(here, here, r.pass_send.at[which], r.pass_recv.at[which], mate)

    most_columns, other_blocks = pl.ds(0, columns - 1), pl.ds(1, columns - 1)
    ring_total = r.matrix.at[other_blocks, pl.ds(0, rows), on_ring]
    grid_total = r.matrix.at[other_blocks, pl.ds(0, (chips - 1) * slab), on_grid]
    slab_total = r.matrix.at[other_blocks, pl.ds(0, slab), on_grid]
    pass_totals = (ring_total, r.matrix.at[other_blocks, pl.ds(0, rows), on_grid])

    rim_rows = 16
    positions = blocks * rows
    rims = [
        remote(
            r.value_in.at[pl.ds(2 * positions - rim_rows, rim_rows), :],
            r.value_rim,
            r.rim_send.at[0],
            r.rim_recv.at[0],
            following,
        ),
        remote(
            r.keys_in.at[pl.ds(positions - rim_rows, rim_rows), :], r.keys_rim, r.rim_send.at[1], r.rim_recv.at[1], following
        ),
    ]
    for rim in rims:
        rim.start()

    def table_copy(offset):
        here = r.tables.at[me_x]
        return remote(here, here, r.table_send.at[0], r.table_recv.at[0], {"tp": column(offset)})

    for i in range(1, columns):
        table_copy(i).start()
    for i in range(1, columns):
        slab_copy(i).start()
    for event in range(min(2, columns - 1)):
        for sub in range(2):
            for way in range(2):
                matrix_ring(way, event, sub).start()
    tables_total = remote(
        r.tables.at[most_columns], r.tables.at[most_columns], r.table_send.at[0], r.table_recv.at[0], right
    )

    def serve_ring(event):
        for sub in range(2):
            for way in range(2):
                matrix_ring(way, event, sub).wait_recv()
                if event + 2 < columns - 1:
                    matrix_ring(way, event + 2, sub).start()
                to_mate(matrix_block(way, event, event // 2 + 1, sub), 0).start()

    def serve_slab():
        remote(slab_total, slab_total, r.slab_send.at[0], r.slab_recv.at[0], right).wait_recv()
        for event in range(2):
            for way in range(2):
                if event < chips - 1:
                    grid_ring(way, event, me_y).start()
        to_mate(r.matrix.at[other_blocks, slab_rows(me_y), on_grid], 1).start()

    def serve_grid(event):
        k = event // 2 + 1
        for way in range(2):
            y = lax.rem(me_y + (chips - k if way == 0 else k), chips)
            grid_ring(way, event, y).wait_recv()
            if event + 2 < chips - 1:
                grid_ring(way, event + 2, y).start()
            to_mate(grid_view(way, event, y), 1).start()

    waiting = [("x", e) for e in range(columns - 1)] + [("y", e) for e in range(chips - 1)]

    def serve(*steps):
        for step in steps:
            if step in waiting:
                waiting.remove(step)
                (serve_ring if step[0] == "x" else serve_grid)(step[1])

    for t in range(dims.tiles):
        span = pl.ds(t * 128, 128)
        for n, weight in enumerate((r.expert_gate_hbm, r.expert_up_hbm)):
            pltpu.make_async_copy(
                weight.at[0, :, span], r.gate_up.at[t, :, pl.ds(n * 128, 128)], r.weight_sem.at[0]
            ).start()
    for p in range(dims.pieces):
        pltpu.make_async_copy(
            r.expert_down_hbm.at[0, :, pl.ds(p * PIECE, PIECE)], r.down.at[p], r.weight_sem.at[1]
        ).start()

    for g in range(2):
        raw = r.raw_ref[g].astype(f32)
        for k in range(blocks):
            r.stride_s[HEADS * k + 2 * g : HEADS * k + 2 * g + 2, :] = raw[:, k * rows : (k + 1) * rows]
    for k in range(blocks):
        r.run_s[HEADS * k : HEADS * k + HEADS, :] = jnp.broadcast_to(r.extra_ref[k : k + 1, :], (HEADS, rows))
    head_of = jnp.bitwise_and(lax.broadcasted_iota(jnp.int32, (HEADS * blocks, rows), 0), HEADS - 1)

    def by_head(table):
        picked = jnp.full((HEADS * blocks, rows), table[1, 1], f32)
        for n in range(3):
            picked = jnp.where(head_of == n, table[n // 2, n % 2], picked)
        return picked

    shifted = r.stride_s[...] + by_head(r.bias_ref)
    stride = jnp.maximum(shifted, 0.0) + jnp.log1p(jnp.exp(-jnp.abs(shifted)))
    log_decay = r.run_s[...] - jnp.exp(by_head(r.log_ref)) * stride
    at_row = lax.broadcasted_iota(jnp.int32, (rows, rows), 0)
    at_lane = lax.broadcasted_iota(jnp.int32, (rows, rows), 1)
    running = jnp.dot(
        log_decay,
        jnp.where(at_row <= at_lane, 1.0, 0.0),
        preferred_element_type=f32,
        precision=lax.Precision.HIGHEST,
    )
    ends = jnp.broadcast_to(running[:, rows - 1 : rows], running.shape)
    r.stride_s[...] = stride
    r.run_s[...] = running
    r.fade_s[...] = jnp.exp(ends - running) * stride
    r.end_s[...] = jnp.exp(ends)
    turned = jnp.transpose(running)
    for k in range(blocks):
        r.cols_s[k, :, 0:HEADS] = turned[:, HEADS * k : HEADS * k + HEADS]

    first_head = at_lane < HEAD_DIM

    def row_pair(table, k, g):
        low = table[pl.ds(HEADS * k + 2 * g, 1), :]
        high = table[pl.ds(HEADS * k + 2 * g + 1, 1), :]
        return jnp.where(first_head[0:1], low, high)

    r.value_wide[rim_rows:, :] = r.value_in[...].astype(f32)
    r.keys_wide[rim_rows:, :] = r.keys_in[...].astype(f32)
    taps = r.value_tap_ref.shape[0] // 2
    value_tap = r.value_tap_ref[...].astype(f32)
    key_tap = r.key_tap_ref[...].astype(f32)
    even = jnp.bitwise_and(lax.broadcasted_iota(jnp.int32, (2 * rows, rows), 0), 1) == 0
    tap_rows = [jnp.where(even, value_tap[2 * j : 2 * j + 1], value_tap[2 * j + 1 : 2 * j + 2]) for j in range(taps)]

    def states_of(k):
        window = r.value_wide[pl.ds(pl.multiple_of(k * 2 * rows, 2 * rows), 2 * rows + rim_rows), :]
        total = jnp.zeros((2 * rows, rows), f32)
        for j in range(taps):
            start = rim_rows - 2 * (taps - 1 - j)
            total = total + window[start : start + 2 * rows] * tap_rows[j]
        r.conv_wide[...] = silu(total).astype(bf16).astype(f32)
        window = r.keys_wide[pl.ds(pl.multiple_of(k * rows, rows), rows + rim_rows), :]
        total = jnp.zeros((rows, r.keys_wide.shape[1]), f32)
        for j in range(taps):
            start = rim_rows - (taps - 1 - j)
            total = total + window[start : start + rows] * key_tap[j : j + 1]
        conv = silu(total).astype(bf16).astype(f32)
        both = conv[:, 0 : 2 * STATE_ONE]
        keys = [jnp.where(first_head, both, 0.0), conv[:, 2 * STATE_ONE : 2 * STATE_ONE + STATE_TWO]]
        asks = [pltpu.roll(both, STATE_ONE, 1), conv[:, 2 * STATE_ONE + STATE_TWO :]]
        for g in range(2):
            x = r.conv_wide[pl.ds(g, rows, stride=2), :].astype(bf16)
            key_t = jnp.transpose(keys[g])
            r.x_s[k, g] = x
            r.kt_s[k, g] = key_t.astype(bf16)
            r.q_s[k, g] = asks[g].astype(bf16)
            faded = jnp.concatenate(
                [key_t * r.fade_s[pl.ds(HEADS * k + 2 * g + h, 1), :] for h in range(2)], axis=0
            ).astype(bf16)
            state = jnp.dot(faded, x, preferred_element_type=f32)
            r.state_s[k, g] = jnp.where(first_head, state[:rows], state[rows:])

    def state_step(i, carry):
        states_of(i)
        return carry

    lax.fori_loop(1, blocks, state_step, 0)
    for rim in rims:
        rim.wait_recv()
    opening = me_s == 0
    r.value_wide[0:rim_rows, :] = jnp.where(opening, 0.0, r.value_rim[...].astype(f32))
    r.keys_wide[0:rim_rows, :] = jnp.where(opening, 0.0, r.keys_rim[...].astype(f32))
    states_of(0)

    packed = STATE_TWO + STATE_ONE
    piece = packed // 2

    def local_end(g):
        total = jnp.zeros((rows, rows), f32)
        faded = jnp.ones((1, rows), f32)
        for k in range(blocks):
            decay = row_pair(r.end_s, k, g)
            total = total * decay + r.state_s[k, g]
            faded = faded * decay
        return total, faded

    end_one, fade_one = local_end(0)
    end_two, fade_two = local_end(1)
    own = jnp.concatenate([end_two, end_one[:STATE_ONE]], axis=0)
    r.own_pack[...] = own.astype(bf16)
    r.own_fade[0:1, :] = fade_one
    r.own_fade[1:2, :] = fade_two
    r.own_fade[2:8, :] = jnp.zeros((6, rows), f32)
    mates = [
        remote(r.own_pack, r.mate_pack, r.mate_send.at[0], r.mate_recv.at[0], mate),
        remote(r.own_fade, r.mate_fade, r.mate_send.at[1], r.mate_recv.at[1], mate),
    ]
    for copy in mates:
        copy.start()
    for copy in mates:
        copy.wait_recv()
    is_low = core == 0
    low = jnp.where(is_low, own, r.mate_pack[...].astype(f32))
    high = jnp.where(is_low, r.mate_pack[...].astype(f32), own)
    mate_rows = r.mate_fade[...]
    own_rows = r.own_fade[...]
    high_rows = jnp.where(is_low, mate_rows, own_rows)
    in_two = lax.broadcasted_iota(jnp.int32, (packed, rows), 0) < STATE_TWO
    r.chip_pack[...] = (low * jnp.where(in_two, high_rows[1:2], high_rows[0:1]) + high).astype(bf16)
    r.chip_fade[...] = own_rows * mate_rows
    my_half = pl.ds(pl.multiple_of(core * piece, 16), piece)

    def to_chip(n, which):
        src = r.chip_pack.at[my_half, :] if which == 0 else r.chip_fade
        dst = r.all_pack.at[me_y] if which == 0 else r.all_fade.at[me_y]
        return remote(src, dst, r.chip_send.at[which, n], r.chip_recv.at[which, n], peer(n))

    for n in range(1, chips):

        @pl.when(me_y + n < chips)
        def _():
            for which in range(2):
                to_chip(n, which).start()


    below = at_row >= at_lane

    def near_step(k, carry):
        cols = r.cols_s[k]
        for g in range(2):
            scores = jnp.dot(r.q_s[k, g], r.kt_s[k, g], preferred_element_type=f32)
            parts = []
            for h in range(2):
                n = 2 * g + h
                gap = cols[:, n : n + 1] - r.run_s[pl.ds(HEADS * k + n, 1), :]
                damping = jnp.exp(jnp.where(below, gap, -1e30))
                parts.append((scores * damping * r.stride_s[pl.ds(HEADS * k + n, 1), :]).astype(bf16))
            near = jnp.dot(jnp.concatenate(parts, axis=0), r.x_s[k, g], preferred_element_type=f32)
            r.near_s[k, g] = jnp.where(first_head, near[:rows], near[rows:])
        return carry

    lax.fori_loop(0, blocks, near_step, 0)
    serve_slab()
    serve(*dims.serving[0])
    main, over, slots = dims.main, dims.over, places * dims.main
    total_slots = slots + over
    slot_row = lax.broadcasted_iota(jnp.int32, (total_slots, over), 0)
    slot_expert = lax.broadcasted_iota(jnp.int32, (total_slots, over), 1)
    spread = jnp.where(
        ((slot_row < slots) & (slot_row >= slot_expert * main) & (slot_row < slot_expert * main + main))
        | (slot_row == slots + slot_expert),
        1.0,
        0.0,
    ).astype(bf16)
    at = lax.broadcasted_iota(jnp.int32, (total_slots, rows), 0)
    turn = jnp.where(at < slots, jnp.bitwise_and(at, main - 1), main).astype(f32)
    expert_at = lax.broadcasted_iota(jnp.int32, (over, rows), 0).astype(f32)
    earlier = jnp.where(at_row < at_lane, 1.0, 0.0).astype(bf16)

    def make_put(col):
        table = r.tables[col]
        named = jnp.where((expert_at == table[0:1]) | (expert_at == table[1:2]), 1.0, 0.0)
        rank = jnp.dot(named.astype(bf16), earlier, preferred_element_type=f32)
        named_x = jnp.dot(spread, named.astype(bf16), preferred_element_type=f32)
        rank_x = jnp.dot(spread, rank.astype(bf16), preferred_element_type=f32)
        r.put[col] = jnp.where(rank_x == turn, named_x, 0.0).astype(bf16)

    tables_total.wait_recv()

    def put_step(col, carry):
        make_put(col)
        return carry

    lax.fori_loop(0, columns, put_step, 0)

    for load in loads[-2:]:
        load.wait()
    serve(*dims.serving[1])
    for n in range(1, chips):

        @pl.when(me_y >= n)
        def _():
            for which in range(2):
                to_chip(n, which).wait_recv()

    row_at = lax.broadcasted_iota(jnp.int32, (piece, rows), 0) + core * piece
    half_two = row_at < STATE_TWO
    entering = jnp.zeros((piece, rows), f32)
    for y in range(chips):
        fades = r.all_fade[y]
        later = entering * jnp.where(half_two, fades[1:2], fades[0:1]) + r.all_pack[y].astype(f32)
        entering = jnp.where(y < me_y, later, entering)
    r.enter_pack[my_half, :] = entering.astype(bf16)
    here = r.enter_pack.at[my_half, :]
    enter_copy = remote(here, here, r.enter_send.at[0], r.enter_recv.at[0], mate)
    enter_copy.start()
    enter_copy.wait_recv()
    chip_state = r.enter_pack[...].astype(f32)
    after_low = chip_state * jnp.where(in_two, mate_rows[1:2], mate_rows[0:1]) + r.mate_pack[...].astype(f32)
    entered = jnp.where(is_low, chip_state, after_low)
    r.carry_s[1] = entered[:STATE_TWO]
    r.carry_s[0] = jnp.zeros((rows, rows), f32)
    r.carry_s[0, 0:STATE_ONE, :] = entered[STATE_TWO:]

    serve(*dims.serving[2])
    def head_copy(col):
        return remote(r.mixed_s.at[col], r.heads_in.at[me_x], r.head_send.at[0], r.head_recv.at[0], {"tp": col})

    def mix_step(k, carry):
        cols = jnp.exp(r.cols_s[k])
        r.gate_wide[...] = r.gate_in[pl.ds(pl.multiple_of(k * 2 * rows, 2 * rows), 2 * rows), :].astype(f32)
        for g in range(2):
            state = r.carry_s[g]
            coarse = state.astype(bf16)
            fine = (state - coarse.astype(f32)).astype(bf16)
            ask = r.q_s[k, g]
            far = jnp.dot(
                jnp.concatenate([ask, ask], axis=1),
                jnp.concatenate([coarse, fine], axis=0),
                preferred_element_type=f32,
            )
            reach = jnp.where(first_head, cols[:, 2 * g : 2 * g + 1], cols[:, 2 * g + 1 : 2 * g + 2])
            skip = jnp.where(first_head[0:1], r.skip_ref[g, 0], r.skip_ref[g, 1])
            mixed = r.near_s[k, g] + far * reach + skip * r.x_s[k, g].astype(f32)
            gated = mixed * silu(r.gate_wide[pl.ds(g, rows, stride=2), :])
            square = gated * gated
            one = jnp.sum(jnp.where(first_head, square, 0.0), axis=1, keepdims=True)
            two = jnp.sum(jnp.where(first_head, 0.0, square), axis=1, keepdims=True)
            scale = lax.rsqrt(jnp.where(first_head, one, two) * (1.0 / HEAD_DIM) + EPSILON)
            r.mixed_s[k, :, g * rows : (g + 1) * rows] = (gated * scale * r.head_gain_ref[g : g + 1, :]).astype(bf16)
            r.carry_s[g] = state * row_pair(r.end_s, k, g) + r.state_s[k, g]

        @pl.when(k != me_x)
        def _():
            head_copy(k).start()

        return carry

    lax.fori_loop(0, blocks, mix_step, 0)
    r.heads_in[me_x] = r.mixed_s[me_x]

    slot_col = lax.broadcasted_iota(jnp.int32, (over, total_slots), 1)
    slot_exp = lax.broadcasted_iota(jnp.int32, (over, total_slots), 0)
    spread_t = jnp.where(
        ((slot_col < slots) & (slot_col >= slot_exp * main) & (slot_col < slot_exp * main + main))
        | (slot_col == slots + slot_exp),
        1.0,
        0.0,
    ).astype(bf16)
    at_t = lax.broadcasted_iota(jnp.int32, (rows, total_slots), 1)
    turn_t = jnp.where(at_t < slots, jnp.bitwise_and(at_t, main - 1), main).astype(f32)
    expert_to = lax.broadcasted_iota(jnp.int32, (rows, over), 1).astype(f32)
    later_t = jnp.where(at_lane < at_row, 1.0, 0.0).astype(bf16)

    def make_pick(col):
        table = jnp.transpose(r.tables[col])
        named = [jnp.where(expert_to == table[:, k : k + 1], 1.0, 0.0) for k in range(2)]
        rank = jnp.dot(later_t, (named[0] + named[1]).astype(bf16), preferred_element_type=f32)
        rank_x = jnp.dot(rank.astype(bf16), spread_t, preferred_element_type=f32)
        for k in range(2):
            named_x = jnp.dot(named[k].astype(bf16), spread_t, preferred_element_type=f32)
            r.pick[col, k] = jnp.where(rank_x == turn_t, named_x, 0.0).astype(bf16)
            r.share_s[col, k] = jnp.broadcast_to(table[:, 2 + k : 3 + k], (rows, rows))

    def product(block, first):
        for n in range(0, width, 512):
            span = slice(n, n + 512)
            part = jnp.dot(r.heads_in[column(block)], r.matrix[block, :, span], preferred_element_type=f32)
            r.acc_s[:, span] = part if first else r.acc_s[:, span] + part

    serve(*dims.serving[3])
    serve(*list(waiting))
    heads_total = remote(
        r.mixed_s.at[most_columns], r.heads_in.at[most_columns], r.head_send.at[0], r.head_recv.at[0], right
    )
    heads_total.wait_recv()
    remote(pass_totals[0], pass_totals[0], r.pass_send.at[0], r.pass_recv.at[0], mate).wait_recv()
    remote(pass_totals[1], pass_totals[1], r.pass_send.at[1], r.pass_recv.at[1], mate).wait_recv()
    for block in range(columns):
        product(block, block == 0)

    stream = (r.residual_in[...].astype(f32) + r.acc_s[...]).astype(bf16)
    r.stream_s[...] = stream
    wide = stream.astype(f32)
    scale = lax.rsqrt(jnp.mean(wide * wide, axis=1, keepdims=True) + EPSILON)
    normed = (wide * scale * r.expert_gain_ref[...]).astype(bf16)

    direct, extra = dims.direct, dims.pieces - dims.direct
    pieces = dims.pieces
    lanes_of = PIECE // 128

    def lines(index):
        return pl.ds(pl.multiple_of(index * main, main), main)

    def far(way, p):
        odd = lax.rem(p, 2) if not isinstance(p, int) else p % 2
        return half - odd if way == 0 else half - 1 + odd

    for q in range(extra):
        r.tokens[me_x, q] = normed[:, (direct + q) * PIECE : (direct + q + 1) * PIECE]

    thin = extra * lanes_of

    def token_ring(way, step, q, col):
        here = r.tokens.at[col, q // lanes_of, :, pl.ds(q % lanes_of * 128, 128)]
        return remote(here, here, r.token_send.at[0], r.token_recv.at[way, step, q], toward(way))

    put_own = r.put[me_x]
    for p in range(direct):
        part = jnp.dot(put_own, normed[:, p * PIECE : (p + 1) * PIECE], preferred_element_type=f32)
        r.outbound[p] = part[:slots].astype(bf16)
        for c in range(lanes_of):
            r.over_out[:, p * lanes_of + c, :] = part[slots:, c * 128 : (c + 1) * 128]
    for q in range(thin):
        for way in range(2):
            token_ring(way, 0, q, me_x).start()

    def send_out(p, carry):
        for i in range(1, places):
            remote(
                r.outbound.at[p, lines(place(i)), :],
                r.chunks.at[me_x, p, lines(me_s), :],
                r.out_send.at[0],
                r.out_recv.at[p],
                {"sp": place(i)},
            ).start()
        r.chunks[me_x, p, lines(me_s), :] = r.outbound[p, lines(me_s), :]
        return carry

    lax.fori_loop(0, direct, send_out, 0)
    for i in range(1, places):
        remote(
            r.over_out.at[place(i)], r.over_in.at[me_s], r.over_send.at[0], r.over_recv.at[0], {"sp": place(i)}
        ).start()
    r.over_in[me_s] = r.over_out[me_s]
    if places < over:
        r.over_in[places:over] = jnp.zeros((over - places, *r.over_in.shape[1:]), f32)
        r.over_ret[places:over] = jnp.zeros((over - places, *r.over_ret.shape[1:]), f32)
        r.xover_in[:, places:over] = jnp.zeros((columns, over - places, *r.xover_in.shape[2:]), f32)
        r.xover_ret[:, places:over] = jnp.zeros((columns, over - places, *r.xover_ret.shape[2:]), f32)

    def route(offset):
        col = column(offset)
        for q in range(extra):
            part = jnp.dot(r.put[col], r.tokens[col, q], preferred_element_type=f32)
            r.xout[col, q] = part[:slots].astype(bf16)
            r.chunks[col, direct + q, lines(me_s), :] = r.xout[col, q, lines(me_s), :]
            for c in range(lanes_of):
                r.xover_out[offset, :, q * lanes_of + c, :] = part[slots:, c * 128 : (c + 1) * 128]
        r.xover_in[offset, me_s] = r.xover_out[offset, me_s]
        for i in range(1, places):
            remote(
                r.xout.at[col, :, lines(place(i)), :],
                r.chunks.at[col, pl.ds(direct, extra), lines(me_s), :],
                r.xout_send.at[0],
                r.xout_recv.at[offset],
                {"sp": place(i)},
            ).start()
            remote(
                r.xover_out.at[offset, place(i)],
                r.xover_in.at[offset, me_s],
                r.xover_send.at[0],
                r.xover_recv.at[0, offset],
                {"sp": place(i)},
            ).start()

    def routed(offset):
        col = column(offset)
        most = pl.ds(0, (places - 1) * main)
        return (
            remote(
                r.xout.at[col, :, most, :],
                r.chunks.at[col, pl.ds(direct, extra), most, :],
                r.xout_send.at[0],
                r.xout_recv.at[offset],
                right,
            ),
            remote(
                r.xover_out.at[offset, 0 : places - 1],
                r.xover_in.at[offset, 0 : places - 1],
                r.xover_send.at[0],
                r.xover_recv.at[0, offset],
                right,
            ),
        )

    def take_routed(offset):
        col = column(offset)
        for copy in routed(offset):
            copy.wait_recv()
        for q in range(extra):
            for c in range(lanes_of):
                r.chunks[col, direct + q, slots:, c * 128 : (c + 1) * 128] = r.xover_in[
                    offset, :, q * lanes_of + c, :
                ].astype(bf16)

    route(0)

    def token_event(k):
        for q in range(thin):
            for way in range(2):
                if k <= far(way, q):
                    col = column(-k if way == 0 else k)
                    token_ring(way, k - 1, q, col).wait_recv()
                    if k < far(way, q):
                        token_ring(way, k, q, col).start()
        if k < half:
            route(columns - k)
        route(k)

    def chunk_ring(way, step, p, col):
        here = r.chunks.at[col, p, pl.ds(0, slots), :]
        return remote(here, here, r.chunk_send.at[0], r.chunk_recv.at[way, step, p], toward(way))

    def over_ring(way, step, col):
        here = r.chunks.at[col, pl.ds(0, direct), pl.ds(slots, over), :]
        return remote(here, here, r.tail_send.at[0], r.tail_recv.at[way, step], toward(way))

    def out_arrived(p):
        most = pl.ds(0, (places - 1) * main)
        return remote(
            r.outbound.at[p, most, :], r.chunks.at[me_x, p, most, :], r.out_send.at[0], r.out_recv.at[p], right
        )

    def start_piece(p):
        out_arrived(p).wait_recv()
        chunk_ring(0, 0, p, me_x).start()
        chunk_ring(1, 0, p, me_x).start()

    def start_over():
        remote(
            r.over_out.at[0 : places - 1], r.over_in.at[0 : places - 1], r.over_send.at[0], r.over_recv.at[0], right
        ).wait_recv()
        for c in range(direct * lanes_of):
            at_lanes = (c % lanes_of) * 128
            r.chunks[me_x, c // lanes_of, slots:, at_lanes : at_lanes + 128] = r.over_in[:, c, :].astype(bf16)
        for way in range(2):
            over_ring(way, 0, me_x).start()

    for copy in rims + mates + [enter_copy]:
        copy.wait_send()
    for n in range(1, chips):

        @pl.when(me_y + n < chips)
        def _():
            for which in range(2):
                to_chip(n, which).wait_send()

    heads_total.wait_send()
    tables_total.wait_send()
    remote(ring_total, ring_total, r.ring_send.at[0], r.ring_recv.at[0, 0, 0], right).wait_send()
    remote(slab_total, slab_total, r.slab_send.at[0], r.slab_recv.at[0], right).wait_send()
    remote(grid_total, grid_total, r.grid_send.at[0], r.grid_recv.at[0, 0], right).wait_send()
    for which in range(2):
        view = pass_totals[which]
        remote(view, view, r.pass_send.at[which], r.pass_recv.at[which], mate).wait_send()

    for step in dims.opening:
        if step > 0:
            token_event(step)
        elif -step < direct:
            start_piece(-step)
    start_over()

    def offset_of(n):
        k = lax.div(n + 1, 2)
        return jnp.where(lax.rem(n, 2) == 1, lax.rem(columns - k, columns), k)

    def unit(n, t):
        offset = offset_of(n)
        col = column(offset)
        pl.when(t == 0)(lambda: take_routed(offset))
        acc = jnp.dot(r.chunks[col, 0], r.gate_up[t, 0:PIECE, :], preferred_element_type=f32)
        for q in range(1, pieces):
            acc = acc + jnp.dot(
                r.chunks[col, q], r.gate_up[t, q * PIECE : (q + 1) * PIECE, :], preferred_element_type=f32
            )
        value = silu(acc[:, 0:128]) * acc[:, 128:256]
        r.hidden[col, :, pl.ds(pl.multiple_of(t * 128, 128), 128)] = value.astype(bf16)
        pl.when(t == dims.tiles - 1)(lambda: give_back(offset))

    def own(col, p):
        return jnp.dot(r.hidden[col], r.down[p], preferred_element_type=f32)

    def give_back(offset):
        col = column(offset)
        for q in range(extra):
            part = own(col, direct + q)
            r.xback[col, q] = part[:slots].astype(bf16)
            r.xret[col, q, lines(me_s), :] = r.xback[col, q, lines(me_s), :]
            for c in range(lanes_of):
                r.xover_back[offset, :, q * lanes_of + c, :] = part[slots:, c * 128 : (c + 1) * 128]
        r.xover_ret[offset, me_s] = r.xover_back[offset, me_s]
        for i in range(1, places):
            remote(
                r.xback.at[col, :, lines(place(i)), :],
                r.xret.at[col, :, lines(me_s), :],
                r.xback_send.at[0],
                r.xback_recv.at[offset],
                {"sp": place(i)},
            ).start()
            remote(
                r.xover_back.at[offset, place(i)],
                r.xover_ret.at[offset, me_s],
                r.xover_send.at[1],
                r.xover_recv.at[1, offset],
                {"sp": place(i)},
            ).start()

    def given_back(offset):
        col = column(offset)
        most = pl.ds(0, (places - 1) * main)
        return (
            remote(
                r.xback.at[col, :, most, :],
                r.xret.at[col, :, most, :],
                r.xback_send.at[0],
                r.xback_recv.at[offset],
                right,
            ),
            remote(
                r.xover_back.at[offset, 0 : places - 1],
                r.xover_ret.at[offset, 0 : places - 1],
                r.xover_send.at[1],
                r.xover_recv.at[1, offset],
                right,
            ),
        )

    for n, weights in enumerate((r.gate_up, r.down)):
        pltpu.make_async_copy(weights, weights, r.weight_sem.at[n]).wait()

    def units(low, high):
        def body(v, carry):
            unit(lax.div(v, dims.tiles), lax.rem(v, dims.tiles))
            return carry

        lax.fori_loop(low, high, body, 0)

    def hop(way, j, p):
        return remote(
            r.sums.at[way, j, p],
            r.sums.at[way, j - 1, p],
            r.sum_send.at[0],
            r.sum_recv.at[way, j - 1, p],
            {"tp": column(1 - 2 * way)},
        )

    def chains(long, step, group):
        j = half - step if long else half - 1 - step

        def body(p, carry):
            odd = lax.rem(p, 2)
            way = 1 - odd if long else odd
            value = own(column(j * (1 - 2 * way)), p)
            if step > 0:
                hop(way, j + 1, p).wait_recv()
                value = value + r.sums[way, j, p].astype(f32)
            r.sums[way, j, p] = value.astype(bf16)
            hop(way, j, p).start()
            return carry

        lax.fori_loop(*group, body, 0)

    share_of = dims.schedule
    for k in range(1, half + 1):
        first, last = share_of[k - 1] * dims.tiles, share_of[k] * dims.tiles

        if k == half and half > 1:
            units(first, last)
            first = last
            for group in dims.groups:
                chains(False, 0, group)

        def pass_on(p, carry, k=k, first=first, last=last):
            for way in range(2):
                col = column(-k if way == 0 else k)

                @pl.when(k <= far(way, p))
                def _():
                    chunk_ring(way, k - 1, p, col).wait_recv()

                if k < half:

                    @pl.when(k < far(way, p))
                    def _():
                        chunk_ring(way, k, p, col).start()

            if last > first:
                units(
                    first + lax.div(p * (last - first), direct), first + lax.div((p + 1) * (last - first), direct)
                )
            return carry

        lax.fori_loop(0, direct, pass_on, 0)
        for way in range(2):
            if k <= far(way, 0):
                col = column(-k if way == 0 else k)
                over_ring(way, k - 1, col).wait_recv()
                if k < far(way, 0):
                    over_ring(way, k, col).start()
        if k == 1:
            lax.fori_loop(0, columns, lambda col, carry: (make_pick(col), carry)[1], 0)
    units(share_of[half] * dims.tiles, columns * dims.tiles)

    def finish(p, carry):
        value = own(me_x, p)
        hop(0, 1, p).wait_recv()
        hop(1, 1, p).wait_recv()
        value = value + r.sums[0, 0, p].astype(f32) + r.sums[1, 0, p].astype(f32)
        r.totals[p] = value[0:slots].astype(bf16)
        r.over_total[p] = value[slots:]
        r.returned[p, lines(me_s), :] = r.totals[p, lines(me_s), :]
        for i in range(1, places):
            remote(
                r.totals.at[p, lines(place(i)), :],
                r.returned.at[p, lines(me_s), :],
                r.back_send.at[0],
                r.back_recv.at[p],
                {"sp": place(i)},
            ).start()
        return carry

    def weighted(col, table):
        one = jnp.dot(r.pick[col, 0], table, preferred_element_type=f32)
        two = jnp.dot(r.pick[col, 1], table, preferred_element_type=f32)
        copies = one.shape[1] // 128
        first, second = (jnp.concatenate([r.share_s[col, k]] * copies, axis=1) for k in range(2))
        return first * one + second * two

    def take_back(offset):
        col = column(offset)
        for copy in given_back(offset):
            copy.wait_recv()
        for q in range(extra):
            for c in range(lanes_of):
                r.xret[col, q, slots:, c * 128 : (c + 1) * 128] = r.xover_ret[
                    offset, :, q * lanes_of + c, :
                ].astype(bf16)

    def token_hop(way, j, q):
        return remote(
            r.xsums.at[way, j, q],
            r.xsums.at[way, j - 1, q],
            r.xsum_send.at[0],
            r.xsum_recv.at[way, j - 1, q],
            toward(way),
        )

    taken = set()

    def thin_part(col, q):
        return weighted(col, r.xret[col, q // lanes_of, :, q % lanes_of * 128 : (q % lanes_of + 1) * 128])

    def token_round(t):
        for q in range(thin):
            for way in range(2):
                j = far(1 - way, q) - t
                if j < 1:
                    continue
                offset = j if way == 0 else columns - j
                if offset not in taken:
                    taken.add(offset)
                    take_back(offset)
                value = thin_part(column(offset), q)
                if t > 0:
                    token_hop(way, j + 1, q).wait_recv()
                    value = value + r.xsums[way, j, q].astype(f32)
                r.xsums[way, j, q] = value.astype(bf16)
                token_hop(way, j, q).start()

    for group in dims.groups:
        chains(True, 0, group)
    def left_by_now(view, send, recv):
        remote(view, view, send, recv, right).wait_send()

    most_places, most_lines = pl.ds(0, places - 1), pl.ds(0, (places - 1) * main)
    chunks_total = r.chunks.at[most_columns, pl.ds(0, direct), pl.ds(0, slots), :]
    left_by_now(r.over_out.at[most_places], r.over_send.at[0], r.over_recv.at[0])
    left_by_now(r.tokens.at[most_columns], r.token_send.at[0], r.token_recv.at[0, 0, 0])
    left_by_now(r.chunks.at[most_columns, pl.ds(0, direct), pl.ds(slots, over), :], r.tail_send.at[0], r.tail_recv.at[0, 0])
    left_by_now(chunks_total, r.chunk_send.at[0], r.chunk_recv.at[0, 0, 0])
    left_by_now(r.outbound.at[:, most_lines, :], r.out_send.at[0], r.out_recv.at[0])
    left_by_now(r.xout.at[:, :, most_lines, :], r.xout_send.at[0], r.xout_recv.at[0])
    left_by_now(r.xover_out.at[:, most_places], r.xover_send.at[0], r.xover_recv.at[0, 0])
    for kind, step, group in dims.closing:
        if kind == "short":
            chains(False, step, group)
        elif kind == "long":
            chains(True, step, group)
        elif kind == "token":
            token_round(step)
        else:
            lax.fori_loop(*group, finish, 0)
    for c in range(direct * lanes_of):
        at_lanes = (c % lanes_of) * 128
        r.over_back[:, c, :] = r.over_total[c // lanes_of, :, at_lanes : at_lanes + 128]
    r.over_ret[me_s] = r.over_back[me_s]
    for i in range(1, places):
        remote(
            r.over_back.at[place(i)], r.over_ret.at[me_s], r.over_send.at[1], r.over_recv.at[1], {"sp": place(i)}
        ).start()

    left_by_now(r.xback.at[:, :, most_lines, :], r.xback_send.at[0], r.xback_recv.at[0])
    left_by_now(r.xover_back.at[:, most_places], r.xover_send.at[1], r.xover_recv.at[1, 0])
    left_by_now(r.chunks.at[most_columns, pl.ds(0, direct)], r.sum_send.at[0], r.sum_recv.at[0, 0, 0])
    token_round(half - 1)
    take_back(0)
    for q in range(thin):
        value = thin_part(me_x, q)
        for way in range(2):
            token_hop(way, 1, q).wait_recv()
            value = value + r.xsums[way, 0, q].astype(f32)
        span = slice(direct * PIECE + q * 128, direct * PIECE + (q + 1) * 128)
        r.out_s[:, span] = (r.stream_s[:, span].astype(f32) + value).astype(bf16)

    def write_out(span):
        return pltpu.make_async_copy(r.out_s.at[:, span], r.out_ref.at[:, span], r.done_sem.at[0])

    write_out(pl.ds(direct * PIECE, extra * PIECE)).start()
    remote(
        r.over_back.at[0 : places - 1], r.over_ret.at[0 : places - 1], r.over_send.at[1], r.over_recv.at[1], right
    ).wait_recv()
    for c in range(direct * lanes_of):
        at_lanes = (c % lanes_of) * 128
        r.returned[c // lanes_of, slots:, at_lanes : at_lanes + 128] = r.over_ret[:, c, :].astype(bf16)

    def back_arrived(p):
        most = pl.ds(0, (places - 1) * main)
        return remote(
            r.totals.at[p, most, :], r.returned.at[p, most, :], r.back_send.at[0], r.back_recv.at[p], right
        )

    def combine(p, carry):
        back_arrived(p).wait_recv()
        span = pl.ds(pl.multiple_of(p * PIECE, PIECE), PIECE)
        value = weighted(me_x, r.returned[p])
        r.out_s[:, span] = (r.stream_s[:, span].astype(f32) + value).astype(bf16)
        write_out(span).start()
        return carry

    lax.fori_loop(0, direct, combine, 0)

    left_by_now(r.over_back.at[most_places], r.over_send.at[1], r.over_recv.at[1])
    left_by_now(r.tokens.at[most_columns], r.xsum_send.at[0], r.xsum_recv.at[0, 0, 0])
    left_by_now(r.totals.at[:, most_lines, :], r.back_send.at[0], r.back_recv.at[0])
    pltpu.make_async_copy(r.out_s, r.out_ref, r.done_sem.at[0]).wait()


def layer(places, columns, **given):
    f32, bf16 = jnp.float32, jnp.bfloat16
    rows, width = given["residual_hbm"].shape
    units = given["expert_gate_hbm"].shape[2]
    lanes = given["keys_hbm"].shape[1]
    positions = columns * BLOCK
    half, chips, blocks = columns // 2, places // 2, columns
    main = 2 * rows // places
    over = -(-places // 16) * 16
    pieces = width // PIECE
    extra = max(1, pieces // 4)
    direct = pieces - extra
    tiles, total = units // 128, places * main + over
    ring_part = width * RING_SHARE // 16 // 128 * 128
    schedule = (0, 0, 1, 5, 7) if half == 4 else (0,) * half + (columns - 1,)
    opening = (1, 0, 2, -1, -2, 3, -3, -4, 4, -5) if half == 4 else (*range(1, half + 1), *range(0, -direct, -1))
    serving = [
        [("x", 0)],
        [("x", 1)],
        [("x", 2)],
        [("x", 3), ("y", 0), ("y", 1), ("y", 2), ("x", 4), ("y", 3), ("y", 4), ("y", 5), ("x", 5), ("x", 6), ("y", 6)],
    ]
    low, high = (0, (direct + 1) // 2), ((direct + 1) // 2, direct)
    groups = [high, low]
    if half == 4:
        closing = [
            ("long", 1, high),
            ("short", 1, high),
            ("long", 1, low),
            ("short", 1, low),
            ("long", 2, low),
            ("long", 2, high),
            ("long", 3, low),
            ("short", 2, low),
            ("token", 0, None),
            ("long", 3, high),
            ("finish", None, low),
            ("short", 2, high),
            ("token", 1, None),
            ("finish", None, high),
            ("token", 2, None),
        ]
    else:
        closing = []
        for step in range(1, half):
            closing += [("short", step, group) for group in groups if step < half - 1]
            closing += [("long", step, group) for group in groups]
            closing.append(("token", step - 1, None))
        closing += [("finish", None, group) for group in groups]
    dims = types.SimpleNamespace(
        places=places, columns=columns, width=width, main=main, over=over, pieces=pieces, direct=direct, tiles=tiles,
        schedule=schedule, opening=opening, groups=groups, closing=closing, ring_part=ring_part, serving=serving,
    )
    packed = STATE_ONE + STATE_TWO
    square = (blocks, 2, BLOCK, BLOCK)
    vmem = lambda *shape, dtype=bf16: pltpu.VMEM(shape, dtype)
    dma = lambda *shape: pltpu.SemaphoreType.DMA(shape)
    spaces = {"ref": pltpu.VMEM, "hbm": pl.ANY}
    in_specs = [
        pl.BlockSpec(memory_space=pltpu.SMEM if a.shape == (2, 2) else spaces[name[-3:]]) for name, a in given.items()
    ]
    lane_rows = PIECE // 128
    scratch = dict(
        residual_in=vmem(rows, width),
        value_in=vmem(2 * positions, BLOCK),
        gate_in=vmem(2 * positions, BLOCK),
        keys_in=vmem(positions, lanes),
        value_rim=vmem(16, BLOCK),
        keys_rim=vmem(16, lanes),
        value_wide=vmem(2 * positions + 16, BLOCK, dtype=f32),
        keys_wide=vmem(positions + 16, lanes, dtype=f32),
        gate_wide=vmem(2 * BLOCK, BLOCK, dtype=f32),
        conv_wide=vmem(2 * BLOCK, BLOCK, dtype=f32),
        x_s=vmem(*square),
        kt_s=vmem(*square),
        q_s=vmem(*square),
        state_s=vmem(*square, dtype=f32),
        near_s=vmem(*square, dtype=f32),
        stride_s=vmem(HEADS * blocks, BLOCK, dtype=f32),
        run_s=vmem(HEADS * blocks, BLOCK, dtype=f32),
        fade_s=vmem(HEADS * blocks, BLOCK, dtype=f32),
        end_s=vmem(HEADS * blocks, BLOCK, dtype=f32),
        cols_s=vmem(blocks, BLOCK, HEADS, dtype=f32),
        own_pack=vmem(packed, BLOCK),
        own_fade=vmem(8, BLOCK, dtype=f32),
        mate_pack=vmem(packed, BLOCK),
        mate_fade=vmem(8, BLOCK, dtype=f32),
        chip_pack=vmem(packed, BLOCK),
        chip_fade=vmem(8, BLOCK, dtype=f32),
        all_pack=vmem(chips, packed // 2, BLOCK),
        all_fade=vmem(chips, 8, BLOCK, dtype=f32),
        enter_pack=vmem(packed, BLOCK),
        carry_s=vmem(2, BLOCK, BLOCK, dtype=f32),
        mixed_s=vmem(columns, BLOCK, 2 * BLOCK),
        heads_in=vmem(columns, BLOCK, 2 * BLOCK),
        matrix=vmem(columns, 2 * BLOCK, width),
        acc_s=vmem(rows, width, dtype=f32),
        stream_s=vmem(rows, width),
        out_s=vmem(rows, width),
        tables=vmem(columns, 8, rows, dtype=f32),
        put=vmem(columns, total, rows),
        pick=vmem(columns, 2, rows, total),
        share_s=vmem(columns, 2, rows, 128, dtype=f32),
        tokens=vmem(columns, extra, rows, PIECE),
        outbound=vmem(direct, places * main, PIECE),
        over_out=vmem(over, direct * lane_rows, 128, dtype=f32),
        over_in=vmem(over, direct * lane_rows, 128, dtype=f32),
        over_back=vmem(over, direct * lane_rows, 128, dtype=f32),
        over_ret=vmem(over, direct * lane_rows, 128, dtype=f32),
        over_total=vmem(direct, over, PIECE, dtype=f32),
        xout=vmem(columns, extra, places * main, PIECE),
        xback=vmem(columns, extra, places * main, PIECE),
        xret=vmem(columns, extra, total, PIECE),
        xover_out=vmem(columns, over, extra * lane_rows, 128, dtype=f32),
        xover_in=vmem(columns, over, extra * lane_rows, 128, dtype=f32),
        xover_back=vmem(columns, over, extra * lane_rows, 128, dtype=f32),
        xover_ret=vmem(columns, over, extra * lane_rows, 128, dtype=f32),
        chunks=vmem(columns, pieces, total, PIECE),
        hidden=vmem(columns, total, units),
        gate_up=vmem(tiles, width, 256),
        down=vmem(pieces, units, PIECE),
        sums=vmem(2, half + 1, direct, total, PIECE),
        xsums=vmem(2, half + 1, extra * lane_rows, rows, 128),
        totals=vmem(direct, places * main, PIECE),
        returned=vmem(direct, total, PIECE),
        load_sem=dma(6),
        weight_sem=dma(2),
        done_sem=dma(1),
    )
    steps = (2, half)
    for name, send, recv in (
        ("rim", (2,), (2,)),
        ("mate", (2,), (2,)),
        ("chip", (2, chips), (2, chips)),
        ("enter", (1,), (1,)),
        ("head", (1,), (1,)),
        ("table", (1,), (1,)),
        ("ring", (1,), (2, columns - 1, 2)),
        ("slab", (1,), (1,)),
        ("grid", (1,), (2, chips - 1)),
        ("pass", (2,), (2,)),
        ("over", (2,), (2,)),
        ("token", (1,), (*steps, extra * lane_rows)),
        ("out", (1,), (direct,)),
        ("xout", (1,), (columns,)),
        ("xover", (2,), (2, columns)),
        ("chunk", (1,), (*steps, direct)),
        ("tail", (1,), steps),
        ("xback", (1,), (columns,)),
        ("sum", (1,), (*steps, direct)),
        ("xsum", (1,), (*steps, extra * lane_rows)),
        ("back", (1,), (direct,)),
    ):
        scratch[name + "_send"], scratch[name + "_recv"] = dma(*send), dma(*recv)
    names = [*given, "out_ref", *scratch]
    return pl.pallas_call(
        functools.partial(layer_kernel, dims, names),
        out_shape=jax.ShapeDtypeStruct((rows, width), bf16),
        in_specs=in_specs,
        out_specs=pl.BlockSpec(memory_space=pl.ANY),
        scratch_shapes=list(scratch.values()),
        compiler_params=pltpu.CompilerParams(
            collective_id=0, has_side_effects=True, vmem_limit_bytes=VMEM_LIMIT
        ),
        name="layer",
    )(*given.values())


def local(
    residual,
    grouped_value_heads,
    output_gate_heads,
    projected_key_query,
    raw_step_size,
    step_size_bias,
    head_decay_logarithm,
    position_extra_decay,
    head_skip_weight,
    value_kernel_taps,
    key_query_kernel,
    head_norm_gain,
    output_matrix,
    expert_norm_gain,
    expert_gate_weight,
    expert_up_weight,
    expert_down_weight,
    token_expert_choice,
    expert_output_weight,
):
    return layer(
        lax.axis_size("sp"),
        lax.axis_size("tp"),
        residual_hbm=residual,
        value_hbm=grouped_value_heads.reshape(-1, BLOCK),
        gate_hbm=output_gate_heads.reshape(-1, BLOCK),
        keys_hbm=projected_key_query,
        raw_ref=raw_step_size.transpose(1, 2, 0),
        bias_ref=step_size_bias,
        log_ref=head_decay_logarithm,
        extra_ref=position_extra_decay.reshape(-1, BLOCK),
        skip_ref=head_skip_weight,
        value_tap_ref=value_kernel_taps.reshape(-1, BLOCK),
        key_tap_ref=key_query_kernel,
        head_gain_ref=head_norm_gain,
        matrix_hbm=output_matrix,
        expert_gain_ref=expert_norm_gain[None],
        choice_ref=token_expert_choice.T,
        share_ref=expert_output_weight.T,
        expert_gate_hbm=expert_gate_weight,
        expert_up_hbm=expert_up_weight,
        expert_down_hbm=expert_down_weight,
    )


def solution(mesh):
    placed = (
        P(("grp", "sp", "tp"), None),
        P(("grp", "sp"), None, "tp"),
        P(("grp", "sp"), None, "tp"),
        P(("grp", "sp"), None),
        P(("grp", "sp"), None, "tp"),
        P(None, "tp"),
        P(None, "tp"),
        P(("grp", "sp")),
        P(None, "tp"),
        P(None, None, "tp"),
        P(),
        P(None, "tp"),
        P(None, "tp", None),
        P(),
        P("sp", None, "tp"),
        P("sp", None, "tp"),
        P("sp", "tp", None),
        P(("grp", "sp", "tp"), None),
        P(("grp", "sp", "tp"), None),
    )
    return jax.shard_map(
        local, mesh=mesh, in_specs=placed, out_specs=P(("grp", "sp", "tp"), None), check_vma=False
    )
```

```python
import functools
import types

import jax
import jax.numpy as jnp
from jax import lax
from jax.experimental import pallas as pl
from jax.experimental.pallas import tpu as pltpu
from jax.sharding import PartitionSpec as P

HEAD_DIM = 64
STATE_ONE = 64
STATE_TWO = 128
BLOCK = 128
EPSILON = 1e-06

MESH = pl.DeviceIdType.MESH
PIECE = 256
HEADS = 4
RING_SHARE = 7
VMEM_LIMIT = 67043328


def remote(src, dst, send, recv, device):
    return pltpu.make_async_remote_copy(
        src_ref=src, dst_ref=dst, send_sem=send, recv_sem=recv, device_id=device, device_id_type=MESH
    )


def silu(a):
    return a * (1.0 / (1.0 + jnp.exp(-a)))


def layer_kernel(dims, names, *refs):
    r = types.SimpleNamespace(**dict(zip(names, refs, strict=True)))
    f32, bf16 = jnp.float32, jnp.bfloat16
    places, columns, width, rows = dims.places, dims.columns, dims.width, BLOCK
    half, chips, blocks = columns // 2, places // 2, columns
    me_x, me_s = lax.axis_index("tp"), lax.axis_index("sp")
    core, me_y = lax.rem(me_s, 2), lax.div(me_s, 2)
    right = {"tp": lax.rem(me_x + 1, columns)}
    left = {"tp": lax.rem(me_x + columns - 1, columns)}
    mate = {"sp": me_s + 1 - 2 * core}
    following = {"sp": lax.rem(me_s + 1, places)}

    def column(offset):
        return lax.rem(me_x + offset + columns, columns)

    def place(offset):
        return lax.rem(me_s + offset, places)

    def peer(offset):
        return {"sp": lax.rem(me_s + 2 * offset, places)}

    def toward(way):
        return right if way == 0 else left

    barrier = pltpu.get_barrier_semaphore()
    peers = [{"tp": column(i)} for i in range(1, columns)] + [{"sp": place(i)} for i in range(1, places)]
    for device in peers:
        pl.semaphore_signal(barrier, inc=1, device_id=device, device_id_type=MESH)

    small = {
        name: pltpu.make_async_copy(getattr(r, name), getattr(r, name[:-5] + "ref"), r.small_sem.at[n])
        for n, name in enumerate(dims.small)
    }
    ring_part, slab = dims.ring_part, rows // chips
    mine = pl.multiple_of(core * rows, rows)

    def slab_rows(y):
        return pl.ds(pl.multiple_of(mine + y * slab, 16), slab)

    on_ring, on_grid = pl.ds(0, ring_part), pl.ds(ring_part, width - ring_part)
    loads = [
        (r.matrix_hbm.at[0], r.matrix.at[0, pl.ds(0, rows), :]),
        (r.matrix_hbm.at[1], r.matrix.at[0, pl.ds(rows, rows), :]),
        (r.value_hbm, r.value_in),
        (r.keys_hbm, r.keys_in),
        (r.gate_hbm, r.gate_in),
        (r.residual_hbm, r.residual_in),
    ]
    loads = [pltpu.make_async_copy(a, b, r.load_sem.at[n]) for n, (a, b) in enumerate(loads)]
    for load in loads[:2] + list(small.values()) + loads[2:]:
        load.start()
    for name in ("choice_small", "share_small"):
        small[name].wait()
    r.tables[me_x] = jnp.zeros((8, rows), f32)
    r.tables[me_x, 0:2, :] = r.choice_ref[...].astype(f32)
    r.tables[me_x, 2:4, :] = r.share_ref[...]

    for load in loads[:2]:
        load.wait()
    pl.semaphore_wait(barrier, len(peers))

    def matrix_block(way, event, k, sub):
        piece = ((event % 2) ^ way) * 2 + sub
        block = (columns - k if way == 0 else k) % columns
        return r.matrix.at[block, pl.ds(pl.multiple_of(mine + piece * (rows // 4), 16), rows // 4), on_ring]

    def matrix_ring(way, event, sub):
        k = event // 2
        return remote(
            matrix_block(way, event, k, sub),
            matrix_block(way, event, k + 1, sub),
            r.ring_send.at[0],
            r.ring_recv.at[event, sub],
            toward(way),
        )

    def slab_copy(offset):
        return remote(
            r.matrix.at[0, slab_rows(me_y), on_grid],
            r.matrix.at[columns - offset, slab_rows(me_y), on_grid],
            r.slab_send.at[0],
            r.slab_recv.at[0],
            {"tp": column(offset)},
        )

    def grid_view(way, event, y):
        blocks_of = pl.ds(1, half) if (event % 2) ^ way == 0 else pl.ds(1 + half, half - 1)
        return r.matrix.at[blocks_of, slab_rows(y), on_grid]

    def grid_ring(way, event, y):
        here = grid_view(way, event, y)
        return remote(
            here, here, r.grid_send.at[0], r.grid_recv.at[event], peer(1) if way == 0 else peer(chips - 1)
        )

    def to_mate(here, which):
        return remote(here, here, r.pass_send.at[which], r.pass_recv.at[which], mate)

    most_columns, other_blocks = pl.ds(0, columns - 1), pl.ds(1, columns - 1)
    ring_total = r.matrix.at[other_blocks, pl.ds(0, rows), on_ring]
    grid_total = r.matrix.at[other_blocks, pl.ds(0, (chips - 1) * slab), on_grid]
    slab_total = r.matrix.at[other_blocks, pl.ds(0, slab), on_grid]
    pass_totals = (ring_total, r.matrix.at[other_blocks, pl.ds(0, rows), on_grid])

    for load in loads[2:4]:
        load.wait()
    rim_rows = 16
    positions = blocks * rows
    rims = [
        remote(
            r.value_in.at[pl.ds(2 * positions - rim_rows, rim_rows), :],
            r.value_rim,
            r.rim_send.at[0],
            r.rim_recv.at[0],
            following,
        ),
        remote(
            r.keys_in.at[pl.ds(positions - rim_rows, rim_rows), :], r.keys_rim, r.rim_send.at[1], r.rim_recv.at[1], following
        ),
    ]
    for rim in rims:
        rim.start()

    def table_copy(offset):
        here = r.tables.at[me_x]
        return remote(here, here, r.table_send.at[0], r.table_recv.at[0], {"tp": column(offset)})

    for i in range(1, columns):
        table_copy(i).start()
    for i in range(1, columns):
        slab_copy(i).start()
    for event in range(min(2, columns - 1)):
        for sub in range(2):
            for way in range(2):
                matrix_ring(way, event, sub).start()
    tables_total = remote(
        r.tables.at[most_columns], r.tables.at[most_columns], r.table_send.at[0], r.table_recv.at[0], right
    )

    def serve_ring(event):
        for sub in range(2):
            both = r.matrix.at[0, pl.ds(0, rows // 2), on_ring]
            remote(both, both, r.ring_send.at[0], r.ring_recv.at[event, sub], right).wait_recv()
            for way in range(2):
                if event + 2 < columns - 1:
                    matrix_ring(way, event + 2, sub).start()
                to_mate(matrix_block(way, event, event // 2 + 1, sub), 0).start()

    def serve_slab():
        remote(slab_total, slab_total, r.slab_send.at[0], r.slab_recv.at[0], right).wait_recv()
        for event in range(2):
            for way in range(2):
                if event < chips - 1:
                    grid_ring(way, event, me_y).start()
        to_mate(r.matrix.at[other_blocks, slab_rows(me_y), on_grid], 1).start()

    def serve_grid(event):
        k = event // 2 + 1
        remote(slab_total, slab_total, r.grid_send.at[0], r.grid_recv.at[event], right).wait_recv()
        for way in range(2):
            y = lax.rem(me_y + (chips - k if way == 0 else k), chips)
            if event + 2 < chips - 1:
                grid_ring(way, event + 2, y).start()
            to_mate(grid_view(way, event, y), 1).start()

    waiting = [("x", e) for e in range(columns - 1)] + [("y", e) for e in range(chips - 1)]

    def serve(*steps):
        for step in steps:
            if step in waiting:
                waiting.remove(step)
                (serve_ring if step[0] == "x" else serve_grid)(step[1])

    for t in range(dims.tiles):
        span = pl.ds(t * 128, 128)
        for n, weight in enumerate((r.expert_gate_hbm, r.expert_up_hbm)):
            pltpu.make_async_copy(
                weight.at[0, :, span], r.gate_up.at[t, :, pl.ds(n * 128, 128)], r.weight_sem.at[0]
            ).start()
    for p in range(dims.pieces):
        pltpu.make_async_copy(
            r.expert_down_hbm.at[0, :, pl.ds(p * PIECE, PIECE)], r.down.at[p], r.weight_sem.at[1]
        ).start()

    for name in dims.small:
        if name not in ("choice_small", "share_small"):
            small[name].wait()
    for g in range(2):
        raw = r.raw_ref[g].astype(f32)
        for k in range(blocks):
            r.stride_s[HEADS * k + 2 * g : HEADS * k + 2 * g + 2, :] = raw[:, k * rows : (k + 1) * rows]
    for k in range(blocks):
        r.run_s[HEADS * k : HEADS * k + HEADS, :] = jnp.broadcast_to(r.extra_ref[k : k + 1, :], (HEADS, rows))
    head_of = jnp.bitwise_and(lax.broadcasted_iota(jnp.int32, (HEADS * blocks, rows), 0), HEADS - 1)

    def by_head(table):
        picked = jnp.full((HEADS * blocks, rows), table[1, 1], f32)
        for n in range(3):
            picked = jnp.where(head_of == n, table[n // 2, n % 2], picked)
        return picked

    shifted = r.stride_s[...] + by_head(r.bias_ref)
    stride = jnp.maximum(shifted, 0.0) + jnp.log1p(jnp.exp(-jnp.abs(shifted)))
    log_decay = r.run_s[...] - jnp.exp(by_head(r.log_ref)) * stride
    at_row = lax.broadcasted_iota(jnp.int32, (rows, rows), 0)
    at_lane = lax.broadcasted_iota(jnp.int32, (rows, rows), 1)
    running = jnp.dot(
        log_decay,
        jnp.where(at_row <= at_lane, 1.0, 0.0),
        preferred_element_type=f32,
        precision=lax.Precision.HIGHEST,
    )
    ends = jnp.broadcast_to(running[:, rows - 1 : rows], running.shape)
    r.stride_s[...] = stride
    r.run_s[...] = running
    r.fade_s[...] = jnp.exp(ends - running) * stride
    r.end_s[...] = jnp.exp(ends)
    turned = jnp.transpose(running)
    for k in range(blocks):
        r.cols_s[k, :, 0:HEADS] = turned[:, HEADS * k : HEADS * k + HEADS]

    first_head = at_lane < HEAD_DIM

    def row_pair(table, k, g):
        low = table[pl.ds(HEADS * k + 2 * g, 1), :]
        high = table[pl.ds(HEADS * k + 2 * g + 1, 1), :]
        return jnp.where(first_head[0:1], low, high)

    r.value_wide[rim_rows:, :] = r.value_in[...].astype(f32)
    r.keys_wide[rim_rows:, :] = r.keys_in[...].astype(f32)
    taps = r.value_tap_ref.shape[0] // 2
    value_tap = r.value_tap_ref[...].astype(f32)
    key_tap = r.key_tap_ref[...].astype(f32)
    even = jnp.bitwise_and(lax.broadcasted_iota(jnp.int32, (2 * rows, rows), 0), 1) == 0
    tap_rows = [jnp.where(even, value_tap[2 * j : 2 * j + 1], value_tap[2 * j + 1 : 2 * j + 2]) for j in range(taps)]

    def states_of(k):
        window = r.value_wide[pl.ds(pl.multiple_of(k * 2 * rows, 2 * rows), 2 * rows + rim_rows), :]
        total = jnp.zeros((2 * rows, rows), f32)
        for j in range(taps):
            start = rim_rows - 2 * (taps - 1 - j)
            total = total + window[start : start + 2 * rows] * tap_rows[j]
        r.conv_wide[...] = silu(total).astype(bf16).astype(f32)
        window = r.keys_wide[pl.ds(pl.multiple_of(k * rows, rows), rows + rim_rows), :]
        total = jnp.zeros((rows, r.keys_wide.shape[1]), f32)
        for j in range(taps):
            start = rim_rows - (taps - 1 - j)
            total = total + window[start : start + rows] * key_tap[j : j + 1]
        conv = silu(total).astype(bf16).astype(f32)
        both = conv[:, 0 : 2 * STATE_ONE]
        keys = [jnp.where(first_head, both, 0.0), conv[:, 2 * STATE_ONE : 2 * STATE_ONE + STATE_TWO]]
        asks = [pltpu.roll(both, STATE_ONE, 1), conv[:, 2 * STATE_ONE + STATE_TWO :]]
        for g in range(2):
            x = r.conv_wide[pl.ds(g, rows, stride=2), :].astype(bf16)
            key_t = jnp.transpose(keys[g])
            r.x_s[k, g] = x
            r.kt_s[k, g] = key_t.astype(bf16)
            r.q_s[k, g] = asks[g].astype(bf16)
            faded = jnp.concatenate(
                [key_t * r.fade_s[pl.ds(HEADS * k + 2 * g + h, 1), :] for h in range(2)], axis=0
            ).astype(bf16)
            state = jnp.dot(faded, x, preferred_element_type=f32)
            r.state_s[k, g] = jnp.where(first_head, state[:rows], state[rows:])

    def state_step(i, carry):
        states_of(i)
        return carry

    lax.fori_loop(1, blocks, state_step, 0)
    for rim in rims:
        rim.wait_recv()
    opening = me_s == 0
    r.value_wide[0:rim_rows, :] = jnp.where(opening, 0.0, r.value_rim[...].astype(f32))
    r.keys_wide[0:rim_rows, :] = jnp.where(opening, 0.0, r.keys_rim[...].astype(f32))
    states_of(0)

    packed = STATE_TWO + STATE_ONE
    piece = packed // 2

    def local_end(g):
        total = jnp.zeros((rows, rows), f32)
        faded = jnp.ones((1, rows), f32)
        for k in range(blocks):
            decay = row_pair(r.end_s, k, g)
            total = total * decay + r.state_s[k, g]
            faded = faded * decay
        return total, faded

    end_one, fade_one = local_end(0)
    end_two, fade_two = local_end(1)
    own = jnp.concatenate([end_two, end_one[:STATE_ONE]], axis=0)
    r.own_pack[...] = own.astype(bf16)
    r.own_fade[0:1, :] = fade_one
    r.own_fade[1:2, :] = fade_two
    r.own_fade[2:8, :] = jnp.zeros((6, rows), f32)
    mates = [
        remote(r.own_pack, r.mate_pack, r.mate_send.at[0], r.mate_recv.at[0], mate),
        remote(r.own_fade, r.mate_fade, r.mate_send.at[1], r.mate_recv.at[1], mate),
    ]
    for copy in mates:
        copy.start()
    for copy in mates:
        copy.wait_recv()
    is_low = core == 0
    low = jnp.where(is_low, own, r.mate_pack[...].astype(f32))
    high = jnp.where(is_low, r.mate_pack[...].astype(f32), own)
    mate_rows = r.mate_fade[...]
    own_rows = r.own_fade[...]
    high_rows = jnp.where(is_low, mate_rows, own_rows)
    in_two = lax.broadcasted_iota(jnp.int32, (packed, rows), 0) < STATE_TWO
    r.chip_pack[...] = (low * jnp.where(in_two, high_rows[1:2], high_rows[0:1]) + high).astype(bf16)
    r.chip_fade[...] = own_rows * mate_rows
    my_half = pl.ds(pl.multiple_of(core * piece, 16), piece)

    def to_chip(n, which):
        src = r.chip_pack.at[my_half, :] if which == 0 else r.chip_fade
        dst = r.all_pack.at[me_y] if which == 0 else r.all_fade.at[me_y]
        return remote(src, dst, r.chip_send.at[n], r.chip_recv.at[n], peer(n))

    def chip_total(n):
        sent = r.own_pack.at[pl.ds(0, piece + 16), :]
        return remote(sent, sent, r.chip_send.at[n], r.chip_recv.at[n], peer(n))

    for n in range(1, chips):

        @pl.when(me_y + n < chips)
        def _():
            for which in range(2):
                to_chip(n, which).start()


    below = at_row >= at_lane

    def near_step(k, carry):
        cols = r.cols_s[k]
        for g in range(2):
            scores = jnp.dot(r.q_s[k, g], r.kt_s[k, g], preferred_element_type=f32)
            parts = []
            for h in range(2):
                n = 2 * g + h
                gap = cols[:, n : n + 1] - r.run_s[pl.ds(HEADS * k + n, 1), :]
                damping = jnp.exp(jnp.where(below, gap, -1e30))
                parts.append((scores * damping * r.stride_s[pl.ds(HEADS * k + n, 1), :]).astype(bf16))
            near = jnp.dot(jnp.concatenate(parts, axis=0), r.x_s[k, g], preferred_element_type=f32)
            r.near_s[k, g] = jnp.where(first_head, near[:rows], near[rows:])
        return carry

    lax.fori_loop(0, blocks, near_step, 0)
    serve_slab()
    serve(*dims.serving[0])
    main, over, slots = dims.main, dims.over, places * dims.main
    total_slots = slots + over
    slot_row = lax.broadcasted_iota(jnp.int32, (total_slots, over), 0)
    slot_expert = lax.broadcasted_iota(jnp.int32, (total_slots, over), 1)
    spread = jnp.where(
        ((slot_row < slots) & (slot_row >= slot_expert * main) & (slot_row < slot_expert * main + main))
        | (slot_row == slots + slot_expert),
        1.0,
        0.0,
    ).astype(bf16)
    at = lax.broadcasted_iota(jnp.int32, (total_slots, rows), 0)
    turn = jnp.where(at < slots, jnp.bitwise_and(at, main - 1), main).astype(f32)
    expert_at = lax.broadcasted_iota(jnp.int32, (over, rows), 0).astype(f32)
    earlier = jnp.where(at_row < at_lane, 1.0, 0.0).astype(bf16)

    def make_put(col):
        table = r.tables[col]
        named = jnp.where((expert_at == table[0:1]) | (expert_at == table[1:2]), 1.0, 0.0)
        rank = jnp.dot(named.astype(bf16), earlier, preferred_element_type=f32)
        named_x = jnp.dot(spread, named.astype(bf16), preferred_element_type=f32)
        rank_x = jnp.dot(spread, rank.astype(bf16), preferred_element_type=f32)
        r.put[col] = jnp.where(rank_x == turn, named_x, 0.0).astype(bf16)

    tables_total.wait_recv()

    def put_step(col, carry):
        make_put(col)
        return carry

    lax.fori_loop(0, columns, put_step, 0)

    for load in loads[-2:]:
        load.wait()
    serve(*dims.serving[1])
    for n in range(1, chips):

        @pl.when(me_y >= n)
        def _():
            chip_total(n).wait_recv()

    row_at = lax.broadcasted_iota(jnp.int32, (piece, rows), 0) + core * piece
    half_two = row_at < STATE_TWO
    entering = jnp.zeros((piece, rows), f32)
    for y in range(chips):
        fades = r.all_fade[y]
        later = entering * jnp.where(half_two, fades[1:2], fades[0:1]) + r.all_pack[y].astype(f32)
        entering = jnp.where(y < me_y, later, entering)
    r.enter_pack[my_half, :] = entering.astype(bf16)
    here = r.enter_pack.at[my_half, :]
    enter_copy = remote(here, here, r.enter_send.at[0], r.enter_recv.at[0], mate)
    enter_copy.start()
    enter_copy.wait_recv()
    chip_state = r.enter_pack[...].astype(f32)
    after_low = chip_state * jnp.where(in_two, mate_rows[1:2], mate_rows[0:1]) + r.mate_pack[...].astype(f32)
    entered = jnp.where(is_low, chip_state, after_low)
    r.carry_s[1] = entered[:STATE_TWO]
    r.carry_s[0] = jnp.zeros((rows, rows), f32)
    r.carry_s[0, 0:STATE_ONE, :] = entered[STATE_TWO:]

    serve(*dims.serving[2])
    def head_copy(col):
        return remote(r.mixed_s.at[col], r.heads_in.at[me_x], r.head_send.at[0], r.head_recv.at[0], {"tp": col})

    def mix_step(k, carry):
        cols = jnp.exp(r.cols_s[k])
        r.gate_wide[...] = r.gate_in[pl.ds(pl.multiple_of(k * 2 * rows, 2 * rows), 2 * rows), :].astype(f32)
        for g in range(2):
            state = r.carry_s[g]
            coarse = state.astype(bf16)
            fine = (state - coarse.astype(f32)).astype(bf16)
            ask = r.q_s[k, g]
            far = jnp.dot(
                jnp.concatenate([ask, ask], axis=1),
                jnp.concatenate([coarse, fine], axis=0),
                preferred_element_type=f32,
            )
            reach = jnp.where(first_head, cols[:, 2 * g : 2 * g + 1], cols[:, 2 * g + 1 : 2 * g + 2])
            skip = jnp.where(first_head[0:1], r.skip_ref[g, 0], r.skip_ref[g, 1])
            mixed = r.near_s[k, g] + far * reach + skip * r.x_s[k, g].astype(f32)
            gated = mixed * silu(r.gate_wide[pl.ds(g, rows, stride=2), :])
            square = gated * gated
            one = jnp.sum(jnp.where(first_head, square, 0.0), axis=1, keepdims=True)
            two = jnp.sum(jnp.where(first_head, 0.0, square), axis=1, keepdims=True)
            scale = lax.rsqrt(jnp.where(first_head, one, two) * (1.0 / HEAD_DIM) + EPSILON)
            r.mixed_s[k, :, g * rows : (g + 1) * rows] = (gated * scale * r.head_gain_ref[g : g + 1, :]).astype(bf16)
            r.carry_s[g] = state * row_pair(r.end_s, k, g) + r.state_s[k, g]

        @pl.when(k != me_x)
        def _():
            head_copy(k).start()

        return carry

    lax.fori_loop(0, blocks, mix_step, 0)
    r.heads_in[me_x] = r.mixed_s[me_x]

    slot_col = lax.broadcasted_iota(jnp.int32, (over, total_slots), 1)
    slot_exp = lax.broadcasted_iota(jnp.int32, (over, total_slots), 0)
    spread_t = jnp.where(
        ((slot_col < slots) & (slot_col >= slot_exp * main) & (slot_col < slot_exp * main + main))
        | (slot_col == slots + slot_exp),
        1.0,
        0.0,
    ).astype(bf16)
    at_t = lax.broadcasted_iota(jnp.int32, (rows, total_slots), 1)
    turn_t = jnp.where(at_t < slots, jnp.bitwise_and(at_t, main - 1), main).astype(f32)
    expert_to = lax.broadcasted_iota(jnp.int32, (rows, over), 1).astype(f32)
    later_t = jnp.where(at_lane < at_row, 1.0, 0.0).astype(bf16)

    def make_pick(col):
        table = jnp.transpose(r.tables[col])
        named = [jnp.where(expert_to == table[:, k : k + 1], 1.0, 0.0) for k in range(2)]
        rank = jnp.dot(later_t, (named[0] + named[1]).astype(bf16), preferred_element_type=f32)
        rank_x = jnp.dot(rank.astype(bf16), spread_t, preferred_element_type=f32)
        for k in range(2):
            named_x = jnp.dot(named[k].astype(bf16), spread_t, preferred_element_type=f32)
            r.pick[col, k] = jnp.where(rank_x == turn_t, named_x, 0.0).astype(bf16)
            r.share_s[col, k] = jnp.broadcast_to(table[:, 2 + k : 3 + k], (rows, rows))

    def product(block, low, high, first):
        for n in range(low, high, 512):
            span = slice(n, min(n + 512, high))
            part = jnp.dot(r.heads_in[column(block)], r.matrix[block, :, span], preferred_element_type=f32)
            r.acc_s[:, span] = part if first else r.acc_s[:, span] + part

    serve(*dims.serving[3])
    serve(*[step for step in waiting if step[0] == "y"])
    heads_total = remote(
        r.mixed_s.at[most_columns], r.heads_in.at[most_columns], r.head_send.at[0], r.head_recv.at[0], right
    )
    heads_total.wait_recv()
    remote(pass_totals[1], pass_totals[1], r.pass_send.at[1], r.pass_recv.at[1], mate).wait_recv()
    for block in range(columns):
        product(block, ring_part, width, block == 0)
    serve(*list(waiting))
    remote(pass_totals[0], pass_totals[0], r.pass_send.at[0], r.pass_recv.at[0], mate).wait_recv()
    for block in range(columns):
        product(block, 0, ring_part, block == 0)

    stream = (r.residual_in[...].astype(f32) + r.acc_s[...]).astype(bf16)
    r.stream_s[...] = stream
    wide = stream.astype(f32)
    scale = lax.rsqrt(jnp.mean(wide * wide, axis=1, keepdims=True) + EPSILON)
    normed = (wide * scale * r.expert_gain_ref[...]).astype(bf16)

    direct, extra = dims.direct, dims.pieces - dims.direct
    pieces = dims.pieces
    lanes_of = PIECE // 128

    def lines(index):
        return pl.ds(pl.multiple_of(index * main, main), main)

    def far(way, p):
        odd = lax.rem(p, 2) if not isinstance(p, int) else p % 2
        return half - odd if way == 0 else half - 1 + odd

    for q in range(extra):
        r.tokens[me_x, q] = normed[:, (direct + q) * PIECE : (direct + q + 1) * PIECE]

    thin = extra * lanes_of

    def token_ring(way, step, q, col):
        here = r.tokens.at[col, q // lanes_of, :, pl.ds(q % lanes_of * 128, 128)]
        return remote(here, here, r.token_send.at[0], r.token_recv.at[step, q], toward(way))

    put_own = r.put[me_x]

    def make_out(p):
        part = jnp.dot(put_own, normed[:, p * PIECE : (p + 1) * PIECE], preferred_element_type=f32)
        r.outbound[p] = part[:slots].astype(bf16)
        for c in range(lanes_of):
            r.over_out[:, p * lanes_of + c, :] = part[slots:, c * 128 : (c + 1) * 128]

    def send_out(p, carry):
        for i in range(1, places):
            remote(
                r.outbound.at[p, lines(place(i)), :],
                r.chunks.at[me_x, p, lines(me_s), :],
                r.out_send.at[0],
                r.out_recv.at[p],
                {"sp": place(i)},
            ).start()
        r.chunks[me_x, p, lines(me_s), :] = r.outbound[p, lines(me_s), :]
        return carry

    make_out(0)
    send_out(0, 0)
    for q in range(thin):
        for way in range(2):
            token_ring(way, 0, q, me_x).start()
    for p in range(1, direct):
        make_out(p)
    lax.fori_loop(1, direct, send_out, 0)
    for i in range(1, places):
        remote(
            r.over_out.at[place(i)], r.over_in.at[me_s], r.over_send.at[0], r.over_recv.at[0], {"sp": place(i)}
        ).start()
    r.over_in[me_s] = r.over_out[me_s]
    if places < over:
        r.over_in[places:over] = jnp.zeros((over - places, *r.over_in.shape[1:]), f32)
        r.over_ret[:, places:over] = jnp.zeros((2, over - places, *r.over_ret.shape[2:]), f32)
        r.xover_in[:, places:over] = jnp.zeros((columns, over - places, *r.xover_in.shape[2:]), f32)
        r.xover_ret[:, places:over] = jnp.zeros((columns, over - places, *r.xover_ret.shape[2:]), f32)

    def route(offset):
        col = column(offset)
        for q in range(extra):
            part = jnp.dot(r.put[col], r.tokens[col, q], preferred_element_type=f32)
            r.xout[col, q] = part[:slots].astype(bf16)
            r.chunks[col, direct + q, lines(me_s), :] = r.xout[col, q, lines(me_s), :]
            for c in range(lanes_of):
                r.xover_out[offset, :, q * lanes_of + c, :] = part[slots:, c * 128 : (c + 1) * 128]
        r.xover_in[offset, me_s] = r.xover_out[offset, me_s]
        for i in range(1, places):
            remote(
                r.xout.at[col, :, lines(place(i)), :],
                r.chunks.at[col, pl.ds(direct, extra), lines(me_s), :],
                r.xout_send.at[0],
                r.xout_recv.at[offset],
                {"sp": place(i)},
            ).start()
            remote(
                r.xover_out.at[offset, place(i)],
                r.xover_in.at[offset, me_s],
                r.xover_send.at[0],
                r.xover_recv.at[0, offset],
                {"sp": place(i)},
            ).start()

    def routed(offset):
        col = column(offset)
        most = pl.ds(0, (places - 1) * main)
        return (
            remote(
                r.xout.at[col, :, most, :],
                r.chunks.at[col, pl.ds(direct, extra), most, :],
                r.xout_send.at[0],
                r.xout_recv.at[offset],
                right,
            ),
            remote(
                r.xover_out.at[offset, 0 : places - 1],
                r.xover_in.at[offset, 0 : places - 1],
                r.xover_send.at[0],
                r.xover_recv.at[0, offset],
                right,
            ),
        )

    def take_routed(offset):
        col = column(offset)
        for copy in routed(offset):
            copy.wait_recv()
        for q in range(extra):
            for c in range(lanes_of):
                r.chunks[col, direct + q, slots:, c * 128 : (c + 1) * 128] = r.xover_in[
                    offset, :, q * lanes_of + c, :
                ].astype(bf16)

    route(0)

    def token_event(k):
        for q in range(thin):
            came = r.tokens.at[pl.ds(0, 2 if k < half else 1), 0, :, pl.ds(0, 128)]
            remote(came, came, r.token_send.at[0], r.token_recv.at[k - 1, q], right).wait_recv()
            for way in range(2):
                if k < far(way, q):
                    token_ring(way, k, q, column(-k if way == 0 else k)).start()
        if k < half:
            route(columns - k)
        route(k)

    def chunk_ring(way, step, p, col):
        here = r.chunks.at[col, p, pl.ds(0, slots), :]
        return remote(here, here, r.chunk_send.at[0], r.chunk_recv.at[step, p], toward(way))

    def over_ring(way, step, col):
        here = r.chunks.at[col, pl.ds(0, direct), pl.ds(slots, over), :]
        return remote(here, here, r.tail_send.at[0], r.tail_recv.at[step], toward(way))

    def out_arrived(p):
        most = pl.ds(0, (places - 1) * main)
        return remote(
            r.outbound.at[p, most, :], r.chunks.at[me_x, p, most, :], r.out_send.at[0], r.out_recv.at[p], right
        )

    def start_piece(p):
        out_arrived(p).wait_recv()
        chunk_ring(0, 0, p, me_x).start()
        chunk_ring(1, 0, p, me_x).start()

    def start_over():
        remote(
            r.over_out.at[0 : places - 1], r.over_in.at[0 : places - 1], r.over_send.at[0], r.over_recv.at[0], right
        ).wait_recv()
        for c in range(direct * lanes_of):
            at_lanes = (c % lanes_of) * 128
            r.chunks[me_x, c // lanes_of, slots:, at_lanes : at_lanes + 128] = r.over_in[:, c, :].astype(bf16)
        for way in range(2):
            over_ring(way, 0, me_x).start()

    for copy in rims + mates + [enter_copy]:
        copy.wait_send()
    for n in range(1, chips):

        @pl.when(me_y + n < chips)
        def _():
            chip_total(n).wait_send()

    heads_total.wait_send()
    tables_total.wait_send()
    remote(ring_total, ring_total, r.ring_send.at[0], r.ring_recv.at[0, 0], right).wait_send()
    remote(slab_total, slab_total, r.slab_send.at[0], r.slab_recv.at[0], right).wait_send()
    remote(grid_total, grid_total, r.grid_send.at[0], r.grid_recv.at[0], right).wait_send()
    for which in range(2):
        view = pass_totals[which]
        remote(view, view, r.pass_send.at[which], r.pass_recv.at[which], mate).wait_send()

    for step in dims.opening:
        if step > 0:
            token_event(step)
        elif -step < direct:
            start_piece(-step)
    start_over()

    def offset_of(n):
        k = lax.div(n + 1, 2)
        return jnp.where(lax.rem(n, 2) == 1, lax.rem(columns - k, columns), k)

    def unit(n, t):
        offset = offset_of(n)
        col = column(offset)
        pl.when(t == 0)(lambda: take_routed(offset))
        acc = jnp.dot(r.chunks[col, 0], r.gate_up[t, 0:PIECE, :], preferred_element_type=f32)
        for q in range(1, pieces):
            acc = acc + jnp.dot(
                r.chunks[col, q], r.gate_up[t, q * PIECE : (q + 1) * PIECE, :], preferred_element_type=f32
            )
        value = silu(acc[:, 0:128]) * acc[:, 128:256]
        r.hidden[col, :, pl.ds(pl.multiple_of(t * 128, 128), 128)] = value.astype(bf16)
        pl.when(t == dims.tiles - 1)(lambda: give_back(offset))

    def own(col, p):
        return jnp.dot(r.hidden[col], r.down[p], preferred_element_type=f32)

    def give_back(offset):
        col = column(offset)
        for q in range(extra):
            part = own(col, direct + q)
            r.xback[col, q] = part[:slots].astype(bf16)
            r.xret[col, q, lines(me_s), :] = r.xback[col, q, lines(me_s), :]
            for c in range(lanes_of):
                r.xover_back[offset, :, q * lanes_of + c, :] = part[slots:, c * 128 : (c + 1) * 128]
        r.xover_ret[offset, me_s] = r.xover_back[offset, me_s]
        for i in range(1, places):
            remote(
                r.xback.at[col, :, lines(place(i)), :],
                r.xret.at[col, :, lines(me_s), :],
                r.xback_send.at[0],
                r.xback_recv.at[offset],
                {"sp": place(i)},
            ).start()
            remote(
                r.xover_back.at[offset, place(i)],
                r.xover_ret.at[offset, me_s],
                r.xover_send.at[1],
                r.xover_recv.at[1, offset],
                {"sp": place(i)},
            ).start()

    def given_back(offset):
        col = column(offset)
        most = pl.ds(0, (places - 1) * main)
        return (
            remote(
                r.xback.at[col, :, most, :],
                r.xret.at[col, :, most, :],
                r.xback_send.at[0],
                r.xback_recv.at[offset],
                right,
            ),
            remote(
                r.xover_back.at[offset, 0 : places - 1],
                r.xover_ret.at[offset, 0 : places - 1],
                r.xover_send.at[1],
                r.xover_recv.at[1, offset],
                right,
            ),
        )

    for n, weights in enumerate((r.gate_up, r.down)):
        pltpu.make_async_copy(weights, weights, r.weight_sem.at[n]).wait()

    def units(low, high):
        def body(v, carry):
            unit(lax.div(v, dims.tiles), lax.rem(v, dims.tiles))
            return carry

        lax.fori_loop(low, high, body, 0)

    def hop(way, j, p):
        return remote(
            r.sums.at[way, j, p],
            r.sums.at[way, j - 1, p],
            r.sum_send.at[0],
            r.sum_recv.at[way, j - 1, p],
            {"tp": column(1 - 2 * way)},
        )

    def chains(long, step, group):
        j = half - step if long else half - 1 - step

        def body(p, carry):
            odd = lax.rem(p, 2)
            way = 1 - odd if long else odd
            value = own(column(j * (1 - 2 * way)), p)
            if step > 0:
                hop(way, j + 1, p).wait_recv()
                value = value + r.sums[way, j, p].astype(f32)
            r.sums[way, j, p] = value.astype(bf16)
            hop(way, j, p).start()
            return carry

        lax.fori_loop(*group, body, 0)

    share_of = dims.schedule
    for k in range(1, half + 1):
        first, last = share_of[k - 1] * dims.tiles, share_of[k] * dims.tiles

        if k == half and half > 1:
            units(first, last)
            first = last
            for group in dims.groups:
                chains(False, 0, group)

        def pass_on(p, carry, k=k, first=first, last=last):
            came = r.chunks.at[pl.ds(0, 2 if k < half else 1), p, pl.ds(0, slots), :]
            remote(came, came, r.chunk_send.at[0], r.chunk_recv.at[k - 1, p], right).wait_recv()
            if k < half:
                for way in range(2):
                    start = lambda way=way: chunk_ring(way, k, p, column(-k if way == 0 else k)).start()
                    if k < half - 1:
                        start()
                    else:
                        pl.when(k < far(way, p))(start)

            if last > first:
                units(
                    first + lax.div(p * (last - first), direct), first + lax.div((p + 1) * (last - first), direct)
                )
            return carry

        lax.fori_loop(0, direct, pass_on, 0)
        came = r.chunks.at[pl.ds(0, 2 if k < half else 1), pl.ds(0, direct), pl.ds(slots, over), :]
        remote(came, came, r.tail_send.at[0], r.tail_recv.at[k - 1], right).wait_recv()
        for way in range(2):
            if k < far(way, 0):
                over_ring(way, k, column(-k if way == 0 else k)).start()
        if k == 1:
            lax.fori_loop(0, columns, lambda col, carry: (make_pick(col), carry)[1], 0)
    units(share_of[half] * dims.tiles, columns * dims.tiles)

    def finish(p, carry):
        value = own(me_x, p)
        hop(0, 1, p).wait_recv()
        hop(1, 1, p).wait_recv()
        value = value + r.sums[0, 0, p].astype(f32) + r.sums[1, 0, p].astype(f32)
        r.totals[p] = value[0:slots].astype(bf16)
        r.over_total[p] = value[slots:]
        r.returned[p, lines(me_s), :] = r.totals[p, lines(me_s), :]
        for i in range(1, places):
            remote(
                r.totals.at[p, lines(place(i)), :],
                r.returned.at[p, lines(me_s), :],
                r.back_send.at[0],
                r.back_recv.at[p],
                {"sp": place(i)},
            ).start()
        return carry

    def weighted(col, table):
        one = jnp.dot(r.pick[col, 0], table, preferred_element_type=f32)
        two = jnp.dot(r.pick[col, 1], table, preferred_element_type=f32)
        copies = one.shape[1] // 128
        first, second = (jnp.concatenate([r.share_s[col, k]] * copies, axis=1) for k in range(2))
        return first * one + second * two

    def take_back(offset):
        col = column(offset)
        for copy in given_back(offset):
            copy.wait_recv()
        for q in range(extra):
            for c in range(lanes_of):
                r.xret[col, q, slots:, c * 128 : (c + 1) * 128] = r.xover_ret[
                    offset, :, q * lanes_of + c, :
                ].astype(bf16)

    def token_hop(way, j, q):
        return remote(
            r.xsums.at[way, j, q],
            r.xsums.at[way, j - 1, q],
            r.xsum_send.at[0],
            r.xsum_recv.at[way, j - 1, q],
            toward(way),
        )

    taken = set()

    def thin_part(col, q):
        return weighted(col, r.xret[col, q // lanes_of, :, q % lanes_of * 128 : (q % lanes_of + 1) * 128])

    def token_round(t):
        for q in range(thin):
            for way in range(2):
                j = far(1 - way, q) - t
                if j < 1:
                    continue
                offset = j if way == 0 else columns - j
                if offset not in taken:
                    taken.add(offset)
                    take_back(offset)
                value = thin_part(column(offset), q)
                if t > 0:
                    token_hop(way, j + 1, q).wait_recv()
                    value = value + r.xsums[way, j, q].astype(f32)
                r.xsums[way, j, q] = value.astype(bf16)
                token_hop(way, j, q).start()

    for group in dims.groups:
        chains(True, 0, group)
    def left_by_now(view, send, recv):
        remote(view, view, send, recv, right).wait_send()

    most_places, most_lines = pl.ds(0, places - 1), pl.ds(0, (places - 1) * main)
    chunks_total = r.chunks.at[most_columns, pl.ds(0, direct), pl.ds(0, slots), :]
    left_by_now(r.over_out.at[most_places], r.over_send.at[0], r.over_recv.at[0])
    left_by_now(r.tokens.at[most_columns], r.token_send.at[0], r.token_recv.at[0, 0])
    left_by_now(r.chunks.at[most_columns, pl.ds(0, direct), pl.ds(slots, over), :], r.tail_send.at[0], r.tail_recv.at[0])
    left_by_now(chunks_total, r.chunk_send.at[0], r.chunk_recv.at[0, 0])
    left_by_now(r.outbound.at[:, most_lines, :], r.out_send.at[0], r.out_recv.at[0])
    left_by_now(r.xout.at[:, :, most_lines, :], r.xout_send.at[0], r.xout_recv.at[0])
    left_by_now(r.xover_out.at[:, most_places], r.xover_send.at[0], r.xover_recv.at[0, 0])
    def over_back_copy(n, to, at):
        return remote(
            r.over_back.at[n, to],
            r.over_ret.at[n, at],
            r.over_send.at[1],
            r.over_recv.at[1 + n],
            {"sp": to},
        )

    def send_over_back(n, group):
        for p in range(*group):
            for c in range(lanes_of):
                r.over_back[n, :, (p - group[0]) * lanes_of + c, :] = r.over_total[p, :, c * 128 : (c + 1) * 128]
        r.over_ret[n, me_s] = r.over_back[n, me_s]
        for i in range(1, places):
            over_back_copy(n, place(i), me_s).start()

    for kind, step, group in dims.closing:
        if kind == "short":
            chains(False, step, group)
        elif kind == "long":
            chains(True, step, group)
        elif kind == "token":
            token_round(step)
        else:
            lax.fori_loop(*group, finish, 0)
            send_over_back(dims.groups.index(group), group)
    left_by_now(r.xback.at[:, :, most_lines, :], r.xback_send.at[0], r.xback_recv.at[0])
    left_by_now(r.xover_back.at[:, most_places], r.xover_send.at[1], r.xover_recv.at[1, 0])
    left_by_now(r.chunks.at[most_columns, pl.ds(0, direct)], r.sum_send.at[0], r.sum_recv.at[0, 0, 0])
    token_round(half - 1)
    def write_out(span):
        return pltpu.make_async_copy(r.out_s.at[:, span], r.out_ref.at[:, span], r.done_sem.at[0])

    def back_arrived(p):
        most = pl.ds(0, (places - 1) * main)
        return remote(
            r.totals.at[p, most, :], r.returned.at[p, most, :], r.back_send.at[0], r.back_recv.at[p], right
        )

    def combine(p, carry):
        back_arrived(p).wait_recv()
        span = pl.ds(pl.multiple_of(p * PIECE, PIECE), PIECE)
        value = weighted(me_x, r.returned[p])
        r.out_s[:, span] = (r.stream_s[:, span].astype(f32) + value).astype(bf16)
        write_out(span).start()
        return carry

    def combine_group(n, group):
        remote(
            r.over_back.at[n, 0 : places - 1],
            r.over_ret.at[n, 0 : places - 1],
            r.over_send.at[1],
            r.over_recv.at[1 + n],
            right,
        ).wait_recv()
        for p in range(*group):
            for c in range(lanes_of):
                r.returned[p, slots:, c * 128 : (c + 1) * 128] = r.over_ret[n, :, (p - group[0]) * lanes_of + c, :].astype(bf16)
        lax.fori_loop(*group, combine, 0)

    combine_group(dims.groups.index(dims.order[0]), dims.order[0])
    take_back(0)
    for q in range(thin):
        value = thin_part(me_x, q)
        for way in range(2):
            token_hop(way, 1, q).wait_recv()
            value = value + r.xsums[way, 0, q].astype(f32)
        span = slice(direct * PIECE + q * 128, direct * PIECE + (q + 1) * 128)
        r.out_s[:, span] = (r.stream_s[:, span].astype(f32) + value).astype(bf16)

    write_out(pl.ds(direct * PIECE, extra * PIECE)).start()
    combine_group(dims.groups.index(dims.order[1]), dims.order[1])

    left_by_now(r.over_back.at[:, most_places], r.over_send.at[1], r.over_recv.at[1])
    left_by_now(r.tokens.at[most_columns], r.xsum_send.at[0], r.xsum_recv.at[0, 0, 0])
    left_by_now(r.totals.at[:, most_lines, :], r.back_send.at[0], r.back_recv.at[0])
    pltpu.make_async_copy(r.out_s, r.out_ref, r.done_sem.at[0]).wait()


def layer(places, columns, **given):
    f32, bf16 = jnp.float32, jnp.bfloat16
    rows, width = given["residual_hbm"].shape
    small = [name for name in given if name.endswith("_small")]
    units = given["expert_gate_hbm"].shape[2]
    lanes = given["keys_hbm"].shape[1]
    positions = columns * BLOCK
    half, chips, blocks = columns // 2, places // 2, columns
    main = 2 * rows // places
    over = -(-places // 16) * 16
    pieces = width // PIECE
    extra = max(1, pieces // 4)
    direct = pieces - extra
    tiles, total = units // 128, places * main + over
    ring_part = width * RING_SHARE // 16 // 128 * 128
    schedule = (0, 0, 1, 5, 7) if half == 4 else (0,) * half + (columns - 1,)
    opening = (1, 0, 2, -1, -2, 3, -3, -4, 4, -5) if half == 4 else (*range(1, half + 1), *range(0, -direct, -1))
    serving = [
        [("x", 0)],
        [("x", 1)],
        [("x", 2)],
        [("x", 3), ("y", 0), ("y", 1), ("y", 2), ("x", 4), ("y", 3), ("y", 4), ("y", 5), ("y", 6), ("x", 5)],
    ]
    low, high = (0, (direct + 1) // 2), ((direct + 1) // 2, direct)
    groups = [high, low]
    if half == 4:
        closing = [
            ("long", 1, high),
            ("short", 1, high),
            ("long", 1, low),
            ("short", 1, low),
            ("long", 2, low),
            ("long", 2, high),
            ("long", 3, low),
            ("short", 2, low),
            ("token", 0, None),
            ("long", 3, high),
            ("finish", None, low),
            ("short", 2, high),
            ("token", 1, None),
            ("finish", None, high),
            ("token", 2, None),
        ]
    else:
        closing = []
        for step in range(1, half):
            closing += [("short", step, group) for group in groups if step < half - 1]
            closing += [("long", step, group) for group in groups]
            closing.append(("token", step - 1, None))
        closing += [("finish", None, group) for group in groups]
    dims = types.SimpleNamespace(
        places=places, columns=columns, width=width, main=main, over=over, pieces=pieces, direct=direct, tiles=tiles,
        schedule=schedule, opening=opening, small=small, groups=groups, order=(low, high), closing=closing, ring_part=ring_part, serving=serving,
    )
    packed = STATE_ONE + STATE_TWO
    square = (blocks, 2, BLOCK, BLOCK)
    vmem = lambda *shape, dtype=bf16: pltpu.VMEM(shape, dtype)
    dma = lambda *shape: pltpu.SemaphoreType.DMA(shape)
    in_specs = [pl.BlockSpec(memory_space=pltpu.SMEM if a.shape == (2, 2) else pl.ANY) for a in given.values()]
    lane_rows = PIECE // 128
    scratch = {name[:-5] + "ref": pltpu.VMEM(given[name].shape, given[name].dtype) for name in small}
    scratch |= dict(
        residual_in=vmem(rows, width),
        value_in=vmem(2 * positions, BLOCK),
        gate_in=vmem(2 * positions, BLOCK),
        keys_in=vmem(positions, lanes),
        value_rim=vmem(16, BLOCK),
        keys_rim=vmem(16, lanes),
        value_wide=vmem(2 * positions + 16, BLOCK, dtype=f32),
        keys_wide=vmem(positions + 16, lanes, dtype=f32),
        gate_wide=vmem(2 * BLOCK, BLOCK, dtype=f32),
        conv_wide=vmem(2 * BLOCK, BLOCK, dtype=f32),
        x_s=vmem(*square),
        kt_s=vmem(*square),
        q_s=vmem(*square),
        state_s=vmem(*square, dtype=f32),
        near_s=vmem(*square, dtype=f32),
        stride_s=vmem(HEADS * blocks, BLOCK, dtype=f32),
        run_s=vmem(HEADS * blocks, BLOCK, dtype=f32),
        fade_s=vmem(HEADS * blocks, BLOCK, dtype=f32),
        end_s=vmem(HEADS * blocks, BLOCK, dtype=f32),
        cols_s=vmem(blocks, BLOCK, HEADS, dtype=f32),
        own_pack=vmem(packed, BLOCK),
        own_fade=vmem(8, BLOCK, dtype=f32),
        mate_pack=vmem(packed, BLOCK),
        mate_fade=vmem(8, BLOCK, dtype=f32),
        chip_pack=vmem(packed, BLOCK),
        chip_fade=vmem(8, BLOCK, dtype=f32),
        all_pack=vmem(chips, packed // 2, BLOCK),
        all_fade=vmem(chips, 8, BLOCK, dtype=f32),
        enter_pack=vmem(packed, BLOCK),
        carry_s=vmem(2, BLOCK, BLOCK, dtype=f32),
        mixed_s=vmem(columns, BLOCK, 2 * BLOCK),
        heads_in=vmem(columns, BLOCK, 2 * BLOCK),
        matrix=vmem(columns, 2 * BLOCK, width),
        acc_s=vmem(rows, width, dtype=f32),
        stream_s=vmem(rows, width),
        out_s=vmem(rows, width),
        tables=vmem(columns, 8, rows, dtype=f32),
        put=vmem(columns, total, rows),
        pick=vmem(columns, 2, rows, total),
        share_s=vmem(columns, 2, rows, 128, dtype=f32),
        tokens=vmem(columns, extra, rows, PIECE),
        outbound=vmem(direct, places * main, PIECE),
        over_out=vmem(over, direct * lane_rows, 128, dtype=f32),
        over_in=vmem(over, direct * lane_rows, 128, dtype=f32),
        over_back=vmem(2, over, (high[1] - low[0] + 1) // 2 * lane_rows, 128, dtype=f32),
        over_ret=vmem(2, over, (high[1] - low[0] + 1) // 2 * lane_rows, 128, dtype=f32),
        over_total=vmem(direct, over, PIECE, dtype=f32),
        xout=vmem(columns, extra, places * main, PIECE),
        xback=vmem(columns, extra, places * main, PIECE),
        xret=vmem(columns, extra, total, PIECE),
        xover_out=vmem(columns, over, extra * lane_rows, 128, dtype=f32),
        xover_in=vmem(columns, over, extra * lane_rows, 128, dtype=f32),
        xover_back=vmem(columns, over, extra * lane_rows, 128, dtype=f32),
        xover_ret=vmem(columns, over, extra * lane_rows, 128, dtype=f32),
        chunks=vmem(columns, pieces, total, PIECE),
        hidden=vmem(columns, total, units),
        gate_up=vmem(tiles, width, 256),
        down=vmem(pieces, units, PIECE),
        sums=vmem(2, half + 1, direct, total, PIECE),
        xsums=vmem(2, half + 1, extra * lane_rows, rows, 128),
        totals=vmem(direct, places * main, PIECE),
        returned=vmem(direct, total, PIECE),
        load_sem=dma(6),
        weight_sem=dma(2),
        done_sem=dma(1),
        small_sem=dma(len(small)),
    )
    steps = (2, half)
    for name, send, recv in (
        ("rim", (2,), (2,)),
        ("mate", (2,), (2,)),
        ("chip", (chips,), (chips,)),
        ("enter", (1,), (1,)),
        ("head", (1,), (1,)),
        ("table", (1,), (1,)),
        ("ring", (1,), (columns - 1, 2)),
        ("slab", (1,), (1,)),
        ("grid", (1,), (chips - 1,)),
        ("pass", (2,), (2,)),
        ("over", (2,), (3,)),
        ("token", (1,), (half, extra * lane_rows)),
        ("out", (1,), (direct,)),
        ("xout", (1,), (columns,)),
        ("xover", (2,), (2, columns)),
        ("chunk", (1,), (half, direct)),
        ("tail", (1,), (half,)),
        ("xback", (1,), (columns,)),
        ("sum", (1,), (*steps, direct)),
        ("xsum", (1,), (*steps, extra * lane_rows)),
        ("back", (1,), (direct,)),
    ):
        scratch[name + "_send"], scratch[name + "_recv"] = dma(*send), dma(*recv)
    names = [*given, "out_ref", *scratch]
    return pl.pallas_call(
        functools.partial(layer_kernel, dims, names),
        out_shape=jax.ShapeDtypeStruct((rows, width), bf16),
        in_specs=in_specs,
        out_specs=pl.BlockSpec(memory_space=pl.ANY),
        scratch_shapes=list(scratch.values()),
        compiler_params=pltpu.CompilerParams(
            collective_id=0, has_side_effects=True, vmem_limit_bytes=VMEM_LIMIT
        ),
        name="layer",
    )(*given.values())


def local(
    residual,
    grouped_value_heads,
    output_gate_heads,
    projected_key_query,
    raw_step_size,
    step_size_bias,
    head_decay_logarithm,
    position_extra_decay,
    head_skip_weight,
    value_kernel_taps,
    key_query_kernel,
    head_norm_gain,
    output_matrix,
    expert_norm_gain,
    expert_gate_weight,
    expert_up_weight,
    expert_down_weight,
    token_expert_choice,
    expert_output_weight,
):
    return layer(
        lax.axis_size("sp"),
        lax.axis_size("tp"),
        residual_hbm=residual,
        value_hbm=grouped_value_heads.reshape(-1, BLOCK),
        gate_hbm=output_gate_heads.reshape(-1, BLOCK),
        keys_hbm=projected_key_query,
        raw_small=raw_step_size.transpose(1, 2, 0),
        bias_ref=step_size_bias,
        log_ref=head_decay_logarithm,
        extra_small=position_extra_decay.reshape(-1, BLOCK),
        skip_ref=head_skip_weight,
        value_tap_small=value_kernel_taps.reshape(-1, BLOCK),
        key_tap_small=key_query_kernel,
        head_gain_small=head_norm_gain,
        matrix_hbm=output_matrix,
        expert_gain_small=expert_norm_gain[None],
        choice_small=token_expert_choice.T,
        share_small=expert_output_weight.T,
        expert_gate_hbm=expert_gate_weight,
        expert_up_hbm=expert_up_weight,
        expert_down_hbm=expert_down_weight,
    )


def solution(mesh):
    placed = (
        P(("grp", "sp", "tp"), None),
        P(("grp", "sp"), None, "tp"),
        P(("grp", "sp"), None, "tp"),
        P(("grp", "sp"), None),
        P(("grp", "sp"), None, "tp"),
        P(None, "tp"),
        P(None, "tp"),
        P(("grp", "sp")),
        P(None, "tp"),
        P(None, None, "tp"),
        P(),
        P(None, "tp"),
        P(None, "tp", None),
        P(),
        P("sp", None, "tp"),
        P("sp", None, "tp"),
        P("sp", "tp", None),
        P(("grp", "sp", "tp"), None),
        P(("grp", "sp", "tp"), None),
    )
    return jax.shard_map(
        local, mesh=mesh, in_specs=placed, out_specs=P(("grp", "sp", "tp"), None), check_vma=False
    )
```

```python
import functools
import types

import jax
import jax.numpy as jnp
from jax import lax
from jax.experimental import pallas as pl
from jax.experimental.pallas import tpu as pltpu
from jax.sharding import PartitionSpec as P

HEAD_DIM = 64
STATE_ONE = 64
STATE_TWO = 128
BLOCK = 128
EPSILON = 1e-06

MESH = pl.DeviceIdType.MESH
PIECE = 256
HEADS = 4
RING_SHARE = 7
VMEM_LIMIT = 67043328


def remote(src, dst, send, recv, device):
    return pltpu.make_async_remote_copy(
        src_ref=src, dst_ref=dst, send_sem=send, recv_sem=recv, device_id=device, device_id_type=MESH
    )


def silu(a):
    return a * (1.0 / (1.0 + jnp.exp(-a)))


def layer_kernel(dims, names, *refs):
    r = types.SimpleNamespace(**dict(zip(names, refs, strict=True)))
    f32, bf16 = jnp.float32, jnp.bfloat16
    places, columns, width, rows = dims.places, dims.columns, dims.width, BLOCK
    half, chips, blocks = columns // 2, places // 2, columns
    me_x, me_s = lax.axis_index("tp"), lax.axis_index("sp")
    core, me_y = lax.rem(me_s, 2), lax.div(me_s, 2)
    right = {"tp": lax.rem(me_x + 1, columns)}
    left = {"tp": lax.rem(me_x + columns - 1, columns)}
    mate = {"sp": me_s + 1 - 2 * core}
    following = {"sp": lax.rem(me_s + 1, places)}

    def column(offset):
        return lax.rem(me_x + offset + columns, columns)

    def place(offset):
        return lax.rem(me_s + offset, places)

    def peer(offset):
        return {"sp": lax.rem(me_s + 2 * offset, places)}

    def toward(way):
        return right if way == 0 else left

    barrier = pltpu.get_barrier_semaphore()
    peers = sorted(
        [(min(i, columns - i), {"tp": column(i)}) for i in range(1, columns)]
        + [(min(i, places - i) / 2, {"sp": place(i)}) for i in range(1, places)],
        key=lambda peer: -peer[0],
    )
    peers = [device for _, device in peers]
    for device in peers:
        pl.semaphore_signal(barrier, inc=1, device_id=device, device_id_type=MESH)

    small = {
        name: pltpu.make_async_copy(getattr(r, name), getattr(r, name[:-5] + "ref"), r.small_sem.at[n])
        for n, name in enumerate(dims.small)
    }
    ring_part, slab = dims.ring_part, rows // chips
    mine = pl.multiple_of(core * rows, rows)

    def slab_rows(y):
        return pl.ds(pl.multiple_of(mine + y * slab, 16), slab)

    on_ring, on_grid = pl.ds(0, ring_part), pl.ds(ring_part, width - ring_part)
    loads = [
        (r.matrix_hbm.at[0], r.matrix.at[0, pl.ds(0, rows), :]),
        (r.matrix_hbm.at[1], r.matrix.at[0, pl.ds(rows, rows), :]),
        (r.value_hbm, r.value_in),
        (r.keys_hbm, r.keys_in),
        (r.gate_hbm, r.gate_in),
        (r.residual_hbm, r.residual_in),
    ]
    loads = [pltpu.make_async_copy(a, b, r.load_sem.at[n]) for n, (a, b) in enumerate(loads)]
    for load in loads[:2] + list(small.values()) + loads[2:4]:
        load.start()
    for name in ("choice_small", "share_small"):
        small[name].wait()
    r.tables[me_x] = jnp.zeros((8, rows), f32)
    r.tables[me_x, 0:2, :] = r.choice_ref[...].astype(f32)
    r.tables[me_x, 2:4, :] = r.share_ref[...]

    for load in loads[:2]:
        load.wait()
    pl.semaphore_wait(barrier, len(peers))

    def matrix_block(way, event, k, sub):
        piece = ((event % 2) ^ way) * 2 + sub
        block = (columns - k if way == 0 else k) % columns
        return r.matrix.at[block, pl.ds(pl.multiple_of(mine + piece * (rows // 4), 16), rows // 4), on_ring]

    def matrix_ring(way, event, sub):
        k = event // 2
        return remote(
            matrix_block(way, event, k, sub),
            matrix_block(way, event, k + 1, sub),
            r.ring_send.at[0],
            r.ring_recv.at[event, sub],
            toward(way),
        )

    def slab_copy(offset):
        return remote(
            r.matrix.at[0, slab_rows(me_y), on_grid],
            r.matrix.at[columns - offset, slab_rows(me_y), on_grid],
            r.slab_send.at[0],
            r.slab_recv.at[0],
            {"tp": column(offset)},
        )

    def grid_view(way, event, y):
        blocks_of = pl.ds(1, half) if (event % 2) ^ way == 0 else pl.ds(1 + half, half - 1)
        return r.matrix.at[blocks_of, slab_rows(y), on_grid]

    def grid_ring(way, event, y):
        here = grid_view(way, event, y)
        return remote(
            here, here, r.grid_send.at[0], r.grid_recv.at[event], peer(1) if way == 0 else peer(chips - 1)
        )

    def to_mate(here, which):
        return remote(here, here, r.pass_send.at[which], r.pass_recv.at[which], mate)

    most_columns, other_blocks = pl.ds(0, columns - 1), pl.ds(1, columns - 1)
    ring_total = r.matrix.at[other_blocks, pl.ds(0, rows), on_ring]
    grid_total = r.matrix.at[other_blocks, pl.ds(0, (chips - 1) * slab), on_grid]
    slab_total = r.matrix.at[other_blocks, pl.ds(0, slab), on_grid]
    pass_totals = (ring_total, r.matrix.at[other_blocks, pl.ds(0, rows), on_grid])

    for load in loads[2:4]:
        load.wait()
    rim_rows = 16
    positions = blocks * rows
    rims = [
        remote(
            r.value_in.at[pl.ds(2 * positions - rim_rows, rim_rows), :],
            r.value_rim,
            r.rim_send.at[0],
            r.rim_recv.at[0],
            following,
        ),
        remote(
            r.keys_in.at[pl.ds(positions - rim_rows, rim_rows), :], r.keys_rim, r.rim_send.at[1], r.rim_recv.at[1], following
        ),
    ]
    for rim in rims:
        rim.start()

    def table_copy(offset):
        here = r.tables.at[me_x]
        return remote(here, here, r.table_send.at[0], r.table_recv.at[0], {"tp": column(offset)})

    for i in range(1, columns):
        table_copy(i).start()
    for i in range(1, columns):
        slab_copy(i).start()
    for event in range(min(2, columns - 1)):
        for sub in range(2):
            for way in range(2):
                matrix_ring(way, event, sub).start()
    tables_total = remote(
        r.tables.at[most_columns], r.tables.at[most_columns], r.table_send.at[0], r.table_recv.at[0], right
    )

    def serve_ring(event):
        for sub in range(2):
            both = r.matrix.at[0, pl.ds(0, rows // 2), on_ring]
            remote(both, both, r.ring_send.at[0], r.ring_recv.at[event, sub], right).wait_recv()
            for way in range(2):
                if event + 2 < columns - 1:
                    matrix_ring(way, event + 2, sub).start()
                to_mate(matrix_block(way, event, event // 2 + 1, sub), 0).start()

    def serve_slab():
        remote(slab_total, slab_total, r.slab_send.at[0], r.slab_recv.at[0], right).wait_recv()
        for event in range(2):
            for way in range(2):
                if event < chips - 1:
                    grid_ring(way, event, me_y).start()
        to_mate(r.matrix.at[other_blocks, slab_rows(me_y), on_grid], 1).start()

    def serve_grid(event):
        k = event // 2 + 1
        remote(slab_total, slab_total, r.grid_send.at[0], r.grid_recv.at[event], right).wait_recv()
        for way in range(2):
            y = lax.rem(me_y + (chips - k if way == 0 else k), chips)
            if event + 2 < chips - 1:
                grid_ring(way, event + 2, y).start()
            to_mate(grid_view(way, event, y), 1).start()

    waiting = [("x", e) for e in range(columns - 1)] + [("y", e) for e in range(chips - 1)]

    def serve(*steps):
        for step in steps:
            if step in waiting:
                waiting.remove(step)
                (serve_ring if step[0] == "x" else serve_grid)(step[1])

    for load in loads[4:]:
        load.start()
    for t in range(dims.tiles):
        span = pl.ds(t * 128, 128)
        for n, weight in enumerate((r.expert_gate_hbm, r.expert_up_hbm)):
            pltpu.make_async_copy(
                weight.at[0, :, span], r.gate_up.at[t, :, pl.ds(n * 128, 128)], r.weight_sem.at[0]
            ).start()
    for p in range(dims.pieces):
        pltpu.make_async_copy(
            r.expert_down_hbm.at[0, :, pl.ds(p * PIECE, PIECE)], r.down.at[p], r.weight_sem.at[1]
        ).start()

    for name in dims.small:
        if name not in ("choice_small", "share_small"):
            small[name].wait()
    for g in range(2):
        raw = r.raw_ref[g].astype(f32)
        for k in range(blocks):
            r.stride_s[HEADS * k + 2 * g : HEADS * k + 2 * g + 2, :] = raw[:, k * rows : (k + 1) * rows]
    for k in range(blocks):
        r.run_s[HEADS * k : HEADS * k + HEADS, :] = jnp.broadcast_to(r.extra_ref[k : k + 1, :], (HEADS, rows))
    head_of = jnp.bitwise_and(lax.broadcasted_iota(jnp.int32, (HEADS * blocks, rows), 0), HEADS - 1)

    def by_head(table):
        picked = jnp.full((HEADS * blocks, rows), table[1, 1], f32)
        for n in range(3):
            picked = jnp.where(head_of == n, table[n // 2, n % 2], picked)
        return picked

    shifted = r.stride_s[...] + by_head(r.bias_ref)
    stride = jnp.maximum(shifted, 0.0) + jnp.log1p(jnp.exp(-jnp.abs(shifted)))
    log_decay = r.run_s[...] - jnp.exp(by_head(r.log_ref)) * stride
    at_row = lax.broadcasted_iota(jnp.int32, (rows, rows), 0)
    at_lane = lax.broadcasted_iota(jnp.int32, (rows, rows), 1)
    running = jnp.dot(
        log_decay,
        jnp.where(at_row <= at_lane, 1.0, 0.0),
        preferred_element_type=f32,
        precision=lax.Precision.HIGHEST,
    )
    ends = jnp.broadcast_to(running[:, rows - 1 : rows], running.shape)
    r.stride_s[...] = stride
    r.run_s[...] = running
    r.fade_s[...] = jnp.exp(ends - running) * stride
    r.end_s[...] = jnp.exp(ends)
    turned = jnp.transpose(running)
    for k in range(blocks):
        r.cols_s[k, :, 0:HEADS] = turned[:, HEADS * k : HEADS * k + HEADS]

    first_head = at_lane < HEAD_DIM

    def row_pair(table, k, g):
        low = table[pl.ds(HEADS * k + 2 * g, 1), :]
        high = table[pl.ds(HEADS * k + 2 * g + 1, 1), :]
        return jnp.where(first_head[0:1], low, high)

    r.value_wide[rim_rows:, :] = r.value_in[...].astype(f32)
    r.keys_wide[rim_rows:, :] = r.keys_in[...].astype(f32)
    taps = r.value_tap_ref.shape[0] // 2
    value_tap = r.value_tap_ref[...].astype(f32)
    key_tap = r.key_tap_ref[...].astype(f32)
    even = jnp.bitwise_and(lax.broadcasted_iota(jnp.int32, (2 * rows, rows), 0), 1) == 0
    tap_rows = [jnp.where(even, value_tap[2 * j : 2 * j + 1], value_tap[2 * j + 1 : 2 * j + 2]) for j in range(taps)]

    def states_of(k):
        window = r.value_wide[pl.ds(pl.multiple_of(k * 2 * rows, 2 * rows), 2 * rows + rim_rows), :]
        total = jnp.zeros((2 * rows, rows), f32)
        for j in range(taps):
            start = rim_rows - 2 * (taps - 1 - j)
            total = total + window[start : start + 2 * rows] * tap_rows[j]
        r.conv_wide[...] = silu(total).astype(bf16).astype(f32)
        window = r.keys_wide[pl.ds(pl.multiple_of(k * rows, rows), rows + rim_rows), :]
        total = jnp.zeros((rows, r.keys_wide.shape[1]), f32)
        for j in range(taps):
            start = rim_rows - (taps - 1 - j)
            total = total + window[start : start + rows] * key_tap[j : j + 1]
        conv = silu(total).astype(bf16).astype(f32)
        both = conv[:, 0 : 2 * STATE_ONE]
        keys = [jnp.where(first_head, both, 0.0), conv[:, 2 * STATE_ONE : 2 * STATE_ONE + STATE_TWO]]
        asks = [pltpu.roll(both, STATE_ONE, 1), conv[:, 2 * STATE_ONE + STATE_TWO :]]
        for g in range(2):
            x = r.conv_wide[pl.ds(g, rows, stride=2), :].astype(bf16)
            key_t = jnp.transpose(keys[g])
            r.x_s[k, g] = x
            r.kt_s[k, g] = key_t.astype(bf16)
            r.q_s[k, g] = asks[g].astype(bf16)
            faded = jnp.concatenate(
                [key_t * r.fade_s[pl.ds(HEADS * k + 2 * g + h, 1), :] for h in range(2)], axis=0
            ).astype(bf16)
            state = jnp.dot(faded, x, preferred_element_type=f32)
            r.state_s[k, g] = jnp.where(first_head, state[:rows], state[rows:])

    def state_step(i, carry):
        states_of(i)
        return carry

    lax.fori_loop(1, blocks, state_step, 0)
    for rim in rims:
        rim.wait_recv()
    opening = me_s == 0
    r.value_wide[0:rim_rows, :] = jnp.where(opening, 0.0, r.value_rim[...].astype(f32))
    r.keys_wide[0:rim_rows, :] = jnp.where(opening, 0.0, r.keys_rim[...].astype(f32))
    states_of(0)

    packed = STATE_TWO + STATE_ONE
    piece = packed // 2

    def local_end(g):
        total = jnp.zeros((rows, rows), f32)
        faded = jnp.ones((1, rows), f32)
        for k in range(blocks):
            decay = row_pair(r.end_s, k, g)
            total = total * decay + r.state_s[k, g]
            faded = faded * decay
        return total, faded

    end_one, fade_one = local_end(0)
    end_two, fade_two = local_end(1)
    own = jnp.concatenate([end_two, end_one[:STATE_ONE]], axis=0)
    r.own_pack[...] = own.astype(bf16)
    r.own_fade[0:1, :] = fade_one
    r.own_fade[1:2, :] = fade_two
    r.own_fade[2:8, :] = jnp.zeros((6, rows), f32)
    mates = [
        remote(r.own_pack, r.mate_pack, r.mate_send.at[0], r.mate_recv.at[0], mate),
        remote(r.own_fade, r.mate_fade, r.mate_send.at[1], r.mate_recv.at[1], mate),
    ]
    for copy in mates:
        copy.start()
    for copy in mates:
        copy.wait_recv()
    is_low = core == 0
    low = jnp.where(is_low, own, r.mate_pack[...].astype(f32))
    high = jnp.where(is_low, r.mate_pack[...].astype(f32), own)
    mate_rows = r.mate_fade[...]
    own_rows = r.own_fade[...]
    high_rows = jnp.where(is_low, mate_rows, own_rows)
    in_two = lax.broadcasted_iota(jnp.int32, (packed, rows), 0) < STATE_TWO
    r.chip_pack[...] = (low * jnp.where(in_two, high_rows[1:2], high_rows[0:1]) + high).astype(bf16)
    r.chip_fade[...] = own_rows * mate_rows
    my_half = pl.ds(pl.multiple_of(core * piece, 16), piece)

    def to_chip(n, which):
        src = r.chip_pack.at[my_half, :] if which == 0 else r.chip_fade
        dst = r.all_pack.at[me_y] if which == 0 else r.all_fade.at[me_y]
        return remote(src, dst, r.chip_send.at[n], r.chip_recv.at[n], peer(n))

    def chip_total(n):
        sent = r.own_pack.at[pl.ds(0, piece + 16), :]
        return remote(sent, sent, r.chip_send.at[n], r.chip_recv.at[n], peer(n))

    for n in range(1, chips):

        @pl.when(me_y + n < chips)
        def _():
            for which in range(2):
                to_chip(n, which).start()


    below = at_row >= at_lane

    def near_step(k, carry):
        cols = r.cols_s[k]
        for g in range(2):
            scores = jnp.dot(r.q_s[k, g], r.kt_s[k, g], preferred_element_type=f32)
            parts = []
            for h in range(2):
                n = 2 * g + h
                gap = cols[:, n : n + 1] - r.run_s[pl.ds(HEADS * k + n, 1), :]
                damping = jnp.exp(jnp.where(below, gap, -1e30))
                parts.append((scores * damping * r.stride_s[pl.ds(HEADS * k + n, 1), :]).astype(bf16))
            near = jnp.dot(jnp.concatenate(parts, axis=0), r.x_s[k, g], preferred_element_type=f32)
            r.near_s[k, g] = jnp.where(first_head, near[:rows], near[rows:])
        return carry

    lax.fori_loop(0, blocks, near_step, 0)
    serve_slab()
    serve(*dims.serving[0])
    main, over, slots = dims.main, dims.over, places * dims.main
    total_slots = slots + over
    slot_row = lax.broadcasted_iota(jnp.int32, (total_slots, over), 0)
    slot_expert = lax.broadcasted_iota(jnp.int32, (total_slots, over), 1)
    spread = jnp.where(
        ((slot_row < slots) & (slot_row >= slot_expert * main) & (slot_row < slot_expert * main + main))
        | (slot_row == slots + slot_expert),
        1.0,
        0.0,
    ).astype(bf16)
    at = lax.broadcasted_iota(jnp.int32, (total_slots, rows), 0)
    turn = jnp.where(at < slots, jnp.bitwise_and(at, main - 1), main).astype(f32)
    expert_at = lax.broadcasted_iota(jnp.int32, (over, rows), 0).astype(f32)
    earlier = jnp.where(at_row < at_lane, 1.0, 0.0).astype(bf16)

    def make_put(col):
        table = r.tables[col]
        named = jnp.where((expert_at == table[0:1]) | (expert_at == table[1:2]), 1.0, 0.0)
        rank = jnp.dot(named.astype(bf16), earlier, preferred_element_type=f32)
        named_x = jnp.dot(spread, named.astype(bf16), preferred_element_type=f32)
        rank_x = jnp.dot(spread, rank.astype(bf16), preferred_element_type=f32)
        r.put[col] = jnp.where(rank_x == turn, named_x, 0.0).astype(bf16)

    tables_total.wait_recv()

    def put_step(col, carry):
        make_put(col)
        return carry

    lax.fori_loop(0, columns, put_step, 0)

    for load in loads[-2:]:
        load.wait()
    serve(*dims.serving[1])
    for n in range(1, chips):

        @pl.when(me_y >= n)
        def _():
            chip_total(n).wait_recv()

    row_at = lax.broadcasted_iota(jnp.int32, (piece, rows), 0) + core * piece
    half_two = row_at < STATE_TWO
    entering = jnp.zeros((piece, rows), f32)
    for y in range(chips):
        fades = r.all_fade[y]
        later = entering * jnp.where(half_two, fades[1:2], fades[0:1]) + r.all_pack[y].astype(f32)
        entering = jnp.where(y < me_y, later, entering)
    r.enter_pack[my_half, :] = entering.astype(bf16)
    here = r.enter_pack.at[my_half, :]
    enter_copy = remote(here, here, r.enter_send.at[0], r.enter_recv.at[0], mate)
    enter_copy.start()
    enter_copy.wait_recv()
    chip_state = r.enter_pack[...].astype(f32)
    after_low = chip_state * jnp.where(in_two, mate_rows[1:2], mate_rows[0:1]) + r.mate_pack[...].astype(f32)
    entered = jnp.where(is_low, chip_state, after_low)
    r.carry_s[1] = entered[:STATE_TWO]
    r.carry_s[0] = jnp.zeros((rows, rows), f32)
    r.carry_s[0, 0:STATE_ONE, :] = entered[STATE_TWO:]

    serve(*dims.serving[2])
    def head_copy(col):
        return remote(r.mixed_s.at[col], r.heads_in.at[me_x], r.head_send.at[0], r.head_recv.at[0], {"tp": col})

    def mix_step(k, carry):
        cols = jnp.exp(r.cols_s[k])
        r.gate_wide[...] = r.gate_in[pl.ds(pl.multiple_of(k * 2 * rows, 2 * rows), 2 * rows), :].astype(f32)
        for g in range(2):
            state = r.carry_s[g]
            coarse = state.astype(bf16)
            fine = (state - coarse.astype(f32)).astype(bf16)
            ask = r.q_s[k, g]
            far = jnp.dot(
                jnp.concatenate([ask, ask], axis=1),
                jnp.concatenate([coarse, fine], axis=0),
                preferred_element_type=f32,
            )
            reach = jnp.where(first_head, cols[:, 2 * g : 2 * g + 1], cols[:, 2 * g + 1 : 2 * g + 2])
            skip = jnp.where(first_head[0:1], r.skip_ref[g, 0], r.skip_ref[g, 1])
            mixed = r.near_s[k, g] + far * reach + skip * r.x_s[k, g].astype(f32)
            gated = mixed * silu(r.gate_wide[pl.ds(g, rows, stride=2), :])
            square = gated * gated
            one = jnp.sum(jnp.where(first_head, square, 0.0), axis=1, keepdims=True)
            two = jnp.sum(jnp.where(first_head, 0.0, square), axis=1, keepdims=True)
            scale = lax.rsqrt(jnp.where(first_head, one, two) * (1.0 / HEAD_DIM) + EPSILON)
            r.mixed_s[k, :, g * rows : (g + 1) * rows] = (gated * scale * r.head_gain_ref[g : g + 1, :]).astype(bf16)
            r.carry_s[g] = state * row_pair(r.end_s, k, g) + r.state_s[k, g]

        @pl.when(k != me_x)
        def _():
            head_copy(k).start()

        return carry

    lax.fori_loop(0, blocks, mix_step, 0)
    r.heads_in[me_x] = r.mixed_s[me_x]

    slot_col = lax.broadcasted_iota(jnp.int32, (over, total_slots), 1)
    slot_exp = lax.broadcasted_iota(jnp.int32, (over, total_slots), 0)
    spread_t = jnp.where(
        ((slot_col < slots) & (slot_col >= slot_exp * main) & (slot_col < slot_exp * main + main))
        | (slot_col == slots + slot_exp),
        1.0,
        0.0,
    ).astype(bf16)
    at_t = lax.broadcasted_iota(jnp.int32, (rows, total_slots), 1)
    turn_t = jnp.where(at_t < slots, jnp.bitwise_and(at_t, main - 1), main).astype(f32)
    expert_to = lax.broadcasted_iota(jnp.int32, (rows, over), 1).astype(f32)
    later_t = jnp.where(at_lane < at_row, 1.0, 0.0).astype(bf16)

    def make_pick(col):
        table = jnp.transpose(r.tables[col])
        named = [jnp.where(expert_to == table[:, k : k + 1], 1.0, 0.0) for k in range(2)]
        rank = jnp.dot(later_t, (named[0] + named[1]).astype(bf16), preferred_element_type=f32)
        rank_x = jnp.dot(rank.astype(bf16), spread_t, preferred_element_type=f32)
        for k in range(2):
            named_x = jnp.dot(named[k].astype(bf16), spread_t, preferred_element_type=f32)
            r.pick[col, k] = jnp.where(rank_x == turn_t, named_x, 0.0).astype(bf16)
            r.share_s[col, k] = jnp.broadcast_to(table[:, 2 + k : 3 + k], (rows, rows))

    def product(block, low, high, first):
        for n in range(low, high, 512):
            span = slice(n, min(n + 512, high))
            part = jnp.dot(r.heads_in[column(block)], r.matrix[block, :, span], preferred_element_type=f32)
            r.acc_s[:, span] = part if first else r.acc_s[:, span] + part

    serve(*dims.serving[3])
    serve(*list(waiting))
    heads_total = remote(
        r.mixed_s.at[most_columns], r.heads_in.at[most_columns], r.head_send.at[0], r.head_recv.at[0], right
    )
    heads_total.wait_recv()
    for which, (low_lane, high_lane) in enumerate(((0, ring_part), (ring_part, width))):
        remote(pass_totals[which], pass_totals[which], r.pass_send.at[which], r.pass_recv.at[which], mate).wait_recv()
        for block in range(columns):
            product(block, low_lane, high_lane, block == 0)

    stream = (r.residual_in[...].astype(f32) + r.acc_s[...]).astype(bf16)
    r.stream_s[...] = stream
    wide = stream.astype(f32)
    scale = lax.rsqrt(jnp.mean(wide * wide, axis=1, keepdims=True) + EPSILON)
    normed = (wide * scale * r.expert_gain_ref[...]).astype(bf16)

    direct, extra = dims.direct, dims.pieces - dims.direct
    pieces = dims.pieces
    lanes_of = PIECE // 128

    def lines(index):
        return pl.ds(pl.multiple_of(index * main, main), main)

    def far(way, p):
        odd = lax.rem(p, 2) if not isinstance(p, int) else p % 2
        return half - odd if way == 0 else half - 1 + odd

    for q in range(extra):
        r.tokens[me_x, q] = normed[:, (direct + q) * PIECE : (direct + q + 1) * PIECE]

    thin = extra * lanes_of

    def token_ring(way, step, q, col):
        here = r.tokens.at[col, q // lanes_of, :, pl.ds(q % lanes_of * 128, 128)]
        return remote(here, here, r.token_send.at[0], r.token_recv.at[step, q], toward(way))

    put_own = r.put[me_x]

    def make_out(p):
        part = jnp.dot(put_own, normed[:, p * PIECE : (p + 1) * PIECE], preferred_element_type=f32)
        r.outbound[p] = part[:slots].astype(bf16)
        for c in range(lanes_of):
            r.over_out[:, p * lanes_of + c, :] = part[slots:, c * 128 : (c + 1) * 128]

    def send_out(p, carry):
        for i in range(1, places):
            remote(
                r.outbound.at[p, lines(place(i)), :],
                r.chunks.at[me_x, p, lines(me_s), :],
                r.out_send.at[0],
                r.out_recv.at[p],
                {"sp": place(i)},
            ).start()
        r.chunks[me_x, p, lines(me_s), :] = r.outbound[p, lines(me_s), :]
        return carry

    make_out(0)
    send_out(0, 0)
    for q in range(thin):
        for way in range(2):
            token_ring(way, 0, q, me_x).start()
    for p in range(1, direct):
        make_out(p)
    lax.fori_loop(1, direct, send_out, 0)
    for i in range(1, places):
        remote(
            r.over_out.at[place(i)], r.over_in.at[me_s], r.over_send.at[0], r.over_recv.at[0], {"sp": place(i)}
        ).start()
    r.over_in[me_s] = r.over_out[me_s]
    if places < over:
        r.over_in[places:over] = jnp.zeros((over - places, *r.over_in.shape[1:]), f32)
        r.over_ret[:, places:over] = jnp.zeros((2, over - places, *r.over_ret.shape[2:]), f32)
        r.xover_in[:, places:over] = jnp.zeros((columns, over - places, *r.xover_in.shape[2:]), f32)
        r.xover_ret[:, places:over] = jnp.zeros((columns, over - places, *r.xover_ret.shape[2:]), f32)

    def route(offset):
        col = column(offset)
        for q in range(extra):
            part = jnp.dot(r.put[col], r.tokens[col, q], preferred_element_type=f32)
            r.xout[col, q] = part[:slots].astype(bf16)
            r.chunks[col, direct + q, lines(me_s), :] = r.xout[col, q, lines(me_s), :]
            for c in range(lanes_of):
                r.xover_out[offset, :, q * lanes_of + c, :] = part[slots:, c * 128 : (c + 1) * 128]
        r.xover_in[offset, me_s] = r.xover_out[offset, me_s]
        for i in range(1, places):
            remote(
                r.xout.at[col, :, lines(place(i)), :],
                r.chunks.at[col, pl.ds(direct, extra), lines(me_s), :],
                r.xout_send.at[0],
                r.xout_recv.at[offset],
                {"sp": place(i)},
            ).start()
            remote(
                r.xover_out.at[offset, place(i)],
                r.xover_in.at[offset, me_s],
                r.xover_send.at[0],
                r.xover_recv.at[0, offset],
                {"sp": place(i)},
            ).start()

    def routed(offset):
        col = column(offset)
        most = pl.ds(0, (places - 1) * main)
        return (
            remote(
                r.xout.at[col, :, most, :],
                r.chunks.at[col, pl.ds(direct, extra), most, :],
                r.xout_send.at[0],
                r.xout_recv.at[offset],
                right,
            ),
            remote(
                r.xover_out.at[offset, 0 : places - 1],
                r.xover_in.at[offset, 0 : places - 1],
                r.xover_send.at[0],
                r.xover_recv.at[0, offset],
                right,
            ),
        )

    def take_routed(offset):
        col = column(offset)
        for copy in routed(offset):
            copy.wait_recv()
        for q in range(extra):
            for c in range(lanes_of):
                r.chunks[col, direct + q, slots:, c * 128 : (c + 1) * 128] = r.xover_in[
                    offset, :, q * lanes_of + c, :
                ].astype(bf16)

    def token_event(k):
        for q in range(thin):
            came = r.tokens.at[pl.ds(0, 2 if k < half else 1), 0, :, pl.ds(0, 128)]
            remote(came, came, r.token_send.at[0], r.token_recv.at[k - 1, q], right).wait_recv()
            for way in range(2):
                if k < far(way, q):
                    token_ring(way, k, q, column(-k if way == 0 else k)).start()

    def chunk_ring(way, step, p, col):
        here = r.chunks.at[col, p, pl.ds(0, slots), :]
        return remote(here, here, r.chunk_send.at[0], r.chunk_recv.at[step, p], toward(way))

    def over_ring(way, step, col):
        here = r.chunks.at[col, pl.ds(0, direct), pl.ds(slots, over), :]
        return remote(here, here, r.tail_send.at[0], r.tail_recv.at[step], toward(way))

    def out_arrived(p):
        most = pl.ds(0, (places - 1) * main)
        return remote(
            r.outbound.at[p, most, :], r.chunks.at[me_x, p, most, :], r.out_send.at[0], r.out_recv.at[p], right
        )

    def start_piece(p):
        out_arrived(p).wait_recv()
        chunk_ring(0, 0, p, me_x).start()
        chunk_ring(1, 0, p, me_x).start()

    def start_over():
        remote(
            r.over_out.at[0 : places - 1], r.over_in.at[0 : places - 1], r.over_send.at[0], r.over_recv.at[0], right
        ).wait_recv()
        for c in range(direct * lanes_of):
            at_lanes = (c % lanes_of) * 128
            r.chunks[me_x, c // lanes_of, slots:, at_lanes : at_lanes + 128] = r.over_in[:, c, :].astype(bf16)
        for way in range(2):
            over_ring(way, 0, me_x).start()

    for copy in rims + mates + [enter_copy]:
        copy.wait_send()
    for n in range(1, chips):

        @pl.when(me_y + n < chips)
        def _():
            chip_total(n).wait_send()

    heads_total.wait_send()
    tables_total.wait_send()
    remote(ring_total, ring_total, r.ring_send.at[0], r.ring_recv.at[0, 0], right).wait_send()
    remote(slab_total, slab_total, r.slab_send.at[0], r.slab_recv.at[0], right).wait_send()
    remote(grid_total, grid_total, r.grid_send.at[0], r.grid_recv.at[0], right).wait_send()
    for which in range(2):
        view = pass_totals[which]
        remote(view, view, r.pass_send.at[which], r.pass_recv.at[which], mate).wait_send()

    def offset_of(n):
        k = (n + 1) // 2 if isinstance(n, int) else lax.div(n + 1, 2)
        if isinstance(n, int):
            return (columns - k) % columns if n % 2 else k
        return jnp.where(lax.rem(n, 2) == 1, lax.rem(columns - k, columns), k)

    opening = {"token": token_event, "piece": start_piece, "route": lambda n: route(offset_of(n)), "over": lambda n: start_over()}
    for kind, n in dims.opening:
        opening[kind](n)

    def unit(n, t):
        offset = offset_of(n)
        col = column(offset)
        pl.when(t == 0)(lambda: take_routed(offset))
        acc = jnp.dot(r.chunks[col, 0], r.gate_up[t, 0:PIECE, :], preferred_element_type=f32)
        for q in range(1, pieces):
            acc = acc + jnp.dot(
                r.chunks[col, q], r.gate_up[t, q * PIECE : (q + 1) * PIECE, :], preferred_element_type=f32
            )
        value = silu(acc[:, 0:128]) * acc[:, 128:256]
        r.hidden[col, :, pl.ds(pl.multiple_of(t * 128, 128), 128)] = value.astype(bf16)
        pl.when(t == dims.tiles - 1)(lambda: give_back(offset))

    def own(col, p):
        return jnp.dot(r.hidden[col], r.down[p], preferred_element_type=f32)

    def give_back(offset):
        col = column(offset)
        for q in range(extra):
            part = own(col, direct + q)
            r.xback[col, q] = part[:slots].astype(bf16)
            r.xret[col, q, lines(me_s), :] = r.xback[col, q, lines(me_s), :]
            for c in range(lanes_of):
                r.xover_back[offset, :, q * lanes_of + c, :] = part[slots:, c * 128 : (c + 1) * 128]
        r.xover_ret[offset, me_s] = r.xover_back[offset, me_s]
        for i in range(1, places):
            remote(
                r.xback.at[col, :, lines(place(i)), :],
                r.xret.at[col, :, lines(me_s), :],
                r.xback_send.at[0],
                r.xback_recv.at[offset],
                {"sp": place(i)},
            ).start()
            remote(
                r.xover_back.at[offset, place(i)],
                r.xover_ret.at[offset, me_s],
                r.xover_send.at[1],
                r.xover_recv.at[1, offset],
                {"sp": place(i)},
            ).start()

    def given_back(offset):
        col = column(offset)
        most = pl.ds(0, (places - 1) * main)
        return (
            remote(
                r.xback.at[col, :, most, :],
                r.xret.at[col, :, most, :],
                r.xback_send.at[0],
                r.xback_recv.at[offset],
                right,
            ),
            remote(
                r.xover_back.at[offset, 0 : places - 1],
                r.xover_ret.at[offset, 0 : places - 1],
                r.xover_send.at[1],
                r.xover_recv.at[1, offset],
                right,
            ),
        )

    for n, weights in enumerate((r.gate_up, r.down)):
        pltpu.make_async_copy(weights, weights, r.weight_sem.at[n]).wait()

    def units(low, high):
        def body(v, carry):
            unit(lax.div(v, dims.tiles), lax.rem(v, dims.tiles))
            return carry

        lax.fori_loop(low, high, body, 0)

    def hop(way, j, p):
        return remote(
            r.sums.at[way, j, p],
            r.sums.at[way, j - 1, p],
            r.sum_send.at[0],
            r.sum_recv.at[way, j - 1, p],
            {"tp": column(1 - 2 * way)},
        )

    def chains(long, step, group):
        j = half - step if long else half - 1 - step

        def body(p, carry):
            odd = lax.rem(p, 2)
            way = 1 - odd if long else odd
            value = own(column(j * (1 - 2 * way)), p)
            if step > 0:
                hop(way, j + 1, p).wait_recv()
                value = value + r.sums[way, j, p].astype(f32)
            r.sums[way, j, p] = value.astype(bf16)
            hop(way, j, p).start()
            return carry

        lax.fori_loop(*group, body, 0)

    share_of = dims.schedule
    for k in range(1, half + 1):
        first, last = share_of[k - 1] * dims.tiles, share_of[k] * dims.tiles

        if k == half and half > 1:
            units(first, last)
            first = last
            for group in dims.groups:
                chains(False, 0, group)

        def pass_on(p, carry, k=k, first=first, last=last):
            came = r.chunks.at[pl.ds(0, 2 if k < half else 1), p, pl.ds(0, slots), :]
            remote(came, came, r.chunk_send.at[0], r.chunk_recv.at[k - 1, p], right).wait_recv()
            if k < half:
                for way in range(2):
                    start = lambda way=way: chunk_ring(way, k, p, column(-k if way == 0 else k)).start()
                    if k < half - 1:
                        start()
                    else:
                        pl.when(k < far(way, p))(start)

            if k == 1 and dims.routed < columns:
                pl.when(p < columns - dims.routed)(lambda: route(offset_of(p + dims.routed)))
            if last > first:
                units(
                    first + lax.div(p * (last - first), direct), first + lax.div((p + 1) * (last - first), direct)
                )
            return carry

        lax.fori_loop(0, direct, pass_on, 0)
        came = r.chunks.at[pl.ds(0, 2 if k < half else 1), pl.ds(0, direct), pl.ds(slots, over), :]
        remote(came, came, r.tail_send.at[0], r.tail_recv.at[k - 1], right).wait_recv()
        for way in range(2):
            if k < far(way, 0):
                over_ring(way, k, column(-k if way == 0 else k)).start()
        if k == 1:
            lax.fori_loop(0, columns, lambda col, carry: (make_pick(col), carry)[1], 0)
    units(share_of[half] * dims.tiles, columns * dims.tiles)

    def finish(p, carry):
        value = own(me_x, p)
        hop(0, 1, p).wait_recv()
        hop(1, 1, p).wait_recv()
        value = value + r.sums[0, 0, p].astype(f32) + r.sums[1, 0, p].astype(f32)
        r.totals[p] = value[0:slots].astype(bf16)
        r.over_total[p] = value[slots:]
        r.returned[p, lines(me_s), :] = r.totals[p, lines(me_s), :]
        for i in range(1, places):
            remote(
                r.totals.at[p, lines(place(i)), :],
                r.returned.at[p, lines(me_s), :],
                r.back_send.at[0],
                r.back_recv.at[p],
                {"sp": place(i)},
            ).start()
        return carry

    def weighted(col, table):
        one = jnp.dot(r.pick[col, 0], table, preferred_element_type=f32)
        two = jnp.dot(r.pick[col, 1], table, preferred_element_type=f32)
        copies = one.shape[1] // 128
        first, second = (jnp.concatenate([r.share_s[col, k]] * copies, axis=1) for k in range(2))
        return first * one + second * two

    def take_back(offset):
        col = column(offset)
        for copy in given_back(offset):
            copy.wait_recv()
        for q in range(extra):
            for c in range(lanes_of):
                r.xret[col, q, slots:, c * 128 : (c + 1) * 128] = r.xover_ret[
                    offset, :, q * lanes_of + c, :
                ].astype(bf16)

    def token_hop(way, j, q):
        return remote(
            r.xsums.at[way, j, q],
            r.xsums.at[way, j - 1, q],
            r.xsum_send.at[0],
            r.xsum_recv.at[way, j - 1, q],
            toward(way),
        )

    taken = set()

    def thin_part(col, q):
        return weighted(col, r.xret[col, q // lanes_of, :, q % lanes_of * 128 : (q % lanes_of + 1) * 128])

    def token_round(t):
        for q in range(thin):
            for way in range(2):
                j = far(1 - way, q) - t
                if j < 1:
                    continue
                offset = j if way == 0 else columns - j
                if offset not in taken:
                    taken.add(offset)
                    take_back(offset)
                value = thin_part(column(offset), q)
                if t > 0:
                    token_hop(way, j + 1, q).wait_recv()
                    value = value + r.xsums[way, j, q].astype(f32)
                r.xsums[way, j, q] = value.astype(bf16)
                token_hop(way, j, q).start()

    for group in dims.groups:
        chains(True, 0, group)
    def left_by_now(view, send, recv):
        remote(view, view, send, recv, right).wait_send()

    most_places, most_lines = pl.ds(0, places - 1), pl.ds(0, (places - 1) * main)
    chunks_total = r.chunks.at[most_columns, pl.ds(0, direct), pl.ds(0, slots), :]
    left_by_now(r.over_out.at[most_places], r.over_send.at[0], r.over_recv.at[0])
    left_by_now(r.tokens.at[most_columns], r.token_send.at[0], r.token_recv.at[0, 0])
    left_by_now(r.chunks.at[most_columns, pl.ds(0, direct), pl.ds(slots, over), :], r.tail_send.at[0], r.tail_recv.at[0])
    left_by_now(chunks_total, r.chunk_send.at[0], r.chunk_recv.at[0, 0])
    left_by_now(r.outbound.at[:, most_lines, :], r.out_send.at[0], r.out_recv.at[0])
    left_by_now(r.xout.at[:, :, most_lines, :], r.xout_send.at[0], r.xout_recv.at[0])
    left_by_now(r.xover_out.at[:, most_places], r.xover_send.at[0], r.xover_recv.at[0, 0])
    def over_back_copy(n, to, at):
        return remote(
            r.over_back.at[n, to],
            r.over_ret.at[n, at],
            r.over_send.at[1],
            r.over_recv.at[1 + n],
            {"sp": to},
        )

    def send_over_back(n, group):
        for p in range(*group):
            for c in range(lanes_of):
                r.over_back[n, :, (p - group[0]) * lanes_of + c, :] = r.over_total[p, :, c * 128 : (c + 1) * 128]
        r.over_ret[n, me_s] = r.over_back[n, me_s]
        for i in range(1, places):
            over_back_copy(n, place(i), me_s).start()

    for kind, step, group in dims.closing:
        if kind == "short":
            chains(False, step, group)
        elif kind == "long":
            chains(True, step, group)
        elif kind == "token":
            token_round(step)
        else:
            lax.fori_loop(*group, finish, 0)
            send_over_back(dims.groups.index(group), group)
    left_by_now(r.xback.at[:, :, most_lines, :], r.xback_send.at[0], r.xback_recv.at[0])
    left_by_now(r.xover_back.at[:, most_places], r.xover_send.at[1], r.xover_recv.at[1, 0])
    left_by_now(r.chunks.at[most_columns, pl.ds(0, direct)], r.sum_send.at[0], r.sum_recv.at[0, 0, 0])
    token_round(half - 1)
    def write_out(span):
        return pltpu.make_async_copy(r.out_s.at[:, span], r.out_ref.at[:, span], r.done_sem.at[0])

    def back_arrived(p):
        most = pl.ds(0, (places - 1) * main)
        return remote(
            r.totals.at[p, most, :], r.returned.at[p, most, :], r.back_send.at[0], r.back_recv.at[p], right
        )

    def combine(p, carry):
        back_arrived(p).wait_recv()
        span = pl.ds(pl.multiple_of(p * PIECE, PIECE), PIECE)
        value = weighted(me_x, r.returned[p])
        r.out_s[:, span] = (r.stream_s[:, span].astype(f32) + value).astype(bf16)
        write_out(span).start()
        return carry

    def combine_group(n, group):
        remote(
            r.over_back.at[n, 0 : places - 1],
            r.over_ret.at[n, 0 : places - 1],
            r.over_send.at[1],
            r.over_recv.at[1 + n],
            right,
        ).wait_recv()
        for p in range(*group):
            for c in range(lanes_of):
                r.returned[p, slots:, c * 128 : (c + 1) * 128] = r.over_ret[n, :, (p - group[0]) * lanes_of + c, :].astype(bf16)
        lax.fori_loop(*group, combine, 0)

    combine_group(dims.groups.index(dims.order[0]), dims.order[0])
    take_back(0)
    for q in range(thin):
        value = thin_part(me_x, q)
        for way in range(2):
            token_hop(way, 1, q).wait_recv()
            value = value + r.xsums[way, 0, q].astype(f32)
        span = slice(direct * PIECE + q * 128, direct * PIECE + (q + 1) * 128)
        r.out_s[:, span] = (r.stream_s[:, span].astype(f32) + value).astype(bf16)

    write_out(pl.ds(direct * PIECE, extra * PIECE)).start()
    combine_group(dims.groups.index(dims.order[1]), dims.order[1])

    left_by_now(r.over_back.at[:, most_places], r.over_send.at[1], r.over_recv.at[1])
    left_by_now(r.tokens.at[most_columns], r.xsum_send.at[0], r.xsum_recv.at[0, 0, 0])
    left_by_now(r.totals.at[:, most_lines, :], r.back_send.at[0], r.back_recv.at[0])
    pltpu.make_async_copy(r.out_s, r.out_ref, r.done_sem.at[0]).wait()


def layer(places, columns, **given):
    f32, bf16 = jnp.float32, jnp.bfloat16
    rows, width = given["residual_hbm"].shape
    small = [name for name in given if name.endswith("_small")]
    units = given["expert_gate_hbm"].shape[2]
    lanes = given["keys_hbm"].shape[1]
    positions = columns * BLOCK
    half, chips, blocks = columns // 2, places // 2, columns
    main = 2 * rows // places
    over = -(-places // 16) * 16
    pieces = width // PIECE
    extra = max(1, pieces // 4)
    direct = pieces - extra
    tiles, total = units // 128, places * main + over
    ring_part = width * RING_SHARE // 16 // 128 * 128
    schedule = (0, 0, 1, 5, 7) if half == 4 else (0,) * half + (columns - 1,)
    if half == 4:
        opening = "token1 piece0 piece1 token2 piece2 route0 piece3 token3 route1 piece4 route2 token4 piece5 over0"
    else:
        opening = " ".join(
            [f"token{n}" for n in range(1, half + 1)]
            + [f"piece{n}" for n in range(direct)]
            + [f"route{n}" for n in range(columns)]
            + ["over0"]
        )
    opening = [(step[:-1], int(step[-1])) for step in opening.split()]
    routed = sum(kind == "route" for kind, _ in opening)
    serving = [
        [("x", 0)],
        [("x", 1)],
        [("x", 2)],
        [("x", 3), ("y", 0), ("y", 1), ("y", 2), ("x", 4), ("y", 3), ("y", 4), ("y", 5), ("x", 5), ("x", 6), ("y", 6)],
    ]
    low, high = (0, (direct + 1) // 2), ((direct + 1) // 2, direct)
    groups = [high, low]
    if half == 4:
        closing = [
            ("long", 1, high),
            ("short", 1, high),
            ("long", 1, low),
            ("short", 1, low),
            ("long", 2, low),
            ("long", 2, high),
            ("long", 3, low),
            ("short", 2, low),
            ("token", 0, None),
            ("long", 3, high),
            ("finish", None, low),
            ("short", 2, high),
            ("token", 1, None),
            ("finish", None, high),
            ("token", 2, None),
        ]
    else:
        closing = []
        for step in range(1, half):
            closing += [("short", step, group) for group in groups if step < half - 1]
            closing += [("long", step, group) for group in groups]
            closing.append(("token", step - 1, None))
        closing += [("finish", None, group) for group in groups]
    dims = types.SimpleNamespace(
        places=places, columns=columns, width=width, main=main, over=over, pieces=pieces, direct=direct, tiles=tiles,
        schedule=schedule, opening=opening, routed=routed, small=small, groups=groups, order=(low, high), closing=closing, ring_part=ring_part, serving=serving,
    )
    packed = STATE_ONE + STATE_TWO
    square = (blocks, 2, BLOCK, BLOCK)
    vmem = lambda *shape, dtype=bf16: pltpu.VMEM(shape, dtype)
    dma = lambda *shape: pltpu.SemaphoreType.DMA(shape)
    in_specs = [pl.BlockSpec(memory_space=pltpu.SMEM if a.shape == (2, 2) else pl.ANY) for a in given.values()]
    lane_rows = PIECE // 128
    scratch = {name[:-5] + "ref": pltpu.VMEM(given[name].shape, given[name].dtype) for name in small}
    scratch |= dict(
        residual_in=vmem(rows, width),
        value_in=vmem(2 * positions, BLOCK),
        gate_in=vmem(2 * positions, BLOCK),
        keys_in=vmem(positions, lanes),
        value_rim=vmem(16, BLOCK),
        keys_rim=vmem(16, lanes),
        value_wide=vmem(2 * positions + 16, BLOCK, dtype=f32),
        keys_wide=vmem(positions + 16, lanes, dtype=f32),
        gate_wide=vmem(2 * BLOCK, BLOCK, dtype=f32),
        conv_wide=vmem(2 * BLOCK, BLOCK, dtype=f32),
        x_s=vmem(*square),
        kt_s=vmem(*square),
        q_s=vmem(*square),
        state_s=vmem(*square, dtype=f32),
        near_s=vmem(*square, dtype=f32),
        stride_s=vmem(HEADS * blocks, BLOCK, dtype=f32),
        run_s=vmem(HEADS * blocks, BLOCK, dtype=f32),
        fade_s=vmem(HEADS * blocks, BLOCK, dtype=f32),
        end_s=vmem(HEADS * blocks, BLOCK, dtype=f32),
        cols_s=vmem(blocks, BLOCK, HEADS, dtype=f32),
        own_pack=vmem(packed, BLOCK),
        own_fade=vmem(8, BLOCK, dtype=f32),
        mate_pack=vmem(packed, BLOCK),
        mate_fade=vmem(8, BLOCK, dtype=f32),
        chip_pack=vmem(packed, BLOCK),
        chip_fade=vmem(8, BLOCK, dtype=f32),
        all_pack=vmem(chips, packed // 2, BLOCK),
        all_fade=vmem(chips, 8, BLOCK, dtype=f32),
        enter_pack=vmem(packed, BLOCK),
        carry_s=vmem(2, BLOCK, BLOCK, dtype=f32),
        mixed_s=vmem(columns, BLOCK, 2 * BLOCK),
        heads_in=vmem(columns, BLOCK, 2 * BLOCK),
        matrix=vmem(columns, 2 * BLOCK, width),
        acc_s=vmem(rows, width, dtype=f32),
        stream_s=vmem(rows, width),
        out_s=vmem(rows, width),
        tables=vmem(columns, 8, rows, dtype=f32),
        put=vmem(columns, total, rows),
        pick=vmem(columns, 2, rows, total),
        share_s=vmem(columns, 2, rows, 128, dtype=f32),
        tokens=vmem(columns, extra, rows, PIECE),
        outbound=vmem(direct, places * main, PIECE),
        over_out=vmem(over, direct * lane_rows, 128, dtype=f32),
        over_in=vmem(over, direct * lane_rows, 128, dtype=f32),
        over_back=vmem(2, over, (high[1] - low[0] + 1) // 2 * lane_rows, 128, dtype=f32),
        over_ret=vmem(2, over, (high[1] - low[0] + 1) // 2 * lane_rows, 128, dtype=f32),
        over_total=vmem(direct, over, PIECE, dtype=f32),
        xout=vmem(columns, extra, places * main, PIECE),
        xback=vmem(columns, extra, places * main, PIECE),
        xret=vmem(columns, extra, total, PIECE),
        xover_out=vmem(columns, over, extra * lane_rows, 128, dtype=f32),
        xover_in=vmem(columns, over, extra * lane_rows, 128, dtype=f32),
        xover_back=vmem(columns, over, extra * lane_rows, 128, dtype=f32),
        xover_ret=vmem(columns, over, extra * lane_rows, 128, dtype=f32),
        chunks=vmem(columns, pieces, total, PIECE),
        hidden=vmem(columns, total, units),
        gate_up=vmem(tiles, width, 256),
        down=vmem(pieces, units, PIECE),
        sums=vmem(2, half + 1, direct, total, PIECE),
        xsums=vmem(2, half + 1, extra * lane_rows, rows, 128),
        totals=vmem(direct, places * main, PIECE),
        returned=vmem(direct, total, PIECE),
        load_sem=dma(6),
        weight_sem=dma(2),
        done_sem=dma(1),
        small_sem=dma(len(small)),
    )
    steps = (2, half)
    for name, send, recv in (
        ("rim", (2,), (2,)),
        ("mate", (2,), (2,)),
        ("chip", (chips,), (chips,)),
        ("enter", (1,), (1,)),
        ("head", (1,), (1,)),
        ("table", (1,), (1,)),
        ("ring", (1,), (columns - 1, 2)),
        ("slab", (1,), (1,)),
        ("grid", (1,), (chips - 1,)),
        ("pass", (2,), (2,)),
        ("over", (2,), (3,)),
        ("token", (1,), (half, extra * lane_rows)),
        ("out", (1,), (direct,)),
        ("xout", (1,), (columns,)),
        ("xover", (2,), (2, columns)),
        ("chunk", (1,), (half, direct)),
        ("tail", (1,), (half,)),
        ("xback", (1,), (columns,)),
        ("sum", (1,), (*steps, direct)),
        ("xsum", (1,), (*steps, extra * lane_rows)),
        ("back", (1,), (direct,)),
    ):
        scratch[name + "_send"], scratch[name + "_recv"] = dma(*send), dma(*recv)
    names = [*given, "out_ref", *scratch]
    return pl.pallas_call(
        functools.partial(layer_kernel, dims, names),
        out_shape=jax.ShapeDtypeStruct((rows, width), bf16),
        in_specs=in_specs,
        out_specs=pl.BlockSpec(memory_space=pl.ANY),
        scratch_shapes=list(scratch.values()),
        compiler_params=pltpu.CompilerParams(
            collective_id=0, has_side_effects=True, vmem_limit_bytes=VMEM_LIMIT
        ),
        name="layer",
    )(*given.values())


def local(
    residual,
    grouped_value_heads,
    output_gate_heads,
    projected_key_query,
    raw_step_size,
    step_size_bias,
    head_decay_logarithm,
    position_extra_decay,
    head_skip_weight,
    value_kernel_taps,
    key_query_kernel,
    head_norm_gain,
    output_matrix,
    expert_norm_gain,
    expert_gate_weight,
    expert_up_weight,
    expert_down_weight,
    token_expert_choice,
    expert_output_weight,
):
    return layer(
        lax.axis_size("sp"),
        lax.axis_size("tp"),
        residual_hbm=residual,
        value_hbm=grouped_value_heads.reshape(-1, BLOCK),
        gate_hbm=output_gate_heads.reshape(-1, BLOCK),
        keys_hbm=projected_key_query,
        raw_small=raw_step_size.transpose(1, 2, 0),
        bias_ref=step_size_bias,
        log_ref=head_decay_logarithm,
        extra_small=position_extra_decay.reshape(-1, BLOCK),
        skip_ref=head_skip_weight,
        value_tap_small=value_kernel_taps.reshape(-1, BLOCK),
        key_tap_small=key_query_kernel,
        head_gain_small=head_norm_gain,
        matrix_hbm=output_matrix,
        expert_gain_small=expert_norm_gain[None],
        choice_small=token_expert_choice.T,
        share_small=expert_output_weight.T,
        expert_gate_hbm=expert_gate_weight,
        expert_up_hbm=expert_up_weight,
        expert_down_hbm=expert_down_weight,
    )


def solution(mesh):
    placed = (
        P(("grp", "sp", "tp"), None),
        P(("grp", "sp"), None, "tp"),
        P(("grp", "sp"), None, "tp"),
        P(("grp", "sp"), None),
        P(("grp", "sp"), None, "tp"),
        P(None, "tp"),
        P(None, "tp"),
        P(("grp", "sp")),
        P(None, "tp"),
        P(None, None, "tp"),
        P(),
        P(None, "tp"),
        P(None, "tp", None),
        P(),
        P("sp", None, "tp"),
        P("sp", None, "tp"),
        P("sp", "tp", None),
        P(("grp", "sp", "tp"), None),
        P(("grp", "sp", "tp"), None),
    )
    return jax.shard_map(
        local, mesh=mesh, in_specs=placed, out_specs=P(("grp", "sp", "tp"), None), check_vma=False
    )
```

```python
import functools
import types

import jax
import jax.numpy as jnp
from jax import lax
from jax.experimental import pallas as pl
from jax.experimental.pallas import tpu as pltpu
from jax.sharding import PartitionSpec as P

HEAD_DIM = 64
STATE_ONE = 64
STATE_TWO = 128
BLOCK = 128
EPSILON = 1e-06

MESH = pl.DeviceIdType.MESH
PIECE = 256
HEADS = 4
RING_SHARE = 7
VMEM_LIMIT = 61600000


def remote(src, dst, send, recv, device):
    return pltpu.make_async_remote_copy(
        src_ref=src, dst_ref=dst, send_sem=send, recv_sem=recv, device_id=device, device_id_type=MESH
    )


def silu(a):
    return a * (1.0 / (1.0 + jnp.exp(-a)))


def layer_kernel(dims, names, *refs):
    r = types.SimpleNamespace(**dict(zip(names, refs, strict=True)))
    f32, bf16 = jnp.float32, jnp.bfloat16
    places, columns, width, rows = dims.places, dims.columns, dims.width, BLOCK
    half, chips, blocks = columns // 2, places // 2, columns
    me_x, me_s = lax.axis_index("tp"), lax.axis_index("sp")
    core, me_y = lax.rem(me_s, 2), lax.div(me_s, 2)
    right = {"tp": lax.rem(me_x + 1, columns)}
    left = {"tp": lax.rem(me_x + columns - 1, columns)}
    mate = {"sp": me_s + 1 - 2 * core}
    following = {"sp": lax.rem(me_s + 1, places)}

    def column(offset):
        return lax.rem(me_x + offset + columns, columns)

    def place(offset):
        return lax.rem(me_s + offset, places)

    def peer(offset):
        return {"sp": lax.rem(me_s + 2 * offset, places)}

    def toward(way):
        return right if way == 0 else left

    barrier = pltpu.get_barrier_semaphore()
    peers = sorted(
        [(min(i, columns - i), {"tp": column(i)}) for i in range(1, columns)]
        + [(min(i, places - i) / 2, {"sp": place(i)}) for i in range(1, places)],
        key=lambda peer: -peer[0],
    )
    peers = [device for _, device in peers]
    for device in peers:
        pl.semaphore_signal(barrier, inc=1, device_id=device, device_id_type=MESH)

    small = {
        name: pltpu.make_async_copy(getattr(r, name), getattr(r, name[:-5] + "ref"), r.small_sem.at[n])
        for n, name in enumerate(dims.small)
    }
    ring_part, slab = dims.ring_part, rows // chips
    rim_rows, positions = 16, blocks * rows
    mine = pl.multiple_of(core * rows, rows)

    def slab_rows(y):
        return pl.ds(pl.multiple_of(mine + y * slab, 16), slab)

    on_ring, on_grid = pl.ds(0, ring_part), pl.ds(ring_part, width - ring_part)
    loads = [
        (r.matrix_hbm.at[0], r.matrix.at[0, pl.ds(0, rows), :]),
        (r.matrix_hbm.at[1], r.matrix.at[0, pl.ds(rows, rows), :]),
        (r.value_hbm, r.value_in.at[pl.ds(rim_rows, 2 * positions), :]),
        (r.keys_hbm, r.keys_in.at[pl.ds(rim_rows, positions), :]),
        (r.gate_hbm, r.gate_in),
        (r.residual_hbm, r.residual_in),
    ]
    loads = [pltpu.make_async_copy(a, b, r.load_sem.at[n]) for n, (a, b) in enumerate(loads)]
    for load in loads[:2] + list(small.values()) + loads[2:4]:
        load.start()
    for name in ("choice_small", "share_small"):
        small[name].wait()
    r.tables[me_x] = jnp.zeros((8, rows), f32)
    r.tables[me_x, 0:2, :] = r.choice_ref[...].astype(f32)
    r.tables[me_x, 2:4, :] = r.share_ref[...]

    for load in loads[:2]:
        load.wait()
    pl.semaphore_wait(barrier, len(peers))

    def matrix_block(way, event, k, sub):
        piece = ((event % 2) ^ way) * 2 + sub
        block = (columns - k if way == 0 else k) % columns
        return r.matrix.at[block, pl.ds(pl.multiple_of(mine + piece * (rows // 4), 16), rows // 4), on_ring]

    def matrix_ring(way, event, sub):
        k = event // 2
        return remote(
            matrix_block(way, event, k, sub),
            matrix_block(way, event, k + 1, sub),
            r.ring_send.at[0],
            r.ring_recv.at[event, sub],
            toward(way),
        )

    def slab_copy(offset):
        return remote(
            r.matrix.at[0, slab_rows(me_y), on_grid],
            r.matrix.at[columns - offset, slab_rows(me_y), on_grid],
            r.slab_send.at[0],
            r.slab_recv.at[0],
            {"tp": column(offset)},
        )

    def grid_view(way, event, y):
        blocks_of = pl.ds(1, half) if (event % 2) ^ way == 0 else pl.ds(1 + half, half - 1)
        return r.matrix.at[blocks_of, slab_rows(y), on_grid]

    def grid_ring(way, event, y):
        here = grid_view(way, event, y)
        return remote(
            here, here, r.grid_send.at[0], r.grid_recv.at[event], peer(1) if way == 0 else peer(chips - 1)
        )

    def to_mate(here, which):
        return remote(here, here, r.pass_send.at[which], r.pass_recv.at[which], mate)

    most_columns, other_blocks = pl.ds(0, columns - 1), pl.ds(1, columns - 1)
    ring_total = r.matrix.at[other_blocks, pl.ds(0, rows), on_ring]
    grid_total = r.matrix.at[other_blocks, pl.ds(0, (chips - 1) * slab), on_grid]
    slab_total = r.matrix.at[other_blocks, pl.ds(0, slab), on_grid]
    pass_totals = (ring_total, r.matrix.at[other_blocks, pl.ds(0, rows), on_grid])

    for load in loads[2:4]:
        load.wait()
    rims = [
        remote(
            r.value_in.at[pl.ds(2 * positions, rim_rows), :],
            r.value_in.at[pl.ds(0, rim_rows), :],
            r.rim_send.at[0],
            r.rim_recv.at[0],
            following,
        ),
        remote(
            r.keys_in.at[pl.ds(positions, rim_rows), :],
            r.keys_in.at[pl.ds(0, rim_rows), :],
            r.rim_send.at[1],
            r.rim_recv.at[1],
            following,
        ),
    ]
    for rim in rims:
        rim.start()

    def table_copy(offset):
        here = r.tables.at[me_x]
        return remote(here, here, r.table_send.at[0], r.table_recv.at[0], {"tp": column(offset)})

    for i in range(1, columns):
        table_copy(i).start()
    for i in range(1, columns):
        slab_copy(i).start()
    for event in range(min(2, columns - 1)):
        for sub in range(2):
            for way in range(2):
                matrix_ring(way, event, sub).start()
    tables_total = remote(
        r.tables.at[most_columns], r.tables.at[most_columns], r.table_send.at[0], r.table_recv.at[0], right
    )

    def serve_ring(event):
        for sub in range(2):
            both = r.matrix.at[0, pl.ds(0, rows // 2), on_ring]
            remote(both, both, r.ring_send.at[0], r.ring_recv.at[event, sub], right).wait_recv()
            for way in range(2):
                if event + 2 < columns - 1:
                    matrix_ring(way, event + 2, sub).start()
                to_mate(matrix_block(way, event, event // 2 + 1, sub), 0).start()

    def serve_slab():
        remote(slab_total, slab_total, r.slab_send.at[0], r.slab_recv.at[0], right).wait_recv()
        for event in range(2):
            for way in range(2):
                if event < chips - 1:
                    grid_ring(way, event, me_y).start()
        to_mate(r.matrix.at[other_blocks, slab_rows(me_y), on_grid], 1).start()

    def serve_grid(event):
        k = event // 2 + 1
        remote(slab_total, slab_total, r.grid_send.at[0], r.grid_recv.at[event], right).wait_recv()
        for way in range(2):
            y = lax.rem(me_y + (chips - k if way == 0 else k), chips)
            if event + 2 < chips - 1:
                grid_ring(way, event + 2, y).start()
            to_mate(grid_view(way, event, y), 1).start()

    waiting = [("x", e) for e in range(columns - 1)] + [("y", e) for e in range(chips - 1)]

    def serve(*steps):
        for step in steps:
            if step in waiting:
                waiting.remove(step)
                (serve_ring if step[0] == "x" else serve_grid)(step[1])

    for load in loads[4:]:
        load.start()
    for t in range(dims.tiles):
        span = pl.ds(t * 128, 128)
        for n, weight in enumerate((r.expert_gate_hbm, r.expert_up_hbm)):
            pltpu.make_async_copy(
                weight.at[0, :, span], r.gate_up.at[t, :, pl.ds(n * 128, 128)], r.weight_sem.at[0]
            ).start()
    for p in range(dims.pieces):
        pltpu.make_async_copy(
            r.expert_down_hbm.at[0, :, pl.ds(p * PIECE, PIECE)], r.down.at[p], r.weight_sem.at[1]
        ).start()

    for name in dims.small:
        if name not in ("choice_small", "share_small"):
            small[name].wait()
    for g in range(2):
        raw = r.raw_ref[g].astype(f32)
        for k in range(blocks):
            r.stride_s[HEADS * k + 2 * g : HEADS * k + 2 * g + 2, :] = raw[:, k * rows : (k + 1) * rows]
    for k in range(blocks):
        r.run_s[HEADS * k : HEADS * k + HEADS, :] = jnp.broadcast_to(r.extra_ref[k : k + 1, :], (HEADS, rows))
    head_of = jnp.bitwise_and(lax.broadcasted_iota(jnp.int32, (HEADS * blocks, rows), 0), HEADS - 1)

    def by_head(table):
        picked = jnp.full((HEADS * blocks, rows), table[1, 1], f32)
        for n in range(3):
            picked = jnp.where(head_of == n, table[n // 2, n % 2], picked)
        return picked

    shifted = r.stride_s[...] + by_head(r.bias_ref)
    stride = jnp.maximum(shifted, 0.0) + jnp.log1p(jnp.exp(-jnp.abs(shifted)))
    log_decay = r.run_s[...] - jnp.exp(by_head(r.log_ref)) * stride
    at_row = lax.broadcasted_iota(jnp.int32, (rows, rows), 0)
    at_lane = lax.broadcasted_iota(jnp.int32, (rows, rows), 1)
    running = jnp.dot(
        log_decay,
        jnp.where(at_row <= at_lane, 1.0, 0.0),
        preferred_element_type=f32,
        precision=lax.Precision.HIGHEST,
    )
    ends = jnp.broadcast_to(running[:, rows - 1 : rows], running.shape)
    r.stride_s[...] = stride
    r.run_s[...] = running
    r.fade_s[...] = jnp.exp(ends - running) * stride
    r.end_s[...] = jnp.exp(ends)
    turned = jnp.transpose(running)
    for k in range(blocks):
        r.cols_s[k, :, 0:HEADS] = turned[:, HEADS * k : HEADS * k + HEADS]

    first_head = at_lane < HEAD_DIM

    def row_pair(table, k, g):
        low = table[pl.ds(HEADS * k + 2 * g, 1), :]
        high = table[pl.ds(HEADS * k + 2 * g + 1, 1), :]
        return jnp.where(first_head[0:1], low, high)

    taps = r.value_tap_ref.shape[0] // 2
    value_tap = r.value_tap_ref[...].astype(f32)
    key_tap = r.key_tap_ref[...].astype(f32)
    even = jnp.bitwise_and(lax.broadcasted_iota(jnp.int32, (2 * rows, rows), 0), 1) == 0
    tap_rows = [jnp.where(even, value_tap[2 * j : 2 * j + 1], value_tap[2 * j + 1 : 2 * j + 2]) for j in range(taps)]

    def states_of(k):
        window = r.value_in[pl.ds(pl.multiple_of(k * 2 * rows, 2 * rows), 2 * rows + rim_rows), :].astype(f32)
        total = jnp.zeros((2 * rows, rows), f32)
        for j in range(taps):
            start = rim_rows - 2 * (taps - 1 - j)
            total = total + window[start : start + 2 * rows] * tap_rows[j]
        r.conv_wide[...] = silu(total).astype(bf16).astype(f32)
        window = r.keys_in[pl.ds(pl.multiple_of(k * rows, rows), rows + rim_rows), :].astype(f32)
        total = jnp.zeros((rows, r.keys_in.shape[1]), f32)
        for j in range(taps):
            start = rim_rows - (taps - 1 - j)
            total = total + window[start : start + rows] * key_tap[j : j + 1]
        conv = silu(total).astype(bf16).astype(f32)
        both = conv[:, 0 : 2 * STATE_ONE]
        keys = [jnp.where(first_head, both, 0.0), conv[:, 2 * STATE_ONE : 2 * STATE_ONE + STATE_TWO]]
        asks = [pltpu.roll(both, STATE_ONE, 1), conv[:, 2 * STATE_ONE + STATE_TWO :]]
        for g in range(2):
            x = r.conv_wide[pl.ds(g, rows, stride=2), :].astype(bf16)
            key_t = jnp.transpose(keys[g])
            r.x_s[k, g] = x
            r.kt_s[k, g] = key_t.astype(bf16)
            r.q_s[k, g] = asks[g].astype(bf16)
            faded = jnp.concatenate(
                [key_t * r.fade_s[pl.ds(HEADS * k + 2 * g + h, 1), :] for h in range(2)], axis=0
            ).astype(bf16)
            state = jnp.dot(faded, x, preferred_element_type=f32)
            r.state_s[k, g] = jnp.where(first_head, state[:rows], state[rows:])

    def state_step(i, carry):
        states_of(i)
        return carry

    lax.fori_loop(1, blocks, state_step, 0)
    for rim in rims:
        rim.wait_recv()
    opening = me_s == 0
    for table in (r.value_in, r.keys_in):
        table[0:rim_rows, :] = jnp.where(opening, 0.0, table[0:rim_rows, :].astype(f32)).astype(bf16)
    states_of(0)

    packed = STATE_TWO + STATE_ONE
    piece = packed // 2

    def local_end(g):
        total = jnp.zeros((rows, rows), f32)
        faded = jnp.ones((1, rows), f32)
        for k in range(blocks):
            decay = row_pair(r.end_s, k, g)
            total = total * decay + r.state_s[k, g]
            faded = faded * decay
        return total, faded

    end_one, fade_one = local_end(0)
    end_two, fade_two = local_end(1)
    own = jnp.concatenate([end_two, end_one[:STATE_ONE]], axis=0)
    r.own_pack[...] = own.astype(bf16)
    r.own_fade[0:1, :] = fade_one
    r.own_fade[1:2, :] = fade_two
    r.own_fade[2:8, :] = jnp.zeros((6, rows), f32)
    mates = [
        remote(r.own_pack, r.mate_pack, r.mate_send.at[0], r.mate_recv.at[0], mate),
        remote(r.own_fade, r.mate_fade, r.mate_send.at[1], r.mate_recv.at[1], mate),
    ]
    for copy in mates:
        copy.start()
    for copy in mates:
        copy.wait_recv()
    is_low = core == 0
    low = jnp.where(is_low, own, r.mate_pack[...].astype(f32))
    high = jnp.where(is_low, r.mate_pack[...].astype(f32), own)
    mate_rows = r.mate_fade[...]
    own_rows = r.own_fade[...]
    high_rows = jnp.where(is_low, mate_rows, own_rows)
    in_two = lax.broadcasted_iota(jnp.int32, (packed, rows), 0) < STATE_TWO
    r.chip_pack[...] = (low * jnp.where(in_two, high_rows[1:2], high_rows[0:1]) + high).astype(bf16)
    r.chip_fade[...] = own_rows * mate_rows
    my_half = pl.ds(pl.multiple_of(core * piece, 16), piece)

    def to_chip(n, which):
        src = r.chip_pack.at[my_half, :] if which == 0 else r.chip_fade
        dst = r.all_pack.at[me_y] if which == 0 else r.all_fade.at[me_y]
        return remote(src, dst, r.chip_send.at[n], r.chip_recv.at[n], peer(n))

    def chip_total(n):
        sent = r.own_pack.at[pl.ds(0, piece + 16), :]
        return remote(sent, sent, r.chip_send.at[n], r.chip_recv.at[n], peer(n))

    for n in range(1, chips):

        @pl.when(me_y + n < chips)
        def _():
            for which in range(2):
                to_chip(n, which).start()


    below = at_row >= at_lane

    def near_step(k, carry):
        cols = r.cols_s[k]
        for g in range(2):
            scores = jnp.dot(r.q_s[k, g], r.kt_s[k, g], preferred_element_type=f32)
            parts = []
            for h in range(2):
                n = 2 * g + h
                gap = cols[:, n : n + 1] - r.run_s[pl.ds(HEADS * k + n, 1), :]
                damping = jnp.exp(jnp.where(below, gap, -1e30))
                parts.append((scores * damping * r.stride_s[pl.ds(HEADS * k + n, 1), :]).astype(bf16))
            near = jnp.dot(jnp.concatenate(parts, axis=0), r.x_s[k, g], preferred_element_type=f32)
            r.near_s[k, g] = jnp.where(first_head, near[:rows], near[rows:])
        return carry

    lax.fori_loop(0, blocks, near_step, 0)
    serve_slab()
    serve(*dims.serving[0])
    main, over, slots = dims.main, dims.over, places * dims.main
    total_slots = slots + over
    slot_row = lax.broadcasted_iota(jnp.int32, (total_slots, over), 0)
    slot_expert = lax.broadcasted_iota(jnp.int32, (total_slots, over), 1)
    spread = jnp.where(
        ((slot_row < slots) & (slot_row >= slot_expert * main) & (slot_row < slot_expert * main + main))
        | (slot_row == slots + slot_expert),
        1.0,
        0.0,
    ).astype(bf16)
    at = lax.broadcasted_iota(jnp.int32, (total_slots, rows), 0)
    turn = jnp.where(at < slots, jnp.bitwise_and(at, main - 1), main).astype(f32)
    expert_at = lax.broadcasted_iota(jnp.int32, (over, rows), 0).astype(f32)
    earlier = jnp.where(at_row < at_lane, 1.0, 0.0).astype(bf16)

    def make_put(col):
        table = r.tables[col]
        named = jnp.where((expert_at == table[0:1]) | (expert_at == table[1:2]), 1.0, 0.0)
        rank = jnp.dot(named.astype(bf16), earlier, preferred_element_type=f32)
        named_x = jnp.dot(spread, named.astype(bf16), preferred_element_type=f32)
        rank_x = jnp.dot(spread, rank.astype(bf16), preferred_element_type=f32)
        r.put[col] = jnp.where(rank_x == turn, named_x, 0.0).astype(bf16)

    tables_total.wait_recv()

    def put_step(col, carry):
        make_put(col)
        return carry

    lax.fori_loop(0, columns, put_step, 0)

    for load in loads[-2:]:
        load.wait()
    serve(*dims.serving[1])
    for n in range(1, chips):

        @pl.when(me_y >= n)
        def _():
            chip_total(n).wait_recv()

    row_at = lax.broadcasted_iota(jnp.int32, (piece, rows), 0) + core * piece
    half_two = row_at < STATE_TWO
    entering = jnp.zeros((piece, rows), f32)
    for y in range(chips):
        fades = r.all_fade[y]
        later = entering * jnp.where(half_two, fades[1:2], fades[0:1]) + r.all_pack[y].astype(f32)
        entering = jnp.where(y < me_y, later, entering)
    r.enter_pack[my_half, :] = entering.astype(bf16)
    here = r.enter_pack.at[my_half, :]
    enter_copy = remote(here, here, r.enter_send.at[0], r.enter_recv.at[0], mate)
    enter_copy.start()
    enter_copy.wait_recv()
    chip_state = r.enter_pack[...].astype(f32)
    after_low = chip_state * jnp.where(in_two, mate_rows[1:2], mate_rows[0:1]) + r.mate_pack[...].astype(f32)
    entered = jnp.where(is_low, chip_state, after_low)
    r.carry_s[1] = entered[:STATE_TWO]
    r.carry_s[0] = jnp.zeros((rows, rows), f32)
    r.carry_s[0, 0:STATE_ONE, :] = entered[STATE_TWO:]

    serve(*dims.serving[2])
    def head_copy(col):
        return remote(r.mixed_s.at[col], r.heads_in.at[me_x], r.head_send.at[0], r.head_recv.at[0], {"tp": col})

    def mix_step(k, carry):
        cols = jnp.exp(r.cols_s[k])
        r.gate_wide[...] = r.gate_in[pl.ds(pl.multiple_of(k * 2 * rows, 2 * rows), 2 * rows), :].astype(f32)
        for g in range(2):
            state = r.carry_s[g]
            coarse = state.astype(bf16)
            fine = (state - coarse.astype(f32)).astype(bf16)
            ask = r.q_s[k, g]
            far = jnp.dot(
                jnp.concatenate([ask, ask], axis=1),
                jnp.concatenate([coarse, fine], axis=0),
                preferred_element_type=f32,
            )
            reach = jnp.where(first_head, cols[:, 2 * g : 2 * g + 1], cols[:, 2 * g + 1 : 2 * g + 2])
            skip = jnp.where(first_head[0:1], r.skip_ref[g, 0], r.skip_ref[g, 1])
            mixed = r.near_s[k, g] + far * reach + skip * r.x_s[k, g].astype(f32)
            gated = mixed * silu(r.gate_wide[pl.ds(g, rows, stride=2), :])
            square = gated * gated
            one = jnp.sum(jnp.where(first_head, square, 0.0), axis=1, keepdims=True)
            two = jnp.sum(jnp.where(first_head, 0.0, square), axis=1, keepdims=True)
            scale = lax.rsqrt(jnp.where(first_head, one, two) * (1.0 / HEAD_DIM) + EPSILON)
            r.mixed_s[k, :, g * rows : (g + 1) * rows] = (gated * scale * r.head_gain_ref[g : g + 1, :]).astype(bf16)
            r.carry_s[g] = state * row_pair(r.end_s, k, g) + r.state_s[k, g]

        @pl.when(k != me_x)
        def _():
            head_copy(k).start()

        return carry

    lax.fori_loop(0, blocks, mix_step, 0)
    r.heads_in[me_x] = r.mixed_s[me_x]

    slot_col = lax.broadcasted_iota(jnp.int32, (over, total_slots), 1)
    slot_exp = lax.broadcasted_iota(jnp.int32, (over, total_slots), 0)
    spread_t = jnp.where(
        ((slot_col < slots) & (slot_col >= slot_exp * main) & (slot_col < slot_exp * main + main))
        | (slot_col == slots + slot_exp),
        1.0,
        0.0,
    ).astype(bf16)
    at_t = lax.broadcasted_iota(jnp.int32, (rows, total_slots), 1)
    turn_t = jnp.where(at_t < slots, jnp.bitwise_and(at_t, main - 1), main).astype(f32)
    expert_to = lax.broadcasted_iota(jnp.int32, (rows, over), 1).astype(f32)
    later_t = jnp.where(at_lane < at_row, 1.0, 0.0).astype(bf16)

    def make_pick(col):
        table = jnp.transpose(r.tables[col])
        named = [jnp.where(expert_to == table[:, k : k + 1], 1.0, 0.0) for k in range(2)]
        rank = jnp.dot(later_t, (named[0] + named[1]).astype(bf16), preferred_element_type=f32)
        rank_x = jnp.dot(rank.astype(bf16), spread_t, preferred_element_type=f32)
        for k in range(2):
            named_x = jnp.dot(named[k].astype(bf16), spread_t, preferred_element_type=f32)
            r.pick[col, k] = jnp.where(rank_x == turn_t, named_x, 0.0).astype(bf16)
            r.share_s[col, k] = jnp.broadcast_to(table[:, 2 + k : 3 + k], (rows, rows))

    def product(block, low, high, first):
        for n in range(low, high, 512):
            span = slice(n, min(n + 512, high))
            part = jnp.dot(r.heads_in[column(block)], r.matrix[block, :, span], preferred_element_type=f32)
            r.acc_s[:, span] = part if first else r.acc_s[:, span] + part

    serve(*dims.serving[3])
    serve(*list(waiting))
    heads_total = remote(
        r.mixed_s.at[most_columns], r.heads_in.at[most_columns], r.head_send.at[0], r.head_recv.at[0], right
    )
    heads_total.wait_recv()
    for which, (low_lane, high_lane) in enumerate(((0, ring_part), (ring_part, width))):
        remote(pass_totals[which], pass_totals[which], r.pass_send.at[which], r.pass_recv.at[which], mate).wait_recv()
        for block in range(columns):
            product(block, low_lane, high_lane, block == 0)

    stream = (r.residual_in[...].astype(f32) + r.acc_s[...]).astype(bf16)
    r.stream_s[...] = stream
    wide = stream.astype(f32)
    scale = lax.rsqrt(jnp.mean(wide * wide, axis=1, keepdims=True) + EPSILON)
    normed = (wide * scale * r.expert_gain_ref[...]).astype(bf16)

    direct, extra = dims.direct, dims.pieces - dims.direct
    pieces = dims.pieces
    lanes_of = PIECE // 128

    def lines(index):
        return pl.ds(pl.multiple_of(index * main, main), main)

    def far(way, p):
        odd = lax.rem(p, 2) if not isinstance(p, int) else p % 2
        return half - odd if way == 0 else half - 1 + odd

    for q in range(extra):
        r.tokens[me_x, q] = normed[:, (direct + q) * PIECE : (direct + q + 1) * PIECE]

    thin = extra * lanes_of

    def token_ring(way, step, q, col):
        here = r.tokens.at[col, q // lanes_of, :, pl.ds(q % lanes_of * 128, 128)]
        return remote(here, here, r.token_send.at[0], r.token_recv.at[step, q], toward(way))

    put_own = r.put[me_x]

    def make_out(p):
        part = jnp.dot(put_own, normed[:, p * PIECE : (p + 1) * PIECE], preferred_element_type=f32)
        r.outbound[p] = part[:slots].astype(bf16)
        for c in range(lanes_of):
            r.over_out[:, p * lanes_of + c, :] = part[slots:, c * 128 : (c + 1) * 128]

    def send_out(p, carry):
        for i in range(1, places):
            remote(
                r.outbound.at[p, lines(place(i)), :],
                r.chunks.at[me_x, p, lines(me_s), :],
                r.out_send.at[0],
                r.out_recv.at[p],
                {"sp": place(i)},
            ).start()
        r.chunks[me_x, p, lines(me_s), :] = r.outbound[p, lines(me_s), :]
        return carry

    make_out(0)
    send_out(0, 0)
    for q in range(thin):
        for way in range(2):
            token_ring(way, 0, q, me_x).start()
    for p in range(1, direct):
        make_out(p)
    lax.fori_loop(1, direct, send_out, 0)
    for i in range(1, places):
        remote(
            r.over_out.at[place(i)], r.over_in.at[me_s], r.over_send.at[0], r.over_recv.at[0], {"sp": place(i)}
        ).start()
    r.over_in[me_s] = r.over_out[me_s]
    if places < over:
        r.over_in[places:over] = jnp.zeros((over - places, *r.over_in.shape[1:]), f32)
        r.over_ret[:, places:over] = jnp.zeros((2, over - places, *r.over_ret.shape[2:]), f32)
        r.xover_in[:, places:over] = jnp.zeros((columns, over - places, *r.xover_in.shape[2:]), f32)
        r.xover_ret[:, places:over] = jnp.zeros((columns, over - places, *r.xover_ret.shape[2:]), f32)

    def route(offset):
        col = column(offset)
        for q in range(extra):
            part = jnp.dot(r.put[col], r.tokens[col, q], preferred_element_type=f32)
            r.xout[col, q] = part[:slots].astype(bf16)
            r.chunks[col, direct + q, lines(me_s), :] = r.xout[col, q, lines(me_s), :]
            for c in range(lanes_of):
                r.xover_out[offset, :, q * lanes_of + c, :] = part[slots:, c * 128 : (c + 1) * 128]
        r.xover_in[offset, me_s] = r.xover_out[offset, me_s]
        for i in range(1, places):
            remote(
                r.xout.at[col, :, lines(place(i)), :],
                r.chunks.at[col, pl.ds(direct, extra), lines(me_s), :],
                r.xout_send.at[0],
                r.xout_recv.at[offset],
                {"sp": place(i)},
            ).start()
            remote(
                r.xover_out.at[offset, place(i)],
                r.xover_in.at[offset, me_s],
                r.xover_send.at[0],
                r.xover_recv.at[0, offset],
                {"sp": place(i)},
            ).start()

    def routed(offset):
        col = column(offset)
        most = pl.ds(0, (places - 1) * main)
        return (
            remote(
                r.xout.at[col, :, most, :],
                r.chunks.at[col, pl.ds(direct, extra), most, :],
                r.xout_send.at[0],
                r.xout_recv.at[offset],
                right,
            ),
            remote(
                r.xover_out.at[offset, 0 : places - 1],
                r.xover_in.at[offset, 0 : places - 1],
                r.xover_send.at[0],
                r.xover_recv.at[0, offset],
                right,
            ),
        )

    def take_routed(offset):
        col = column(offset)
        for copy in routed(offset):
            copy.wait_recv()
        for q in range(extra):
            for c in range(lanes_of):
                r.chunks[col, direct + q, slots:, c * 128 : (c + 1) * 128] = r.xover_in[
                    offset, :, q * lanes_of + c, :
                ].astype(bf16)

    def token_event(k):
        for q in range(thin):
            came = r.tokens.at[pl.ds(0, 2 if k < half else 1), 0, :, pl.ds(0, 128)]
            remote(came, came, r.token_send.at[0], r.token_recv.at[k - 1, q], right).wait_recv()
            for way in range(2):
                if k < far(way, q):
                    token_ring(way, k, q, column(-k if way == 0 else k)).start()

    def chunk_ring(way, step, p, col):
        here = r.chunks.at[col, p, pl.ds(0, slots), :]
        return remote(here, here, r.chunk_send.at[0], r.chunk_recv.at[step, p], toward(way))

    def over_ring(way, step, col):
        here = r.chunks.at[col, pl.ds(0, direct), pl.ds(slots, over), :]
        return remote(here, here, r.tail_send.at[0], r.tail_recv.at[step], toward(way))

    def out_arrived(p):
        most = pl.ds(0, (places - 1) * main)
        return remote(
            r.outbound.at[p, most, :], r.chunks.at[me_x, p, most, :], r.out_send.at[0], r.out_recv.at[p], right
        )

    def start_piece(p):
        out_arrived(p).wait_recv()
        chunk_ring(0, 0, p, me_x).start()
        chunk_ring(1, 0, p, me_x).start()

    def start_over():
        remote(
            r.over_out.at[0 : places - 1], r.over_in.at[0 : places - 1], r.over_send.at[0], r.over_recv.at[0], right
        ).wait_recv()
        for c in range(direct * lanes_of):
            at_lanes = (c % lanes_of) * 128
            r.chunks[me_x, c // lanes_of, slots:, at_lanes : at_lanes + 128] = r.over_in[:, c, :].astype(bf16)
        for way in range(2):
            over_ring(way, 0, me_x).start()

    for copy in rims + mates + [enter_copy]:
        copy.wait_send()
    for n in range(1, chips):

        @pl.when(me_y + n < chips)
        def _():
            chip_total(n).wait_send()

    heads_total.wait_send()
    tables_total.wait_send()
    remote(ring_total, ring_total, r.ring_send.at[0], r.ring_recv.at[0, 0], right).wait_send()
    remote(slab_total, slab_total, r.slab_send.at[0], r.slab_recv.at[0], right).wait_send()
    remote(grid_total, grid_total, r.grid_send.at[0], r.grid_recv.at[0], right).wait_send()
    for which in range(2):
        view = pass_totals[which]
        remote(view, view, r.pass_send.at[which], r.pass_recv.at[which], mate).wait_send()

    def offset_of(n):
        k = (n + 1) // 2 if isinstance(n, int) else lax.div(n + 1, 2)
        if isinstance(n, int):
            return (columns - k) % columns if n % 2 else k
        return jnp.where(lax.rem(n, 2) == 1, lax.rem(columns - k, columns), k)

    opening = {"token": token_event, "piece": start_piece, "route": lambda n: route(offset_of(n)), "over": lambda n: start_over()}
    for kind, n in dims.opening:
        opening[kind](n)

    def unit(n, t):
        offset = offset_of(n)
        col = column(offset)
        pl.when(t == 0)(lambda: take_routed(offset))
        acc = jnp.dot(r.chunks[col, 0], r.gate_up[t, 0:PIECE, :], preferred_element_type=f32)
        for q in range(1, pieces):
            acc = acc + jnp.dot(
                r.chunks[col, q], r.gate_up[t, q * PIECE : (q + 1) * PIECE, :], preferred_element_type=f32
            )
        value = silu(acc[:, 0:128]) * acc[:, 128:256]
        r.hidden[col, :, pl.ds(pl.multiple_of(t * 128, 128), 128)] = value.astype(bf16)
        pl.when(t == dims.tiles - 1)(lambda: give_back(offset))

    def own(col, p):
        return jnp.dot(r.hidden[col], r.down[p], preferred_element_type=f32)

    def give_back(offset):
        col = column(offset)
        for q in range(extra):
            part = own(col, direct + q)
            r.xback[col, q] = part[:slots].astype(bf16)
            r.xret[col, q, lines(me_s), :] = r.xback[col, q, lines(me_s), :]
            for c in range(lanes_of):
                r.xover_back[offset, :, q * lanes_of + c, :] = part[slots:, c * 128 : (c + 1) * 128]
        r.xover_ret[offset, me_s] = r.xover_back[offset, me_s]
        for i in range(1, places):
            remote(
                r.xback.at[col, :, lines(place(i)), :],
                r.xret.at[col, :, lines(me_s), :],
                r.xback_send.at[0],
                r.xback_recv.at[offset],
                {"sp": place(i)},
            ).start()
            remote(
                r.xover_back.at[offset, place(i)],
                r.xover_ret.at[offset, me_s],
                r.xover_send.at[1],
                r.xover_recv.at[1, offset],
                {"sp": place(i)},
            ).start()

    def given_back(offset):
        col = column(offset)
        most = pl.ds(0, (places - 1) * main)
        return (
            remote(
                r.xback.at[col, :, most, :],
                r.xret.at[col, :, most, :],
                r.xback_send.at[0],
                r.xback_recv.at[offset],
                right,
            ),
            remote(
                r.xover_back.at[offset, 0 : places - 1],
                r.xover_ret.at[offset, 0 : places - 1],
                r.xover_send.at[1],
                r.xover_recv.at[1, offset],
                right,
            ),
        )

    for n, weights in enumerate((r.gate_up, r.down)):
        pltpu.make_async_copy(weights, weights, r.weight_sem.at[n]).wait()

    def units(low, high):
        def body(v, carry):
            unit(lax.div(v, dims.tiles), lax.rem(v, dims.tiles))
            return carry

        lax.fori_loop(low, high, body, 0)

    def hop(way, j, p):
        return remote(
            r.sums.at[way, j, p],
            r.sums.at[way, j - 1, p],
            r.sum_send.at[0],
            r.sum_recv.at[way, j - 1, p],
            {"tp": column(1 - 2 * way)},
        )

    def chains(long, step, group):
        j = half - step if long else half - 1 - step

        def body(p, carry):
            odd = lax.rem(p, 2)
            way = 1 - odd if long else odd
            value = own(column(j * (1 - 2 * way)), p)
            if step > 0:
                hop(way, j + 1, p).wait_recv()
                value = value + r.sums[way, j, p].astype(f32)
            r.sums[way, j, p] = value.astype(bf16)
            hop(way, j, p).start()
            return carry

        lax.fori_loop(*group, body, 0)

    share_of = dims.schedule
    for k in range(1, half + 1):
        first, last = share_of[k - 1] * dims.tiles, share_of[k] * dims.tiles

        if k == half and half > 1:
            units(first, last)
            first = last
            for group in dims.groups:
                chains(False, 0, group)

        def pass_on(p, carry, k=k, first=first, last=last):
            came = r.chunks.at[pl.ds(0, 2 if k < half else 1), p, pl.ds(0, slots), :]
            remote(came, came, r.chunk_send.at[0], r.chunk_recv.at[k - 1, p], right).wait_recv()
            if k < half:
                for way in range(2):
                    start = lambda way=way: chunk_ring(way, k, p, column(-k if way == 0 else k)).start()
                    if k < half - 1:
                        start()
                    else:
                        pl.when(k < far(way, p))(start)

            if k == 1 and dims.routed < columns:
                pl.when(p < columns - dims.routed)(lambda: route(offset_of(p + dims.routed)))
            if last > first:
                units(
                    first + lax.div(p * (last - first), direct), first + lax.div((p + 1) * (last - first), direct)
                )
            return carry

        lax.fori_loop(0, direct, pass_on, 0)
        came = r.chunks.at[pl.ds(0, 2 if k < half else 1), pl.ds(0, direct), pl.ds(slots, over), :]
        remote(came, came, r.tail_send.at[0], r.tail_recv.at[k - 1], right).wait_recv()
        for way in range(2):
            if k < far(way, 0):
                over_ring(way, k, column(-k if way == 0 else k)).start()
        if k == 1:
            lax.fori_loop(0, columns, lambda col, carry: (make_pick(col), carry)[1], 0)
    units(share_of[half] * dims.tiles, columns * dims.tiles)

    def finish(p, carry):
        value = own(me_x, p)
        hop(0, 1, p).wait_recv()
        hop(1, 1, p).wait_recv()
        value = value + r.sums[0, 0, p].astype(f32) + r.sums[1, 0, p].astype(f32)
        r.totals[p] = value[0:slots].astype(bf16)
        r.over_total[p] = value[slots:]
        r.returned[p, lines(me_s), :] = r.totals[p, lines(me_s), :]
        for i in range(1, places):
            remote(
                r.totals.at[p, lines(place(i)), :],
                r.returned.at[p, lines(me_s), :],
                r.back_send.at[0],
                r.back_recv.at[p],
                {"sp": place(i)},
            ).start()
        return carry

    def weighted(col, table):
        one = jnp.dot(r.pick[col, 0], table, preferred_element_type=f32)
        two = jnp.dot(r.pick[col, 1], table, preferred_element_type=f32)
        copies = one.shape[1] // 128
        first, second = (jnp.concatenate([r.share_s[col, k]] * copies, axis=1) for k in range(2))
        return first * one + second * two

    def take_back(offset):
        col = column(offset)
        for copy in given_back(offset):
            copy.wait_recv()
        for q in range(extra):
            for c in range(lanes_of):
                r.xret[col, q, slots:, c * 128 : (c + 1) * 128] = r.xover_ret[
                    offset, :, q * lanes_of + c, :
                ].astype(bf16)

    def token_hop(way, j, q):
        return remote(
            r.xsums.at[way, j, q],
            r.xsums.at[way, j - 1, q],
            r.xsum_send.at[0],
            r.xsum_recv.at[way, j - 1, q],
            toward(way),
        )

    taken = set()

    def thin_part(col, q):
        return weighted(col, r.xret[col, q // lanes_of, :, q % lanes_of * 128 : (q % lanes_of + 1) * 128])

    def token_round(t):
        for q in range(thin):
            for way in range(2):
                j = far(1 - way, q) - t
                if j < 1:
                    continue
                offset = j if way == 0 else columns - j
                if offset not in taken:
                    taken.add(offset)
                    take_back(offset)
                value = thin_part(column(offset), q)
                if t > 0:
                    token_hop(way, j + 1, q).wait_recv()
                    value = value + r.xsums[way, j, q].astype(f32)
                r.xsums[way, j, q] = value.astype(bf16)
                token_hop(way, j, q).start()

    for group in dims.groups:
        chains(True, 0, group)
    def left_by_now(view, send, recv):
        remote(view, view, send, recv, right).wait_send()

    most_places, most_lines = pl.ds(0, places - 1), pl.ds(0, (places - 1) * main)
    chunks_total = r.chunks.at[most_columns, pl.ds(0, direct), pl.ds(0, slots), :]
    left_by_now(r.over_out.at[most_places], r.over_send.at[0], r.over_recv.at[0])
    left_by_now(r.tokens.at[most_columns], r.token_send.at[0], r.token_recv.at[0, 0])
    left_by_now(r.chunks.at[most_columns, pl.ds(0, direct), pl.ds(slots, over), :], r.tail_send.at[0], r.tail_recv.at[0])
    left_by_now(chunks_total, r.chunk_send.at[0], r.chunk_recv.at[0, 0])
    left_by_now(r.outbound.at[:, most_lines, :], r.out_send.at[0], r.out_recv.at[0])
    left_by_now(r.xout.at[:, :, most_lines, :], r.xout_send.at[0], r.xout_recv.at[0])
    left_by_now(r.xover_out.at[:, most_places], r.xover_send.at[0], r.xover_recv.at[0, 0])
    def over_back_copy(n, to, at):
        return remote(
            r.over_back.at[n, to],
            r.over_ret.at[n, at],
            r.over_send.at[1],
            r.over_recv.at[1 + n],
            {"sp": to},
        )

    def send_over_back(n, group):
        for p in range(*group):
            for c in range(lanes_of):
                r.over_back[n, :, (p - group[0]) * lanes_of + c, :] = r.over_total[p, :, c * 128 : (c + 1) * 128]
        r.over_ret[n, me_s] = r.over_back[n, me_s]
        for i in range(1, places):
            over_back_copy(n, place(i), me_s).start()

    for kind, step, group in dims.closing:
        if kind == "short":
            chains(False, step, group)
        elif kind == "long":
            chains(True, step, group)
        elif kind == "token":
            token_round(step)
        else:
            lax.fori_loop(*group, finish, 0)
            send_over_back(dims.groups.index(group), group)
    left_by_now(r.xback.at[:, :, most_lines, :], r.xback_send.at[0], r.xback_recv.at[0])
    left_by_now(r.xover_back.at[:, most_places], r.xover_send.at[1], r.xover_recv.at[1, 0])
    left_by_now(r.chunks.at[most_columns, pl.ds(0, direct)], r.sum_send.at[0], r.sum_recv.at[0, 0, 0])
    token_round(half - 1)
    def back_arrived(p):
        most = pl.ds(0, (places - 1) * main)
        return remote(
            r.totals.at[p, most, :], r.returned.at[p, most, :], r.back_send.at[0], r.back_recv.at[p], right
        )

    def combine(p, carry):
        back_arrived(p).wait_recv()
        span = pl.ds(pl.multiple_of(p * PIECE, PIECE), PIECE)
        value = weighted(me_x, r.returned[p])
        r.out_ref[:, span] = (r.stream_s[:, span].astype(f32) + value).astype(bf16)
        return carry

    def combine_group(n, group):
        remote(
            r.over_back.at[n, 0 : places - 1],
            r.over_ret.at[n, 0 : places - 1],
            r.over_send.at[1],
            r.over_recv.at[1 + n],
            right,
        ).wait_recv()
        for p in range(*group):
            for c in range(lanes_of):
                r.returned[p, slots:, c * 128 : (c + 1) * 128] = r.over_ret[n, :, (p - group[0]) * lanes_of + c, :].astype(bf16)
        lax.fori_loop(*group, combine, 0)

    combine_group(dims.groups.index(dims.order[0]), dims.order[0])
    take_back(0)
    for q in range(thin):
        value = thin_part(me_x, q)
        for way in range(2):
            token_hop(way, 1, q).wait_recv()
            value = value + r.xsums[way, 0, q].astype(f32)
        span = slice(direct * PIECE + q * 128, direct * PIECE + (q + 1) * 128)
        r.out_ref[:, span] = (r.stream_s[:, span].astype(f32) + value).astype(bf16)

    combine_group(dims.groups.index(dims.order[1]), dims.order[1])

    left_by_now(r.over_back.at[:, most_places], r.over_send.at[1], r.over_recv.at[1])
    left_by_now(r.tokens.at[most_columns], r.xsum_send.at[0], r.xsum_recv.at[0, 0, 0])
    left_by_now(r.totals.at[:, most_lines, :], r.back_send.at[0], r.back_recv.at[0])


def layer(places, columns, **given):
    f32, bf16 = jnp.float32, jnp.bfloat16
    rows, width = given["residual_hbm"].shape
    small = [name for name in given if name.endswith("_small")]
    units = given["expert_gate_hbm"].shape[2]
    lanes = given["keys_hbm"].shape[1]
    positions = columns * BLOCK
    half, chips, blocks = columns // 2, places // 2, columns
    main = 2 * rows // places
    over = -(-places // 16) * 16
    pieces = width // PIECE
    extra = max(1, pieces // 4)
    direct = pieces - extra
    tiles, total = units // 128, places * main + over
    ring_part = width * RING_SHARE // 16 // 128 * 128
    schedule = (0, 0, 1, 5, 7) if half == 4 else (0,) * half + (columns - 1,)
    if half == 4:
        opening = [("token", 1), ("piece", 0), ("piece", 1), ("token", 2), ("piece", 2), ("route", 0), ("piece", 3)]
        opening += [("token", 3), ("route", 1), ("piece", 4), ("route", 2), ("token", 4), ("piece", 5), ("over", 0)]
    else:
        opening = [("token", n) for n in range(1, half + 1)] + [("piece", n) for n in range(direct)]
        opening += [("route", n) for n in range(columns)] + [("over", 0)]
    routed = sum(kind == "route" for kind, _ in opening)
    serving = [
        [("x", 0)],
        [("x", 1)],
        [("x", 2)],
        [("x", 3), ("y", 0), ("y", 1), ("y", 2), ("x", 4), ("y", 3), ("y", 4), ("y", 5), ("x", 5), ("x", 6), ("y", 6)],
    ]
    low, high = (0, (direct + 1) // 2), ((direct + 1) // 2, direct)
    groups = [high, low]
    if half == 4:
        closing = [
            ("long", 1, high),
            ("short", 1, high),
            ("long", 1, low),
            ("short", 1, low),
            ("long", 2, low),
            ("long", 2, high),
            ("long", 3, low),
            ("short", 2, low),
            ("token", 0, None),
            ("long", 3, high),
            ("finish", None, low),
            ("short", 2, high),
            ("token", 1, None),
            ("finish", None, high),
            ("token", 2, None),
        ]
    else:
        closing = []
        for step in range(1, half):
            closing += [("short", step, group) for group in groups if step < half - 1]
            closing += [("long", step, group) for group in groups]
            closing.append(("token", step - 1, None))
        closing += [("finish", None, group) for group in groups]
    dims = types.SimpleNamespace(
        places=places, columns=columns, width=width, main=main, over=over, pieces=pieces, direct=direct, tiles=tiles,
        schedule=schedule, opening=opening, routed=routed, small=small, groups=groups, order=(low, high), closing=closing, ring_part=ring_part, serving=serving,
    )
    packed = STATE_ONE + STATE_TWO
    square = (blocks, 2, BLOCK, BLOCK)
    vmem = lambda *shape, dtype=bf16: pltpu.VMEM(shape, dtype)
    dma = lambda *shape: pltpu.SemaphoreType.DMA(shape)
    in_specs = [pl.BlockSpec(memory_space=pltpu.SMEM if a.shape == (2, 2) else pl.ANY) for a in given.values()]
    lane_rows = PIECE // 128
    scratch = {name[:-5] + "ref": pltpu.VMEM(given[name].shape, given[name].dtype) for name in small}
    scratch |= dict(
        residual_in=vmem(rows, width),
        value_in=vmem(2 * positions + 16, BLOCK),
        gate_in=vmem(2 * positions, BLOCK),
        keys_in=vmem(positions + 16, lanes),
        gate_wide=vmem(2 * BLOCK, BLOCK, dtype=f32),
        conv_wide=vmem(2 * BLOCK, BLOCK, dtype=f32),
        x_s=vmem(*square),
        kt_s=vmem(*square),
        q_s=vmem(*square),
        state_s=vmem(*square, dtype=f32),
        near_s=vmem(*square, dtype=f32),
        stride_s=vmem(HEADS * blocks, BLOCK, dtype=f32),
        run_s=vmem(HEADS * blocks, BLOCK, dtype=f32),
        fade_s=vmem(HEADS * blocks, BLOCK, dtype=f32),
        end_s=vmem(HEADS * blocks, BLOCK, dtype=f32),
        cols_s=vmem(blocks, BLOCK, HEADS, dtype=f32),
        own_pack=vmem(packed, BLOCK),
        own_fade=vmem(8, BLOCK, dtype=f32),
        mate_pack=vmem(packed, BLOCK),
        mate_fade=vmem(8, BLOCK, dtype=f32),
        chip_pack=vmem(packed, BLOCK),
        chip_fade=vmem(8, BLOCK, dtype=f32),
        all_pack=vmem(chips, packed // 2, BLOCK),
        all_fade=vmem(chips, 8, BLOCK, dtype=f32),
        enter_pack=vmem(packed, BLOCK),
        carry_s=vmem(2, BLOCK, BLOCK, dtype=f32),
        mixed_s=vmem(columns, BLOCK, 2 * BLOCK),
        heads_in=vmem(columns, BLOCK, 2 * BLOCK),
        matrix=vmem(columns, 2 * BLOCK, width),
        acc_s=vmem(rows, width, dtype=f32),
        stream_s=vmem(rows, width),
        tables=vmem(columns, 8, rows, dtype=f32),
        put=vmem(columns, total, rows),
        pick=vmem(columns, 2, rows, total),
        share_s=vmem(columns, 2, rows, 128, dtype=f32),
        tokens=vmem(columns, extra, rows, PIECE),
        outbound=vmem(direct, places * main, PIECE),
        over_out=vmem(over, direct * lane_rows, 128, dtype=f32),
        over_in=vmem(over, direct * lane_rows, 128, dtype=f32),
        over_back=vmem(2, over, (high[1] - low[0] + 1) // 2 * lane_rows, 128, dtype=f32),
        over_ret=vmem(2, over, (high[1] - low[0] + 1) // 2 * lane_rows, 128, dtype=f32),
        over_total=vmem(direct, over, PIECE, dtype=f32),
        xout=vmem(columns, extra, places * main, PIECE),
        xback=vmem(columns, extra, places * main, PIECE),
        xret=vmem(columns, extra, total, PIECE),
        xover_out=vmem(columns, over, extra * lane_rows, 128, dtype=f32),
        xover_in=vmem(columns, over, extra * lane_rows, 128, dtype=f32),
        xover_back=vmem(columns, over, extra * lane_rows, 128, dtype=f32),
        xover_ret=vmem(columns, over, extra * lane_rows, 128, dtype=f32),
        chunks=vmem(columns, pieces, total, PIECE),
        hidden=vmem(columns, total, units),
        gate_up=vmem(tiles, width, 256),
        down=vmem(pieces, units, PIECE),
        sums=vmem(2, half + 1, direct, total, PIECE),
        xsums=vmem(2, half + 1, extra * lane_rows, rows, 128),
        totals=vmem(direct, places * main, PIECE),
        returned=vmem(direct, total, PIECE),
        load_sem=dma(6),
        weight_sem=dma(2),
        small_sem=dma(len(small)),
    )
    steps = (2, half)
    for name, send, recv in (
        ("rim", (2,), (2,)),
        ("mate", (2,), (2,)),
        ("chip", (chips,), (chips,)),
        ("enter", (1,), (1,)),
        ("head", (1,), (1,)),
        ("table", (1,), (1,)),
        ("ring", (1,), (columns - 1, 2)),
        ("slab", (1,), (1,)),
        ("grid", (1,), (chips - 1,)),
        ("pass", (2,), (2,)),
        ("over", (2,), (3,)),
        ("token", (1,), (half, extra * lane_rows)),
        ("out", (1,), (direct,)),
        ("xout", (1,), (columns,)),
        ("xover", (2,), (2, columns)),
        ("chunk", (1,), (half, direct)),
        ("tail", (1,), (half,)),
        ("xback", (1,), (columns,)),
        ("sum", (1,), (*steps, direct)),
        ("xsum", (1,), (*steps, extra * lane_rows)),
        ("back", (1,), (direct,)),
    ):
        scratch[name + "_send"], scratch[name + "_recv"] = dma(*send), dma(*recv)
    names = [*given, "out_ref", *scratch]
    return pl.pallas_call(
        functools.partial(layer_kernel, dims, names),
        out_shape=pltpu.VMEM((rows, width), bf16),
        in_specs=in_specs,
        out_specs=pl.BlockSpec(memory_space=pltpu.VMEM),
        scratch_shapes=list(scratch.values()),
        compiler_params=pltpu.CompilerParams(
            collective_id=0, has_side_effects=True, vmem_limit_bytes=VMEM_LIMIT
        ),
        name="layer",
    )(*given.values())


def local(
    residual,
    grouped_value_heads,
    output_gate_heads,
    projected_key_query,
    raw_step_size,
    step_size_bias,
    head_decay_logarithm,
    position_extra_decay,
    head_skip_weight,
    value_kernel_taps,
    key_query_kernel,
    head_norm_gain,
    output_matrix,
    expert_norm_gain,
    expert_gate_weight,
    expert_up_weight,
    expert_down_weight,
    token_expert_choice,
    expert_output_weight,
):
    return layer(
        lax.axis_size("sp"),
        lax.axis_size("tp"),
        residual_hbm=residual,
        value_hbm=grouped_value_heads.reshape(-1, BLOCK),
        gate_hbm=output_gate_heads.reshape(-1, BLOCK),
        keys_hbm=projected_key_query,
        raw_small=raw_step_size.transpose(1, 2, 0),
        bias_ref=step_size_bias,
        log_ref=head_decay_logarithm,
        extra_small=position_extra_decay.reshape(-1, BLOCK),
        skip_ref=head_skip_weight,
        value_tap_small=value_kernel_taps.reshape(-1, BLOCK),
        key_tap_small=key_query_kernel,
        head_gain_small=head_norm_gain,
        matrix_hbm=output_matrix,
        expert_gain_small=expert_norm_gain[None],
        choice_small=token_expert_choice.T,
        share_small=expert_output_weight.T,
        expert_gate_hbm=expert_gate_weight,
        expert_up_hbm=expert_up_weight,
        expert_down_hbm=expert_down_weight,
    )


def solution(mesh):
    placed = (
        P(("grp", "sp", "tp"), None),
        P(("grp", "sp"), None, "tp"),
        P(("grp", "sp"), None, "tp"),
        P(("grp", "sp"), None),
        P(("grp", "sp"), None, "tp"),
        P(None, "tp"),
        P(None, "tp"),
        P(("grp", "sp")),
        P(None, "tp"),
        P(None, None, "tp"),
        P(),
        P(None, "tp"),
        P(None, "tp", None),
        P(),
        P("sp", None, "tp"),
        P("sp", None, "tp"),
        P("sp", "tp", None),
        P(("grp", "sp", "tp"), None),
        P(("grp", "sp", "tp"), None),
    )
    return jax.shard_map(
        local, mesh=mesh, in_specs=placed, out_specs=P(("grp", "sp", "tp"), None), check_vma=False
    )
```

```python
import functools
import types

import jax
import jax.numpy as jnp
from jax import lax
from jax.experimental import pallas as pl
from jax.experimental.pallas import tpu as pltpu
from jax.sharding import PartitionSpec as P

HEAD_DIM = 64
STATE_ONE = 64
STATE_TWO = 128
BLOCK = 128
EPSILON = 1e-06

MESH = pl.DeviceIdType.MESH
PIECE = 256
HEADS = 4
RING_SHARE = 7
VMEM_LIMIT = 61600000


def remote(src, dst, send, recv, device):
    return pltpu.make_async_remote_copy(
        src_ref=src, dst_ref=dst, send_sem=send, recv_sem=recv, device_id=device, device_id_type=MESH
    )


def silu(a):
    return a * (1.0 / (1.0 + jnp.exp(-a)))


def layer_kernel(dims, names, *refs):
    r = types.SimpleNamespace(**dict(zip(names, refs, strict=True)))
    f32, bf16 = jnp.float32, jnp.bfloat16
    places, columns, width, rows = dims.places, dims.columns, dims.width, BLOCK
    half, chips, blocks = columns // 2, places // 2, columns
    me_x, me_s = lax.axis_index("tp"), lax.axis_index("sp")
    core, me_y = lax.rem(me_s, 2), lax.div(me_s, 2)
    right = {"tp": lax.rem(me_x + 1, columns)}
    left = {"tp": lax.rem(me_x + columns - 1, columns)}
    mate = {"sp": me_s + 1 - 2 * core}
    following = {"sp": lax.rem(me_s + 1, places)}

    def column(offset):
        return lax.rem(me_x + offset + columns, columns)

    def place(offset):
        return lax.rem(me_s + offset, places)

    def peer(offset):
        return {"sp": lax.rem(me_s + 2 * offset, places)}

    def toward(way):
        return right if way == 0 else left

    barrier = pltpu.get_barrier_semaphore()
    peers = sorted(
        [(min(i, columns - i), {"tp": column(i)}) for i in range(1, columns)]
        + [(min(i, places - i) / 2, {"sp": place(i)}) for i in range(1, places) if i % 2 == 0 or i in (1, places - 1)],
        key=lambda peer: -peer[0],
    )
    peers = [device for _, device in peers]
    for device in peers:
        pl.semaphore_signal(barrier, inc=1, device_id=device, device_id_type=MESH)

    small = {
        name: pltpu.make_async_copy(getattr(r, name), getattr(r, name[:-5] + "ref"), r.small_sem.at[n])
        for n, name in enumerate(dims.small)
    }
    ring_part, slab = dims.ring_part, rows // chips
    rim_rows, positions = 16, blocks * rows
    mine = pl.multiple_of(core * rows, rows)

    def slab_rows(y):
        return pl.ds(pl.multiple_of(mine + y * slab, 16), slab)

    on_ring, on_grid = pl.ds(0, ring_part), pl.ds(ring_part, width - ring_part)
    loads = [
        (r.matrix_hbm.at[0], r.matrix.at[0, pl.ds(0, rows), :]),
        (r.matrix_hbm.at[1], r.matrix.at[0, pl.ds(rows, rows), :]),
        (r.value_hbm, r.value_in.at[pl.ds(rim_rows, 2 * positions), :]),
        (r.keys_hbm, r.keys_in.at[pl.ds(rim_rows, positions), :]),
        (r.gate_hbm, r.gate_in),
        (r.residual_hbm, r.residual_in),
    ]
    loads = [pltpu.make_async_copy(a, b, r.load_sem.at[n]) for n, (a, b) in enumerate(loads)]
    for load in loads[:2] + list(small.values()) + loads[2:4]:
        load.start()
    for name in ("choice_small", "share_small"):
        small[name].wait()
    r.tables[me_x] = jnp.zeros((8, rows), f32)
    r.tables[me_x, 0:2, :] = r.choice_ref[...].astype(f32)
    r.tables[me_x, 2:4, :] = r.share_ref[...]

    for load in loads[:2]:
        load.wait()
    pl.semaphore_wait(barrier, len(peers))

    def matrix_block(way, event, k, sub):
        piece = ((event % 2) ^ way) * 2 + sub
        block = (columns - k if way == 0 else k) % columns
        return r.matrix.at[block, pl.ds(pl.multiple_of(mine + piece * (rows // 4), 16), rows // 4), on_ring]

    def matrix_ring(way, event, sub):
        k = event // 2
        return remote(
            matrix_block(way, event, k, sub),
            matrix_block(way, event, k + 1, sub),
            r.ring_send.at[0],
            r.ring_recv.at[event, sub],
            toward(way),
        )

    def slab_copy(offset):
        return remote(
            r.matrix.at[0, slab_rows(me_y), on_grid],
            r.matrix.at[columns - offset, slab_rows(me_y), on_grid],
            r.slab_send.at[0],
            r.slab_recv.at[0],
            {"tp": column(offset)},
        )

    def grid_view(way, event, y):
        blocks_of = pl.ds(1, half) if (event % 2) ^ way == 0 else pl.ds(1 + half, half - 1)
        return r.matrix.at[blocks_of, slab_rows(y), on_grid]

    def grid_ring(way, event, y):
        here = grid_view(way, event, y)
        return remote(
            here, here, r.grid_send.at[0], r.grid_recv.at[event], peer(1) if way == 0 else peer(chips - 1)
        )

    def to_mate(here, which):
        return remote(here, here, r.pass_send.at[which], r.pass_recv.at[which], mate)

    most_columns, other_blocks = pl.ds(0, columns - 1), pl.ds(1, columns - 1)
    ring_total = r.matrix.at[other_blocks, pl.ds(0, rows), on_ring]
    grid_total = r.matrix.at[other_blocks, pl.ds(0, (chips - 1) * slab), on_grid]
    slab_total = r.matrix.at[other_blocks, pl.ds(0, slab), on_grid]
    pass_totals = (ring_total, r.matrix.at[other_blocks, pl.ds(0, rows), on_grid])

    for load in loads[2:4]:
        load.wait()
    rims = [
        remote(
            r.value_in.at[pl.ds(2 * positions, rim_rows), :],
            r.value_in.at[pl.ds(0, rim_rows), :],
            r.rim_send.at[0],
            r.rim_recv.at[0],
            following,
        ),
        remote(
            r.keys_in.at[pl.ds(positions, rim_rows), :],
            r.keys_in.at[pl.ds(0, rim_rows), :],
            r.rim_send.at[1],
            r.rim_recv.at[1],
            following,
        ),
    ]
    for rim in rims:
        rim.start()

    def table_copy(offset):
        here = r.tables.at[me_x]
        return remote(here, here, r.table_send.at[0], r.table_recv.at[0], {"tp": column(offset)})

    for i in range(1, columns):
        table_copy(i).start()
    for i in range(1, columns):
        slab_copy(i).start()
    for event in range(min(2, columns - 1)):
        for sub in range(2):
            for way in range(2):
                matrix_ring(way, event, sub).start()
    tables_total = remote(
        r.tables.at[most_columns], r.tables.at[most_columns], r.table_send.at[0], r.table_recv.at[0], right
    )

    def serve_ring(event):
        for sub in range(2):
            both = r.matrix.at[0, pl.ds(0, rows // 2), on_ring]
            remote(both, both, r.ring_send.at[0], r.ring_recv.at[event, sub], right).wait_recv()
            for way in range(2):
                if event + 2 < columns - 1:
                    matrix_ring(way, event + 2, sub).start()
                to_mate(matrix_block(way, event, event // 2 + 1, sub), 0).start()

    def serve_slab():
        remote(slab_total, slab_total, r.slab_send.at[0], r.slab_recv.at[0], right).wait_recv()
        for event in range(2):
            for way in range(2):
                if event < chips - 1:
                    grid_ring(way, event, me_y).start()
        to_mate(r.matrix.at[other_blocks, slab_rows(me_y), on_grid], 1).start()

    def serve_grid(event):
        k = event // 2 + 1
        remote(slab_total, slab_total, r.grid_send.at[0], r.grid_recv.at[event], right).wait_recv()
        for way in range(2):
            y = lax.rem(me_y + (chips - k if way == 0 else k), chips)
            if event + 2 < chips - 1:
                grid_ring(way, event + 2, y).start()
            to_mate(grid_view(way, event, y), 1).start()

    waiting = [("x", e) for e in range(columns - 1)] + [("y", e) for e in range(chips - 1)]

    def serve(*steps):
        for step in steps:
            if step in waiting:
                waiting.remove(step)
                (serve_ring if step[0] == "x" else serve_grid)(step[1])

    for load in loads[4:]:
        load.start()
    for t in range(dims.tiles):
        span = pl.ds(t * 128, 128)
        for n, weight in enumerate((r.expert_gate_hbm, r.expert_up_hbm)):
            pltpu.make_async_copy(
                weight.at[0, :, span], r.gate_up.at[t, :, pl.ds(n * 128, 128)], r.weight_sem.at[0]
            ).start()
    for p in range(dims.pieces):
        pltpu.make_async_copy(
            r.expert_down_hbm.at[0, :, pl.ds(p * PIECE, PIECE)], r.down.at[p], r.weight_sem.at[1]
        ).start()

    for name in dims.small:
        if name not in ("choice_small", "share_small"):
            small[name].wait()
    for g in range(2):
        raw = r.raw_ref[g].astype(f32)
        for k in range(blocks):
            r.stride_s[HEADS * k + 2 * g : HEADS * k + 2 * g + 2, :] = raw[:, k * rows : (k + 1) * rows]
    for k in range(blocks):
        r.run_s[HEADS * k : HEADS * k + HEADS, :] = jnp.broadcast_to(r.extra_ref[k : k + 1, :], (HEADS, rows))
    head_of = jnp.bitwise_and(lax.broadcasted_iota(jnp.int32, (HEADS * blocks, rows), 0), HEADS - 1)

    def by_head(table):
        picked = jnp.full((HEADS * blocks, rows), table[1, 1], f32)
        for n in range(3):
            picked = jnp.where(head_of == n, table[n // 2, n % 2], picked)
        return picked

    shifted = r.stride_s[...] + by_head(r.bias_ref)
    stride = jnp.maximum(shifted, 0.0) + jnp.log1p(jnp.exp(-jnp.abs(shifted)))
    log_decay = r.run_s[...] - jnp.exp(by_head(r.log_ref)) * stride
    at_row = lax.broadcasted_iota(jnp.int32, (rows, rows), 0)
    at_lane = lax.broadcasted_iota(jnp.int32, (rows, rows), 1)
    running = jnp.dot(
        log_decay,
        jnp.where(at_row <= at_lane, 1.0, 0.0),
        preferred_element_type=f32,
        precision=lax.Precision.HIGHEST,
    )
    ends = jnp.broadcast_to(running[:, rows - 1 : rows], running.shape)
    r.stride_s[...] = stride
    r.run_s[...] = running
    r.fade_s[...] = jnp.exp(ends - running) * stride
    r.end_s[...] = jnp.exp(ends)
    turned = jnp.transpose(running)
    for k in range(blocks):
        r.cols_s[k, :, 0:HEADS] = turned[:, HEADS * k : HEADS * k + HEADS]

    first_head = at_lane < HEAD_DIM

    def row_pair(table, k, g):
        low = table[pl.ds(HEADS * k + 2 * g, 1), :]
        high = table[pl.ds(HEADS * k + 2 * g + 1, 1), :]
        return jnp.where(first_head[0:1], low, high)

    taps = r.value_tap_ref.shape[0] // 2
    value_tap = r.value_tap_ref[...].astype(f32)
    key_tap = r.key_tap_ref[...].astype(f32)
    even = jnp.bitwise_and(lax.broadcasted_iota(jnp.int32, (2 * rows, rows), 0), 1) == 0
    tap_rows = [jnp.where(even, value_tap[2 * j : 2 * j + 1], value_tap[2 * j + 1 : 2 * j + 2]) for j in range(taps)]

    def states_of(k):
        window = r.value_in[pl.ds(pl.multiple_of(k * 2 * rows, 2 * rows), 2 * rows + rim_rows), :].astype(f32)
        total = jnp.zeros((2 * rows, rows), f32)
        for j in range(taps):
            start = rim_rows - 2 * (taps - 1 - j)
            total = total + window[start : start + 2 * rows] * tap_rows[j]
        r.conv_wide[...] = silu(total).astype(bf16).astype(f32)
        window = r.keys_in[pl.ds(pl.multiple_of(k * rows, rows), rows + rim_rows), :].astype(f32)
        total = jnp.zeros((rows, r.keys_in.shape[1]), f32)
        for j in range(taps):
            start = rim_rows - (taps - 1 - j)
            total = total + window[start : start + rows] * key_tap[j : j + 1]
        conv = silu(total).astype(bf16).astype(f32)
        both = conv[:, 0 : 2 * STATE_ONE]
        keys = [jnp.where(first_head, both, 0.0), conv[:, 2 * STATE_ONE : 2 * STATE_ONE + STATE_TWO]]
        asks = [pltpu.roll(both, STATE_ONE, 1), conv[:, 2 * STATE_ONE + STATE_TWO :]]
        for g in range(2):
            x = r.conv_wide[pl.ds(g, rows, stride=2), :].astype(bf16)
            key_t = jnp.transpose(keys[g])
            r.x_s[k, g] = x
            r.kt_s[k, g] = key_t.astype(bf16)
            r.q_s[k, g] = asks[g].astype(bf16)
            faded = jnp.concatenate(
                [key_t * r.fade_s[pl.ds(HEADS * k + 2 * g + h, 1), :] for h in range(2)], axis=0
            ).astype(bf16)
            state = jnp.dot(faded, x, preferred_element_type=f32)
            r.state_s[k, g] = jnp.where(first_head, state[:rows], state[rows:])

    def state_step(i, carry):
        states_of(i)
        return carry

    lax.fori_loop(1, blocks, state_step, 0)
    for rim in rims:
        rim.wait_recv()
    opening = me_s == 0
    for table in (r.value_in, r.keys_in):
        table[0:rim_rows, :] = jnp.where(opening, 0.0, table[0:rim_rows, :].astype(f32)).astype(bf16)
    states_of(0)

    packed = STATE_TWO + STATE_ONE
    piece = packed // 2

    def local_end(g):
        total = jnp.zeros((rows, rows), f32)
        faded = jnp.ones((1, rows), f32)
        for k in range(blocks):
            decay = row_pair(r.end_s, k, g)
            total = total * decay + r.state_s[k, g]
            faded = faded * decay
        return total, faded

    end_one, fade_one = local_end(0)
    end_two, fade_two = local_end(1)
    own = jnp.concatenate([end_two, end_one[:STATE_ONE]], axis=0)
    r.own_pack[...] = own.astype(bf16)
    r.own_fade[0:1, :] = fade_one
    r.own_fade[1:2, :] = fade_two
    r.own_fade[2:8, :] = jnp.zeros((6, rows), f32)
    mates = [
        remote(r.own_pack, r.mate_pack, r.mate_send.at[0], r.mate_recv.at[0], mate),
        remote(r.own_fade, r.mate_fade, r.mate_send.at[1], r.mate_recv.at[1], mate),
    ]
    for copy in mates:
        copy.start()
    for copy in mates:
        copy.wait_recv()
    is_low = core == 0
    low = jnp.where(is_low, own, r.mate_pack[...].astype(f32))
    high = jnp.where(is_low, r.mate_pack[...].astype(f32), own)
    mate_rows = r.mate_fade[...]
    own_rows = r.own_fade[...]
    high_rows = jnp.where(is_low, mate_rows, own_rows)
    in_two = lax.broadcasted_iota(jnp.int32, (packed, rows), 0) < STATE_TWO
    r.chip_pack[...] = (low * jnp.where(in_two, high_rows[1:2], high_rows[0:1]) + high).astype(bf16)
    r.chip_fade[...] = own_rows * mate_rows
    my_half = pl.ds(pl.multiple_of(core * piece, 16), piece)

    def to_chip(n, which):
        src = r.chip_pack.at[my_half, :] if which == 0 else r.chip_fade
        dst = r.all_pack.at[me_y] if which == 0 else r.all_fade.at[me_y]
        return remote(src, dst, r.chip_send.at[n], r.chip_recv.at[n], peer(n))

    def chip_total(n):
        sent = r.own_pack.at[pl.ds(0, piece + 16), :]
        return remote(sent, sent, r.chip_send.at[n], r.chip_recv.at[n], peer(n))

    for n in range(1, chips):

        @pl.when(me_y + n < chips)
        def _():
            for which in range(2):
                to_chip(n, which).start()


    below = at_row >= at_lane

    def near_step(k, carry):
        cols = r.cols_s[k]
        for g in range(2):
            scores = jnp.dot(r.q_s[k, g], r.kt_s[k, g], preferred_element_type=f32)
            parts = []
            for h in range(2):
                n = 2 * g + h
                gap = cols[:, n : n + 1] - r.run_s[pl.ds(HEADS * k + n, 1), :]
                damping = jnp.exp(jnp.where(below, gap, -1e30))
                parts.append((scores * damping * r.stride_s[pl.ds(HEADS * k + n, 1), :]).astype(bf16))
            near = jnp.dot(jnp.concatenate(parts, axis=0), r.x_s[k, g], preferred_element_type=f32)
            r.near_s[k, g] = jnp.where(first_head, near[:rows], near[rows:])
        return carry

    lax.fori_loop(0, blocks, near_step, 0)
    serve_slab()
    serve(*dims.serving[0])
    main, over, slots = dims.main, dims.over, places * dims.main
    total_slots = slots + over
    slot_row = lax.broadcasted_iota(jnp.int32, (total_slots, over), 0)
    slot_expert = lax.broadcasted_iota(jnp.int32, (total_slots, over), 1)
    spread = jnp.where(
        ((slot_row < slots) & (slot_row >= slot_expert * main) & (slot_row < slot_expert * main + main))
        | (slot_row == slots + slot_expert),
        1.0,
        0.0,
    ).astype(bf16)
    at = lax.broadcasted_iota(jnp.int32, (total_slots, rows), 0)
    turn = jnp.where(at < slots, jnp.bitwise_and(at, main - 1), main).astype(f32)
    expert_at = lax.broadcasted_iota(jnp.int32, (over, rows), 0).astype(f32)
    earlier = jnp.where(at_row < at_lane, 1.0, 0.0).astype(bf16)

    def make_put(col):
        table = r.tables[col]
        named = jnp.where((expert_at == table[0:1]) | (expert_at == table[1:2]), 1.0, 0.0)
        rank = jnp.dot(named.astype(bf16), earlier, preferred_element_type=f32)
        named_x = jnp.dot(spread, named.astype(bf16), preferred_element_type=f32)
        rank_x = jnp.dot(spread, rank.astype(bf16), preferred_element_type=f32)
        r.put[col] = jnp.where(rank_x == turn, named_x, 0.0).astype(bf16)

    tables_total.wait_recv()

    def put_step(col, carry):
        make_put(col)
        return carry

    lax.fori_loop(0, columns, put_step, 0)

    for load in loads[-2:]:
        load.wait()
    serve(*dims.serving[1])
    for n in range(1, chips):

        @pl.when(me_y >= n)
        def _():
            chip_total(n).wait_recv()

    row_at = lax.broadcasted_iota(jnp.int32, (piece, rows), 0) + core * piece
    half_two = row_at < STATE_TWO
    entering = jnp.zeros((piece, rows), f32)
    for y in range(chips):
        fades = r.all_fade[y]
        later = entering * jnp.where(half_two, fades[1:2], fades[0:1]) + r.all_pack[y].astype(f32)
        entering = jnp.where(y < me_y, later, entering)
    r.enter_pack[my_half, :] = entering.astype(bf16)
    here = r.enter_pack.at[my_half, :]
    enter_copy = remote(here, here, r.enter_send.at[0], r.enter_recv.at[0], mate)
    enter_copy.start()
    enter_copy.wait_recv()
    chip_state = r.enter_pack[...].astype(f32)
    after_low = chip_state * jnp.where(in_two, mate_rows[1:2], mate_rows[0:1]) + r.mate_pack[...].astype(f32)
    entered = jnp.where(is_low, chip_state, after_low)
    r.carry_s[1] = entered[:STATE_TWO]
    r.carry_s[0] = jnp.zeros((rows, rows), f32)
    r.carry_s[0, 0:STATE_ONE, :] = entered[STATE_TWO:]

    serve(*dims.serving[2])
    def head_copy(col):
        return remote(r.mixed_s.at[col], r.heads_in.at[me_x], r.head_send.at[0], r.head_recv.at[0], {"tp": col})

    def mix_step(k, carry):
        cols = jnp.exp(r.cols_s[k])
        r.gate_wide[...] = r.gate_in[pl.ds(pl.multiple_of(k * 2 * rows, 2 * rows), 2 * rows), :].astype(f32)
        for g in range(2):
            state = r.carry_s[g]
            coarse = state.astype(bf16)
            fine = (state - coarse.astype(f32)).astype(bf16)
            ask = r.q_s[k, g]
            far = jnp.dot(
                jnp.concatenate([ask, ask], axis=1),
                jnp.concatenate([coarse, fine], axis=0),
                preferred_element_type=f32,
            )
            reach = jnp.where(first_head, cols[:, 2 * g : 2 * g + 1], cols[:, 2 * g + 1 : 2 * g + 2])
            skip = jnp.where(first_head[0:1], r.skip_ref[g, 0], r.skip_ref[g, 1])
            mixed = r.near_s[k, g] + far * reach + skip * r.x_s[k, g].astype(f32)
            gated = mixed * silu(r.gate_wide[pl.ds(g, rows, stride=2), :])
            square = gated * gated
            one = jnp.sum(jnp.where(first_head, square, 0.0), axis=1, keepdims=True)
            two = jnp.sum(jnp.where(first_head, 0.0, square), axis=1, keepdims=True)
            scale = lax.rsqrt(jnp.where(first_head, one, two) * (1.0 / HEAD_DIM) + EPSILON)
            r.mixed_s[k, :, g * rows : (g + 1) * rows] = (gated * scale * r.head_gain_ref[g : g + 1, :]).astype(bf16)
            r.carry_s[g] = state * row_pair(r.end_s, k, g) + r.state_s[k, g]

        @pl.when(k != me_x)
        def _():
            head_copy(k).start()

        return carry

    lax.fori_loop(0, blocks, mix_step, 0)
    r.heads_in[me_x] = r.mixed_s[me_x]

    slot_col = lax.broadcasted_iota(jnp.int32, (over, total_slots), 1)
    slot_exp = lax.broadcasted_iota(jnp.int32, (over, total_slots), 0)
    spread_t = jnp.where(
        ((slot_col < slots) & (slot_col >= slot_exp * main) & (slot_col < slot_exp * main + main))
        | (slot_col == slots + slot_exp),
        1.0,
        0.0,
    ).astype(bf16)
    at_t = lax.broadcasted_iota(jnp.int32, (rows, total_slots), 1)
    turn_t = jnp.where(at_t < slots, jnp.bitwise_and(at_t, main - 1), main).astype(f32)
    expert_to = lax.broadcasted_iota(jnp.int32, (rows, over), 1).astype(f32)
    later_t = jnp.where(at_lane < at_row, 1.0, 0.0).astype(bf16)

    def make_pick(col):
        table = jnp.transpose(r.tables[col])
        named = [jnp.where(expert_to == table[:, k : k + 1], 1.0, 0.0) for k in range(2)]
        rank = jnp.dot(later_t, (named[0] + named[1]).astype(bf16), preferred_element_type=f32)
        rank_x = jnp.dot(rank.astype(bf16), spread_t, preferred_element_type=f32)
        for k in range(2):
            named_x = jnp.dot(named[k].astype(bf16), spread_t, preferred_element_type=f32)
            r.pick[col, k] = jnp.where(rank_x == turn_t, named_x, 0.0).astype(bf16)
            r.share_s[col, k] = jnp.broadcast_to(table[:, 2 + k : 3 + k], (rows, rows))

    def product(block, low, high, first):
        for n in range(low, high, 512):
            span = slice(n, min(n + 512, high))
            part = jnp.dot(r.heads_in[column(block)], r.matrix[block, :, span], preferred_element_type=f32)
            r.acc_s[:, span] = part if first else r.acc_s[:, span] + part

    serve(*dims.serving[3])
    serve(*list(waiting))
    heads_total = remote(
        r.mixed_s.at[most_columns], r.heads_in.at[most_columns], r.head_send.at[0], r.head_recv.at[0], right
    )
    heads_total.wait_recv()
    for which, (low_lane, high_lane) in enumerate(((0, ring_part), (ring_part, width))):
        remote(pass_totals[which], pass_totals[which], r.pass_send.at[which], r.pass_recv.at[which], mate).wait_recv()
        for block in range(columns):
            product(block, low_lane, high_lane, block == 0)

    stream = (r.residual_in[...].astype(f32) + r.acc_s[...]).astype(bf16)
    r.stream_s[...] = stream
    wide = stream.astype(f32)
    scale = lax.rsqrt(jnp.mean(wide * wide, axis=1, keepdims=True) + EPSILON)
    normed = (wide * scale * r.expert_gain_ref[...]).astype(bf16)

    direct, extra = dims.direct, dims.pieces - dims.direct
    pieces = dims.pieces
    lanes_of = PIECE // 128

    def lines(index):
        return pl.ds(pl.multiple_of(index * main, main), main)

    def far(way, p):
        odd = lax.rem(p, 2) if not isinstance(p, int) else p % 2
        return half - odd if way == 0 else half - 1 + odd

    for q in range(extra):
        r.tokens[me_x, q] = normed[:, (direct + q) * PIECE : (direct + q + 1) * PIECE]

    thin = extra * lanes_of

    def token_ring(way, step, q, col):
        here = r.tokens.at[col, q // lanes_of, :, pl.ds(q % lanes_of * 128, 128)]
        return remote(here, here, r.token_send.at[0], r.token_recv.at[step, q], toward(way))

    put_own = r.put[me_x]

    def make_out(p):
        part = jnp.dot(put_own, normed[:, p * PIECE : (p + 1) * PIECE], preferred_element_type=f32)
        r.outbound[p] = part[:slots].astype(bf16)
        for c in range(lanes_of):
            r.over_out[:, p * lanes_of + c, :] = part[slots:, c * 128 : (c + 1) * 128]

    def send_out(p, carry):
        for i in range(1, places):
            remote(
                r.outbound.at[p, lines(place(i)), :],
                r.chunks.at[me_x, p, lines(me_s), :],
                r.out_send.at[0],
                r.out_recv.at[p],
                {"sp": place(i)},
            ).start()
        r.chunks[me_x, p, lines(me_s), :] = r.outbound[p, lines(me_s), :]
        return carry

    make_out(0)
    send_out(0, 0)
    for q in range(thin):
        for way in range(2):
            token_ring(way, 0, q, me_x).start()
    for p in range(1, direct):
        make_out(p)
    lax.fori_loop(1, direct, send_out, 0)
    for i in range(1, places):
        remote(
            r.over_out.at[place(i)], r.over_in.at[me_s], r.over_send.at[0], r.over_recv.at[0], {"sp": place(i)}
        ).start()
    r.over_in[me_s] = r.over_out[me_s]
    if places < over:
        r.over_in[places:over] = jnp.zeros((over - places, *r.over_in.shape[1:]), f32)
        r.over_ret[:, places:over] = jnp.zeros((2, over - places, *r.over_ret.shape[2:]), f32)
        r.xover_in[:, places:over] = jnp.zeros((columns, over - places, *r.xover_in.shape[2:]), f32)
        r.xover_ret[:, places:over] = jnp.zeros((columns, over - places, *r.xover_ret.shape[2:]), f32)

    def route(offset):
        col = column(offset)
        for q in range(extra):
            part = jnp.dot(r.put[col], r.tokens[col, q], preferred_element_type=f32)
            r.xout[col, q] = part[:slots].astype(bf16)
            r.chunks[col, direct + q, lines(me_s), :] = r.xout[col, q, lines(me_s), :]
            for c in range(lanes_of):
                r.xover_out[offset, :, q * lanes_of + c, :] = part[slots:, c * 128 : (c + 1) * 128]
        r.xover_in[offset, me_s] = r.xover_out[offset, me_s]
        for i in range(1, places):
            remote(
                r.xout.at[col, :, lines(place(i)), :],
                r.chunks.at[col, pl.ds(direct, extra), lines(me_s), :],
                r.xout_send.at[0],
                r.xout_recv.at[offset],
                {"sp": place(i)},
            ).start()
            remote(
                r.xover_out.at[offset, place(i)],
                r.xover_in.at[offset, me_s],
                r.xover_send.at[0],
                r.xover_recv.at[0, offset],
                {"sp": place(i)},
            ).start()

    def routed(offset):
        col = column(offset)
        most = pl.ds(0, (places - 1) * main)
        return (
            remote(
                r.xout.at[col, :, most, :],
                r.chunks.at[col, pl.ds(direct, extra), most, :],
                r.xout_send.at[0],
                r.xout_recv.at[offset],
                right,
            ),
            remote(
                r.xover_out.at[offset, 0 : places - 1],
                r.xover_in.at[offset, 0 : places - 1],
                r.xover_send.at[0],
                r.xover_recv.at[0, offset],
                right,
            ),
        )

    def take_routed(offset):
        col = column(offset)
        for copy in routed(offset):
            copy.wait_recv()
        for q in range(extra):
            for c in range(lanes_of):
                r.chunks[col, direct + q, slots:, c * 128 : (c + 1) * 128] = r.xover_in[
                    offset, :, q * lanes_of + c, :
                ].astype(bf16)

    def token_event(k):
        for q in range(thin):
            came = r.tokens.at[pl.ds(0, 2 if k < half else 1), 0, :, pl.ds(0, 128)]
            remote(came, came, r.token_send.at[0], r.token_recv.at[k - 1, q], right).wait_recv()
            for way in range(2):
                if k < far(way, q):
                    token_ring(way, k, q, column(-k if way == 0 else k)).start()

    def chunk_ring(way, step, p, col):
        here = r.chunks.at[col, p, pl.ds(0, slots), :]
        return remote(here, here, r.chunk_send.at[0], r.chunk_recv.at[step, p], toward(way))

    def over_ring(way, step, col):
        here = r.chunks.at[col, pl.ds(0, direct), pl.ds(slots, over), :]
        return remote(here, here, r.tail_send.at[0], r.tail_recv.at[step], toward(way))

    def out_arrived(p):
        most = pl.ds(0, (places - 1) * main)
        return remote(
            r.outbound.at[p, most, :], r.chunks.at[me_x, p, most, :], r.out_send.at[0], r.out_recv.at[p], right
        )

    def start_piece(p):
        out_arrived(p).wait_recv()
        chunk_ring(0, 0, p, me_x).start()
        chunk_ring(1, 0, p, me_x).start()

    def start_over():
        remote(
            r.over_out.at[0 : places - 1], r.over_in.at[0 : places - 1], r.over_send.at[0], r.over_recv.at[0], right
        ).wait_recv()
        for c in range(direct * lanes_of):
            at_lanes = (c % lanes_of) * 128
            r.chunks[me_x, c // lanes_of, slots:, at_lanes : at_lanes + 128] = r.over_in[:, c, :].astype(bf16)
        for way in range(2):
            over_ring(way, 0, me_x).start()

    for copy in rims + mates + [enter_copy]:
        copy.wait_send()
    for n in range(1, chips):

        @pl.when(me_y + n < chips)
        def _():
            chip_total(n).wait_send()

    heads_total.wait_send()
    tables_total.wait_send()
    remote(ring_total, ring_total, r.ring_send.at[0], r.ring_recv.at[0, 0], right).wait_send()
    remote(slab_total, slab_total, r.slab_send.at[0], r.slab_recv.at[0], right).wait_send()
    remote(grid_total, grid_total, r.grid_send.at[0], r.grid_recv.at[0], right).wait_send()
    for which in range(2):
        view = pass_totals[which]
        remote(view, view, r.pass_send.at[which], r.pass_recv.at[which], mate).wait_send()

    def offset_of(n):
        k = (n + 1) // 2 if isinstance(n, int) else lax.div(n + 1, 2)
        if isinstance(n, int):
            return (columns - k) % columns if n % 2 else k
        return jnp.where(lax.rem(n, 2) == 1, lax.rem(columns - k, columns), k)

    opening = {"token": token_event, "piece": start_piece, "route": lambda n: route(offset_of(n)), "over": lambda n: start_over()}
    for kind, n in dims.opening:
        opening[kind](n)

    def unit(n, t):
        offset = offset_of(n)
        col = column(offset)
        pl.when(t == 0)(lambda: take_routed(offset))
        acc = jnp.dot(r.chunks[col, 0], r.gate_up[t, 0:PIECE, :], preferred_element_type=f32)
        for q in range(1, pieces):
            acc = acc + jnp.dot(
                r.chunks[col, q], r.gate_up[t, q * PIECE : (q + 1) * PIECE, :], preferred_element_type=f32
            )
        value = silu(acc[:, 0:128]) * acc[:, 128:256]
        r.hidden[col, :, pl.ds(pl.multiple_of(t * 128, 128), 128)] = value.astype(bf16)
        pl.when(t == dims.tiles - 1)(lambda: give_back(offset))

    def own(col, p):
        return jnp.dot(r.hidden[col], r.down[p], preferred_element_type=f32)

    def give_back(offset):
        col = column(offset)
        for q in range(extra):
            part = own(col, direct + q)
            r.xback[col, q] = part[:slots].astype(bf16)
            r.xret[col, q, lines(me_s), :] = r.xback[col, q, lines(me_s), :]
            for c in range(lanes_of):
                r.xover_back[offset, :, q * lanes_of + c, :] = part[slots:, c * 128 : (c + 1) * 128]
        r.xover_ret[offset, me_s] = r.xover_back[offset, me_s]
        for i in range(1, places):
            remote(
                r.xback.at[col, :, lines(place(i)), :],
                r.xret.at[col, :, lines(me_s), :],
                r.xback_send.at[0],
                r.xback_recv.at[offset],
                {"sp": place(i)},
            ).start()
            remote(
                r.xover_back.at[offset, place(i)],
                r.xover_ret.at[offset, me_s],
                r.xover_send.at[1],
                r.xover_recv.at[1, offset],
                {"sp": place(i)},
            ).start()

    def given_back(offset):
        col = column(offset)
        most = pl.ds(0, (places - 1) * main)
        return (
            remote(
                r.xback.at[col, :, most, :],
                r.xret.at[col, :, most, :],
                r.xback_send.at[0],
                r.xback_recv.at[offset],
                right,
            ),
            remote(
                r.xover_back.at[offset, 0 : places - 1],
                r.xover_ret.at[offset, 0 : places - 1],
                r.xover_send.at[1],
                r.xover_recv.at[1, offset],
                right,
            ),
        )

    for n, weights in enumerate((r.gate_up, r.down)):
        pltpu.make_async_copy(weights, weights, r.weight_sem.at[n]).wait()

    def units(low, high):
        def body(v, carry):
            unit(lax.div(v, dims.tiles), lax.rem(v, dims.tiles))
            return carry

        lax.fori_loop(low, high, body, 0)

    def hop(way, j, p):
        return remote(
            r.sums.at[way, j, p],
            r.sums.at[way, j - 1, p],
            r.sum_send.at[0],
            r.sum_recv.at[way, j - 1, p],
            {"tp": column(1 - 2 * way)},
        )

    def chains(long, step, group):
        j = half - step if long else half - 1 - step

        def body(p, carry):
            odd = lax.rem(p, 2)
            way = 1 - odd if long else odd
            value = own(column(j * (1 - 2 * way)), p)
            if step > 0:
                hop(way, j + 1, p).wait_recv()
                value = value + r.sums[way, j, p].astype(f32)
            r.sums[way, j, p] = value.astype(bf16)
            hop(way, j, p).start()
            return carry

        lax.fori_loop(*group, body, 0)

    share_of = dims.schedule
    for k in range(1, half + 1):
        first, last = share_of[k - 1] * dims.tiles, share_of[k] * dims.tiles

        if k == half and half > 1:
            units(first, last)
            first = last
            for group in dims.groups:
                chains(False, 0, group)

        def pass_on(p, carry, k=k, first=first, last=last):
            came = r.chunks.at[pl.ds(0, 2 if k < half else 1), p, pl.ds(0, slots), :]
            remote(came, came, r.chunk_send.at[0], r.chunk_recv.at[k - 1, p], right).wait_recv()
            if k < half:
                for way in range(2):
                    start = lambda way=way: chunk_ring(way, k, p, column(-k if way == 0 else k)).start()
                    if k < half - 1:
                        start()
                    else:
                        pl.when(k < far(way, p))(start)

            if k == 1 and dims.routed < columns:
                pl.when(p < columns - dims.routed)(lambda: route(offset_of(p + dims.routed)))
            if last > first:
                units(
                    first + lax.div(p * (last - first), direct), first + lax.div((p + 1) * (last - first), direct)
                )
            return carry

        lax.fori_loop(0, direct, pass_on, 0)
        came = r.chunks.at[pl.ds(0, 2 if k < half else 1), pl.ds(0, direct), pl.ds(slots, over), :]
        remote(came, came, r.tail_send.at[0], r.tail_recv.at[k - 1], right).wait_recv()
        for way in range(2):
            if k < far(way, 0):
                over_ring(way, k, column(-k if way == 0 else k)).start()
        if k == 1:
            lax.fori_loop(0, columns, lambda col, carry: (make_pick(col), carry)[1], 0)
    units(share_of[half] * dims.tiles, columns * dims.tiles)

    def finish(p, carry):
        value = own(me_x, p)
        hop(0, 1, p).wait_recv()
        hop(1, 1, p).wait_recv()
        value = value + r.sums[0, 0, p].astype(f32) + r.sums[1, 0, p].astype(f32)
        r.totals[p] = value[0:slots].astype(bf16)
        r.over_total[p] = value[slots:]
        r.returned[p, lines(me_s), :] = r.totals[p, lines(me_s), :]
        for i in range(1, places):
            remote(
                r.totals.at[p, lines(place(i)), :],
                r.returned.at[p, lines(me_s), :],
                r.back_send.at[0],
                r.back_recv.at[p],
                {"sp": place(i)},
            ).start()
        return carry

    def weighted(col, table):
        one = jnp.dot(r.pick[col, 0], table, preferred_element_type=f32)
        two = jnp.dot(r.pick[col, 1], table, preferred_element_type=f32)
        copies = one.shape[1] // 128
        first, second = (jnp.concatenate([r.share_s[col, k]] * copies, axis=1) for k in range(2))
        return first * one + second * two

    def take_back(offset):
        col = column(offset)
        for copy in given_back(offset):
            copy.wait_recv()
        for q in range(extra):
            for c in range(lanes_of):
                r.xret[col, q, slots:, c * 128 : (c + 1) * 128] = r.xover_ret[
                    offset, :, q * lanes_of + c, :
                ].astype(bf16)

    def token_hop(way, j, q):
        return remote(
            r.xsums.at[way, j, q],
            r.xsums.at[way, j - 1, q],
            r.xsum_send.at[0],
            r.xsum_recv.at[way, j - 1, q],
            toward(way),
        )

    taken = set()

    def thin_part(col, q):
        return weighted(col, r.xret[col, q // lanes_of, :, q % lanes_of * 128 : (q % lanes_of + 1) * 128])

    def token_round(t):
        for q in range(thin):
            for way in range(2):
                j = far(1 - way, q) - t
                if j < 1:
                    continue
                offset = j if way == 0 else columns - j
                if offset not in taken:
                    taken.add(offset)
                    take_back(offset)
                value = thin_part(column(offset), q)
                if t > 0:
                    token_hop(way, j + 1, q).wait_recv()
                    value = value + r.xsums[way, j, q].astype(f32)
                r.xsums[way, j, q] = value.astype(bf16)
                token_hop(way, j, q).start()

    for group in dims.groups:
        chains(True, 0, group)
    def left_by_now(view, send, recv):
        remote(view, view, send, recv, right).wait_send()

    most_places, most_lines = pl.ds(0, places - 1), pl.ds(0, (places - 1) * main)
    chunks_total = r.chunks.at[most_columns, pl.ds(0, direct), pl.ds(0, slots), :]
    left_by_now(r.over_out.at[most_places], r.over_send.at[0], r.over_recv.at[0])
    left_by_now(r.tokens.at[most_columns], r.token_send.at[0], r.token_recv.at[0, 0])
    left_by_now(r.chunks.at[most_columns, pl.ds(0, direct), pl.ds(slots, over), :], r.tail_send.at[0], r.tail_recv.at[0])
    left_by_now(chunks_total, r.chunk_send.at[0], r.chunk_recv.at[0, 0])
    left_by_now(r.outbound.at[:, most_lines, :], r.out_send.at[0], r.out_recv.at[0])
    left_by_now(r.xout.at[:, :, most_lines, :], r.xout_send.at[0], r.xout_recv.at[0])
    left_by_now(r.xover_out.at[:, most_places], r.xover_send.at[0], r.xover_recv.at[0, 0])
    def over_back_copy(n, to, at):
        return remote(
            r.over_back.at[n, to],
            r.over_ret.at[n, at],
            r.over_send.at[1],
            r.over_recv.at[1 + n],
            {"sp": to},
        )

    def send_over_back(n, group):
        for p in range(*group):
            for c in range(lanes_of):
                r.over_back[n, :, (p - group[0]) * lanes_of + c, :] = r.over_total[p, :, c * 128 : (c + 1) * 128]
        r.over_ret[n, me_s] = r.over_back[n, me_s]
        for i in range(1, places):
            over_back_copy(n, place(i), me_s).start()

    for kind, step, group in dims.closing:
        if kind == "short":
            chains(False, step, group)
        elif kind == "long":
            chains(True, step, group)
        elif kind == "token":
            token_round(step)
        else:
            lax.fori_loop(*group, finish, 0)
            send_over_back(dims.groups.index(group), group)
    left_by_now(r.xback.at[:, :, most_lines, :], r.xback_send.at[0], r.xback_recv.at[0])
    left_by_now(r.xover_back.at[:, most_places], r.xover_send.at[1], r.xover_recv.at[1, 0])
    left_by_now(r.chunks.at[most_columns, pl.ds(0, direct)], r.sum_send.at[0], r.sum_recv.at[0, 0, 0])
    token_round(half - 1)
    def back_arrived(p):
        most = pl.ds(0, (places - 1) * main)
        return remote(
            r.totals.at[p, most, :], r.returned.at[p, most, :], r.back_send.at[0], r.back_recv.at[p], right
        )

    def combine(p, carry):
        back_arrived(p).wait_recv()
        span = pl.ds(pl.multiple_of(p * PIECE, PIECE), PIECE)
        value = weighted(me_x, r.returned[p])
        r.out_ref[:, span] = (r.stream_s[:, span].astype(f32) + value).astype(bf16)
        return carry

    def combine_group(n, group):
        remote(
            r.over_back.at[n, 0 : places - 1],
            r.over_ret.at[n, 0 : places - 1],
            r.over_send.at[1],
            r.over_recv.at[1 + n],
            right,
        ).wait_recv()
        for p in range(*group):
            for c in range(lanes_of):
                r.returned[p, slots:, c * 128 : (c + 1) * 128] = r.over_ret[n, :, (p - group[0]) * lanes_of + c, :].astype(bf16)
        lax.fori_loop(*group, combine, 0)

    combine_group(dims.groups.index(dims.order[0]), dims.order[0])
    take_back(0)
    for q in range(thin):
        value = thin_part(me_x, q)
        for way in range(2):
            token_hop(way, 1, q).wait_recv()
            value = value + r.xsums[way, 0, q].astype(f32)
        span = slice(direct * PIECE + q * 128, direct * PIECE + (q + 1) * 128)
        r.out_ref[:, span] = (r.stream_s[:, span].astype(f32) + value).astype(bf16)

    combine_group(dims.groups.index(dims.order[1]), dims.order[1])

    left_by_now(r.over_back.at[:, most_places], r.over_send.at[1], r.over_recv.at[1])
    left_by_now(r.tokens.at[most_columns], r.xsum_send.at[0], r.xsum_recv.at[0, 0, 0])
    left_by_now(r.totals.at[:, most_lines, :], r.back_send.at[0], r.back_recv.at[0])


def layer(places, columns, **given):
    f32, bf16 = jnp.float32, jnp.bfloat16
    rows, width = given["residual_hbm"].shape
    small = [name for name in given if name.endswith("_small")]
    units = given["expert_gate_hbm"].shape[2]
    lanes = given["keys_hbm"].shape[1]
    positions = columns * BLOCK
    half, chips, blocks = columns // 2, places // 2, columns
    main = 2 * rows // places
    over = -(-places // 16) * 16
    pieces = width // PIECE
    extra = max(1, pieces // 4)
    direct = pieces - extra
    tiles, total = units // 128, places * main + over
    ring_part = width * RING_SHARE // 16 // 128 * 128
    schedule = (0, 0, 1, 5, 7) if half == 4 else (0,) * half + (columns - 1,)
    if half == 4:
        opening = [("token", 1), ("piece", 0), ("token", 2), ("piece", 1), ("piece", 2), ("token", 3), ("piece", 3)]
        opening += [("route", 0), ("piece", 4), ("token", 4), ("piece", 5), ("route", 1), ("route", 2), ("over", 0)]
    else:
        opening = [("token", n) for n in range(1, half + 1)] + [("piece", n) for n in range(direct)]
        opening += [("route", n) for n in range(columns)] + [("over", 0)]
    routed = sum(kind == "route" for kind, _ in opening)
    serving = [
        [("x", 0)],
        [("x", 1)],
        [("x", 2)],
        [("x", 3), ("y", 0), ("y", 1), ("y", 2), ("x", 4), ("y", 3), ("y", 4), ("y", 5), ("x", 5), ("x", 6), ("y", 6)],
    ]
    low, high = (0, (direct + 1) // 2), ((direct + 1) // 2, direct)
    groups = [high, low]
    if half == 4:
        closing = [
            ("long", 1, high),
            ("short", 1, high),
            ("long", 1, low),
            ("short", 1, low),
            ("long", 2, low),
            ("long", 2, high),
            ("long", 3, low),
            ("short", 2, low),
            ("token", 0, None),
            ("long", 3, high),
            ("short", 2, high),
            ("finish", None, low),
            ("token", 1, None),
            ("finish", None, high),
            ("token", 2, None),
        ]
    else:
        closing = []
        for step in range(1, half):
            closing += [("short", step, group) for group in groups if step < half - 1]
            closing += [("long", step, group) for group in groups]
            closing.append(("token", step - 1, None))
        closing += [("finish", None, group) for group in groups]
    dims = types.SimpleNamespace(
        places=places, columns=columns, width=width, main=main, over=over, pieces=pieces, direct=direct, tiles=tiles,
        schedule=schedule, opening=opening, routed=routed, small=small, groups=groups, order=(low, high), closing=closing, ring_part=ring_part, serving=serving,
    )
    packed = STATE_ONE + STATE_TWO
    square = (blocks, 2, BLOCK, BLOCK)
    vmem = lambda *shape, dtype=bf16: pltpu.VMEM(shape, dtype)
    dma = lambda *shape: pltpu.SemaphoreType.DMA(shape)
    in_specs = [pl.BlockSpec(memory_space=pltpu.SMEM if a.shape == (2, 2) else pl.ANY) for a in given.values()]
    lane_rows = PIECE // 128
    scratch = {name[:-5] + "ref": pltpu.VMEM(given[name].shape, given[name].dtype) for name in small}
    scratch |= dict(
        residual_in=vmem(rows, width),
        value_in=vmem(2 * positions + 16, BLOCK),
        gate_in=vmem(2 * positions, BLOCK),
        keys_in=vmem(positions + 16, lanes),
        gate_wide=vmem(2 * BLOCK, BLOCK, dtype=f32),
        conv_wide=vmem(2 * BLOCK, BLOCK, dtype=f32),
        x_s=vmem(*square),
        kt_s=vmem(*square),
        q_s=vmem(*square),
        state_s=vmem(*square, dtype=f32),
        near_s=vmem(*square, dtype=f32),
        stride_s=vmem(HEADS * blocks, BLOCK, dtype=f32),
        run_s=vmem(HEADS * blocks, BLOCK, dtype=f32),
        fade_s=vmem(HEADS * blocks, BLOCK, dtype=f32),
        end_s=vmem(HEADS * blocks, BLOCK, dtype=f32),
        cols_s=vmem(blocks, BLOCK, HEADS, dtype=f32),
        own_pack=vmem(packed, BLOCK),
        own_fade=vmem(8, BLOCK, dtype=f32),
        mate_pack=vmem(packed, BLOCK),
        mate_fade=vmem(8, BLOCK, dtype=f32),
        chip_pack=vmem(packed, BLOCK),
        chip_fade=vmem(8, BLOCK, dtype=f32),
        all_pack=vmem(chips, packed // 2, BLOCK),
        all_fade=vmem(chips, 8, BLOCK, dtype=f32),
        enter_pack=vmem(packed, BLOCK),
        carry_s=vmem(2, BLOCK, BLOCK, dtype=f32),
        mixed_s=vmem(columns, BLOCK, 2 * BLOCK),
        heads_in=vmem(columns, BLOCK, 2 * BLOCK),
        matrix=vmem(columns, 2 * BLOCK, width),
        acc_s=vmem(rows, width, dtype=f32),
        stream_s=vmem(rows, width),
        tables=vmem(columns, 8, rows, dtype=f32),
        put=vmem(columns, total, rows),
        pick=vmem(columns, 2, rows, total),
        share_s=vmem(columns, 2, rows, 128, dtype=f32),
        tokens=vmem(columns, extra, rows, PIECE),
        outbound=vmem(direct, places * main, PIECE),
        over_out=vmem(over, direct * lane_rows, 128, dtype=f32),
        over_in=vmem(over, direct * lane_rows, 128, dtype=f32),
        over_back=vmem(2, over, (high[1] - low[0] + 1) // 2 * lane_rows, 128, dtype=f32),
        over_ret=vmem(2, over, (high[1] - low[0] + 1) // 2 * lane_rows, 128, dtype=f32),
        over_total=vmem(direct, over, PIECE, dtype=f32),
        xout=vmem(columns, extra, places * main, PIECE),
        xback=vmem(columns, extra, places * main, PIECE),
        xret=vmem(columns, extra, total, PIECE),
        xover_out=vmem(columns, over, extra * lane_rows, 128, dtype=f32),
        xover_in=vmem(columns, over, extra * lane_rows, 128, dtype=f32),
        xover_back=vmem(columns, over, extra * lane_rows, 128, dtype=f32),
        xover_ret=vmem(columns, over, extra * lane_rows, 128, dtype=f32),
        chunks=vmem(columns, pieces, total, PIECE),
        hidden=vmem(columns, total, units),
        gate_up=vmem(tiles, width, 256),
        down=vmem(pieces, units, PIECE),
        sums=vmem(2, half + 1, direct, total, PIECE),
        xsums=vmem(2, half + 1, extra * lane_rows, rows, 128),
        totals=vmem(direct, places * main, PIECE),
        returned=vmem(direct, total, PIECE),
        load_sem=dma(6),
        weight_sem=dma(2),
        small_sem=dma(len(small)),
    )
    steps = (2, half)
    for name, send, recv in (
        ("rim", (2,), (2,)),
        ("mate", (2,), (2,)),
        ("chip", (chips,), (chips,)),
        ("enter", (1,), (1,)),
        ("head", (1,), (1,)),
        ("table", (1,), (1,)),
        ("ring", (1,), (columns - 1, 2)),
        ("slab", (1,), (1,)),
        ("grid", (1,), (chips - 1,)),
        ("pass", (2,), (2,)),
        ("over", (2,), (3,)),
        ("token", (1,), (half, extra * lane_rows)),
        ("out", (1,), (direct,)),
        ("xout", (1,), (columns,)),
        ("xover", (2,), (2, columns)),
        ("chunk", (1,), (half, direct)),
        ("tail", (1,), (half,)),
        ("xback", (1,), (columns,)),
        ("sum", (1,), (*steps, direct)),
        ("xsum", (1,), (*steps, extra * lane_rows)),
        ("back", (1,), (direct,)),
    ):
        scratch[name + "_send"], scratch[name + "_recv"] = dma(*send), dma(*recv)
    names = [*given, "out_ref", *scratch]
    return pl.pallas_call(
        functools.partial(layer_kernel, dims, names),
        out_shape=pltpu.VMEM((rows, width), bf16),
        in_specs=in_specs,
        out_specs=pl.BlockSpec(memory_space=pltpu.VMEM),
        scratch_shapes=list(scratch.values()),
        compiler_params=pltpu.CompilerParams(
            collective_id=0, has_side_effects=True, vmem_limit_bytes=VMEM_LIMIT
        ),
        name="layer",
    )(*given.values())


def local(
    residual,
    grouped_value_heads,
    output_gate_heads,
    projected_key_query,
    raw_step_size,
    step_size_bias,
    head_decay_logarithm,
    position_extra_decay,
    head_skip_weight,
    value_kernel_taps,
    key_query_kernel,
    head_norm_gain,
    output_matrix,
    expert_norm_gain,
    expert_gate_weight,
    expert_up_weight,
    expert_down_weight,
    token_expert_choice,
    expert_output_weight,
):
    return layer(
        lax.axis_size("sp"),
        lax.axis_size("tp"),
        residual_hbm=residual,
        value_hbm=grouped_value_heads.reshape(-1, BLOCK),
        gate_hbm=output_gate_heads.reshape(-1, BLOCK),
        keys_hbm=projected_key_query,
        raw_small=raw_step_size.transpose(1, 2, 0),
        bias_ref=step_size_bias,
        log_ref=head_decay_logarithm,
        extra_small=position_extra_decay.reshape(-1, BLOCK),
        skip_ref=head_skip_weight,
        value_tap_small=value_kernel_taps.reshape(-1, BLOCK),
        key_tap_small=key_query_kernel,
        head_gain_small=head_norm_gain,
        matrix_hbm=output_matrix,
        expert_gain_small=expert_norm_gain[None],
        choice_small=token_expert_choice.T,
        share_small=expert_output_weight.T,
        expert_gate_hbm=expert_gate_weight,
        expert_up_hbm=expert_up_weight,
        expert_down_hbm=expert_down_weight,
    )


def solution(mesh):
    placed = (
        P(("grp", "sp", "tp"), None),
        P(("grp", "sp"), None, "tp"),
        P(("grp", "sp"), None, "tp"),
        P(("grp", "sp"), None),
        P(("grp", "sp"), None, "tp"),
        P(None, "tp"),
        P(None, "tp"),
        P(("grp", "sp")),
        P(None, "tp"),
        P(None, None, "tp"),
        P(),
        P(None, "tp"),
        P(None, "tp", None),
        P(),
        P("sp", None, "tp"),
        P("sp", None, "tp"),
        P("sp", "tp", None),
        P(("grp", "sp", "tp"), None),
        P(("grp", "sp", "tp"), None),
    )
    return jax.shard_map(
        local, mesh=mesh, in_specs=placed, out_specs=P(("grp", "sp", "tp"), None), check_vma=False
    )
```

```python
import functools
import types

import jax
import jax.numpy as jnp
from jax import lax
from jax.experimental import pallas as pl
from jax.experimental.pallas import tpu as pltpu
from jax.sharding import PartitionSpec as P

HEAD_DIM = 64
STATE_ONE = 64
STATE_TWO = 128
BLOCK = 128
EPSILON = 1e-06

MESH = pl.DeviceIdType.MESH
PIECE = 256
HEADS = 4
RING_SHARE = 7
VMEM_LIMIT = 61600000


def remote(src, dst, send, recv, device):
    return pltpu.make_async_remote_copy(
        src_ref=src, dst_ref=dst, send_sem=send, recv_sem=recv, device_id=device, device_id_type=MESH
    )


def silu(a):
    return a * (1.0 / (1.0 + jnp.exp(-a)))


def layer_kernel(dims, names, *refs):
    r = types.SimpleNamespace(**dict(zip(names, refs, strict=True)))
    f32, bf16 = jnp.float32, jnp.bfloat16
    places, columns, width, rows = dims.places, dims.columns, dims.width, BLOCK
    half, chips, blocks = columns // 2, places // 2, columns
    me_x, me_s = lax.axis_index("tp"), lax.axis_index("sp")
    core, me_y = lax.rem(me_s, 2), lax.div(me_s, 2)
    right = {"tp": lax.rem(me_x + 1, columns)}
    left = {"tp": lax.rem(me_x + columns - 1, columns)}
    mate = {"sp": me_s + 1 - 2 * core}
    following = {"sp": lax.rem(me_s + 1, places)}

    def column(offset):
        return lax.rem(me_x + offset + columns, columns)

    def place(offset):
        return lax.rem(me_s + offset, places)

    def peer(offset):
        return {"sp": lax.rem(me_s + 2 * offset, places)}

    def toward(way):
        return right if way == 0 else left

    barrier = pltpu.get_barrier_semaphore()
    peers = sorted(
        [(min(i, columns - i), {"tp": column(i)}) for i in range(1, columns)]
        + [(min(i, places - i) / 2, {"sp": place(i)}) for i in sorted({1, 2, places - 2, places - 1})],
        key=lambda peer: -peer[0],
    )
    peers = [device for _, device in peers]
    later = 0
    for n in range(2, chips - 1):
        later = later + jnp.where(me_y + n < chips, 1, 0)

        @pl.when(me_y + n >= chips)
        def _():
            pl.semaphore_signal(barrier, inc=1, device_id=peer(n), device_id_type=MESH)

    for device in peers:
        pl.semaphore_signal(barrier, inc=1, device_id=device, device_id_type=MESH)

    small = {
        name: pltpu.make_async_copy(getattr(r, name), getattr(r, name[:-5] + "ref"), r.small_sem.at[n])
        for n, name in enumerate(dims.small)
    }
    ring_part, slab = dims.ring_part, rows // chips
    rim_rows, positions = 16, blocks * rows
    mine = pl.multiple_of(core * rows, rows)

    def slab_rows(y):
        return pl.ds(pl.multiple_of(mine + y * slab, 16), slab)

    on_ring, on_grid = pl.ds(0, ring_part), pl.ds(ring_part, width - ring_part)
    loads = [
        (r.matrix_hbm.at[0], r.matrix.at[0, pl.ds(0, rows), :]),
        (r.matrix_hbm.at[1], r.matrix.at[0, pl.ds(rows, rows), :]),
        (r.value_hbm, r.value_in.at[pl.ds(rim_rows, 2 * positions), :]),
        (r.keys_hbm, r.keys_in.at[pl.ds(rim_rows, positions), :]),
        (r.gate_hbm, r.gate_in),
        (r.residual_hbm, r.residual_in),
    ]
    loads = [pltpu.make_async_copy(a, b, r.load_sem.at[n]) for n, (a, b) in enumerate(loads)]
    for load in loads[:2] + list(small.values()) + loads[2:4]:
        load.start()
    for name in ("choice_small", "share_small"):
        small[name].wait()
    r.tables[me_x] = jnp.zeros((8, rows), f32)
    r.tables[me_x, 0:2, :] = r.choice_ref[...].astype(f32)
    r.tables[me_x, 2:4, :] = r.share_ref[...]

    for load in loads[:2]:
        load.wait()
    pl.semaphore_wait(barrier, len(peers) + later)

    def matrix_block(way, event, k, sub):
        piece = ((event % 2) ^ way) * 2 + sub
        block = (columns - k if way == 0 else k) % columns
        return r.matrix.at[block, pl.ds(pl.multiple_of(mine + piece * (rows // 4), 16), rows // 4), on_ring]

    def matrix_ring(way, event, sub):
        k = event // 2
        return remote(
            matrix_block(way, event, k, sub),
            matrix_block(way, event, k + 1, sub),
            r.ring_send.at[0],
            r.ring_recv.at[event, sub],
            toward(way),
        )

    def slab_copy(offset):
        return remote(
            r.matrix.at[0, slab_rows(me_y), on_grid],
            r.matrix.at[columns - offset, slab_rows(me_y), on_grid],
            r.slab_send.at[0],
            r.slab_recv.at[0],
            {"tp": column(offset)},
        )

    def grid_view(way, event, y):
        blocks_of = pl.ds(1, half) if (event % 2) ^ way == 0 else pl.ds(1 + half, half - 1)
        return r.matrix.at[blocks_of, slab_rows(y), on_grid]

    def grid_ring(way, event, y):
        here = grid_view(way, event, y)
        return remote(
            here, here, r.grid_send.at[0], r.grid_recv.at[event], peer(1) if way == 0 else peer(chips - 1)
        )

    def to_mate(here, which):
        return remote(here, here, r.pass_send.at[which], r.pass_recv.at[which], mate)

    most_columns, other_blocks = pl.ds(0, columns - 1), pl.ds(1, columns - 1)
    ring_total = r.matrix.at[other_blocks, pl.ds(0, rows), on_ring]
    grid_total = r.matrix.at[other_blocks, pl.ds(0, (chips - 1) * slab), on_grid]
    slab_total = r.matrix.at[other_blocks, pl.ds(0, slab), on_grid]
    pass_totals = (ring_total, r.matrix.at[other_blocks, pl.ds(0, rows), on_grid])

    for load in loads[2:4]:
        load.wait()
    rims = [
        remote(
            r.value_in.at[pl.ds(2 * positions, rim_rows), :],
            r.value_in.at[pl.ds(0, rim_rows), :],
            r.rim_send.at[0],
            r.rim_recv.at[0],
            following,
        ),
        remote(
            r.keys_in.at[pl.ds(positions, rim_rows), :],
            r.keys_in.at[pl.ds(0, rim_rows), :],
            r.rim_send.at[1],
            r.rim_recv.at[1],
            following,
        ),
    ]
    for rim in rims:
        rim.start()

    def table_copy(offset):
        here = r.tables.at[me_x]
        return remote(here, here, r.table_send.at[0], r.table_recv.at[0], {"tp": column(offset)})

    for i in range(1, columns):
        table_copy(i).start()
    for i in range(1, columns):
        slab_copy(i).start()
    for event in range(min(2, columns - 1)):
        for sub in range(2):
            for way in range(2):
                matrix_ring(way, event, sub).start()
    tables_total = remote(
        r.tables.at[most_columns], r.tables.at[most_columns], r.table_send.at[0], r.table_recv.at[0], right
    )

    def serve_ring(event):
        for sub in range(2):
            both = r.matrix.at[0, pl.ds(0, rows // 2), on_ring]
            remote(both, both, r.ring_send.at[0], r.ring_recv.at[event, sub], right).wait_recv()
            for way in range(2):
                if event + 2 < columns - 1:
                    matrix_ring(way, event + 2, sub).start()
                to_mate(matrix_block(way, event, event // 2 + 1, sub), 0).start()

    def serve_slab():
        remote(slab_total, slab_total, r.slab_send.at[0], r.slab_recv.at[0], right).wait_recv()
        for event in range(2):
            for way in range(2):
                if event < chips - 1:
                    grid_ring(way, event, me_y).start()
        to_mate(r.matrix.at[other_blocks, slab_rows(me_y), on_grid], 1).start()

    def serve_grid(event):
        k = event // 2 + 1
        remote(slab_total, slab_total, r.grid_send.at[0], r.grid_recv.at[event], right).wait_recv()
        for way in range(2):
            y = lax.rem(me_y + (chips - k if way == 0 else k), chips)
            if event + 2 < chips - 1:
                grid_ring(way, event + 2, y).start()
            to_mate(grid_view(way, event, y), 1).start()

    waiting = [("x", e) for e in range(columns - 1)] + [("y", e) for e in range(chips - 1)]

    def serve(*steps):
        for step in steps:
            if step in waiting:
                waiting.remove(step)
                (serve_ring if step[0] == "x" else serve_grid)(step[1])

    for load in loads[4:]:
        load.start()
    for t in range(dims.tiles):
        span = pl.ds(t * 128, 128)
        for n, weight in enumerate((r.expert_gate_hbm, r.expert_up_hbm)):
            pltpu.make_async_copy(
                weight.at[0, :, span], r.gate_up.at[t, :, pl.ds(n * 128, 128)], r.weight_sem.at[0]
            ).start()
    for p in range(dims.pieces):
        pltpu.make_async_copy(
            r.expert_down_hbm.at[0, :, pl.ds(p * PIECE, PIECE)], r.down.at[p], r.weight_sem.at[1]
        ).start()

    for name in dims.small:
        if name not in ("choice_small", "share_small"):
            small[name].wait()
    for g in range(2):
        raw = r.raw_ref[g].astype(f32)
        for k in range(blocks):
            r.stride_s[HEADS * k + 2 * g : HEADS * k + 2 * g + 2, :] = raw[:, k * rows : (k + 1) * rows]
    for k in range(blocks):
        r.run_s[HEADS * k : HEADS * k + HEADS, :] = jnp.broadcast_to(r.extra_ref[k : k + 1, :], (HEADS, rows))
    head_of = jnp.bitwise_and(lax.broadcasted_iota(jnp.int32, (HEADS * blocks, rows), 0), HEADS - 1)

    def by_head(table):
        picked = jnp.full((HEADS * blocks, rows), table[1, 1], f32)
        for n in range(3):
            picked = jnp.where(head_of == n, table[n // 2, n % 2], picked)
        return picked

    shifted = r.stride_s[...] + by_head(r.bias_ref)
    stride = jnp.maximum(shifted, 0.0) + jnp.log1p(jnp.exp(-jnp.abs(shifted)))
    log_decay = r.run_s[...] - jnp.exp(by_head(r.log_ref)) * stride
    at_row = lax.broadcasted_iota(jnp.int32, (rows, rows), 0)
    at_lane = lax.broadcasted_iota(jnp.int32, (rows, rows), 1)
    running = jnp.dot(
        log_decay,
        jnp.where(at_row <= at_lane, 1.0, 0.0),
        preferred_element_type=f32,
        precision=lax.Precision.HIGHEST,
    )
    ends = jnp.broadcast_to(running[:, rows - 1 : rows], running.shape)
    r.stride_s[...] = stride
    r.run_s[...] = running
    r.fade_s[...] = jnp.exp(ends - running) * stride
    r.end_s[...] = jnp.exp(ends)
    turned = jnp.transpose(running)
    for k in range(blocks):
        r.cols_s[k, :, 0:HEADS] = turned[:, HEADS * k : HEADS * k + HEADS]

    first_head = at_lane < HEAD_DIM

    def row_pair(table, k, g):
        low = table[pl.ds(HEADS * k + 2 * g, 1), :]
        high = table[pl.ds(HEADS * k + 2 * g + 1, 1), :]
        return jnp.where(first_head[0:1], low, high)

    taps = r.value_tap_ref.shape[0] // 2
    value_tap = r.value_tap_ref[...].astype(f32)
    key_tap = r.key_tap_ref[...].astype(f32)
    even = jnp.bitwise_and(lax.broadcasted_iota(jnp.int32, (2 * rows, rows), 0), 1) == 0
    tap_rows = [jnp.where(even, value_tap[2 * j : 2 * j + 1], value_tap[2 * j + 1 : 2 * j + 2]) for j in range(taps)]

    def states_of(k):
        window = r.value_in[pl.ds(pl.multiple_of(k * 2 * rows, 2 * rows), 2 * rows + rim_rows), :].astype(f32)
        total = jnp.zeros((2 * rows, rows), f32)
        for j in range(taps):
            start = rim_rows - 2 * (taps - 1 - j)
            total = total + window[start : start + 2 * rows] * tap_rows[j]
        r.conv_wide[...] = silu(total).astype(bf16).astype(f32)
        window = r.keys_in[pl.ds(pl.multiple_of(k * rows, rows), rows + rim_rows), :].astype(f32)
        total = jnp.zeros((rows, r.keys_in.shape[1]), f32)
        for j in range(taps):
            start = rim_rows - (taps - 1 - j)
            total = total + window[start : start + rows] * key_tap[j : j + 1]
        conv = silu(total).astype(bf16).astype(f32)
        both = conv[:, 0 : 2 * STATE_ONE]
        keys = [jnp.where(first_head, both, 0.0), conv[:, 2 * STATE_ONE : 2 * STATE_ONE + STATE_TWO]]
        asks = [pltpu.roll(both, STATE_ONE, 1), conv[:, 2 * STATE_ONE + STATE_TWO :]]
        for g in range(2):
            x = r.conv_wide[pl.ds(g, rows, stride=2), :].astype(bf16)
            key_t = jnp.transpose(keys[g])
            r.x_s[k, g] = x
            r.kt_s[k, g] = key_t.astype(bf16)
            r.q_s[k, g] = asks[g].astype(bf16)
            faded = jnp.concatenate(
                [key_t * r.fade_s[pl.ds(HEADS * k + 2 * g + h, 1), :] for h in range(2)], axis=0
            ).astype(bf16)
            state = jnp.dot(faded, x, preferred_element_type=f32)
            r.state_s[k, g] = jnp.where(first_head, state[:rows], state[rows:])

    def state_step(i, carry):
        states_of(i)
        return carry

    lax.fori_loop(1, blocks, state_step, 0)
    for rim in rims:
        rim.wait_recv()
    opening = me_s == 0
    for table in (r.value_in, r.keys_in):
        table[0:rim_rows, :] = jnp.where(opening, 0.0, table[0:rim_rows, :].astype(f32)).astype(bf16)
    states_of(0)

    packed = STATE_TWO + STATE_ONE
    piece = packed // 2

    def local_end(g):
        total = jnp.zeros((rows, rows), f32)
        faded = jnp.ones((1, rows), f32)
        for k in range(blocks):
            decay = row_pair(r.end_s, k, g)
            total = total * decay + r.state_s[k, g]
            faded = faded * decay
        return total, faded

    end_one, fade_one = local_end(0)
    end_two, fade_two = local_end(1)
    own = jnp.concatenate([end_two, end_one[:STATE_ONE]], axis=0)
    r.own_pack[...] = own.astype(bf16)
    r.own_fade[0:1, :] = fade_one
    r.own_fade[1:2, :] = fade_two
    r.own_fade[2:8, :] = jnp.zeros((6, rows), f32)
    mates = [
        remote(r.own_pack, r.mate_pack, r.mate_send.at[0], r.mate_recv.at[0], mate),
        remote(r.own_fade, r.mate_fade, r.mate_send.at[1], r.mate_recv.at[1], mate),
    ]
    for copy in mates:
        copy.start()
    for copy in mates:
        copy.wait_recv()
    is_low = core == 0
    low = jnp.where(is_low, own, r.mate_pack[...].astype(f32))
    high = jnp.where(is_low, r.mate_pack[...].astype(f32), own)
    mate_rows = r.mate_fade[...]
    own_rows = r.own_fade[...]
    high_rows = jnp.where(is_low, mate_rows, own_rows)
    in_two = lax.broadcasted_iota(jnp.int32, (packed, rows), 0) < STATE_TWO
    r.chip_pack[...] = (low * jnp.where(in_two, high_rows[1:2], high_rows[0:1]) + high).astype(bf16)
    r.chip_fade[...] = own_rows * mate_rows
    my_half = pl.ds(pl.multiple_of(core * piece, 16), piece)

    def to_chip(n, which):
        src = r.chip_pack.at[my_half, :] if which == 0 else r.chip_fade
        dst = r.all_pack.at[me_y] if which == 0 else r.all_fade.at[me_y]
        return remote(src, dst, r.chip_send.at[n], r.chip_recv.at[n], peer(n))

    def chip_total(n):
        sent = r.own_pack.at[pl.ds(0, piece + 16), :]
        return remote(sent, sent, r.chip_send.at[n], r.chip_recv.at[n], peer(n))

    for n in range(1, chips):

        @pl.when(me_y + n < chips)
        def _():
            for which in range(2):
                to_chip(n, which).start()


    below = at_row >= at_lane

    def near_step(k, carry):
        cols = r.cols_s[k]
        for g in range(2):
            scores = jnp.dot(r.q_s[k, g], r.kt_s[k, g], preferred_element_type=f32)
            parts = []
            for h in range(2):
                n = 2 * g + h
                gap = cols[:, n : n + 1] - r.run_s[pl.ds(HEADS * k + n, 1), :]
                damping = jnp.exp(jnp.where(below, gap, -1e30))
                parts.append((scores * damping * r.stride_s[pl.ds(HEADS * k + n, 1), :]).astype(bf16))
            near = jnp.dot(jnp.concatenate(parts, axis=0), r.x_s[k, g], preferred_element_type=f32)
            r.near_s[k, g] = jnp.where(first_head, near[:rows], near[rows:])
        return carry

    lax.fori_loop(0, blocks, near_step, 0)
    serve_slab()
    serve(*dims.serving[0])
    main, over, slots = dims.main, dims.over, places * dims.main
    total_slots = slots + over
    slot_row = lax.broadcasted_iota(jnp.int32, (total_slots, over), 0)
    slot_expert = lax.broadcasted_iota(jnp.int32, (total_slots, over), 1)
    spread = jnp.where(
        ((slot_row < slots) & (slot_row >= slot_expert * main) & (slot_row < slot_expert * main + main))
        | (slot_row == slots + slot_expert),
        1.0,
        0.0,
    ).astype(bf16)
    at = lax.broadcasted_iota(jnp.int32, (total_slots, rows), 0)
    turn = jnp.where(at < slots, jnp.bitwise_and(at, main - 1), main).astype(f32)
    expert_at = lax.broadcasted_iota(jnp.int32, (over, rows), 0).astype(f32)
    earlier = jnp.where(at_row < at_lane, 1.0, 0.0).astype(bf16)

    def make_put(col):
        table = r.tables[col]
        named = jnp.where((expert_at == table[0:1]) | (expert_at == table[1:2]), 1.0, 0.0)
        rank = jnp.dot(named.astype(bf16), earlier, preferred_element_type=f32)
        named_x = jnp.dot(spread, named.astype(bf16), preferred_element_type=f32)
        rank_x = jnp.dot(spread, rank.astype(bf16), preferred_element_type=f32)
        r.put[col] = jnp.where(rank_x == turn, named_x, 0.0).astype(bf16)

    tables_total.wait_recv()

    def put_step(col, carry):
        make_put(col)
        return carry

    lax.fori_loop(0, columns, put_step, 0)

    for load in loads[-2:]:
        load.wait()
    serve(*dims.serving[1])
    for n in range(1, chips):

        @pl.when(me_y >= n)
        def _():
            chip_total(n).wait_recv()

    row_at = lax.broadcasted_iota(jnp.int32, (piece, rows), 0) + core * piece
    half_two = row_at < STATE_TWO
    entering = jnp.zeros((piece, rows), f32)
    for y in range(chips):
        fades = r.all_fade[y]
        later = entering * jnp.where(half_two, fades[1:2], fades[0:1]) + r.all_pack[y].astype(f32)
        entering = jnp.where(y < me_y, later, entering)
    r.enter_pack[my_half, :] = entering.astype(bf16)
    here = r.enter_pack.at[my_half, :]
    enter_copy = remote(here, here, r.enter_send.at[0], r.enter_recv.at[0], mate)
    enter_copy.start()
    enter_copy.wait_recv()
    chip_state = r.enter_pack[...].astype(f32)
    after_low = chip_state * jnp.where(in_two, mate_rows[1:2], mate_rows[0:1]) + r.mate_pack[...].astype(f32)
    entered = jnp.where(is_low, chip_state, after_low)
    r.carry_s[1] = entered[:STATE_TWO]
    r.carry_s[0] = jnp.zeros((rows, rows), f32)
    r.carry_s[0, 0:STATE_ONE, :] = entered[STATE_TWO:]

    serve(*dims.serving[2])
    def head_copy(col):
        return remote(r.mixed_s.at[col], r.heads_in.at[me_x], r.head_send.at[0], r.head_recv.at[0], {"tp": col})

    def mix_step(k, carry):
        cols = jnp.exp(r.cols_s[k])
        r.gate_wide[...] = r.gate_in[pl.ds(pl.multiple_of(k * 2 * rows, 2 * rows), 2 * rows), :].astype(f32)
        for g in range(2):
            state = r.carry_s[g]
            coarse = state.astype(bf16)
            fine = (state - coarse.astype(f32)).astype(bf16)
            ask = r.q_s[k, g]
            far = jnp.dot(
                jnp.concatenate([ask, ask], axis=1),
                jnp.concatenate([coarse, fine], axis=0),
                preferred_element_type=f32,
            )
            reach = jnp.where(first_head, cols[:, 2 * g : 2 * g + 1], cols[:, 2 * g + 1 : 2 * g + 2])
            skip = jnp.where(first_head[0:1], r.skip_ref[g, 0], r.skip_ref[g, 1])
            mixed = r.near_s[k, g] + far * reach + skip * r.x_s[k, g].astype(f32)
            gated = mixed * silu(r.gate_wide[pl.ds(g, rows, stride=2), :])
            square = gated * gated
            one = jnp.sum(jnp.where(first_head, square, 0.0), axis=1, keepdims=True)
            two = jnp.sum(jnp.where(first_head, 0.0, square), axis=1, keepdims=True)
            scale = lax.rsqrt(jnp.where(first_head, one, two) * (1.0 / HEAD_DIM) + EPSILON)
            r.mixed_s[k, :, g * rows : (g + 1) * rows] = (gated * scale * r.head_gain_ref[g : g + 1, :]).astype(bf16)
            r.carry_s[g] = state * row_pair(r.end_s, k, g) + r.state_s[k, g]

        @pl.when(k != me_x)
        def _():
            head_copy(k).start()

        return carry

    lax.fori_loop(0, blocks, mix_step, 0)
    r.heads_in[me_x] = r.mixed_s[me_x]

    slot_col = lax.broadcasted_iota(jnp.int32, (over, total_slots), 1)
    slot_exp = lax.broadcasted_iota(jnp.int32, (over, total_slots), 0)
    spread_t = jnp.where(
        ((slot_col < slots) & (slot_col >= slot_exp * main) & (slot_col < slot_exp * main + main))
        | (slot_col == slots + slot_exp),
        1.0,
        0.0,
    ).astype(bf16)
    at_t = lax.broadcasted_iota(jnp.int32, (rows, total_slots), 1)
    turn_t = jnp.where(at_t < slots, jnp.bitwise_and(at_t, main - 1), main).astype(f32)
    expert_to = lax.broadcasted_iota(jnp.int32, (rows, over), 1).astype(f32)
    later_t = jnp.where(at_lane < at_row, 1.0, 0.0).astype(bf16)

    def make_pick(col):
        table = jnp.transpose(r.tables[col])
        named = [jnp.where(expert_to == table[:, k : k + 1], 1.0, 0.0) for k in range(2)]
        rank = jnp.dot(later_t, (named[0] + named[1]).astype(bf16), preferred_element_type=f32)
        rank_x = jnp.dot(rank.astype(bf16), spread_t, preferred_element_type=f32)
        for k in range(2):
            named_x = jnp.dot(named[k].astype(bf16), spread_t, preferred_element_type=f32)
            r.pick[col, k] = jnp.where(rank_x == turn_t, named_x, 0.0).astype(bf16)
            r.share_s[col, k] = jnp.broadcast_to(table[:, 2 + k : 3 + k], (rows, rows))

    def product(block, low, high, first):
        for n in range(low, high, 512):
            span = slice(n, min(n + 512, high))
            part = jnp.dot(r.heads_in[column(block)], r.matrix[block, :, span], preferred_element_type=f32)
            r.acc_s[:, span] = part if first else r.acc_s[:, span] + part

    serve(*dims.serving[3])
    serve(*list(waiting))
    heads_total = remote(
        r.mixed_s.at[most_columns], r.heads_in.at[most_columns], r.head_send.at[0], r.head_recv.at[0], right
    )
    heads_total.wait_recv()
    for which, (low_lane, high_lane) in enumerate(((0, ring_part), (ring_part, width))):
        remote(pass_totals[which], pass_totals[which], r.pass_send.at[which], r.pass_recv.at[which], mate).wait_recv()
        for block in range(columns):
            product(block, low_lane, high_lane, block == 0)

    stream = (r.residual_in[...].astype(f32) + r.acc_s[...]).astype(bf16)
    r.stream_s[...] = stream
    wide = stream.astype(f32)
    scale = lax.rsqrt(jnp.mean(wide * wide, axis=1, keepdims=True) + EPSILON)
    normed = (wide * scale * r.expert_gain_ref[...]).astype(bf16)

    direct, extra = dims.direct, dims.pieces - dims.direct
    pieces = dims.pieces
    lanes_of = PIECE // 128

    def lines(index):
        return pl.ds(pl.multiple_of(index * main, main), main)

    def far(way, p):
        odd = lax.rem(p, 2) if not isinstance(p, int) else p % 2
        return half - odd if way == 0 else half - 1 + odd

    for q in range(extra):
        r.tokens[me_x, q] = normed[:, (direct + q) * PIECE : (direct + q + 1) * PIECE]

    thin = extra * lanes_of

    def token_ring(way, step, q, col):
        here = r.tokens.at[col, q // lanes_of, :, pl.ds(q % lanes_of * 128, 128)]
        return remote(here, here, r.token_send.at[0], r.token_recv.at[step, q], toward(way))

    put_own = r.put[me_x]

    def make_out(p):
        part = jnp.dot(put_own, normed[:, p * PIECE : (p + 1) * PIECE], preferred_element_type=f32)
        r.outbound[p] = part[:slots].astype(bf16)
        for c in range(lanes_of):
            r.over_out[:, p * lanes_of + c, :] = part[slots:, c * 128 : (c + 1) * 128]

    def send_out(p, carry):
        for i in range(1, places):
            remote(
                r.outbound.at[p, lines(place(i)), :],
                r.chunks.at[me_x, p, lines(me_s), :],
                r.out_send.at[0],
                r.out_recv.at[p],
                {"sp": place(i)},
            ).start()
        r.chunks[me_x, p, lines(me_s), :] = r.outbound[p, lines(me_s), :]
        return carry

    make_out(0)
    send_out(0, 0)
    for q in range(thin):
        for way in range(2):
            token_ring(way, 0, q, me_x).start()
    for p in range(1, direct):
        make_out(p)
    lax.fori_loop(1, direct, send_out, 0)
    for i in range(1, places):
        remote(
            r.over_out.at[place(i)], r.over_in.at[me_s], r.over_send.at[0], r.over_recv.at[0], {"sp": place(i)}
        ).start()
    r.over_in[me_s] = r.over_out[me_s]
    if places < over:
        r.over_in[places:over] = jnp.zeros((over - places, *r.over_in.shape[1:]), f32)
        r.over_ret[:, places:over] = jnp.zeros((2, over - places, *r.over_ret.shape[2:]), f32)
        r.xover_in[:, places:over] = jnp.zeros((columns, over - places, *r.xover_in.shape[2:]), f32)
        r.xover_ret[:, places:over] = jnp.zeros((columns, over - places, *r.xover_ret.shape[2:]), f32)

    def route(offset):
        col = column(offset)
        for q in range(extra):
            part = jnp.dot(r.put[col], r.tokens[col, q], preferred_element_type=f32)
            r.xout[col, q] = part[:slots].astype(bf16)
            r.chunks[col, direct + q, lines(me_s), :] = r.xout[col, q, lines(me_s), :]
            for c in range(lanes_of):
                r.xover_out[offset, :, q * lanes_of + c, :] = part[slots:, c * 128 : (c + 1) * 128]
        r.xover_in[offset, me_s] = r.xover_out[offset, me_s]
        for i in range(1, places):
            remote(
                r.xout.at[col, :, lines(place(i)), :],
                r.chunks.at[col, pl.ds(direct, extra), lines(me_s), :],
                r.xout_send.at[0],
                r.xout_recv.at[offset],
                {"sp": place(i)},
            ).start()
            remote(
                r.xover_out.at[offset, place(i)],
                r.xover_in.at[offset, me_s],
                r.xover_send.at[0],
                r.xover_recv.at[0, offset],
                {"sp": place(i)},
            ).start()

    def routed(offset):
        col = column(offset)
        most = pl.ds(0, (places - 1) * main)
        return (
            remote(
                r.xout.at[col, :, most, :],
                r.chunks.at[col, pl.ds(direct, extra), most, :],
                r.xout_send.at[0],
                r.xout_recv.at[offset],
                right,
            ),
            remote(
                r.xover_out.at[offset, 0 : places - 1],
                r.xover_in.at[offset, 0 : places - 1],
                r.xover_send.at[0],
                r.xover_recv.at[0, offset],
                right,
            ),
        )

    def take_routed(offset):
        col = column(offset)
        for copy in routed(offset):
            copy.wait_recv()
        for q in range(extra):
            for c in range(lanes_of):
                r.chunks[col, direct + q, slots:, c * 128 : (c + 1) * 128] = r.xover_in[
                    offset, :, q * lanes_of + c, :
                ].astype(bf16)

    def token_event(k):
        for q in range(thin):
            came = r.tokens.at[pl.ds(0, 2 if k < half else 1), 0, :, pl.ds(0, 128)]
            remote(came, came, r.token_send.at[0], r.token_recv.at[k - 1, q], right).wait_recv()
            for way in range(2):
                if k < far(way, q):
                    token_ring(way, k, q, column(-k if way == 0 else k)).start()

    def chunk_ring(way, step, p, col):
        here = r.chunks.at[col, p, pl.ds(0, slots), :]
        return remote(here, here, r.chunk_send.at[0], r.chunk_recv.at[step, p], toward(way))

    def over_ring(way, step, col):
        here = r.chunks.at[col, pl.ds(0, direct), pl.ds(slots, over), :]
        return remote(here, here, r.tail_send.at[0], r.tail_recv.at[step], toward(way))

    def out_arrived(p):
        most = pl.ds(0, (places - 1) * main)
        return remote(
            r.outbound.at[p, most, :], r.chunks.at[me_x, p, most, :], r.out_send.at[0], r.out_recv.at[p], right
        )

    def start_piece(p):
        out_arrived(p).wait_recv()
        chunk_ring(0, 0, p, me_x).start()
        chunk_ring(1, 0, p, me_x).start()

    def start_over():
        remote(
            r.over_out.at[0 : places - 1], r.over_in.at[0 : places - 1], r.over_send.at[0], r.over_recv.at[0], right
        ).wait_recv()
        for c in range(direct * lanes_of):
            at_lanes = (c % lanes_of) * 128
            r.chunks[me_x, c // lanes_of, slots:, at_lanes : at_lanes + 128] = r.over_in[:, c, :].astype(bf16)
        for way in range(2):
            over_ring(way, 0, me_x).start()

    for copy in rims + mates + [enter_copy]:
        copy.wait_send()
    for n in range(1, chips):

        @pl.when(me_y + n < chips)
        def _():
            chip_total(n).wait_send()

    heads_total.wait_send()
    tables_total.wait_send()
    remote(ring_total, ring_total, r.ring_send.at[0], r.ring_recv.at[0, 0], right).wait_send()
    remote(slab_total, slab_total, r.slab_send.at[0], r.slab_recv.at[0], right).wait_send()
    remote(grid_total, grid_total, r.grid_send.at[0], r.grid_recv.at[0], right).wait_send()
    for which in range(2):
        view = pass_totals[which]
        remote(view, view, r.pass_send.at[which], r.pass_recv.at[which], mate).wait_send()

    def offset_of(n):
        k = (n + 1) // 2 if isinstance(n, int) else lax.div(n + 1, 2)
        if isinstance(n, int):
            return (columns - k) % columns if n % 2 else k
        return jnp.where(lax.rem(n, 2) == 1, lax.rem(columns - k, columns), k)

    opening = {"token": token_event, "piece": start_piece, "route": lambda n: route(offset_of(n)), "over": lambda n: start_over()}
    for kind, n in dims.opening:
        opening[kind](n)

    def unit(n, t):
        offset = offset_of(n)
        col = column(offset)
        pl.when(t == 0)(lambda: take_routed(offset))
        acc = jnp.dot(r.chunks[col, 0], r.gate_up[t, 0:PIECE, :], preferred_element_type=f32)
        for q in range(1, pieces):
            acc = acc + jnp.dot(
                r.chunks[col, q], r.gate_up[t, q * PIECE : (q + 1) * PIECE, :], preferred_element_type=f32
            )
        value = silu(acc[:, 0:128]) * acc[:, 128:256]
        r.hidden[col, :, pl.ds(pl.multiple_of(t * 128, 128), 128)] = value.astype(bf16)
        pl.when(t == dims.tiles - 1)(lambda: give_back(offset))

    def own(col, p):
        return jnp.dot(r.hidden[col], r.down[p], preferred_element_type=f32)

    def give_back(offset):
        col = column(offset)
        for q in range(extra):
            part = own(col, direct + q)
            r.xback[col, q] = part[:slots].astype(bf16)
            r.xret[col, q, lines(me_s), :] = r.xback[col, q, lines(me_s), :]
            for c in range(lanes_of):
                r.xover_back[offset, :, q * lanes_of + c, :] = part[slots:, c * 128 : (c + 1) * 128]
        r.xover_ret[offset, me_s] = r.xover_back[offset, me_s]
        for i in range(1, places):
            remote(
                r.xback.at[col, :, lines(place(i)), :],
                r.xret.at[col, :, lines(me_s), :],
                r.xback_send.at[0],
                r.xback_recv.at[offset],
                {"sp": place(i)},
            ).start()
            remote(
                r.xover_back.at[offset, place(i)],
                r.xover_ret.at[offset, me_s],
                r.xover_send.at[1],
                r.xover_recv.at[1, offset],
                {"sp": place(i)},
            ).start()

    def given_back(offset):
        col = column(offset)
        most = pl.ds(0, (places - 1) * main)
        return (
            remote(
                r.xback.at[col, :, most, :],
                r.xret.at[col, :, most, :],
                r.xback_send.at[0],
                r.xback_recv.at[offset],
                right,
            ),
            remote(
                r.xover_back.at[offset, 0 : places - 1],
                r.xover_ret.at[offset, 0 : places - 1],
                r.xover_send.at[1],
                r.xover_recv.at[1, offset],
                right,
            ),
        )

    for n, weights in enumerate((r.gate_up, r.down)):
        pltpu.make_async_copy(weights, weights, r.weight_sem.at[n]).wait()

    def units(low, high):
        def body(v, carry):
            unit(lax.div(v, dims.tiles), lax.rem(v, dims.tiles))
            return carry

        lax.fori_loop(low, high, body, 0)

    def hop(way, j, p):
        return remote(
            r.sums.at[way, j, p],
            r.sums.at[way, j - 1, p],
            r.sum_send.at[0],
            r.sum_recv.at[way, j - 1, p],
            {"tp": column(1 - 2 * way)},
        )

    def chains(long, step, group):
        j = half - step if long else half - 1 - step

        def body(p, carry):
            odd = lax.rem(p, 2)
            way = 1 - odd if long else odd
            value = own(column(j * (1 - 2 * way)), p)
            if step > 0:
                hop(way, j + 1, p).wait_recv()
                value = value + r.sums[way, j, p].astype(f32)
            r.sums[way, j, p] = value.astype(bf16)
            hop(way, j, p).start()
            return carry

        lax.fori_loop(*group, body, 0)

    share_of = dims.schedule
    for k in range(1, half + 1):
        first, last = share_of[k - 1] * dims.tiles, share_of[k] * dims.tiles

        if k == half and half > 1:
            units(first, last)
            first = last
            for group in dims.groups:
                chains(False, 0, group)

        def pass_on(p, carry, k=k, first=first, last=last):
            came = r.chunks.at[pl.ds(0, 2 if k < half else 1), p, pl.ds(0, slots), :]
            remote(came, came, r.chunk_send.at[0], r.chunk_recv.at[k - 1, p], right).wait_recv()
            if k < half:
                for way in range(2):
                    start = lambda way=way: chunk_ring(way, k, p, column(-k if way == 0 else k)).start()
                    if k < half - 1:
                        start()
                    else:
                        pl.when(k < far(way, p))(start)

            if k == 1 and dims.routed < columns:
                pl.when(p < columns - dims.routed)(lambda: route(offset_of(p + dims.routed)))
            if last > first:
                units(
                    first + lax.div(p * (last - first), direct), first + lax.div((p + 1) * (last - first), direct)
                )
            return carry

        lax.fori_loop(0, direct, pass_on, 0)
        came = r.chunks.at[pl.ds(0, 2 if k < half else 1), pl.ds(0, direct), pl.ds(slots, over), :]
        remote(came, came, r.tail_send.at[0], r.tail_recv.at[k - 1], right).wait_recv()
        for way in range(2):
            if k < far(way, 0):
                over_ring(way, k, column(-k if way == 0 else k)).start()
        if k == 1:
            lax.fori_loop(0, columns, lambda col, carry: (make_pick(col), carry)[1], 0)
    units(share_of[half] * dims.tiles, columns * dims.tiles)

    def finish(p, carry):
        value = own(me_x, p)
        hop(0, 1, p).wait_recv()
        hop(1, 1, p).wait_recv()
        value = value + r.sums[0, 0, p].astype(f32) + r.sums[1, 0, p].astype(f32)
        r.totals[p] = value[0:slots].astype(bf16)
        r.over_total[p] = value[slots:]
        r.returned[p, lines(me_s), :] = r.totals[p, lines(me_s), :]
        for i in range(1, places):
            remote(
                r.totals.at[p, lines(place(i)), :],
                r.returned.at[p, lines(me_s), :],
                r.back_send.at[0],
                r.back_recv.at[p],
                {"sp": place(i)},
            ).start()
        return carry

    def weighted(col, table):
        one = jnp.dot(r.pick[col, 0], table, preferred_element_type=f32)
        two = jnp.dot(r.pick[col, 1], table, preferred_element_type=f32)
        copies = one.shape[1] // 128
        first, second = (jnp.concatenate([r.share_s[col, k]] * copies, axis=1) for k in range(2))
        return first * one + second * two

    def take_back(offset):
        col = column(offset)
        for copy in given_back(offset):
            copy.wait_recv()
        for q in range(extra):
            for c in range(lanes_of):
                r.xret[col, q, slots:, c * 128 : (c + 1) * 128] = r.xover_ret[
                    offset, :, q * lanes_of + c, :
                ].astype(bf16)

    def token_hop(way, j, q):
        return remote(
            r.xsums.at[way, j, q],
            r.xsums.at[way, j - 1, q],
            r.xsum_send.at[0],
            r.xsum_recv.at[way, j - 1, q],
            toward(way),
        )

    taken = set()

    def thin_part(col, q):
        return weighted(col, r.xret[col, q // lanes_of, :, q % lanes_of * 128 : (q % lanes_of + 1) * 128])

    def token_round(t):
        for q in range(thin):
            for way in range(2):
                j = far(1 - way, q) - t
                if j < 1:
                    continue
                offset = j if way == 0 else columns - j
                if offset not in taken:
                    taken.add(offset)
                    take_back(offset)
                value = thin_part(column(offset), q)
                if t > 0:
                    token_hop(way, j + 1, q).wait_recv()
                    value = value + r.xsums[way, j, q].astype(f32)
                r.xsums[way, j, q] = value.astype(bf16)
                token_hop(way, j, q).start()

    for group in dims.groups:
        chains(True, 0, group)
    def left_by_now(view, send, recv):
        remote(view, view, send, recv, right).wait_send()

    most_places, most_lines = pl.ds(0, places - 1), pl.ds(0, (places - 1) * main)
    chunks_total = r.chunks.at[most_columns, pl.ds(0, direct), pl.ds(0, slots), :]
    left_by_now(r.over_out.at[most_places], r.over_send.at[0], r.over_recv.at[0])
    left_by_now(r.tokens.at[most_columns], r.token_send.at[0], r.token_recv.at[0, 0])
    left_by_now(r.chunks.at[most_columns, pl.ds(0, direct), pl.ds(slots, over), :], r.tail_send.at[0], r.tail_recv.at[0])
    left_by_now(chunks_total, r.chunk_send.at[0], r.chunk_recv.at[0, 0])
    left_by_now(r.outbound.at[:, most_lines, :], r.out_send.at[0], r.out_recv.at[0])
    left_by_now(r.xout.at[:, :, most_lines, :], r.xout_send.at[0], r.xout_recv.at[0])
    left_by_now(r.xover_out.at[:, most_places], r.xover_send.at[0], r.xover_recv.at[0, 0])
    def over_back_copy(n, to, at):
        return remote(
            r.over_back.at[n, to],
            r.over_ret.at[n, at],
            r.over_send.at[1],
            r.over_recv.at[1 + n],
            {"sp": to},
        )

    def send_over_back(n, group):
        for p in range(*group):
            for c in range(lanes_of):
                r.over_back[n, :, (p - group[0]) * lanes_of + c, :] = r.over_total[p, :, c * 128 : (c + 1) * 128]
        r.over_ret[n, me_s] = r.over_back[n, me_s]
        for i in range(1, places):
            over_back_copy(n, place(i), me_s).start()

    for kind, step, group in dims.closing:
        if kind == "short":
            chains(False, step, group)
        elif kind == "long":
            chains(True, step, group)
        elif kind == "token":
            token_round(step)
        else:
            lax.fori_loop(*group, finish, 0)
            send_over_back(dims.groups.index(group), group)
    left_by_now(r.xback.at[:, :, most_lines, :], r.xback_send.at[0], r.xback_recv.at[0])
    left_by_now(r.xover_back.at[:, most_places], r.xover_send.at[1], r.xover_recv.at[1, 0])
    left_by_now(r.chunks.at[most_columns, pl.ds(0, direct)], r.sum_send.at[0], r.sum_recv.at[0, 0, 0])
    token_round(half - 1)
    def back_arrived(p):
        most = pl.ds(0, (places - 1) * main)
        return remote(
            r.totals.at[p, most, :], r.returned.at[p, most, :], r.back_send.at[0], r.back_recv.at[p], right
        )

    def combine(p, carry):
        back_arrived(p).wait_recv()
        span = pl.ds(pl.multiple_of(p * PIECE, PIECE), PIECE)
        value = weighted(me_x, r.returned[p])
        r.out_ref[:, span] = (r.stream_s[:, span].astype(f32) + value).astype(bf16)
        return carry

    def combine_group(n, group):
        remote(
            r.over_back.at[n, 0 : places - 1],
            r.over_ret.at[n, 0 : places - 1],
            r.over_send.at[1],
            r.over_recv.at[1 + n],
            right,
        ).wait_recv()
        for p in range(*group):
            for c in range(lanes_of):
                r.returned[p, slots:, c * 128 : (c + 1) * 128] = r.over_ret[n, :, (p - group[0]) * lanes_of + c, :].astype(bf16)
        lax.fori_loop(*group, combine, 0)

    combine_group(dims.groups.index(dims.order[0]), dims.order[0])
    take_back(0)
    for q in range(thin):
        value = thin_part(me_x, q)
        for way in range(2):
            token_hop(way, 1, q).wait_recv()
            value = value + r.xsums[way, 0, q].astype(f32)
        span = slice(direct * PIECE + q * 128, direct * PIECE + (q + 1) * 128)
        r.out_ref[:, span] = (r.stream_s[:, span].astype(f32) + value).astype(bf16)

    combine_group(dims.groups.index(dims.order[1]), dims.order[1])

    left_by_now(r.over_back.at[:, most_places], r.over_send.at[1], r.over_recv.at[1])
    left_by_now(r.tokens.at[most_columns], r.xsum_send.at[0], r.xsum_recv.at[0, 0, 0])
    left_by_now(r.totals.at[:, most_lines, :], r.back_send.at[0], r.back_recv.at[0])


def layer(places, columns, **given):
    f32, bf16 = jnp.float32, jnp.bfloat16
    rows, width = given["residual_hbm"].shape
    small = [name for name in given if name.endswith("_small")]
    units = given["expert_gate_hbm"].shape[2]
    lanes = given["keys_hbm"].shape[1]
    positions = columns * BLOCK
    half, chips, blocks = columns // 2, places // 2, columns
    main = 2 * rows // places
    over = -(-places // 16) * 16
    pieces = width // PIECE
    extra = max(1, pieces // 4)
    direct = pieces - extra
    tiles, total = units // 128, places * main + over
    ring_part = width * RING_SHARE // 16 // 128 * 128
    schedule = (0, 0, 1, 5, 7) if half == 4 else (0,) * half + (columns - 1,)
    if half == 4:
        opening = [("token", 1), ("piece", 0), ("token", 2), ("piece", 1), ("piece", 2), ("token", 3), ("piece", 3)]
        opening += [("route", 0), ("piece", 4), ("token", 4), ("piece", 5), ("route", 1), ("route", 2), ("over", 0)]
    else:
        opening = [("token", n) for n in range(1, half + 1)] + [("piece", n) for n in range(direct)]
        opening += [("route", n) for n in range(columns)] + [("over", 0)]
    routed = sum(kind == "route" for kind, _ in opening)
    serving = [
        [("x", 0)],
        [("x", 1)],
        [("x", 2)],
        [("x", 3), ("y", 0), ("y", 1), ("y", 2), ("x", 4), ("y", 3), ("y", 4), ("y", 5), ("x", 5), ("x", 6), ("y", 6)],
    ]
    low, high = (0, (direct + 1) // 2), ((direct + 1) // 2, direct)
    groups = [high, low]
    if half == 4:
        closing = [
            ("long", 1, high),
            ("short", 1, high),
            ("long", 1, low),
            ("short", 1, low),
            ("long", 2, low),
            ("long", 2, high),
            ("long", 3, low),
            ("short", 2, low),
            ("token", 0, None),
            ("long", 3, high),
            ("short", 2, high),
            ("finish", None, low),
            ("token", 1, None),
            ("finish", None, high),
            ("token", 2, None),
        ]
    else:
        closing = []
        for step in range(1, half):
            closing += [("short", step, group) for group in groups if step < half - 1]
            closing += [("long", step, group) for group in groups]
            closing.append(("token", step - 1, None))
        closing += [("finish", None, group) for group in groups]
    dims = types.SimpleNamespace(
        places=places, columns=columns, width=width, main=main, over=over, pieces=pieces, direct=direct, tiles=tiles,
        schedule=schedule, opening=opening, routed=routed, small=small, groups=groups, order=(low, high), closing=closing, ring_part=ring_part, serving=serving,
    )
    packed = STATE_ONE + STATE_TWO
    square = (blocks, 2, BLOCK, BLOCK)
    vmem = lambda *shape, dtype=bf16: pltpu.VMEM(shape, dtype)
    dma = lambda *shape: pltpu.SemaphoreType.DMA(shape)
    in_specs = [pl.BlockSpec(memory_space=pltpu.SMEM if a.shape == (2, 2) else pl.ANY) for a in given.values()]
    lane_rows = PIECE // 128
    scratch = {name[:-5] + "ref": pltpu.VMEM(given[name].shape, given[name].dtype) for name in small}
    scratch |= dict(
        residual_in=vmem(rows, width),
        value_in=vmem(2 * positions + 16, BLOCK),
        gate_in=vmem(2 * positions, BLOCK),
        keys_in=vmem(positions + 16, lanes),
        gate_wide=vmem(2 * BLOCK, BLOCK, dtype=f32),
        conv_wide=vmem(2 * BLOCK, BLOCK, dtype=f32),
        x_s=vmem(*square),
        kt_s=vmem(*square),
        q_s=vmem(*square),
        state_s=vmem(*square, dtype=f32),
        near_s=vmem(*square, dtype=f32),
        stride_s=vmem(HEADS * blocks, BLOCK, dtype=f32),
        run_s=vmem(HEADS * blocks, BLOCK, dtype=f32),
        fade_s=vmem(HEADS * blocks, BLOCK, dtype=f32),
        end_s=vmem(HEADS * blocks, BLOCK, dtype=f32),
        cols_s=vmem(blocks, BLOCK, HEADS, dtype=f32),
        own_pack=vmem(packed, BLOCK),
        own_fade=vmem(8, BLOCK, dtype=f32),
        mate_pack=vmem(packed, BLOCK),
        mate_fade=vmem(8, BLOCK, dtype=f32),
        chip_pack=vmem(packed, BLOCK),
        chip_fade=vmem(8, BLOCK, dtype=f32),
        all_pack=vmem(chips, packed // 2, BLOCK),
        all_fade=vmem(chips, 8, BLOCK, dtype=f32),
        enter_pack=vmem(packed, BLOCK),
        carry_s=vmem(2, BLOCK, BLOCK, dtype=f32),
        mixed_s=vmem(columns, BLOCK, 2 * BLOCK),
        heads_in=vmem(columns, BLOCK, 2 * BLOCK),
        matrix=vmem(columns, 2 * BLOCK, width),
        acc_s=vmem(rows, width, dtype=f32),
        stream_s=vmem(rows, width),
        tables=vmem(columns, 8, rows, dtype=f32),
        put=vmem(columns, total, rows),
        pick=vmem(columns, 2, rows, total),
        share_s=vmem(columns, 2, rows, 128, dtype=f32),
        tokens=vmem(columns, extra, rows, PIECE),
        outbound=vmem(direct, places * main, PIECE),
        over_out=vmem(over, direct * lane_rows, 128, dtype=f32),
        over_in=vmem(over, direct * lane_rows, 128, dtype=f32),
        over_back=vmem(2, over, (high[1] - low[0] + 1) // 2 * lane_rows, 128, dtype=f32),
        over_ret=vmem(2, over, (high[1] - low[0] + 1) // 2 * lane_rows, 128, dtype=f32),
        over_total=vmem(direct, over, PIECE, dtype=f32),
        xout=vmem(columns, extra, places * main, PIECE),
        xback=vmem(columns, extra, places * main, PIECE),
        xret=vmem(columns, extra, total, PIECE),
        xover_out=vmem(columns, over, extra * lane_rows, 128, dtype=f32),
        xover_in=vmem(columns, over, extra * lane_rows, 128, dtype=f32),
        xover_back=vmem(columns, over, extra * lane_rows, 128, dtype=f32),
        xover_ret=vmem(columns, over, extra * lane_rows, 128, dtype=f32),
        chunks=vmem(columns, pieces, total, PIECE),
        hidden=vmem(columns, total, units),
        gate_up=vmem(tiles, width, 256),
        down=vmem(pieces, units, PIECE),
        sums=vmem(2, half + 1, direct, total, PIECE),
        xsums=vmem(2, half + 1, extra * lane_rows, rows, 128),
        totals=vmem(direct, places * main, PIECE),
        returned=vmem(direct, total, PIECE),
        load_sem=dma(6),
        weight_sem=dma(2),
        small_sem=dma(len(small)),
    )
    steps = (2, half)
    for name, send, recv in (
        ("rim", (2,), (2,)),
        ("mate", (2,), (2,)),
        ("chip", (chips,), (chips,)),
        ("enter", (1,), (1,)),
        ("head", (1,), (1,)),
        ("table", (1,), (1,)),
        ("ring", (1,), (columns - 1, 2)),
        ("slab", (1,), (1,)),
        ("grid", (1,), (chips - 1,)),
        ("pass", (2,), (2,)),
        ("over", (2,), (3,)),
        ("token", (1,), (half, extra * lane_rows)),
        ("out", (1,), (direct,)),
        ("xout", (1,), (columns,)),
        ("xover", (2,), (2, columns)),
        ("chunk", (1,), (half, direct)),
        ("tail", (1,), (half,)),
        ("xback", (1,), (columns,)),
        ("sum", (1,), (*steps, direct)),
        ("xsum", (1,), (*steps, extra * lane_rows)),
        ("back", (1,), (direct,)),
    ):
        scratch[name + "_send"], scratch[name + "_recv"] = dma(*send), dma(*recv)
    names = [*given, "out_ref", *scratch]
    return pl.pallas_call(
        functools.partial(layer_kernel, dims, names),
        out_shape=pltpu.VMEM((rows, width), bf16),
        in_specs=in_specs,
        out_specs=pl.BlockSpec(memory_space=pltpu.VMEM),
        scratch_shapes=list(scratch.values()),
        compiler_params=pltpu.CompilerParams(
            collective_id=0, has_side_effects=True, vmem_limit_bytes=VMEM_LIMIT
        ),
        name="layer",
    )(*given.values())


def local(
    residual,
    grouped_value_heads,
    output_gate_heads,
    projected_key_query,
    raw_step_size,
    step_size_bias,
    head_decay_logarithm,
    position_extra_decay,
    head_skip_weight,
    value_kernel_taps,
    key_query_kernel,
    head_norm_gain,
    output_matrix,
    expert_norm_gain,
    expert_gate_weight,
    expert_up_weight,
    expert_down_weight,
    token_expert_choice,
    expert_output_weight,
):
    return layer(
        lax.axis_size("sp"),
        lax.axis_size("tp"),
        residual_hbm=residual,
        value_hbm=grouped_value_heads.reshape(-1, BLOCK),
        gate_hbm=output_gate_heads.reshape(-1, BLOCK),
        keys_hbm=projected_key_query,
        raw_small=raw_step_size.transpose(1, 2, 0),
        bias_ref=step_size_bias,
        log_ref=head_decay_logarithm,
        extra_small=position_extra_decay.reshape(-1, BLOCK),
        skip_ref=head_skip_weight,
        value_tap_small=value_kernel_taps.reshape(-1, BLOCK),
        key_tap_small=key_query_kernel,
        head_gain_small=head_norm_gain,
        matrix_hbm=output_matrix,
        expert_gain_small=expert_norm_gain[None],
        choice_small=token_expert_choice.T,
        share_small=expert_output_weight.T,
        expert_gate_hbm=expert_gate_weight,
        expert_up_hbm=expert_up_weight,
        expert_down_hbm=expert_down_weight,
    )


def solution(mesh):
    placed = (
        P(("grp", "sp", "tp"), None),
        P(("grp", "sp"), None, "tp"),
        P(("grp", "sp"), None, "tp"),
        P(("grp", "sp"), None),
        P(("grp", "sp"), None, "tp"),
        P(None, "tp"),
        P(None, "tp"),
        P(("grp", "sp")),
        P(None, "tp"),
        P(None, None, "tp"),
        P(),
        P(None, "tp"),
        P(None, "tp", None),
        P(),
        P("sp", None, "tp"),
        P("sp", None, "tp"),
        P("sp", "tp", None),
        P(("grp", "sp", "tp"), None),
        P(("grp", "sp", "tp"), None),
    )
    return jax.shard_map(
        local, mesh=mesh, in_specs=placed, out_specs=P(("grp", "sp", "tp"), None), check_vma=False
    )
```
